512 devices in a mesh: ep: 32 (over z, x), tp: 16 (over y, core).
Axes of the slice: x: 4, y: 8, z: 8, core: 2. Of those that a mesh axis runs over, the one named last changes fastest.
Arguments:
- tokens: bfloat16 [256, 4096], P('ep', 'tp'), may hold values from -6 to 6
- norm_gain: float32 [4096], replicated, may hold values from 0.1 to 1.9
- route_experts: int32 [256, 2], P('ep'), may hold values from 0 to 63, all different within a row; in each aligned block of 8 rows (0 to 7, 8 to 15, ...) at most 2 rows name the same one
- route_logits: float32 [256, 2], P('ep'), may hold values from -4 to 4
- expert_gate: bfloat16 [64, 4096, 1024], P('ep', None, 'tp'), may hold values from -0.09375 to 0.09375
- expert_up: bfloat16 [64, 4096, 1024], P('ep', None, 'tp'), may hold values from -0.09375 to 0.09375
- expert_down: bfloat16 [64, 1024, 4096], P('ep', 'tp'), may hold values from -0.1875 to 0.1875
- dense_gate: bfloat16 [4096, 1024], P(None, 'tp'), may hold values from -0.09375 to 0.09375
- dense_up: bfloat16 [4096, 1024], P(None, 'tp'), may hold values from -0.09375 to 0.09375
- dense_down: bfloat16 [1024, 4096], P('tp'), may hold values from -0.1875 to 0.1875
- mix_weight: float32 [4096], replicated, may hold values from -0.09375 to 0.09375
- out_gain: float32 [4096], P('tp'), may hold values from 0.1 to 1.9
Outputs:
- result: bfloat16 [256, 4096], P('ep', 'tp')
The draws below stay inside these ranges and needn't reach their ends.
Inputs may be any that keep to these rules, and one draw needn't show every extreme that they name: `route_experts`: each row names 2 different experts; the 8 rows of one index of ep (aligned blocks) name any one expert at most 2 times, and some block names some expert exactly 2 times; every expert is named somewhere.
All inputs are finite; a program needn't handle non-finite values.
Results may differ from the reference program's by a relative error of at most 0.0025.
Values may be sent and summed in bfloat16 or wider, within the bound.
A program may use at most 64 MiB of HBM per device.

```python
import math
import jax
import jax.numpy as jnp
import numpy as np
from jax import lax

D = 4096
FFE = 1024
DENSE_FF = 1024
TOP = 2
CAP = 2
TOK_DEV = 8
EXPERTS = 64
TOKENS = 256
N_EP = 32


def levels(rng, dims, pieces, low, high):
    level = 1.0
    for dim, shards_of in pieces:
        draws = jax.random.uniform(jax.random.fold_in(jax.random.fold_in(rng, 6), dim), (shards_of,), jnp.float32, low / len(pieces), high / len(pieces))
        level = level * jnp.repeat(jnp.exp(draws), dims[dim] // shards_of).reshape((-1,) + (1,) * (len(dims) - 1 - dim))
    return level


def shared_out(key, own, number, rows, amount, top, reach, lean):
    sequence = jax.random.permutation(key, amount)
    crowded, usual = load_shares(amount, rows * top, reach, lean, True), load_shares(amount, rows * top, reach, lean, False)
    places = jnp.arange(amount)

    def named(tallies, offset_by):
        used = int((tallies > 0).sum())
        fixed = max(1, used // 4)
        shifted = fixed + (places - fixed + offset_by * (used - fixed)) % max(1, amount - fixed)
        return jnp.zeros((amount,), jnp.int32).at[sequence[jnp.where(places < fixed, places, shifted)]].set(jnp.asarray(tallies, jnp.int32))

    tallies = jnp.where(number % 4 == 0, named(crowded, number // 4), named(usual, number - number // 4 - 1))
    mixed = jax.random.permutation(jax.random.fold_in(own, 3), amount)
    donor, taker = mixed[0:amount // 2 * 2:2], mixed[1:amount // 2 * 2:2]
    margin = jnp.minimum(tallies[donor] - 1, reach - tallies[taker]) // 2
    margin = jnp.where((donor == sequence[0]) | (taker == sequence[0]) | (tallies[taker] == 0), 0, jnp.maximum(margin, 0))
    shifted = jax.random.randint(jax.random.fold_in(own, 4), (amount // 2,), 0, 1 << 20) % (margin + 1)
    tallies = tallies.at[donor].add(-shifted).at[taker].add(shifted)
    items = jnp.searchsorted(jnp.cumsum(tallies), jnp.arange(rows * top), side="right").astype(jnp.int32)
    table = items.reshape(top, rows).T
    table = table[jax.random.permutation(jax.random.fold_in(own, 1), rows)]
    offset_by = jax.random.randint(jax.random.fold_in(own, 2), (rows, 1), 0, top)
    return jnp.take_along_axis(table, (jnp.arange(top)[None, :] + offset_by) % top, axis=1)


def load_shares(number_of, total, reach, slope, full):
    loads = [(1 << 20) // math.isqrt(grade ** slope) + 1 for grade in range(1, number_of + 1)]
    largest = reach if full else min(reach, max(-(-total // number_of), total * loads[0] // sum(loads)))
    least = 1 if total - largest >= number_of - 1 else 0
    holding, surplus = [largest] + [least] * (number_of - 1), total - largest - least * (number_of - 1)
    while surplus > 0:
        free = [i for i in range(1, number_of) if holding[i] < largest] or [i for i in range(1, number_of) if holding[i] < reach]
        mass, remaining = sum([loads[i] for i in free]), surplus
        for i in free:
            addition = min(reach - holding[i], max(1, remaining * loads[i] // mass), surplus)
            holding[i] = holding[i] + addition
            surplus = surplus - addition
    return np.array(holding)


def centred(rng, dims, scale, limit, shards=(), held_as=jnp.bfloat16):
    result = jax.random.normal(rng, dims, jnp.float32) * scale
    if len(shards) > 0:
        result = levels(rng, dims, shards, -0.22, 0.18) * result
    return jnp.clip(result, min=-limit, max=limit).astype(held_as)


def setup_inputs(seed: int = 0) -> dict:
    seeds = jax.random.split(jax.random.key(seed), 13)
    tokens = centred(seeds[0], (TOKENS, D), 1.0, 6.0, ((0, 32), (1, 16)))
    norm_gain = jnp.clip(1.0 + 0.18 * jax.random.normal(seeds[1], (D,), jnp.float32), 0.1, 1.9)
    route_experts_keys = jax.random.split(jax.random.fold_in(seeds[2], 1), TOKENS // TOK_DEV)
    route_experts_turns = jax.random.permutation(jax.random.fold_in(seeds[2], 3), TOKENS // TOK_DEV)
    route_experts = jax.vmap(lambda own, number: shared_out(jax.random.fold_in(seeds[2], 2), own, number, TOK_DEV, EXPERTS, TOP, CAP, 2))(route_experts_keys, route_experts_turns).reshape((TOKENS, TOP))
    route_logits = centred(seeds[3], (TOKENS, TOP), 1.0, 4.0, ((0, 32),), jnp.float32)
    expert_gate = centred(seeds[4], (EXPERTS, D, FFE), D ** -0.5, 0.09375, ((0, 32), (2, 16)))
    expert_up = centred(seeds[5], (EXPERTS, D, FFE), D ** -0.5, 0.09375, ((0, 32), (2, 16)))
    expert_down = centred(seeds[6], (EXPERTS, FFE, D), FFE ** -0.5, 0.1875, ((0, 32), (1, 16)))
    dense_gate = centred(seeds[7], (D, DENSE_FF), D ** -0.5, 0.09375, ((1, 16),))
    dense_up = centred(seeds[8], (D, DENSE_FF), D ** -0.5, 0.09375, ((1, 16),))
    dense_down = centred(seeds[9], (DENSE_FF, D), DENSE_FF ** -0.5, 0.1875, ((0, 16),))
    mix_weight = centred(seeds[10], (D,), D ** -0.5, 0.09375, (), jnp.float32)
    out_gain = jnp.clip(1.0 + 0.18 * jax.random.normal(seeds[11], (D,), jnp.float32), 0.1, 1.9)
    return dict(tokens=tokens, norm_gain=norm_gain, route_experts=route_experts, route_logits=route_logits, expert_gate=expert_gate, expert_up=expert_up, expert_down=expert_down, dense_gate=dense_gate, dense_up=dense_up, dense_down=dense_down, mix_weight=mix_weight, out_gain=out_gain)


norm_eps = 1e-06

def reference(tokens, norm_gain, route_experts, route_logits, expert_gate, expert_up, expert_down, dense_gate, dense_up, dense_down, mix_weight, out_gain):
    values = tokens.astype(jnp.float32)
    normed = (values * lax.rsqrt(lax.optimization_barrier(jnp.mean(values * values, axis=1, keepdims=True)) + norm_eps) * norm_gain).astype(jnp.bfloat16)
    weights = jax.nn.softmax(route_logits, axis=-1)
    rows_cap = N_EP * CAP

    def per_expert(running, expert):
        route_hits = route_experts == expert
        routed = jnp.any(route_hits, axis=1)
        row_index = jnp.nonzero(routed, size=rows_cap, fill_value=0)[0].astype(jnp.int32)
        row_count = jnp.sum(routed.astype(jnp.int32))
        usable = (jnp.arange(rows_cap, dtype=jnp.int32) < row_count).astype(jnp.float32)
        picked = normed[row_index]
        gate_act = jnp.dot(picked, expert_gate[expert], preferred_element_type=jnp.float32)
        up_act = jnp.dot(picked, expert_up[expert], preferred_element_type=jnp.float32)
        hidden = (jax.nn.silu(gate_act) * up_act).astype(jnp.bfloat16)
        produced = jnp.dot(hidden, expert_down[expert], preferred_element_type=jnp.float32)
        factor = lax.optimization_barrier(jnp.sum(jnp.where(route_hits, weights, jnp.zeros_like(weights)), axis=1))[row_index] * usable
        return (running.at[row_index].add(factor[:, None] * produced), None)
    expert_mix, _ = lax.scan(per_expert, jnp.zeros((TOKENS, D), jnp.float32), jnp.arange(EXPERTS, dtype=jnp.int32))
    dense_hidden = (jax.nn.silu(jnp.dot(normed, dense_gate, preferred_element_type=jnp.float32)) * jnp.dot(normed, dense_up, preferred_element_type=jnp.float32)).astype(jnp.bfloat16)
    dense_out = jnp.dot(dense_hidden, dense_down, preferred_element_type=jnp.float32)
    mix_gate = jax.nn.sigmoid(jnp.dot(normed.astype(jnp.float32), mix_weight, precision=lax.Precision.HIGHEST))
    combined = expert_mix + mix_gate[:, None] * dense_out
    scaled = combined * lax.rsqrt(lax.optimization_barrier(jnp.mean(combined * combined, axis=1, keepdims=True)) + norm_eps) * out_gain
    return scaled.astype(jnp.bfloat16)
```

```python
import functools

import jax
import jax.numpy as jnp
from jax import lax
from jax.experimental import pallas as pl
from jax.experimental.pallas import tpu as pltpu
from jax.sharding import PartitionSpec as P

MESH = pl.DeviceIdType.MESH
F32 = jnp.float32
BF16 = jnp.bfloat16
EPS = 1e-06

NX, NZ, NY = 4, 8, 8
NEP = NX * NZ
NTP = 2 * NY
ROWS = 128
PART = 256
WIDTH = 4096


def rcopy(src, dst, send_sem, recv_sem, device):
    return pltpu.make_async_remote_copy(
        src_ref=src,
        dst_ref=dst,
        send_sem=send_sem,
        recv_sem=recv_sem,
        device_id=device,
        device_id_type=MESH,
    )


def nt_dot(a, b):
    return lax.dot_general(a, b, (((1,), (1,)), ((), ())), preferred_element_type=F32)


def silu(v):
    return v / (1.0 + jnp.exp(-v))


def kernel(
    tok,
    gain,
    routes,
    logits,
    wg,
    wu,
    wd,
    dg,
    du,
    dd,
    mixw,
    ogain,
    out,
    w_gu,
    wd_own,
    wd_par,
    w_dense,
    d_down,
    a2a_out,
    a2a_in,
    gathered,
    tok_all,
    dense_out,
    dense_in,
    comb,
    h_own,
    h_par,
    q_out,
    q_in,
    s_out,
    s_in,
    kept,
    ret_out,
    ret_in,
    sq_out,
    sq_in,
    ssq,
    gate_ref,
    w_sem,
    wp_ssem,
    wp_rsem,
    a2a_ssem,
    a2a_rsem,
    tok_ssem,
    tok_rsem,
    dense_ssem,
    dense_rsem,
    ag_ssem,
    ag_rsem,
    pf_ssem,
    pf_rsem,
    h_ssem,
    h_rsem,
    q_ssem,
    q_rsem,
    sc_ssem,
    sc_rsem,
    ret_ssem,
    ret_rsem,
    sq_ssem,
    sq_rsem,
):
    me_e = lax.axis_index("ep")
    me_t = lax.axis_index("tp")
    z, x = me_e // NX, me_e % NX
    y, core = me_t // 2, me_t % 2
    partner = (me_e, y * 2 + 1 - core)

    def ydev(step):
        return (me_e, ((y + step + NY) % NY) * 2 + core)

    def ysrc(step, c):
        return ((y + step + NY) % NY) * 2 + c

    def ep_peer(i):
        zi, xi = i // NX, i % NX
        dz, dx = (zi + 1) // 2, (xi + 1) // 2
        dz = 4 + dz * (1 - 2 * (zi % 2))
        dx = 2 + dx * (1 - 2 * (xi % 2))
        return ((z + dz) % NZ) * NX + (x + dx) % NX

    barrier = pltpu.get_barrier_semaphore()

    def greet_ep(k, carry):
        pl.semaphore_signal(barrier, inc=1, device_id=(ep_peer(k), me_t), device_id_type=MESH)
        return carry

    def greet_tp(k, carry):
        pl.semaphore_signal(
            barrier, inc=1, device_id=(me_e, (me_t + k) % NTP), device_id_type=MESH
        )
        return carry

    lax.fori_loop(0, NEP - 1, greet_ep, 0)
    lax.fori_loop(1, NTP, greet_tp, 0)

    loads = [
        pltpu.make_async_copy(dg, w_dense.at[pl.ds(0, 64)], w_sem.at[0]),
        pltpu.make_async_copy(du, w_dense.at[pl.ds(64, 64)], w_sem.at[1]),
        pltpu.make_async_copy(dd, d_down, w_sem.at[2]),
        pltpu.make_async_copy(wg, w_gu.at[pl.ds(0, 2)], w_sem.at[3]),
        pltpu.make_async_copy(wu, w_gu.at[pl.ds(2, 2)], w_sem.at[4]),
    ]
    for k in range(NY):
        columns = pl.ds(pl.multiple_of((2 * k + core) * PART, PART), PART)
        loads.append(pltpu.make_async_copy(wd.at[:, :, columns], wd_own.at[k], w_sem.at[5 + k]))
    for load in loads:
        load.start()

    lane = lax.broadcasted_iota(jnp.int32, (8, 256), 1)
    sub = lax.broadcasted_iota(jnp.int32, (8, 256), 0)
    expert = 2 * (lane // 8) + (lane // 2) % 2
    half = (lane // 4) % 2
    r0 = jnp.zeros((8, 256), jnp.int32)
    r1 = jnp.zeros((8, 256), jnp.int32)
    l0 = jnp.zeros((8, 256), F32)
    l1 = jnp.zeros((8, 256), F32)
    for t in range(8):
        r0 = jnp.where(sub == t, routes[0, t], r0)
        r1 = jnp.where(sub == t, routes[1, t], r1)
        l0 = jnp.where(sub == t, logits[0, t], l0)
        l1 = jnp.where(sub == t, logits[1, t], l1)
    top = jnp.maximum(l0, l1)
    e0, e1 = jnp.exp(l0 - top), jnp.exp(l1 - top)
    is0, is1 = (r0 == expert), (r1 == expert)
    hit = jnp.where(is0, 1.0, 0.0) + jnp.where(is1, 1.0, 0.0)
    before = jnp.zeros((8, 256), F32)
    for t in range(7):
        before = before + jnp.where(sub > t, hit[t : t + 1, :], 0.0)
    placed = jnp.where(before == (lane % 2).astype(F32), hit, 0.0)
    weight = (jnp.where(is0, e0, 0.0) + jnp.where(is1, e1, 0.0)) / (e0 + e1) * placed
    comb[0:8, :] = jnp.where(half == 0, weight, 0.0)
    comb[8:16, :] = jnp.where(half == 1, weight, 0.0)
    place = jnp.concatenate(
        [jnp.where(half == 0, placed, 0.0), jnp.where(half == 1, placed, 0.0)], axis=0
    ).astype(BF16)
    tok_value = tok[...]
    halves = jnp.concatenate(
        [tok_value[:, 0:128].astype(F32), tok_value[:, 128:256].astype(F32)], axis=0
    ).astype(BF16)
    a2a_out[...] = (
        lax.dot_general(place, halves, (((0,), (0,)), ((), ())), preferred_element_type=F32)
        .astype(BF16)
        .reshape(NEP, 8, 128)
    )

    pl.semaphore_wait(barrier, NEP - 1 + NTP - 1)

    def send_a2a(k, carry):
        peer = ep_peer(k)
        rcopy(a2a_out.at[peer], a2a_in.at[me_e], a2a_ssem, a2a_rsem, (peer, me_t)).start()
        return carry

    lax.fori_loop(0, NEP - 1, send_a2a, 0)

    def send_tok(k, carry):
        to = (me_t + k) % NTP
        rcopy(tok, tok_all.at[me_t], tok_ssem, tok_rsem, (me_e, to)).start()
        return carry

    lax.fori_loop(1, NTP, send_tok, 0)
    tok_all[me_t] = tok_value
    a2a_in[me_e] = a2a_out[me_e]

    wparts = []
    for k in range(NY):
        columns = pl.ds(pl.multiple_of((2 * k + 1 - core) * PART, PART), PART)
        copy = rcopy(wd.at[:, :, columns], wd_par.at[k], wp_ssem.at[k], wp_rsem.at[k], partner)
        copy.start()
        wparts.append(copy)

    rcopy(
        tok_all.at[pl.ds(0, NTP - 1)],
        tok_all.at[pl.ds(0, NTP - 1)],
        tok_ssem,
        tok_rsem,
        partner,
    ).wait_recv()
    squares = jnp.zeros((8, PART), F32)
    for j in range(NTP):
        v = tok_all[j].astype(F32)
        squares = squares + v * v
    scale = lax.rsqrt(jnp.sum(squares, axis=1, keepdims=True) / WIDTH + EPS)
    for load in loads[0:3]:
        load.wait()
    act = jnp.zeros((8, 128), F32)
    mix_acc = jnp.zeros((8, PART), F32)
    for j in range(NTP):
        cols = slice(j * PART, (j + 1) * PART)
        n = (tok_all[j].astype(F32) * scale * gain[:, cols]).astype(BF16)
        mix_acc = mix_acc + n.astype(F32) * mixw[:, cols]
        act = act + nt_dot(n, w_dense[:, cols])
    gate_ref[...] = jnp.broadcast_to(
        jax.nn.sigmoid(jnp.sum(mix_acc, axis=1, keepdims=True)), (8, 128)
    )
    dense_h = (silu(act[:, 0:64]) * act[:, 64:128]).astype(BF16)
    for j in range(NTP):
        cols = slice(j * PART, (j + 1) * PART)
        dense_out[j] = jnp.dot(dense_h, d_down[:, cols], preferred_element_type=F32)

    def send_dense(k, carry):
        to = (me_t + k) % NTP
        rcopy(
            dense_out.at[to], dense_in.at[me_t], dense_ssem, dense_rsem, (me_e, to)
        ).start()
        return carry

    lax.fori_loop(1, NTP, send_dense, 0)
    dense_in[me_t] = dense_out[me_t]

    rcopy(
        a2a_out.at[pl.ds(0, NEP - 1)],
        a2a_in.at[pl.ds(0, NEP - 1)],
        a2a_ssem,
        a2a_rsem,
        partner,
    ).wait_recv()
    pairs = a2a_in[...].astype(F32).reshape(16, 2, 8, 128)
    even, odd = pairs[:, 0], pairs[:, 1]
    sub3 = lax.broadcasted_iota(jnp.int32, (16, 8, 128), 1)
    left = jnp.where(sub3 < 4, even, pltpu.roll(odd, 4, 1)).reshape(ROWS, 128)
    right = jnp.where(sub3 < 4, pltpu.roll(even, 4, 1), odd).reshape(ROWS, 128)
    gathered[me_t, :, 0:128] = left.astype(BF16)
    gathered[me_t, :, 128:256] = right.astype(BF16)

    sends = []

    def ag_send(slot, rows, sem, device):
        ref = gathered.at[slot, rows]
        copy = rcopy(ref, ref, ag_ssem.at[len(sends)], ag_rsem.at[sem], device)
        copy.start()
        sends.append(copy)

    def ag_wait(slot, rows, sem):
        ref = gathered.at[slot, rows]
        rcopy(ref, ref, ag_ssem.at[0], ag_rsem.at[sem], partner).wait_recv()

    passes = []

    def pass_on(rel):
        ref = gathered.at[ysrc(rel, core)]
        copy = rcopy(ref, ref, pf_ssem.at[rel], pf_rsem.at[rel], partner)
        copy.start()
        passes.append(copy)

    whole, low, high = pl.ds(0, ROWS), pl.ds(0, ROWS // 2), pl.ds(ROWS // 2, ROWS // 2)
    ag_send(me_t, whole, 6, ydev(2))
    ag_send(me_t, whole, 2, ydev(-2))
    ag_send(me_t, whole, 7, ydev(1))
    ag_send(me_t, whole, 1, ydev(-1))
    pass_on(0)
    ssq[...] = left * left + right * right

    def add_squares(slot):
        v = gathered[slot].astype(F32)
        v = v * v
        ssq[...] += v[:, 0:128] + v[:, 128:256]

    s6, s2 = ysrc(6, core), ysrc(2, core)
    ag_wait(s6, whole, 6)
    ag_send(s6, low, 4, ydev(2))
    ag_send(s6, whole, 5, ydev(1))
    ag_wait(s2, whole, 2)
    ag_send(s2, high, 8, ydev(-2))
    ag_send(s2, whole, 3, ydev(-1))
    pass_on(6)
    pass_on(2)
    for rel in (7, 1):
        ag_wait(ysrc(rel, core), whole, rel)
        pass_on(rel)
    for rel in (6, 2, 7, 1):
        add_squares(ysrc(rel, core))
    for rel in (5, 3):
        ag_wait(ysrc(rel, core), whole, rel)
        pass_on(rel)
        add_squares(ysrc(rel, core))
    s4 = ysrc(4, core)
    ag_wait(s4, low, 4)
    ag_wait(s4, high, 8)
    pass_on(4)
    add_squares(s4)
    for rel in (0, 6, 2, 7, 1, 5, 3, 4):
        slot = ysrc(rel, 1 - core)
        ref = gathered.at[slot]
        rcopy(ref, ref, pf_ssem.at[rel], pf_rsem.at[rel], partner).wait_recv()
        add_squares(slot)

    row_scale = lax.rsqrt(jnp.sum(ssq[...], axis=1, keepdims=True) / WIDTH + EPS)
    loads[3].wait()
    loads[4].wait()
    acts = jnp.zeros((ROWS, 256), F32)
    for j in range(NTP):
        cols = slice(j * PART, (j + 1) * PART)
        n = (gathered[j].astype(F32) * row_scale * gain[:, cols]).astype(BF16)
        acts = acts + nt_dot(n, w_gu[:, :, cols].reshape(256, PART))
    hidden = silu(acts[:, 0:128]) * acts[:, 128:256]
    row = lax.broadcasted_iota(jnp.int32, (ROWS, 128), 0)
    col = lax.broadcasted_iota(jnp.int32, (ROWS, 128), 1)
    hidden = jnp.where((row // 2) % 2 == col // 64, hidden, 0.0).astype(BF16)
    h_own[...] = hidden
    h_copy = rcopy(h_own, h_par, h_ssem, h_rsem, partner)
    h_copy.start()
    for load in loads[5:]:
        load.wait()
    for copy in wparts:
        copy.wait_recv()
    h_copy.wait_recv()

    diagonal = row == col

    def partial(rel):
        k = (y + rel) % NY
        return jnp.dot(
            h_own[...], wd_own[k].reshape(128, PART), preferred_element_type=F32
        ) + jnp.dot(h_par[...], wd_par[k].reshape(128, PART), preferred_element_type=F32)

    def pack(value, slot):
        most = jnp.maximum(jnp.max(jnp.abs(value), axis=1, keepdims=True), 1e-30)
        q_out[slot] = jnp.round(value * (32767.0 / most)).astype(jnp.int16)
        s_out[slot] = jnp.sum(
            jnp.where(diagonal, most * (1.0 / 32767.0), 0.0), axis=0, keepdims=True
        )

    def unpack(slot, sslot):
        unit = jnp.sum(jnp.where(diagonal, s_in[sslot], 0.0), axis=1, keepdims=True)
        return q_in[slot].astype(F32) * unit

    qsends = []

    def q_send(slot, rows, sem, device):
        copy = rcopy(
            q_out.at[slot, rows], q_in.at[slot, rows], q_ssem.at[sem], q_rsem.at[sem], device
        )
        copy.start()
        qsends.append(copy)
        copy = rcopy(s_out.at[slot], s_in.at[sem], sc_ssem.at[sem], sc_rsem.at[sem], device)
        copy.start()
        qsends.append(copy)

    def q_wait(slot, rows, sem):
        rcopy(
            q_out.at[slot, rows], q_in.at[slot, rows], q_ssem.at[sem], q_rsem.at[sem], partner
        ).wait_recv()
        rcopy(s_out.at[slot], s_in.at[sem], sc_ssem.at[sem], sc_rsem.at[sem], partner).wait_recv()

    pack(partial(4), 2)
    q_send(2, low, 2, ydev(2))
    q_send(2, high, 7, ydev(-2))
    pack(partial(3), 0)
    q_send(0, whole, 0, ydev(1))
    pack(partial(5), 1)
    q_send(1, whole, 1, ydev(-1))
    pack(partial(1), 3)
    q_send(3, whole, 3, ydev(1))
    pack(partial(7), 4)
    q_send(4, whole, 4, ydev(-1))
    kept[0] = partial(2)
    kept[1] = partial(6)
    kept[2] = partial(0)
    q_wait(0, whole, 0)
    q_wait(2, low, 2)
    total = kept[0] + unpack(0, 0)
    far = jnp.where(lax.broadcasted_iota(jnp.int32, (ROWS, PART), 0) < ROWS // 2, 1.0, 0.0)
    q_wait(2, high, 7)
    q_wait(1, whole, 1)
    pack(total + unpack(2, 2) * far, 5)
    q_send(5, whole, 5, ydev(2))
    pack(kept[1] + unpack(1, 1) + unpack(2, 7) * (1.0 - far), 6)
    q_send(6, whole, 6, ydev(-2))
    q_wait(3, whole, 3)
    q_wait(4, whole, 4)
    kept[2] += unpack(3, 3) + unpack(4, 4)
    q_wait(5, whole, 5)
    q_wait(6, whole, 6)
    summed = kept[2] + unpack(5, 5) + unpack(6, 6)

    left = summed[:, 0:128].reshape(16, 8, 128)
    right = summed[:, 128:256].reshape(16, 8, 128)
    even = jnp.where(sub3 < 4, left, pltpu.roll(right, 4, 1))
    odd = jnp.where(sub3 < 4, pltpu.roll(left, 4, 1), right)
    ret_out[...] = jnp.stack([even, odd], axis=1).reshape(NEP, 8, 128)

    def send_ret(k, carry):
        peer = ep_peer(k)
        rcopy(ret_out.at[peer], ret_in.at[me_e], ret_ssem, ret_rsem, (peer, me_t)).start()
        return carry

    lax.fori_loop(0, NEP - 1, send_ret, 0)
    ret_in[me_e] = ret_out[me_e]

    rcopy(
        dense_out.at[pl.ds(0, NTP - 1)],
        dense_in.at[pl.ds(0, NTP - 1)],
        dense_ssem,
        dense_rsem,
        partner,
    ).wait_recv()
    dense = dense_in[0]
    for j in range(1, NTP):
        dense = dense + dense_in[j]
    gate = gate_ref[...]
    dense = jnp.concatenate([gate, gate], axis=1) * dense

    rcopy(
        ret_out.at[pl.ds(0, NEP - 1)],
        ret_in.at[pl.ds(0, NEP - 1)],
        ret_ssem,
        ret_rsem,
        partner,
    ).wait_recv()
    mixed = jnp.dot(
        comb[...],
        ret_in[...].reshape(256, 128),
        preferred_element_type=F32,
        precision=lax.Precision.HIGHEST,
    )
    combined = jnp.concatenate([mixed[0:8], mixed[8:16]], axis=1) + dense
    own = combined * combined
    own = own[:, 0:128] + own[:, 128:256]
    sq_out[...] = own

    def send_sq(k, carry):
        to = (me_t + k) % NTP
        rcopy(sq_out, sq_in.at[me_t], sq_ssem, sq_rsem, (me_e, to)).start()
        return carry

    lax.fori_loop(1, NTP, send_sq, 0)
    sq_in[me_t] = own
    rcopy(
        sq_in.at[pl.ds(0, NTP - 1)], sq_in.at[pl.ds(0, NTP - 1)], sq_ssem, sq_rsem, partner
    ).wait_recv()
    total_sq = sq_in[0]
    for j in range(1, NTP):
        total_sq = total_sq + sq_in[j]
    final = lax.rsqrt(jnp.sum(total_sq, axis=1, keepdims=True) / WIDTH + EPS)
    out[...] = (combined * final * ogain[...]).astype(BF16)

    for copy in wparts + sends + passes + [h_copy] + qsends:
        copy.wait_send()
    for ref, ssem, rsem, n in (
        (a2a_out, a2a_ssem, a2a_rsem, NEP - 1),
        (tok_all, tok_ssem, tok_rsem, NTP - 1),
        (dense_out, dense_ssem, dense_rsem, NTP - 1),
        (ret_out, ret_ssem, ret_rsem, NEP - 1),
        (sq_in, sq_ssem, sq_rsem, NTP - 1),
    ):
        part = ref.at[pl.ds(0, n)]
        rcopy(part, part, ssem, rsem, partner).wait_send()


def local(
    tokens,
    norm_gain,
    route_experts,
    route_logits,
    expert_gate,
    expert_up,
    expert_down,
    dense_gate,
    dense_up,
    dense_down,
    mix_weight,
    out_gain,
):
    vmem = pl.BlockSpec(memory_space=pltpu.VMEM)
    smem = pl.BlockSpec(memory_space=pltpu.SMEM)
    hbm = pl.BlockSpec(memory_space=pl.ANY)
    dma = pltpu.SemaphoreType.DMA
    return pl.pallas_call(
        kernel,
        out_shape=jax.ShapeDtypeStruct((8, PART), BF16),
        in_specs=[vmem, vmem, smem, smem, hbm, hbm, hbm, hbm, hbm, hbm, vmem, vmem],
        out_specs=vmem,
        scratch_shapes=[
            pltpu.VMEM((4, 64, WIDTH), BF16),
            pltpu.VMEM((NY, 2, 64, PART), BF16),
            pltpu.VMEM((NY, 2, 64, PART), BF16),
            pltpu.VMEM((128, WIDTH), BF16),
            pltpu.VMEM((64, WIDTH), BF16),
            pltpu.VMEM((NEP, 8, 128), BF16),
            pltpu.VMEM((NEP, 8, 128), BF16),
            pltpu.VMEM((NTP, ROWS, PART), BF16),
            pltpu.VMEM((NTP, 8, PART), BF16),
            pltpu.VMEM((NTP, 8, PART), F32),
            pltpu.VMEM((NTP, 8, PART), F32),
            pltpu.VMEM((16, 256), F32),
            pltpu.VMEM((ROWS, 128), BF16),
            pltpu.VMEM((ROWS, 128), BF16),
            pltpu.VMEM((7, ROWS, PART), jnp.int16),
            pltpu.VMEM((7, ROWS, PART), jnp.int16),
            pltpu.VMEM((7, 1, 128), F32),
            pltpu.VMEM((8, 1, 128), F32),
            pltpu.VMEM((3, ROWS, PART), F32),
            pltpu.VMEM((NEP, 8, 128), F32),
            pltpu.VMEM((NEP, 8, 128), F32),
            pltpu.VMEM((8, 128), F32),
            pltpu.VMEM((NTP, 8, 128), F32),
            pltpu.VMEM((ROWS, 128), F32),
            pltpu.VMEM((8, 128), F32),
            dma((13,)),
            dma((NY,)),
            dma((NY,)),
            dma,
            dma,
            dma,
            dma,
            dma,
            dma,
            dma((8,)),
            dma((9,)),
            dma((8,)),
            dma((8,)),
            dma,
            dma,
            dma((8,)),
            dma((8,)),
            dma((8,)),
            dma((8,)),
            dma,
            dma,
            dma,
            dma,
        ],
        compiler_params=pltpu.CompilerParams(collective_id=0, has_side_effects=True),
    )(
        tokens,
        norm_gain.reshape(1, WIDTH),
        route_experts.T,
        route_logits.T,
        jnp.swapaxes(expert_gate, 1, 2),
        jnp.swapaxes(expert_up, 1, 2),
        expert_down,
        dense_gate.T,
        dense_up.T,
        dense_down,
        mix_weight.reshape(1, WIDTH),
        out_gain.reshape(1, PART),
    )


def solution(mesh):
    tp = "tp"
    in_specs = (
        P("ep", tp),
        P(),
        P("ep", None),
        P("ep", None),
        P("ep", None, tp),
        P("ep", None, tp),
        P("ep", tp, None),
        P(None, tp),
        P(None, tp),
        P(tp, None),
        P(),
        P(tp),
    )
    return jax.shard_map(
        local, mesh=mesh, in_specs=in_specs, out_specs=P("ep", tp), check_vma=False
    )
```

```python
import functools

import jax
import jax.numpy as jnp
from jax import lax
from jax.experimental import pallas as pl
from jax.experimental.pallas import tpu as pltpu
from jax.sharding import PartitionSpec as P

MESH = pl.DeviceIdType.MESH
F32 = jnp.float32
BF16 = jnp.bfloat16
EPS = 1e-06

NX, NZ, NY = 4, 8, 8
NEP = NX * NZ
NTP = 2 * NY
ROWS = 128
PART = 256
WIDTH = 4096


def rcopy(src, dst, send_sem, recv_sem, device):
    return pltpu.make_async_remote_copy(
        src_ref=src,
        dst_ref=dst,
        send_sem=send_sem,
        recv_sem=recv_sem,
        device_id=device,
        device_id_type=MESH,
    )


def nt_dot(a, b):
    return lax.dot_general(a, b, (((1,), (1,)), ((), ())), preferred_element_type=F32)


def silu(v):
    return v / (1.0 + jnp.exp(-v))


def kernel(
    tok_hbm,
    gain_hbm,
    routes_hbm,
    logits_hbm,
    wg,
    wu,
    wd,
    dg,
    du,
    dd,
    mixw_hbm,
    ogain_hbm,
    out,
    tok,
    gain,
    routes,
    logits,
    mixw,
    ogain,
    w_gu,
    wd_own,
    wd_par,
    w_dense,
    dd_own,
    dd_par,
    a2a_out,
    a2a_in,
    gathered,
    tok_all,
    dense_out,
    dense_in,
    dh_own,
    dh_par,
    comb,
    h_own,
    h_par,
    q_out,
    q_in,
    s_out,
    s_in,
    kept,
    ret_out,
    ret_in,
    sq_out,
    sq_in,
    ssq,
    gate_ref,
    i_sem,
    w_sem,
    wp_ssem,
    wp_rsem,
    a2a_ssem,
    a2a_rsem,
    tok_ssem,
    tok_rsem,
    tp_ssem,
    tp_rsem,
    dh_ssem,
    dh_rsem,
    dense_ssem,
    dense_rsem,
    ag_ssem,
    ag_rsem,
    pf_ssem,
    pf_rsem,
    h_ssem,
    h_rsem,
    q_ssem,
    q_rsem,
    sc_ssem,
    sc_rsem,
    ret_ssem,
    ret_rsem,
    sq_ssem,
    sq_rsem,
):
    me_e = lax.axis_index("ep")
    me_t = lax.axis_index("tp")
    z, x = lax.div(me_e, NX), lax.rem(me_e, NX)
    y, core = lax.div(me_t, 2), lax.rem(me_t, 2)
    other = 1 - core
    partner = (me_e, y * 2 + other)
    zs = [lax.rem(z + k, NZ) * NX for k in range(NZ)]
    xs = [lax.rem(x + k, NX) for k in range(NX)]
    ys = [lax.rem(y + k, NY) for k in range(NY)]
    peers = [zs[dz] + xs[dx] for dz in (4, 3, 5, 2, 6, 1, 7, 0) for dx in (2, 1, 3, 0)][:-1]
    y_order = (4, 3, 5, 2, 6, 1, 7)

    def ydev(step):
        return (me_e, ys[step % NY] * 2 + core)

    barrier = pltpu.get_barrier_semaphore()
    for peer in peers:
        pl.semaphore_signal(barrier, inc=1, device_id=(peer, me_t), device_id_type=MESH)
    for step in y_order:
        for c in range(2):
            pl.semaphore_signal(
                barrier, inc=1, device_id=(me_e, ys[step] * 2 + c), device_id_type=MESH
            )
    pl.semaphore_signal(barrier, inc=1, device_id=partner, device_id_type=MESH)

    smalls = [
        pltpu.make_async_copy(routes_hbm, routes, i_sem.at[0]),
        pltpu.make_async_copy(logits_hbm, logits, i_sem.at[1]),
        pltpu.make_async_copy(tok_hbm, tok, i_sem.at[2]),
        pltpu.make_async_copy(gain_hbm, gain, i_sem.at[3]),
        pltpu.make_async_copy(mixw_hbm, mixw, i_sem.at[4]),
        pltpu.make_async_copy(ogain_hbm, ogain, i_sem.at[5]),
    ]
    loads = [
        pltpu.make_async_copy(dg, w_dense.at[pl.ds(0, 64)], w_sem.at[0]),
        pltpu.make_async_copy(du, w_dense.at[pl.ds(64, 64)], w_sem.at[1]),
        pltpu.make_async_copy(wg, w_gu.at[pl.ds(0, 2)], w_sem.at[2]),
        pltpu.make_async_copy(wu, w_gu.at[pl.ds(2, 2)], w_sem.at[3]),
    ]

    def columns(k, c):
        return pl.ds(pl.multiple_of((2 * k + c) * PART, PART), PART)

    for k in range(NY):
        loads.append(
            pltpu.make_async_copy(dd.at[:, columns(k, core)], dd_own.at[k], w_sem.at[4 + k])
        )
    for k in range(NY):
        loads.append(
            pltpu.make_async_copy(wd.at[:, :, columns(k, core)], wd_own.at[k], w_sem.at[12 + k])
        )
    for load in smalls + loads:
        load.start()

    for load in smalls[0:3]:
        load.wait()
    lane = lax.broadcasted_iota(jnp.int32, (8, 256), 1)
    sub = lax.broadcasted_iota(jnp.int32, (8, 256), 0)
    expert = 2 * (lane // 8) + (lane // 2) % 2
    half = (lane // 4) % 2
    r0 = jnp.zeros((8, 256), jnp.int32)
    r1 = jnp.zeros((8, 256), jnp.int32)
    l0 = jnp.zeros((8, 256), F32)
    l1 = jnp.zeros((8, 256), F32)
    for t in range(8):
        r0 = jnp.where(sub == t, routes[0, t], r0)
        r1 = jnp.where(sub == t, routes[1, t], r1)
        l0 = jnp.where(sub == t, logits[0, t], l0)
        l1 = jnp.where(sub == t, logits[1, t], l1)
    top = jnp.maximum(l0, l1)
    e0, e1 = jnp.exp(l0 - top), jnp.exp(l1 - top)
    is0, is1 = (r0 == expert), (r1 == expert)
    hit = jnp.where(is0, 1.0, 0.0) + jnp.where(is1, 1.0, 0.0)
    before = jnp.zeros((8, 256), F32)
    for t in range(7):
        before = before + jnp.where(sub > t, hit[t : t + 1, :], 0.0)
    placed = jnp.where(before == (lane % 2).astype(F32), hit, 0.0)
    weight = (jnp.where(is0, e0, 0.0) + jnp.where(is1, e1, 0.0)) / (e0 + e1) * placed
    comb[0:8, :] = jnp.where(half == 0, weight, 0.0)
    comb[8:16, :] = jnp.where(half == 1, weight, 0.0)
    place = jnp.concatenate(
        [jnp.where(half == 0, placed, 0.0), jnp.where(half == 1, placed, 0.0)], axis=0
    ).astype(BF16)
    tok_value = tok[...]
    halves = jnp.concatenate(
        [tok_value[:, 0:128].astype(F32), tok_value[:, 128:256].astype(F32)], axis=0
    ).astype(BF16)
    a2a_out[...] = (
        lax.dot_general(place, halves, (((0,), (0,)), ((), ())), preferred_element_type=F32)
        .astype(BF16)
        .reshape(NEP, 8, 128)
    )
    a2a_in[me_e] = a2a_out[me_e]
    tok_all[core, y] = tok_value

    pl.semaphore_wait(barrier, NEP - 1 + NTP - 1)

    for peer in peers:
        rcopy(a2a_out.at[peer], a2a_in.at[me_e], a2a_ssem, a2a_rsem, (peer, me_t)).start()

    for step in y_order:
        rcopy(tok, tok_all.at[core, y], tok_ssem, tok_rsem, ydev(step)).start()

    wparts = []
    for k in range(NY):
        copy = rcopy(
            dd.at[:, columns(k, other)], dd_par.at[k], wp_ssem.at[k], wp_rsem.at[k], partner
        )
        copy.start()
        wparts.append(copy)
    for k in range(NY):
        copy = rcopy(
            wd.at[:, :, columns(k, other)],
            wd_par.at[k],
            wp_ssem.at[NY + k],
            wp_rsem.at[NY + k],
            partner,
        )
        copy.start()
        wparts.append(copy)

    rcopy(
        a2a_out.at[pl.ds(0, NEP - 1)],
        a2a_in.at[pl.ds(0, NEP - 1)],
        a2a_ssem,
        a2a_rsem,
        partner,
    ).wait_recv()
    pairs = a2a_in[...].astype(F32).reshape(16, 2, 8, 128)
    even, odd = pairs[:, 0], pairs[:, 1]
    sub3 = lax.broadcasted_iota(jnp.int32, (16, 8, 128), 1)
    left = jnp.where(sub3 < 4, even, pltpu.roll(odd, 4, 1)).reshape(ROWS, 128)
    right = jnp.where(sub3 < 4, pltpu.roll(even, 4, 1), odd).reshape(ROWS, 128)
    gathered[core, y, :, 0:128] = left.astype(BF16)
    gathered[core, y, :, 128:256] = right.astype(BF16)

    sends = []
    whole, low, high = pl.ds(0, ROWS), pl.ds(0, ROWS // 2), pl.ds(ROWS // 2, ROWS // 2)

    def ag_send(rel, rows, sem, step):
        ref = gathered.at[core, ys[rel], rows]
        copy = rcopy(ref, ref, ag_ssem.at[len(sends)], ag_rsem.at[sem], ydev(step))
        copy.start()
        sends.append(copy)

    def ag_wait(rel, rows, sem):
        ref = gathered.at[core, ys[rel], rows]
        rcopy(ref, ref, ag_ssem.at[0], ag_rsem.at[sem], partner).wait_recv()

    passes = []

    def pass_on(rel):
        ref = gathered.at[core, ys[rel]]
        copy = rcopy(ref, ref, pf_ssem.at[rel], pf_rsem.at[rel], partner)
        copy.start()
        passes.append(copy)

    def pass_wait(rel):
        ref = gathered.at[other, ys[rel]]
        rcopy(ref, ref, pf_ssem.at[rel], pf_rsem.at[rel], partner).wait_recv()

    def add_squares(c, rel):
        v = gathered[c, ys[rel]].astype(F32)
        v = v * v
        ssq[...] += v[:, 0:128] + v[:, 128:256]

    ag_send(0, low, 12, 2)
    ag_send(0, low, 4, -2)
    ag_send(0, high, 13, 2)
    ag_send(0, high, 5, -2)
    ag_send(0, whole, 14, 1)
    ag_send(0, whole, 2, -1)
    pass_on(0)
    ssq[...] = left * left + right * right

    tok_step = rcopy(
        tok_all.at[0, pl.ds(0, NY - 1)], tok_all.at[0, pl.ds(0, NY - 1)], tok_ssem, tok_rsem, partner
    )
    tok_step.wait_recv()
    tok_pass = rcopy(tok_all.at[core], tok_all.at[core], tp_ssem, tp_rsem, partner)
    tok_pass.start()
    for load in smalls[3:6] + loads[0:2]:
        load.wait()
    rcopy(tok_all.at[other], tok_all.at[other], tp_ssem, tp_rsem, partner).wait_recv()

    squares = jnp.zeros((8, PART), F32)
    for j in range(NTP):
        v = tok_all[j % 2, j // 2].astype(F32)
        squares = squares + v * v
    scale = lax.rsqrt(jnp.sum(squares, axis=1, keepdims=True) / WIDTH + EPS)
    act = jnp.zeros((8, 128), F32)
    mix_acc = jnp.zeros((8, PART), F32)
    for j in range(NTP):
        cols = slice(j * PART, (j + 1) * PART)
        n = (tok_all[j % 2, j // 2].astype(F32) * scale * gain[:, cols]).astype(BF16)
        mix_acc = mix_acc + n.astype(F32) * mixw[:, cols]
        act = act + nt_dot(n, w_dense[:, cols])
    gate_ref[...] = jnp.broadcast_to(
        jax.nn.sigmoid(jnp.sum(mix_acc, axis=1, keepdims=True)), (8, 128)
    )
    dh_own[...] = (silu(act[:, 0:64]) * act[:, 64:128]).astype(BF16)
    dh_copy = rcopy(dh_own, dh_par, dh_ssem, dh_rsem, partner)
    dh_copy.start()

    ag_wait(6, low, 12)
    ag_send(6, low, 8, 2)
    ag_send(6, low, 10, 1)
    ag_wait(2, low, 4)
    ag_send(2, low, 6, -1)
    ag_wait(6, high, 13)
    ag_send(6, high, 11, 1)
    ag_wait(2, high, 5)
    ag_send(2, high, 9, -2)
    ag_send(2, high, 7, -1)
    pass_on(6)
    pass_on(2)
    for load in loads[4:12]:
        load.wait()
    for copy in wparts[0:NY]:
        copy.wait_recv()
    dh_copy.wait_recv()
    for k in range(NY):
        dense_out[k] = jnp.dot(
            dh_own[...], dd_own[k], preferred_element_type=F32
        ) + jnp.dot(dh_par[...], dd_par[k], preferred_element_type=F32)
    dense_in[y] = dense_out[y]
    add_squares(core, 6)
    add_squares(core, 2)
    for rel in (7, 1):
        ag_wait(rel, whole, 2 * rel)
        pass_on(rel)
    for rel in (7, 1):
        add_squares(core, rel)
    for step in y_order:
        rcopy(
            dense_out.at[ys[step]], dense_in.at[y], dense_ssem, dense_rsem, ydev(step)
        ).start()
    for rel in (5, 3):
        ag_wait(rel, low, 2 * rel)
        ag_wait(rel, high, 2 * rel + 1)
        pass_on(rel)
    for rel in (0, 6, 2, 7, 1):
        pass_wait(rel)
        add_squares(other, rel)
    for rel in (5, 3):
        add_squares(core, rel)
    ag_wait(4, low, 8)
    ag_wait(4, high, 9)
    pass_on(4)
    add_squares(core, 4)
    for rel in (5, 3, 4):
        pass_wait(rel)
        add_squares(other, rel)

    row_scale = lax.rsqrt(jnp.sum(ssq[...], axis=1, keepdims=True) / WIDTH + EPS)
    loads[2].wait()
    loads[3].wait()
    acts = jnp.zeros((ROWS, 256), F32)
    for j in range(NTP):
        cols = slice(j * PART, (j + 1) * PART)
        n = (gathered[j % 2, j // 2].astype(F32) * row_scale * gain[:, cols]).astype(BF16)
        acts = acts + nt_dot(n, w_gu[:, :, cols].reshape(256, PART))
    hidden = silu(acts[:, 0:128]) * acts[:, 128:256]
    row = lax.broadcasted_iota(jnp.int32, (ROWS, 128), 0)
    col = lax.broadcasted_iota(jnp.int32, (ROWS, 128), 1)
    hidden = jnp.where((row // 2) % 2 == col // 64, hidden, 0.0).astype(BF16)
    h_own[...] = hidden
    h_copy = rcopy(h_own, h_par, h_ssem, h_rsem, partner)
    h_copy.start()
    for load in loads[12:]:
        load.wait()
    for copy in wparts[NY:]:
        copy.wait_recv()
    h_copy.wait_recv()

    diagonal = row == col

    def partial(rel):
        k = ys[rel]
        return jnp.dot(
            h_own[...], wd_own[k].reshape(128, PART), preferred_element_type=F32
        ) + jnp.dot(h_par[...], wd_par[k].reshape(128, PART), preferred_element_type=F32)

    def pack(value, slot):
        most = jnp.maximum(jnp.max(jnp.abs(value), axis=1, keepdims=True), 1e-30)
        q_out[slot] = jnp.round(value * (32767.0 / most)).astype(jnp.int16)
        s_out[slot] = jnp.sum(
            jnp.where(diagonal, most * (1.0 / 32767.0), 0.0), axis=0, keepdims=True
        )

    def unpack(slot, sslot):
        unit = jnp.sum(jnp.where(diagonal, s_in[sslot], 0.0), axis=1, keepdims=True)
        return q_in[slot].astype(F32) * unit

    qsends = []

    def q_send(slot, rows, sem, step):
        device = ydev(step)
        copy = rcopy(
            q_out.at[slot, rows], q_in.at[slot, rows], q_ssem.at[sem], q_rsem.at[sem], device
        )
        copy.start()
        qsends.append(copy)
        copy = rcopy(s_out.at[slot], s_in.at[sem], sc_ssem.at[sem], sc_rsem.at[sem], device)
        copy.start()
        qsends.append(copy)

    def q_wait(slot, rows, sem):
        rcopy(
            q_out.at[slot, rows], q_in.at[slot, rows], q_ssem.at[sem], q_rsem.at[sem], partner
        ).wait_recv()
        rcopy(s_out.at[slot], s_in.at[sem], sc_ssem.at[sem], sc_rsem.at[sem], partner).wait_recv()

    pack(partial(4), 2)
    q_send(2, low, 2, 2)
    q_send(2, high, 7, -2)
    pack(partial(3), 0)
    q_send(0, whole, 0, 1)
    pack(partial(5), 1)
    q_send(1, whole, 1, -1)
    pack(partial(1), 3)
    q_send(3, whole, 3, 1)
    pack(partial(7), 4)
    q_send(4, whole, 4, -1)
    kept[0] = partial(2)
    kept[1] = partial(6)
    kept[2] = partial(0)
    dense_step = rcopy(
        dense_out.at[pl.ds(0, NY - 1)],
        dense_in.at[pl.ds(0, NY - 1)],
        dense_ssem,
        dense_rsem,
        partner,
    )
    dense_step.wait_recv()
    dense = dense_in[0]
    for k in range(1, NY):
        dense = dense + dense_in[k]
    gate = gate_ref[...]
    dense = jnp.concatenate([gate, gate], axis=1) * dense
    q_wait(0, whole, 0)
    q_wait(2, low, 2)
    total = kept[0] + unpack(0, 0)
    far = jnp.where(lax.broadcasted_iota(jnp.int32, (ROWS, PART), 0) < ROWS // 2, 1.0, 0.0)
    q_wait(2, high, 7)
    q_wait(1, whole, 1)
    pack(total + unpack(2, 2) * far, 5)
    q_send(5, whole, 5, 2)
    pack(kept[1] + unpack(1, 1) + unpack(2, 7) * (1.0 - far), 6)
    q_send(6, whole, 6, -2)
    q_wait(3, whole, 3)
    q_wait(4, whole, 4)
    kept[2] += unpack(3, 3) + unpack(4, 4)
    q_wait(5, whole, 5)
    q_wait(6, whole, 6)
    summed = kept[2] + unpack(5, 5) + unpack(6, 6)

    left = summed[:, 0:128].reshape(16, 8, 128)
    right = summed[:, 128:256].reshape(16, 8, 128)
    even = jnp.where(sub3 < 4, left, pltpu.roll(right, 4, 1))
    odd = jnp.where(sub3 < 4, pltpu.roll(left, 4, 1), right)
    ret_out[...] = jnp.stack([even, odd], axis=1).reshape(NEP, 8, 128)
    for peer in peers:
        rcopy(ret_out.at[peer], ret_in.at[me_e], ret_ssem, ret_rsem, (peer, me_t)).start()
    ret_in[me_e] = ret_out[me_e]
    rcopy(
        ret_out.at[pl.ds(0, NEP - 1)],
        ret_in.at[pl.ds(0, NEP - 1)],
        ret_ssem,
        ret_rsem,
        partner,
    ).wait_recv()
    mixed = jnp.dot(
        comb[...],
        ret_in[...].reshape(256, 128),
        preferred_element_type=F32,
        precision=lax.Precision.HIGHEST,
    )
    combined = jnp.concatenate([mixed[0:8], mixed[8:16]], axis=1) + dense
    token_diagonal = (
        lax.broadcasted_iota(jnp.int32, (8, 128), 0)
        == lax.broadcasted_iota(jnp.int32, (8, 128), 1)
    )
    own = jnp.sum(
        jnp.where(token_diagonal, jnp.sum(combined * combined, axis=1, keepdims=True), 0.0),
        axis=0,
        keepdims=True,
    )
    sq_out[...] = own
    for step in y_order:
        for c in range(2):
            rcopy(sq_out, sq_in.at[me_t], sq_ssem, sq_rsem, (me_e, ys[step] * 2 + c)).start()
    rcopy(sq_out, sq_in.at[me_t], sq_ssem, sq_rsem, partner).start()
    sq_in[me_t] = own
    sq_step = rcopy(
        sq_in.at[pl.ds(0, NTP - 1)], sq_in.at[pl.ds(0, NTP - 1)], sq_ssem, sq_rsem, partner
    )
    sq_step.wait_recv()
    total_sq = sq_in[0]
    for j in range(1, NTP):
        total_sq = total_sq + sq_in[j]
    final = lax.rsqrt(
        jnp.sum(jnp.where(token_diagonal, total_sq, 0.0), axis=1, keepdims=True) / WIDTH + EPS
    )
    out[...] = (combined * final * ogain[...]).astype(BF16)

    for copy in wparts + sends + passes + [tok_pass, dh_copy, h_copy] + qsends:
        copy.wait_send()
    tok_step.wait_send()
    dense_step.wait_send()
    sq_step.wait_send()
    for ref, ssem, rsem in ((a2a_out, a2a_ssem, a2a_rsem), (ret_out, ret_ssem, ret_rsem)):
        part = ref.at[pl.ds(0, NEP - 1)]
        rcopy(part, part, ssem, rsem, partner).wait_send()


def local(
    tokens,
    norm_gain,
    route_experts,
    route_logits,
    expert_gate,
    expert_up,
    expert_down,
    dense_gate,
    dense_up,
    dense_down,
    mix_weight,
    out_gain,
):
    vmem = pl.BlockSpec(memory_space=pltpu.VMEM)
    dma = pltpu.SemaphoreType.DMA
    return pl.pallas_call(
        kernel,
        out_shape=jax.ShapeDtypeStruct((8, PART), BF16),
        in_specs=[pl.BlockSpec(memory_space=pl.ANY)] * 12,
        out_specs=vmem,
        scratch_shapes=[
            pltpu.VMEM((8, PART), BF16),
            pltpu.VMEM((1, WIDTH), F32),
            pltpu.SMEM((2, 8), jnp.int32),
            pltpu.SMEM((2, 8), F32),
            pltpu.VMEM((1, WIDTH), F32),
            pltpu.VMEM((1, PART), F32),
            pltpu.VMEM((4, 64, WIDTH), BF16),
            pltpu.VMEM((NY, 2, 64, PART), BF16),
            pltpu.VMEM((NY, 2, 64, PART), BF16),
            pltpu.VMEM((128, WIDTH), BF16),
            pltpu.VMEM((NY, 64, PART), BF16),
            pltpu.VMEM((NY, 64, PART), BF16),
            pltpu.VMEM((NEP, 8, 128), BF16),
            pltpu.VMEM((NEP, 8, 128), BF16),
            pltpu.VMEM((2, NY, ROWS, PART), BF16),
            pltpu.VMEM((2, NY, 8, PART), BF16),
            pltpu.VMEM((NY, 8, PART), F32),
            pltpu.VMEM((NY, 8, PART), F32),
            pltpu.VMEM((8, 64), BF16),
            pltpu.VMEM((8, 64), BF16),
            pltpu.VMEM((16, 256), F32),
            pltpu.VMEM((ROWS, 128), BF16),
            pltpu.VMEM((ROWS, 128), BF16),
            pltpu.VMEM((7, ROWS, PART), jnp.int16),
            pltpu.VMEM((7, ROWS, PART), jnp.int16),
            pltpu.VMEM((7, 1, 128), F32),
            pltpu.VMEM((8, 1, 128), F32),
            pltpu.VMEM((3, ROWS, PART), F32),
            pltpu.VMEM((NEP, 8, 128), F32),
            pltpu.VMEM((NEP, 8, 128), F32),
            pltpu.VMEM((1, 128), F32),
            pltpu.VMEM((NTP, 1, 128), F32),
            pltpu.VMEM((ROWS, 128), F32),
            pltpu.VMEM((8, 128), F32),
            dma((6,)),
            dma((20,)),
            dma((2 * NY,)),
            dma((2 * NY,)),
            dma,
            dma,
            dma,
            dma,
            dma,
            dma,
            dma,
            dma,
            dma,
            dma,
            dma((14,)),
            dma((16,)),
            dma((8,)),
            dma((8,)),
            dma,
            dma,
            dma((8,)),
            dma((8,)),
            dma((8,)),
            dma((8,)),
            dma,
            dma,
            dma,
            dma,
        ],
        compiler_params=pltpu.CompilerParams(collective_id=0, has_side_effects=True),
    )(
        tokens,
        norm_gain.reshape(1, WIDTH),
        route_experts.T,
        route_logits.T,
        jnp.swapaxes(expert_gate, 1, 2),
        jnp.swapaxes(expert_up, 1, 2),
        expert_down,
        dense_gate.T,
        dense_up.T,
        dense_down,
        mix_weight.reshape(1, WIDTH),
        out_gain.reshape(1, PART),
    )


def solution(mesh):
    tp = "tp"
    in_specs = (
        P("ep", tp),
        P(),
        P("ep", None),
        P("ep", None),
        P("ep", None, tp),
        P("ep", None, tp),
        P("ep", tp, None),
        P(None, tp),
        P(None, tp),
        P(tp, None),
        P(),
        P(tp),
    )
    return jax.shard_map(
        local, mesh=mesh, in_specs=in_specs, out_specs=P("ep", tp), check_vma=False
    )
```

```python
import functools

import jax
import jax.numpy as jnp
from jax import lax
from jax.experimental import pallas as pl
from jax.experimental.pallas import tpu as pltpu
from jax.sharding import PartitionSpec as P

MESH = pl.DeviceIdType.MESH
F32 = jnp.float32
BF16 = jnp.bfloat16
EPS = 1e-06

NX, NZ, NY = 4, 8, 8
NEP = NX * NZ
NTP = 2 * NY
ROWS = 128
HALF = ROWS // 2
PART = 256
WIDTH = 4096


def rcopy(src, dst, send_sem, recv_sem, device):
    return pltpu.make_async_remote_copy(
        src_ref=src,
        dst_ref=dst,
        send_sem=send_sem,
        recv_sem=recv_sem,
        device_id=device,
        device_id_type=MESH,
    )


def nt_dot(a, b):
    return lax.dot_general(a, b, (((1,), (1,)), ((), ())), preferred_element_type=F32)


def silu(v):
    return v / (1.0 + jnp.exp(-v))


def kernel(
    tok_hbm,
    gain_hbm,
    routes_hbm,
    logits_hbm,
    wg,
    wu,
    wd,
    dg,
    du,
    dd,
    mixw_hbm,
    ogain_hbm,
    out,
    tok,
    gain,
    routes,
    logits,
    mixw,
    ogain,
    w_gu,
    wd_all,
    w_dense,
    dd_own,
    dd_par,
    a2a_out,
    a2a_in,
    gathered,
    tok_all,
    dense_out,
    dense_in,
    dh_own,
    dh_par,
    comb,
    slots,
    r_out,
    r_in,
    acts,
    hid,
    q_out,
    q_in,
    s_out,
    s_in,
    kept,
    ret_out,
    ret_in,
    sq_out,
    sq_in,
    gate_ref,
    i_sem,
    w_sem,
    wp_ssem,
    wp_rsem,
    a2a_ssem,
    a2a_rsem,
    tok_ssem,
    tok_rsem,
    tp_ssem,
    tp_rsem,
    dh_ssem,
    dh_rsem,
    dense_ssem,
    dense_rsem,
    ag_ssem,
    ag_rsem,
    pf_ssem,
    pf_rsem,
    r_ssem,
    r_rsem,
    q_ssem,
    q_rsem,
    sc_ssem,
    sc_rsem,
    ret_ssem,
    ret_rsem,
    sq_ssem,
    sq_rsem,
):
    me_e = lax.axis_index("ep")
    me_t = lax.axis_index("tp")
    z, x = lax.div(me_e, NX), lax.rem(me_e, NX)
    y, core = lax.div(me_t, 2), lax.rem(me_t, 2)
    other = 1 - core
    partner = (me_e, y * 2 + other)
    zs = [lax.rem(z + k, NZ) * NX for k in range(NZ)]
    xs = [lax.rem(x + k, NX) for k in range(NX)]
    ys = [lax.rem(y + k, NY) for k in range(NY)]
    peers = [zs[dz] + xs[dx] for dz in (4, 3, 5, 2, 6, 1, 7, 0) for dx in (2, 1, 3, 0)][:-1]
    y_order = (4, 3, 5, 2, 6, 1, 7)

    def ydev(step):
        return (me_e, ys[step % NY] * 2 + core)

    barrier = pltpu.get_barrier_semaphore()
    for peer in peers:
        pl.semaphore_signal(barrier, inc=1, device_id=(peer, me_t), device_id_type=MESH)
    for step in y_order:
        for c in range(2):
            pl.semaphore_signal(
                barrier, inc=1, device_id=(me_e, ys[step] * 2 + c), device_id_type=MESH
            )
    pl.semaphore_signal(barrier, inc=1, device_id=partner, device_id_type=MESH)

    smalls = [
        pltpu.make_async_copy(routes_hbm, routes, i_sem.at[0]),
        pltpu.make_async_copy(logits_hbm, logits, i_sem.at[1]),
        pltpu.make_async_copy(tok_hbm, tok, i_sem.at[2]),
        pltpu.make_async_copy(gain_hbm, gain, i_sem.at[3]),
        pltpu.make_async_copy(mixw_hbm, mixw, i_sem.at[4]),
        pltpu.make_async_copy(ogain_hbm, ogain, i_sem.at[5]),
    ]
    loads = [
        pltpu.make_async_copy(dg, w_dense.at[pl.ds(0, 64)], w_sem.at[0]),
        pltpu.make_async_copy(du, w_dense.at[pl.ds(64, 64)], w_sem.at[1]),
        pltpu.make_async_copy(wg, w_gu.at[0, pl.ds(0, 2)], w_sem.at[2]),
        pltpu.make_async_copy(wu, w_gu.at[0, pl.ds(2, 2)], w_sem.at[3]),
    ]

    def columns(k, c):
        return pl.ds(pl.multiple_of((2 * k + c) * PART, PART), PART)

    for k in range(NY):
        loads.append(
            pltpu.make_async_copy(dd.at[:, columns(k, core)], dd_own.at[k], w_sem.at[4 + k])
        )
    for k in range(NY):
        loads.append(
            pltpu.make_async_copy(wd.at[:, :, columns(k, core)], wd_all.at[k, 0], w_sem.at[12 + k])
        )
    for load in smalls + loads:
        load.start()

    for load in smalls[0:3]:
        load.wait()
    lane = lax.broadcasted_iota(jnp.int32, (8, 256), 1)
    sub = lax.broadcasted_iota(jnp.int32, (8, 256), 0)
    expert = 2 * (lane // 8) + (lane // 2) % 2
    half = (lane // 4) % 2
    r0 = jnp.zeros((8, 256), jnp.int32)
    r1 = jnp.zeros((8, 256), jnp.int32)
    l0 = jnp.zeros((8, 256), F32)
    l1 = jnp.zeros((8, 256), F32)
    for t in range(8):
        r0 = jnp.where(sub == t, routes[0, t], r0)
        r1 = jnp.where(sub == t, routes[1, t], r1)
        l0 = jnp.where(sub == t, logits[0, t], l0)
        l1 = jnp.where(sub == t, logits[1, t], l1)
    top = jnp.maximum(l0, l1)
    e0, e1 = jnp.exp(l0 - top), jnp.exp(l1 - top)
    is0, is1 = (r0 == expert), (r1 == expert)
    hit = jnp.where(is0, 1.0, 0.0) + jnp.where(is1, 1.0, 0.0)
    before = jnp.zeros((8, 256), F32)
    for t in range(7):
        before = before + jnp.where(sub > t, hit[t : t + 1, :], 0.0)
    placed = jnp.where(before == (lane % 2).astype(F32), hit, 0.0)
    weight = (jnp.where(is0, e0, 0.0) + jnp.where(is1, e1, 0.0)) / (e0 + e1) * placed
    comb[0:8, :] = jnp.where(half == 0, weight, 0.0)
    comb[8:16, :] = jnp.where(half == 1, weight, 0.0)
    slots[...] = placed
    place = jnp.concatenate(
        [jnp.where(half == 0, placed, 0.0), jnp.where(half == 1, placed, 0.0)], axis=0
    ).astype(BF16)
    tok_value = tok[...]
    halves = jnp.concatenate(
        [tok_value[:, 0:128].astype(F32), tok_value[:, 128:256].astype(F32)], axis=0
    ).astype(BF16)
    a2a_out[...] = (
        lax.dot_general(place, halves, (((0,), (0,)), ((), ())), preferred_element_type=F32)
        .astype(BF16)
        .reshape(NEP, 8, 128)
    )
    a2a_in[me_e] = a2a_out[me_e]
    tok_all[core, y] = tok_value

    pl.semaphore_wait(barrier, NEP - 1 + NTP - 1)

    for peer in peers:
        rcopy(a2a_out.at[peer], a2a_in.at[me_e], a2a_ssem, a2a_rsem, (peer, me_t)).start()

    for step in y_order:
        rcopy(tok, tok_all.at[core, y], tok_ssem, tok_rsem, ydev(step)).start()

    wparts = []
    for k in range(NY):
        copy = rcopy(
            dd.at[:, columns(k, other)], dd_par.at[k], wp_ssem.at[k], wp_rsem.at[k], partner
        )
        copy.start()
        wparts.append(copy)
    for k in range(NY):
        copy = rcopy(
            wd.at[:, :, columns(k, other)],
            wd_all.at[k, 1],
            wp_ssem.at[NY + k],
            wp_rsem.at[NY + k],
            partner,
        )
        copy.start()
        wparts.append(copy)
    for k, ref in enumerate((wg, wu)):
        copy = rcopy(
            ref,
            w_gu.at[1, pl.ds(2 * k, 2)],
            wp_ssem.at[2 * NY + k],
            wp_rsem.at[2 * NY + k],
            partner,
        )
        copy.start()
        wparts.append(copy)

    rcopy(
        a2a_out.at[pl.ds(0, NEP - 1)],
        a2a_in.at[pl.ds(0, NEP - 1)],
        a2a_ssem,
        a2a_rsem,
        partner,
    ).wait_recv()
    pairs = a2a_in[...].astype(F32).reshape(16, 2, 8, 128)
    even, odd = pairs[:, 0], pairs[:, 1]
    sub3 = lax.broadcasted_iota(jnp.int32, (16, 8, 128), 1)
    left = jnp.where(sub3 < 4, even, pltpu.roll(odd, 4, 1)).reshape(ROWS, 128)
    right = jnp.where(sub3 < 4, pltpu.roll(even, 4, 1), odd).reshape(ROWS, 128)
    gathered[core, y, :, 0:128] = left.astype(BF16)
    gathered[core, y, :, 128:256] = right.astype(BF16)

    sends = []
    whole, low, high = pl.ds(0, ROWS), pl.ds(0, ROWS // 2), pl.ds(ROWS // 2, ROWS // 2)

    def ag_send(rel, rows, sem, step):
        ref = gathered.at[core, ys[rel], rows]
        copy = rcopy(ref, ref, ag_ssem.at[len(sends)], ag_rsem.at[sem], ydev(step))
        copy.start()
        sends.append(copy)

    def ag_wait(rel, rows, sem):
        ref = gathered.at[core, ys[rel], rows]
        rcopy(ref, ref, ag_ssem.at[0], ag_rsem.at[sem], partner).wait_recv()

    passes = []

    def pass_on(rel):
        ref = gathered.at[core, ys[rel]]
        copy = rcopy(ref, ref, pf_ssem.at[rel], pf_rsem.at[rel], partner)
        copy.start()
        passes.append(copy)

    def pass_wait(rel):
        ref = gathered.at[other, ys[rel]]
        rcopy(ref, ref, pf_ssem.at[rel], pf_rsem.at[rel], partner).wait_recv()

    ag_send(0, low, 12, 2)
    ag_send(0, low, 4, -2)
    ag_send(0, high, 13, 2)
    ag_send(0, high, 5, -2)
    ag_send(0, whole, 14, 1)
    ag_send(0, whole, 2, -1)
    pass_on(0)

    tok_step = rcopy(
        tok_all.at[0, pl.ds(0, NY - 1)], tok_all.at[0, pl.ds(0, NY - 1)], tok_ssem, tok_rsem, partner
    )
    tok_step.wait_recv()
    tok_pass = rcopy(tok_all.at[core], tok_all.at[core], tp_ssem, tp_rsem, partner)
    tok_pass.start()
    for load in smalls[3:6] + loads[0:2]:
        load.wait()
    rcopy(tok_all.at[other], tok_all.at[other], tp_ssem, tp_rsem, partner).wait_recv()

    squares = jnp.zeros((8, PART), F32)
    for j in range(NTP):
        v = tok_all[j % 2, j // 2].astype(F32)
        squares = squares + v * v
    scale = lax.rsqrt(jnp.sum(squares, axis=1, keepdims=True) / WIDTH + EPS)
    r_out[...] = jnp.sum(slots[...] * scale, axis=0, keepdims=True)
    for peer in peers:
        rcopy(r_out, r_in.at[me_e], r_ssem, r_rsem, (peer, me_t)).start()
    r_in[me_e] = r_out[...]
    act = jnp.zeros((8, 128), F32)
    mix_acc = jnp.zeros((8, PART), F32)
    for j in range(NTP):
        cols = slice(j * PART, (j + 1) * PART)
        n = (tok_all[j % 2, j // 2].astype(F32) * scale * gain[:, cols]).astype(BF16)
        mix_acc = mix_acc + n.astype(F32) * mixw[:, cols]
        act = act + nt_dot(n, w_dense[:, cols])
    gate_ref[...] = jnp.broadcast_to(
        jax.nn.sigmoid(jnp.sum(mix_acc, axis=1, keepdims=True)), (8, 128)
    )
    dh_own[...] = (silu(act[:, 0:64]) * act[:, 64:128]).astype(BF16)
    dh_copy = rcopy(dh_own, dh_par, dh_ssem, dh_rsem, partner)
    dh_copy.start()

    ag_wait(6, low, 12)
    ag_send(6, low, 8, 2)
    ag_send(6, low, 10, 1)
    ag_wait(2, low, 4)
    ag_send(2, low, 6, -1)
    ag_wait(6, high, 13)
    ag_send(6, high, 11, 1)
    ag_wait(2, high, 5)
    ag_send(2, high, 9, -2)
    ag_send(2, high, 7, -1)
    pass_on(6)
    pass_on(2)
    for load in loads[4:12]:
        load.wait()
    for copy in wparts[0:NY]:
        copy.wait_recv()
    dh_copy.wait_recv()
    for k in range(NY):
        dense_out[k] = jnp.dot(
            dh_own[...], dd_own[k], preferred_element_type=F32
        ) + jnp.dot(dh_par[...], dd_par[k], preferred_element_type=F32)
    dense_in[y] = dense_out[y]
    for rel in (7, 1):
        ag_wait(rel, whole, 2 * rel)
        pass_on(rel)
    for step in y_order:
        rcopy(
            dense_out.at[ys[step]], dense_in.at[y], dense_ssem, dense_rsem, ydev(step)
        ).start()
    loads[2].wait()
    loads[3].wait()
    for copy in wparts[2 * NY :]:
        copy.wait_recv()
    rcopy(
        r_in.at[pl.ds(0, NEP - 1)], r_in.at[pl.ds(0, NEP - 1)], r_ssem, r_rsem, partner
    ).wait_recv()
    picked = (
        lax.broadcasted_iota(jnp.int32, (ROWS, NEP), 0) // 4
        == lax.broadcasted_iota(jnp.int32, (ROWS, NEP), 1)
    )
    spread = jnp.dot(
        jnp.where(picked, 1.0, 0.0),
        r_in[...].reshape(NEP, 256),
        preferred_element_type=F32,
        precision=lax.Precision.HIGHEST,
    )
    wanted = me_e * 8 + lax.broadcasted_iota(jnp.int32, (ROWS, 256), 0) % 4
    here = lax.broadcasted_iota(jnp.int32, (ROWS, 256), 1) == wanted
    row_scale = jnp.sum(jnp.where(here, spread, 0.0), axis=1, keepdims=True)

    def project(c, rel, first=False):
        cols = pl.ds(pl.multiple_of((2 * ys[rel] + c) * PART, PART), PART)
        n = (gathered[c, ys[rel]].astype(F32) * row_scale * gain[:, cols]).astype(BF16)
        for k in range(2):
            v = nt_dot(n, w_gu[k, :, :, cols].reshape(256, PART))
            acts[k] = v if first else acts[k] + v

    project(core, 0, True)
    for rel in (6, 2, 7, 1):
        project(core, rel)
    for rel in (0, 6, 2, 7, 1):
        pass_wait(rel)
        project(other, rel)
    for rel in (5, 3):
        ag_wait(rel, low, 2 * rel)
        ag_wait(rel, high, 2 * rel + 1)
        pass_on(rel)
    ag_wait(4, low, 8)
    ag_wait(4, high, 9)
    pass_on(4)
    for rel in (5, 3, 4):
        project(core, rel)
    for rel in (5, 3, 4):
        pass_wait(rel)
        project(other, rel)

    row = lax.broadcasted_iota(jnp.int32, (ROWS, 128), 0)
    col = lax.broadcasted_iota(jnp.int32, (ROWS, 128), 1)
    mine = (row // 2) % 2 == col // 64
    for k in range(2):
        v = acts[k]
        hidden = silu(v[:, 0:128]) * v[:, 128:256]
        hid[:, k * 128 : (k + 1) * 128] = jnp.where(mine, hidden, 0.0).astype(BF16)
    for load in loads[12:]:
        load.wait()
    for copy in wparts[NY : 2 * NY]:
        copy.wait_recv()

    diagonal = (
        lax.broadcasted_iota(jnp.int32, (HALF, 128), 0)
        == lax.broadcasted_iota(jnp.int32, (HALF, 128), 1)
    )

    def partial(rel):
        return jnp.dot(
            hid[...], wd_all[ys[rel]].reshape(256, PART), preferred_element_type=F32
        )

    def pack(value, slot, h):
        most = jnp.maximum(jnp.max(jnp.abs(value), axis=1, keepdims=True), 1e-30)
        q_out[slot, h] = jnp.round(value * (32767.0 / most)).astype(jnp.int16)
        s_out[slot, h] = jnp.sum(
            jnp.where(diagonal, most * (1.0 / 32767.0), 0.0), axis=0, keepdims=True
        )

    def unpack(slot, h):
        unit = jnp.sum(jnp.where(diagonal, s_in[slot, h], 0.0), axis=1, keepdims=True)
        return q_in[slot, h].astype(F32) * unit

    qsends = []

    def q_copies(slot, h, device):
        at = (slot, h)
        return (
            rcopy(q_out.at[at], q_in.at[at], q_ssem.at[at], q_rsem.at[at], device),
            rcopy(s_out.at[at], s_in.at[at], sc_ssem.at[at], sc_rsem.at[at], device),
        )

    def q_send(value, slot, h, step):
        pack(value, slot, h)
        for copy in q_copies(slot, h, ydev(step)):
            copy.start()
            qsends.append(copy)

    def q_get(slot, h):
        for copy in q_copies(slot, h, partner):
            copy.wait_recv()
        return unpack(slot, h)

    v = partial(4)
    q_send(v[:HALF], 2, 0, 2)
    q_send(v[HALF:], 2, 1, -2)
    v, w = partial(3), partial(5)
    q_send(v[:HALF], 0, 0, 1)
    q_send(w[HALF:], 1, 1, -1)
    q_send(v[HALF:], 0, 1, 1)
    q_send(w[:HALF], 1, 0, -1)
    v, w = partial(1), partial(7)
    for h in range(2):
        q_send(v[h * HALF : (h + 1) * HALF], 3, h, 1)
        q_send(w[h * HALF : (h + 1) * HALF], 4, h, -1)
    kept[0] = partial(2)
    kept[1] = partial(6)
    kept[2] = partial(0)
    dense_step = rcopy(
        dense_out.at[pl.ds(0, NY - 1)],
        dense_in.at[pl.ds(0, NY - 1)],
        dense_ssem,
        dense_rsem,
        partner,
    )
    dense_step.wait_recv()
    dense = dense_in[0]
    for k in range(1, NY):
        dense = dense + dense_in[k]
    gate = gate_ref[...]
    dense = jnp.concatenate([gate, gate], axis=1) * dense
    q_send(kept[0, :HALF] + q_get(2, 0) + q_get(0, 0), 5, 0, 2)
    q_send(kept[1, HALF:] + q_get(2, 1) + q_get(1, 1), 6, 1, -2)
    q_send(kept[0, HALF:] + q_get(0, 1), 5, 1, 2)
    q_send(kept[1, :HALF] + q_get(1, 0), 6, 0, -2)
    for h in range(2):
        kept[2, h * HALF : (h + 1) * HALF] += q_get(3, h) + q_get(4, h)
    summed = kept[2] + jnp.concatenate(
        [q_get(5, 0) + q_get(6, 0), q_get(6, 1) + q_get(5, 1)], axis=0
    )
    left = summed[:, 0:128].reshape(16, 8, 128)
    right = summed[:, 128:256].reshape(16, 8, 128)
    even = jnp.where(sub3 < 4, left, pltpu.roll(right, 4, 1))
    odd = jnp.where(sub3 < 4, pltpu.roll(left, 4, 1), right)
    ret_out[...] = jnp.stack([even, odd], axis=1).reshape(NEP, 8, 128)
    for peer in peers:
        rcopy(ret_out.at[peer], ret_in.at[me_e], ret_ssem, ret_rsem, (peer, me_t)).start()
    ret_in[me_e] = ret_out[me_e]
    rcopy(
        ret_out.at[pl.ds(0, NEP - 1)],
        ret_in.at[pl.ds(0, NEP - 1)],
        ret_ssem,
        ret_rsem,
        partner,
    ).wait_recv()
    mixed = jnp.dot(
        comb[...],
        ret_in[...].reshape(256, 128),
        preferred_element_type=F32,
        precision=lax.Precision.HIGHEST,
    )
    combined = jnp.concatenate([mixed[0:8], mixed[8:16]], axis=1) + dense
    token_diagonal = (
        lax.broadcasted_iota(jnp.int32, (8, 128), 0)
        == lax.broadcasted_iota(jnp.int32, (8, 128), 1)
    )
    own = jnp.sum(
        jnp.where(token_diagonal, jnp.sum(combined * combined, axis=1, keepdims=True), 0.0),
        axis=0,
        keepdims=True,
    )
    sq_out[...] = own
    for step in y_order:
        for c in range(2):
            rcopy(sq_out, sq_in.at[me_t], sq_ssem, sq_rsem, (me_e, ys[step] * 2 + c)).start()
    rcopy(sq_out, sq_in.at[me_t], sq_ssem, sq_rsem, partner).start()
    sq_in[me_t] = own
    sq_step = rcopy(
        sq_in.at[pl.ds(0, NTP - 1)], sq_in.at[pl.ds(0, NTP - 1)], sq_ssem, sq_rsem, partner
    )
    sq_step.wait_recv()
    total_sq = sq_in[0]
    for j in range(1, NTP):
        total_sq = total_sq + sq_in[j]
    final = lax.rsqrt(
        jnp.sum(jnp.where(token_diagonal, total_sq, 0.0), axis=1, keepdims=True) / WIDTH + EPS
    )
    out[...] = (combined * final * ogain[...]).astype(BF16)

    for copy in wparts + sends + passes + [tok_pass, dh_copy] + qsends:
        copy.wait_send()
    tok_step.wait_send()
    dense_step.wait_send()
    sq_step.wait_send()
    for ref, ssem, rsem in (
        (a2a_out, a2a_ssem, a2a_rsem),
        (r_in, r_ssem, r_rsem),
        (ret_out, ret_ssem, ret_rsem),
    ):
        part = ref.at[pl.ds(0, NEP - 1)]
        rcopy(part, part, ssem, rsem, partner).wait_send()


def local(
    tokens,
    norm_gain,
    route_experts,
    route_logits,
    expert_gate,
    expert_up,
    expert_down,
    dense_gate,
    dense_up,
    dense_down,
    mix_weight,
    out_gain,
):
    vmem = pl.BlockSpec(memory_space=pltpu.VMEM)
    dma = pltpu.SemaphoreType.DMA
    return pl.pallas_call(
        kernel,
        out_shape=pltpu.VMEM((8, PART), BF16),
        in_specs=[pl.BlockSpec(memory_space=pl.ANY)] * 12,
        out_specs=vmem,
        scratch_shapes=[
            pltpu.VMEM((8, PART), BF16),
            pltpu.VMEM((1, WIDTH), F32),
            pltpu.SMEM((2, 8), jnp.int32),
            pltpu.SMEM((2, 8), F32),
            pltpu.VMEM((1, WIDTH), F32),
            pltpu.VMEM((1, PART), F32),
            pltpu.VMEM((2, 4, 64, WIDTH), BF16),
            pltpu.VMEM((NY, 2, 2, 64, PART), BF16),
            pltpu.VMEM((128, WIDTH), BF16),
            pltpu.VMEM((NY, 64, PART), BF16),
            pltpu.VMEM((NY, 64, PART), BF16),
            pltpu.VMEM((NEP, 8, 128), BF16),
            pltpu.VMEM((NEP, 8, 128), BF16),
            pltpu.VMEM((2, NY, ROWS, PART), BF16),
            pltpu.VMEM((2, NY, 8, PART), BF16),
            pltpu.VMEM((NY, 8, PART), F32),
            pltpu.VMEM((NY, 8, PART), F32),
            pltpu.VMEM((8, 64), BF16),
            pltpu.VMEM((8, 64), BF16),
            pltpu.VMEM((16, 256), F32),
            pltpu.VMEM((8, 256), F32),
            pltpu.VMEM((1, 256), F32),
            pltpu.VMEM((NEP, 1, 256), F32),
            pltpu.VMEM((2, ROWS, 256), F32),
            pltpu.VMEM((ROWS, 256), BF16),
            pltpu.VMEM((7, 2, HALF, PART), jnp.int16),
            pltpu.VMEM((7, 2, HALF, PART), jnp.int16),
            pltpu.VMEM((7, 2, 1, 128), F32),
            pltpu.VMEM((7, 2, 1, 128), F32),
            pltpu.VMEM((3, ROWS, PART), F32),
            pltpu.VMEM((NEP, 8, 128), F32),
            pltpu.VMEM((NEP, 8, 128), F32),
            pltpu.VMEM((1, 128), F32),
            pltpu.VMEM((NTP, 1, 128), F32),
            pltpu.VMEM((8, 128), F32),
            dma((6,)),
            dma((20,)),
            dma((2 * NY + 2,)),
            dma((2 * NY + 2,)),
            dma,
            dma,
            dma,
            dma,
            dma,
            dma,
            dma,
            dma,
            dma,
            dma,
            dma((14,)),
            dma((16,)),
            dma((8,)),
            dma((8,)),
            dma,
            dma,
            dma((7, 2)),
            dma((7, 2)),
            dma((7, 2)),
            dma((7, 2)),
            dma,
            dma,
            dma,
            dma,
        ],
        compiler_params=pltpu.CompilerParams(
            collective_id=0, has_side_effects=True, vmem_limit_bytes=56650000
        ),
    )(
        tokens,
        norm_gain.reshape(1, WIDTH),
        route_experts.T,
        route_logits.T,
        jnp.swapaxes(expert_gate, 1, 2),
        jnp.swapaxes(expert_up, 1, 2),
        expert_down,
        dense_gate.T,
        dense_up.T,
        dense_down,
        mix_weight.reshape(1, WIDTH),
        out_gain.reshape(1, PART),
    )


def solution(mesh):
    tp = "tp"
    in_specs = (
        P("ep", tp),
        P(),
        P("ep", None),
        P("ep", None),
        P("ep", None, tp),
        P("ep", None, tp),
        P("ep", tp, None),
        P(None, tp),
        P(None, tp),
        P(tp, None),
        P(),
        P(tp),
    )
    return jax.shard_map(
        local, mesh=mesh, in_specs=in_specs, out_specs=P("ep", tp), check_vma=False
    )
```

```python
import functools

import jax
import jax.numpy as jnp
from jax import lax
from jax.experimental import pallas as pl
from jax.experimental.pallas import tpu as pltpu
from jax.sharding import PartitionSpec as P

MESH = pl.DeviceIdType.MESH
F32 = jnp.float32
BF16 = jnp.bfloat16
EPS = 1e-06

NX, NZ, NY = 4, 8, 8
NEP = NX * NZ
NTP = 2 * NY
ROWS = 128
FAR = (3, 4, 5)
NEAR = (2, 6, 1, 7)
PART = 256
WIDTH = 4096


def rcopy(src, dst, send_sem, recv_sem, device):
    return pltpu.make_async_remote_copy(
        src_ref=src,
        dst_ref=dst,
        send_sem=send_sem,
        recv_sem=recv_sem,
        device_id=device,
        device_id_type=MESH,
    )


def nt_dot(a, b):
    return lax.dot_general(a, b, (((1,), (1,)), ((), ())), preferred_element_type=F32)


def silu(v):
    return v / (1.0 + jnp.exp(-v))


def kernel(
    tok_hbm,
    gain_hbm,
    routes_hbm,
    logits_hbm,
    wg,
    wu,
    wd,
    dg,
    du,
    dd,
    mixw_hbm,
    ogain_hbm,
    out,
    tok,
    gain,
    routes,
    logits,
    mixw,
    ogain,
    w_gu,
    wd_all,
    w_dense,
    dd_own,
    dd_par,
    a2a_out,
    a2a_in,
    far_out,
    far_in,
    gathered,
    tok_all,
    dense_out,
    dense_in,
    dh_own,
    dh_par,
    comb,
    place,
    slots,
    r_out,
    r_in,
    acts,
    hid,
    q_out,
    q_in,
    s_out,
    s_in,
    fq_out,
    fq_in,
    fs_out,
    fs_in,
    fy_out,
    fy_in,
    kept,
    ret_out,
    ret_in,
    sq_out,
    sq_in,
    gate_ref,
    i_sem,
    w_sem,
    wp_ssem,
    wp_rsem,
    a2a_ssem,
    a2a_rsem,
    far_ssem,
    far_rsem,
    tok_ssem,
    tok_rsem,
    dh_ssem,
    dh_rsem,
    dense_ssem,
    dense_rsem,
    ag_ssem,
    ag_rsem,
    pf_ssem,
    pf_rsem,
    r_ssem,
    r_rsem,
    q_ssem,
    q_rsem,
    sc_ssem,
    sc_rsem,
    fq_ssem,
    fq_rsem,
    fs_ssem,
    fs_rsem,
    fy_ssem,
    fy_rsem,
    ret_ssem,
    ret_rsem,
    sq_ssem,
    sq_rsem,
):
    me_e = lax.axis_index("ep")
    me_t = lax.axis_index("tp")
    z, x = lax.div(me_e, NX), lax.rem(me_e, NX)
    y, core = lax.div(me_t, 2), lax.rem(me_t, 2)
    other = 1 - core
    partner = (me_e, y * 2 + other)
    zs = [lax.rem(z + k, NZ) * NX for k in range(NZ)]
    xs = [lax.rem(x + k, NX) for k in range(NX)]
    ys = [lax.rem(y + k, NY) for k in range(NY)]
    peers = [zs[dz] + xs[dx] for dz in (4, 3, 5, 2, 6, 1, 7, 0) for dx in (2, 1, 3, 0)][:-1]
    y_order = (4, 3, 5, 2, 6, 1, 7)

    def ydev(step):
        return (me_e, ys[step % NY] * 2 + core)

    barrier = pltpu.get_barrier_semaphore()
    for peer in peers:
        pl.semaphore_signal(barrier, inc=1, device_id=(peer, me_t), device_id_type=MESH)
    for step in y_order:
        for c in range(2):
            pl.semaphore_signal(
                barrier, inc=1, device_id=(me_e, ys[step] * 2 + c), device_id_type=MESH
            )
    pl.semaphore_signal(barrier, inc=1, device_id=partner, device_id_type=MESH)

    smalls = [
        pltpu.make_async_copy(routes_hbm, routes, i_sem.at[0]),
        pltpu.make_async_copy(logits_hbm, logits, i_sem.at[1]),
        pltpu.make_async_copy(tok_hbm, tok, i_sem.at[2]),
        pltpu.make_async_copy(gain_hbm, gain, i_sem.at[3]),
        pltpu.make_async_copy(mixw_hbm, mixw, i_sem.at[4]),
        pltpu.make_async_copy(ogain_hbm, ogain, i_sem.at[5]),
    ]
    loads = [
        pltpu.make_async_copy(dg, w_dense.at[pl.ds(0, 64)], w_sem.at[0]),
        pltpu.make_async_copy(du, w_dense.at[pl.ds(64, 64)], w_sem.at[1]),
        pltpu.make_async_copy(wg, w_gu.at[0, pl.ds(0, 2)], w_sem.at[2]),
        pltpu.make_async_copy(wu, w_gu.at[0, pl.ds(2, 2)], w_sem.at[3]),
    ]

    def columns(k, c):
        return pl.ds(pl.multiple_of((2 * k + c) * PART, PART), PART)

    for k in range(NY):
        loads.append(
            pltpu.make_async_copy(dd.at[:, columns(k, core)], dd_own.at[k], w_sem.at[4 + k])
        )
    for k in range(NY):
        loads.append(
            pltpu.make_async_copy(wd.at[:, :, columns(k, core)], wd_all.at[k, 0], w_sem.at[12 + k])
        )
    for load in smalls + loads:
        load.start()

    for load in smalls[0:3]:
        load.wait()
    lane = lax.broadcasted_iota(jnp.int32, (8, 256), 1)
    sub = lax.broadcasted_iota(jnp.int32, (8, 256), 0)
    expert = 2 * (lane // 8) + (lane // 2) % 2
    half = (lane // 4) % 2
    r0 = jnp.zeros((8, 256), jnp.int32)
    r1 = jnp.zeros((8, 256), jnp.int32)
    l0 = jnp.zeros((8, 256), F32)
    l1 = jnp.zeros((8, 256), F32)
    for t in range(8):
        r0 = jnp.where(sub == t, routes[0, t], r0)
        r1 = jnp.where(sub == t, routes[1, t], r1)
        l0 = jnp.where(sub == t, logits[0, t], l0)
        l1 = jnp.where(sub == t, logits[1, t], l1)
    top = jnp.maximum(l0, l1)
    e0, e1 = jnp.exp(l0 - top), jnp.exp(l1 - top)
    is0, is1 = (r0 == expert), (r1 == expert)
    hit = jnp.where(is0, 1.0, 0.0) + jnp.where(is1, 1.0, 0.0)
    before = jnp.zeros((8, 256), F32)
    for t in range(7):
        before = before + jnp.where(sub > t, hit[t : t + 1, :], 0.0)
    placed = jnp.where(before == (lane % 2).astype(F32), hit, 0.0)
    weight = (jnp.where(is0, e0, 0.0) + jnp.where(is1, e1, 0.0)) / (e0 + e1) * placed
    comb[0:8, :] = jnp.where(half == 0, weight, 0.0)
    comb[8:16, :] = jnp.where(half == 1, weight, 0.0)
    slots[...] = placed
    place[...] = jnp.concatenate(
        [jnp.where(half == 0, placed, 0.0), jnp.where(half == 1, placed, 0.0)], axis=0
    ).astype(BF16)

    def placed_rows(value):
        halves = jnp.concatenate(
            [value[:, 0:128].astype(F32), value[:, 128:256].astype(F32)], axis=0
        ).astype(BF16)
        rows = lax.dot_general(
            place[...], halves, (((0,), (0,)), ((), ())), preferred_element_type=F32
        )
        return rows.astype(BF16).reshape(NEP, 8, 128)

    tok_value = tok[...]
    a2a_out[...] = placed_rows(tok_value)
    a2a_in[me_e] = a2a_out[me_e]
    tok_all[me_t] = tok_value

    pl.semaphore_wait(barrier, NEP - 1 + NTP - 1)

    for step in y_order:
        for c in range(2):
            rcopy(
                tok, tok_all.at[me_t], tok_ssem, tok_rsem, (me_e, ys[step] * 2 + c)
            ).start()
    rcopy(tok, tok_all.at[me_t], tok_ssem, tok_rsem, partner).start()

    for peer in peers:
        rcopy(a2a_out.at[peer], a2a_in.at[me_e], a2a_ssem, a2a_rsem, (peer, me_t)).start()

    wparts = []
    for k in range(NY):
        copy = rcopy(
            dd.at[:, columns(k, other)], dd_par.at[k], wp_ssem.at[k], wp_rsem.at[k], partner
        )
        copy.start()
        wparts.append(copy)
    for k in range(NY):
        copy = rcopy(
            wd.at[:, :, columns(k, other)],
            wd_all.at[k, 1],
            wp_ssem.at[NY + k],
            wp_rsem.at[NY + k],
            partner,
        )
        copy.start()
        wparts.append(copy)
    for k, ref in enumerate((wg, wu)):
        copy = rcopy(
            ref,
            w_gu.at[1, pl.ds(2 * k, 2)],
            wp_ssem.at[2 * NY + k],
            wp_rsem.at[2 * NY + k],
            partner,
        )
        copy.start()
        wparts.append(copy)

    def arrived(src, dst, ssem, rsem, n):
        part = pl.ds(0, n)
        copy = rcopy(src.at[part], dst.at[part], ssem, rsem, partner)
        copy.wait_recv()
        return copy

    done = [arrived(tok_all, tok_all, tok_ssem, tok_rsem, NTP - 1)]
    squares = jnp.zeros((8, PART), F32)
    for j in range(NTP):
        v = tok_all[j].astype(F32)
        squares = squares + v * v
    scale = lax.rsqrt(jnp.sum(squares, axis=1, keepdims=True) / WIDTH + EPS)
    r_out[...] = jnp.sum(slots[...] * scale, axis=0, keepdims=True)
    for peer in peers:
        rcopy(r_out, r_in.at[me_e], r_ssem, r_rsem, (peer, me_t)).start()
    r_in[me_e] = r_out[...]
    for i, rel in enumerate(FAR):
        far_out[:, i] = placed_rows(tok_all[ys[rel] * 2 + core])
    for peer in peers:
        rcopy(far_out.at[peer], far_in.at[me_e], far_ssem, far_rsem, (peer, me_t)).start()
    far_in[me_e] = far_out[me_e]

    done.append(arrived(a2a_out, a2a_in, a2a_ssem, a2a_rsem, NEP - 1))
    sub3 = lax.broadcasted_iota(jnp.int32, (16, 8, 128), 1)

    def keep_rows(value, rel):
        pairs = value.astype(F32).reshape(16, 2, 8, 128)
        even, odd = pairs[:, 0], pairs[:, 1]
        left = jnp.where(sub3 < 4, even, pltpu.roll(odd, 4, 1)).reshape(ROWS, 128)
        right = jnp.where(sub3 < 4, pltpu.roll(even, 4, 1), odd).reshape(ROWS, 128)
        gathered[core, ys[rel], :, 0:128] = left.astype(BF16)
        gathered[core, ys[rel], :, 128:256] = right.astype(BF16)

    keep_rows(a2a_in[...], 0)

    sends = []

    def ag_copy(slot, k, rel, device):
        ref = gathered.at[core, ys[slot]]
        return rcopy(ref, ref, ag_ssem.at[k], ag_rsem.at[rel], device)

    for k, (rel, step) in enumerate(((6, 2), (2, -2), (7, 1), (1, -1))):
        copy = ag_copy(0, k, rel, ydev(step))
        copy.start()
        sends.append(copy)

    def pass_on(rel):
        ref = gathered.at[core, ys[rel]]
        copy = rcopy(ref, ref, pf_ssem.at[rel], pf_rsem.at[rel], partner)
        copy.start()
        sends.append(copy)

    def pass_wait(rel):
        ref = gathered.at[other, ys[rel]]
        rcopy(ref, ref, pf_ssem.at[rel], pf_rsem.at[rel], partner).wait_recv()

    pass_on(0)

    for load in smalls[3:6] + loads[0:2]:
        load.wait()
    act = jnp.zeros((8, 128), F32)
    mix_acc = jnp.zeros((8, PART), F32)
    for j in range(NTP):
        cols = slice(j * PART, (j + 1) * PART)
        n = (tok_all[j].astype(F32) * scale * gain[:, cols]).astype(BF16)
        mix_acc = mix_acc + n.astype(F32) * mixw[:, cols]
        act = act + nt_dot(n, w_dense[:, cols])
    gate_ref[...] = jnp.broadcast_to(
        jax.nn.sigmoid(jnp.sum(mix_acc, axis=1, keepdims=True)), (8, 128)
    )
    dh_own[...] = (silu(act[:, 0:64]) * act[:, 64:128]).astype(BF16)
    dh_copy = rcopy(dh_own, dh_par, dh_ssem, dh_rsem, partner)
    dh_copy.start()

    for rel in (6, 2):
        ag_copy(rel, 0, rel, partner).wait_recv()
        pass_on(rel)
    for load in loads[4:12]:
        load.wait()
    for copy in wparts[0:NY]:
        copy.wait_recv()
    dh_copy.wait_recv()
    for k in range(NY):
        dense_out[k] = jnp.dot(
            dh_own[...], dd_own[k], preferred_element_type=F32
        ) + jnp.dot(dh_par[...], dd_par[k], preferred_element_type=F32)
    dense_in[y] = dense_out[y]
    for rel in (7, 1):
        ag_copy(rel, 0, rel, partner).wait_recv()
        pass_on(rel)
    for step in y_order:
        rcopy(
            dense_out.at[ys[step]], dense_in.at[y], dense_ssem, dense_rsem, ydev(step)
        ).start()
    loads[2].wait()
    loads[3].wait()
    for copy in wparts[2 * NY :]:
        copy.wait_recv()
    done.append(arrived(r_in, r_in, r_ssem, r_rsem, NEP - 1))
    picked = (
        lax.broadcasted_iota(jnp.int32, (ROWS, NEP), 0) // 4
        == lax.broadcasted_iota(jnp.int32, (ROWS, NEP), 1)
    )
    spread = jnp.dot(
        jnp.where(picked, 1.0, 0.0),
        r_in[...].reshape(NEP, 256),
        preferred_element_type=F32,
        precision=lax.Precision.HIGHEST,
    )
    wanted = me_e * 8 + lax.broadcasted_iota(jnp.int32, (ROWS, 256), 0) % 4
    here = lax.broadcasted_iota(jnp.int32, (ROWS, 256), 1) == wanted
    row_scale = jnp.sum(jnp.where(here, spread, 0.0), axis=1, keepdims=True)

    def project(c, rel, first=False):
        cols = pl.ds(pl.multiple_of((2 * ys[rel] + c) * PART, PART), PART)
        n = (gathered[c, ys[rel]].astype(F32) * row_scale * gain[:, cols]).astype(BF16)
        for k in range(2):
            v = nt_dot(n, w_gu[k, :, :, cols].reshape(256, PART))
            acts[k] = v if first else acts[k] + v

    project(core, 0, True)
    for rel in NEAR:
        project(core, rel)
    for rel in (0,) + NEAR:
        pass_wait(rel)
        project(other, rel)
    done.append(arrived(far_out, far_in, far_ssem, far_rsem, NEP - 1))
    for i, rel in enumerate(FAR):
        keep_rows(far_in[:, i], rel)
        pass_on(rel)
    for rel in FAR:
        project(core, rel)
    for rel in FAR:
        pass_wait(rel)
        project(other, rel)

    row = lax.broadcasted_iota(jnp.int32, (ROWS, 128), 0)
    col = lax.broadcasted_iota(jnp.int32, (ROWS, 128), 1)
    mine = (row // 2) % 2 == col // 64
    for k in range(2):
        v = acts[k]
        hidden = silu(v[:, 0:128]) * v[:, 128:256]
        hid[:, k * 128 : (k + 1) * 128] = jnp.where(mine, hidden, 0.0).astype(BF16)
    for load in loads[12:]:
        load.wait()
    for copy in wparts[NY : 2 * NY]:
        copy.wait_recv()

    diagonal = row == col

    def partial(rel):
        return jnp.dot(
            hid[...], wd_all[ys[rel]].reshape(256, PART), preferred_element_type=F32
        )

    def column(value):
        return jnp.sum(jnp.where(diagonal, value, 0.0), axis=0, keepdims=True)

    def messages(value):
        left = value[:, 0:128].reshape(16, 8, 128)
        right = value[:, 128:256].reshape(16, 8, 128)
        even = jnp.where(sub3 < 4, left, pltpu.roll(right, 4, 1))
        odd = jnp.where(sub3 < 4, pltpu.roll(left, 4, 1), right)
        return jnp.stack([even, odd], axis=1).reshape(NEP, 8, 128)

    def q_copies(k, device):
        return (
            rcopy(q_out.at[k], q_in.at[k], q_ssem.at[k], q_rsem.at[k], device),
            rcopy(s_out.at[k], s_in.at[k], sc_ssem.at[k], sc_rsem.at[k], device),
        )

    def q_send(k):
        value = partial(NEAR[k])
        most = jnp.maximum(jnp.max(jnp.abs(value), axis=1, keepdims=True), 1e-30)
        q_out[k] = jnp.round(value * (32767.0 / most)).astype(jnp.int16)
        s_out[k] = column(most * (1.0 / 32767.0))
        for copy in q_copies(k, ydev(NEAR[k])):
            copy.start()
            sends.append(copy)

    def q_get(k):
        for copy in q_copies(k, partner):
            copy.wait_recv()
        unit = jnp.sum(jnp.where(diagonal, s_in[k], 0.0), axis=1, keepdims=True)
        return q_in[k].astype(F32) * unit

    values = [partial(rel) for rel in FAR]
    most = jnp.maximum(jnp.maximum(jnp.abs(values[0]), jnp.abs(values[1])), jnp.abs(values[2]))
    most = jnp.maximum(jnp.max(most, axis=1, keepdims=True), 1e-30)
    fs_out[...] = column(most * (1.0 / 32767.0))
    for i in range(3):
        fq_out[:, i] = messages(jnp.round(values[i] * (32767.0 / most))).astype(jnp.int16)
    for peer in peers:
        rcopy(fq_out.at[peer], fq_in.at[me_e], fq_ssem, fq_rsem, (peer, me_t)).start()
        rcopy(fs_out, fs_in.at[me_e], fs_ssem, fs_rsem, (peer, me_t)).start()
    for k in range(4):
        q_send(k)
    fq_in[me_e] = fq_out[me_e]
    fs_in[me_e] = fs_out[...]
    kept[...] = partial(0)
    done.append(arrived(dense_out, dense_in, dense_ssem, dense_rsem, NY - 1))
    dense = dense_in[0]
    for k in range(1, NY):
        dense = dense + dense_in[k]
    gate = gate_ref[...]
    dense = jnp.concatenate([gate, gate], axis=1) * dense
    summed = kept[...]
    for k in (2, 3, 0, 1):
        summed = summed + q_get(k)
    ret_out[...] = messages(summed)
    for peer in peers:
        rcopy(ret_out.at[peer], ret_in.at[me_e], ret_ssem, ret_rsem, (peer, me_t)).start()
    ret_in[me_e] = ret_out[me_e]
    done.append(arrived(fq_out, fq_in, fq_ssem, fq_rsem, NEP - 1))
    done.append(arrived(fs_in, fs_in, fs_ssem, fs_rsem, NEP - 1))
    lane2 = lax.broadcasted_iota(jnp.int32, (128, 256), 1)
    mine4 = lax.broadcasted_iota(jnp.int32, (128, 256), 0) == me_e * 4 + lane2 % 4
    unit = jnp.dot(
        fs_in[...].reshape(NEP, 128),
        jnp.where(mine4, 1.0, 0.0),
        preferred_element_type=F32,
        precision=lax.Precision.HIGHEST,
    )
    source = lax.broadcasted_iota(jnp.int32, (NEP, 256), 0)
    source = source == lax.broadcasted_iota(jnp.int32, (NEP, 256), 1) // 8
    unit = jnp.sum(jnp.where(source, unit, 0.0), axis=0, keepdims=True)
    far_sum = jnp.dot(
        comb[...] * unit,
        jnp.concatenate(
            [fq_in[:, i].astype(F32).reshape(256, 128) for i in range(3)], axis=1
        ),
        preferred_element_type=F32,
        precision=lax.Precision.HIGHEST,
    )
    for i, rel in enumerate(FAR):
        cols = slice(i * 128, (i + 1) * 128)
        fy_out[i, :, 0:128] = far_sum[0:8, cols]
        fy_out[i, :, 128:256] = far_sum[8:16, cols]
        copy = rcopy(fy_out.at[i], fy_in.at[i], fy_ssem.at[i], fy_rsem.at[i], ydev(rel))
        copy.start()
        sends.append(copy)
    done.append(arrived(ret_out, ret_in, ret_ssem, ret_rsem, NEP - 1))
    mixed = jnp.dot(
        comb[...],
        ret_in[...].reshape(256, 128),
        preferred_element_type=F32,
        precision=lax.Precision.HIGHEST,
    )
    combined = jnp.concatenate([mixed[0:8], mixed[8:16]], axis=1) + dense
    for i in range(3):
        rcopy(fy_out.at[i], fy_in.at[i], fy_ssem.at[i], fy_rsem.at[i], partner).wait_recv()
        combined = combined + fy_in[i]
    token_diagonal = (
        lax.broadcasted_iota(jnp.int32, (8, 128), 0)
        == lax.broadcasted_iota(jnp.int32, (8, 128), 1)
    )
    own = jnp.sum(
        jnp.where(token_diagonal, jnp.sum(combined * combined, axis=1, keepdims=True), 0.0),
        axis=0,
        keepdims=True,
    )
    sq_out[...] = own
    for step in y_order:
        for c in range(2):
            rcopy(sq_out, sq_in.at[me_t], sq_ssem, sq_rsem, (me_e, ys[step] * 2 + c)).start()
    rcopy(sq_out, sq_in.at[me_t], sq_ssem, sq_rsem, partner).start()
    sq_in[me_t] = own
    done.append(arrived(sq_in, sq_in, sq_ssem, sq_rsem, NTP - 1))
    total_sq = sq_in[0]
    for j in range(1, NTP):
        total_sq = total_sq + sq_in[j]
    final = lax.rsqrt(
        jnp.sum(jnp.where(token_diagonal, total_sq, 0.0), axis=1, keepdims=True) / WIDTH + EPS
    )
    out[...] = (combined * final * ogain[...]).astype(BF16)

    for copy in wparts + sends + [dh_copy] + done:
        copy.wait_send()


def local(
    tokens,
    norm_gain,
    route_experts,
    route_logits,
    expert_gate,
    expert_up,
    expert_down,
    dense_gate,
    dense_up,
    dense_down,
    mix_weight,
    out_gain,
):
    vmem = pl.BlockSpec(memory_space=pltpu.VMEM)
    dma = pltpu.SemaphoreType.DMA
    return pl.pallas_call(
        kernel,
        out_shape=pltpu.VMEM((8, PART), BF16),
        in_specs=[pl.BlockSpec(memory_space=pl.ANY)] * 12,
        out_specs=vmem,
        scratch_shapes=[
            pltpu.VMEM((8, PART), BF16),
            pltpu.VMEM((1, WIDTH), F32),
            pltpu.SMEM((2, 8), jnp.int32),
            pltpu.SMEM((2, 8), F32),
            pltpu.VMEM((1, WIDTH), F32),
            pltpu.VMEM((1, PART), F32),
            pltpu.VMEM((2, 4, 64, WIDTH), BF16),
            pltpu.VMEM((NY, 2, 2, 64, PART), BF16),
            pltpu.VMEM((128, WIDTH), BF16),
            pltpu.VMEM((NY, 64, PART), BF16),
            pltpu.VMEM((NY, 64, PART), BF16),
            pltpu.VMEM((NEP, 8, 128), BF16),
            pltpu.VMEM((NEP, 8, 128), BF16),
            pltpu.VMEM((NEP, 3, 8, 128), BF16),
            pltpu.VMEM((NEP, 3, 8, 128), BF16),
            pltpu.VMEM((2, NY, ROWS, PART), BF16),
            pltpu.VMEM((NTP, 8, PART), BF16),
            pltpu.VMEM((NY, 8, PART), F32),
            pltpu.VMEM((NY, 8, PART), F32),
            pltpu.VMEM((8, 64), BF16),
            pltpu.VMEM((8, 64), BF16),
            pltpu.VMEM((16, 256), F32),
            pltpu.VMEM((16, 256), BF16),
            pltpu.VMEM((8, 256), F32),
            pltpu.VMEM((1, 256), F32),
            pltpu.VMEM((NEP, 1, 256), F32),
            pltpu.VMEM((2, ROWS, 256), F32),
            pltpu.VMEM((ROWS, 256), BF16),
            pltpu.VMEM((4, ROWS, PART), jnp.int16),
            pltpu.VMEM((4, ROWS, PART), jnp.int16),
            pltpu.VMEM((4, 1, 128), F32),
            pltpu.VMEM((4, 1, 128), F32),
            pltpu.VMEM((NEP, 3, 8, 128), jnp.int16),
            pltpu.VMEM((NEP, 3, 8, 128), jnp.int16),
            pltpu.VMEM((1, 128), F32),
            pltpu.VMEM((NEP, 1, 128), F32),
            pltpu.VMEM((3, 8, PART), F32),
            pltpu.VMEM((3, 8, PART), F32),
            pltpu.VMEM((ROWS, PART), F32),
            pltpu.VMEM((NEP, 8, 128), F32),
            pltpu.VMEM((NEP, 8, 128), F32),
            pltpu.VMEM((1, 128), F32),
            pltpu.VMEM((NTP, 1, 128), F32),
            pltpu.VMEM((8, 128), F32),
            dma((6,)),
            dma((20,)),
            dma((2 * NY + 2,)),
            dma((2 * NY + 2,)),
            dma,
            dma,
            dma,
            dma,
            dma,
            dma,
            dma,
            dma,
            dma,
            dma,
            dma((4,)),
            dma((8,)),
            dma((8,)),
            dma((8,)),
            dma,
            dma,
            dma((4,)),
            dma((4,)),
            dma((4,)),
            dma((4,)),
            dma,
            dma,
            dma,
            dma,
            dma((3,)),
            dma((3,)),
            dma,
            dma,
            dma,
            dma,
        ],
        compiler_params=pltpu.CompilerParams(
            collective_id=0, has_side_effects=True, vmem_limit_bytes=56650000
        ),
    )(
        tokens,
        norm_gain.reshape(1, WIDTH),
        route_experts.T,
        route_logits.T,
        jnp.swapaxes(expert_gate, 1, 2),
        jnp.swapaxes(expert_up, 1, 2),
        expert_down,
        dense_gate.T,
        dense_up.T,
        dense_down,
        mix_weight.reshape(1, WIDTH),
        out_gain.reshape(1, PART),
    )


def solution(mesh):
    tp = "tp"
    in_specs = (
        P("ep", tp),
        P(),
        P("ep", None),
        P("ep", None),
        P("ep", None, tp),
        P("ep", None, tp),
        P("ep", tp, None),
        P(None, tp),
        P(None, tp),
        P(tp, None),
        P(),
        P(tp),
    )
    return jax.shard_map(
        local, mesh=mesh, in_specs=in_specs, out_specs=P("ep", tp), check_vma=False
    )
```

```python
import functools

import jax
import jax.numpy as jnp
from jax import lax
from jax.experimental import pallas as pl
from jax.experimental.pallas import tpu as pltpu
from jax.sharding import PartitionSpec as P

MESH = pl.DeviceIdType.MESH
F32 = jnp.float32
BF16 = jnp.bfloat16
EPS = 1e-06

NX, NZ, NY = 4, 8, 8
NEP = NX * NZ
NTP = 2 * NY
ROWS = 128
FAR = (3, 4, 5)
NEAR = (2, 6, 1, 7)
PART = 256
WIDTH = 4096


def rcopy(src, dst, send_sem, recv_sem, device):
    return pltpu.make_async_remote_copy(
        src_ref=src,
        dst_ref=dst,
        send_sem=send_sem,
        recv_sem=recv_sem,
        device_id=device,
        device_id_type=MESH,
    )


def nt_dot(a, b):
    return lax.dot_general(a, b, (((1,), (1,)), ((), ())), preferred_element_type=F32)


def silu(v):
    return v / (1.0 + jnp.exp(-v))


def kernel(
    tok_hbm,
    gain_hbm,
    routes_hbm,
    logits_hbm,
    wg,
    wu,
    wd,
    dg,
    du,
    dd,
    mixw_hbm,
    ogain_hbm,
    out,
    tok,
    gain,
    routes,
    logits,
    mixw,
    ogain,
    w_gu,
    wd_all,
    w_dense,
    dd_own,
    dd_par,
    a2a_out,
    a2a_in,
    far_out,
    far_in,
    gathered,
    tok_all,
    dense_out,
    dense_in,
    dh_own,
    dh_par,
    comb,
    place,
    slots,
    r_out,
    r_in,
    acts,
    hid,
    q_out,
    q_in,
    s_out,
    s_in,
    fq_out,
    fq_in,
    fs_out,
    fs_in,
    fy_out,
    fy_in,
    kept,
    ret_out,
    ret_in,
    sq_out,
    sq_in,
    gate_ref,
    i_sem,
    w_sem,
    wp_ssem,
    wp_rsem,
    a2a_ssem,
    a2a_rsem,
    far_ssem,
    far_rsem,
    tok_ssem,
    tok_rsem,
    dh_ssem,
    dh_rsem,
    dense_ssem,
    dense_rsem,
    ag_ssem,
    ag_rsem,
    pf_ssem,
    pf_rsem,
    r_ssem,
    r_rsem,
    q_ssem,
    q_rsem,
    sc_ssem,
    sc_rsem,
    fq_ssem,
    fq_rsem,
    fs_ssem,
    fs_rsem,
    fy_ssem,
    fy_rsem,
    ret_ssem,
    ret_rsem,
    sq_ssem,
    sq_rsem,
):
    me_e = lax.axis_index("ep")
    me_t = lax.axis_index("tp")
    z, x = lax.div(me_e, NX), lax.rem(me_e, NX)
    y, core = lax.div(me_t, 2), lax.rem(me_t, 2)
    other = 1 - core
    partner = (me_e, y * 2 + other)
    zs = [lax.rem(z + k, NZ) * NX for k in range(NZ)]
    xs = [lax.rem(x + k, NX) for k in range(NX)]
    ys = [lax.rem(y + k, NY) for k in range(NY)]
    peers = [zs[dz] + xs[dx] for dz in (4, 3, 5, 2, 6, 1, 7, 0) for dx in (2, 1, 3, 0)][:-1]
    y_order = (4, 3, 5, 2, 6, 1, 7)

    def ydev(step):
        return (me_e, ys[step % NY] * 2 + core)

    barrier = pltpu.get_barrier_semaphore()
    for peer in peers:
        pl.semaphore_signal(barrier, inc=1, device_id=(peer, me_t), device_id_type=MESH)
    for step in y_order:
        for c in range(2):
            pl.semaphore_signal(
                barrier, inc=1, device_id=(me_e, ys[step] * 2 + c), device_id_type=MESH
            )
    pl.semaphore_signal(barrier, inc=1, device_id=partner, device_id_type=MESH)

    smalls = [
        pltpu.make_async_copy(routes_hbm, routes, i_sem.at[0]),
        pltpu.make_async_copy(logits_hbm, logits, i_sem.at[1]),
        pltpu.make_async_copy(tok_hbm, tok, i_sem.at[2]),
        pltpu.make_async_copy(gain_hbm, gain, i_sem.at[3]),
        pltpu.make_async_copy(mixw_hbm, mixw, i_sem.at[4]),
        pltpu.make_async_copy(ogain_hbm, ogain, i_sem.at[5]),
    ]
    loads = [
        pltpu.make_async_copy(dg, w_dense.at[pl.ds(0, 64)], w_sem.at[0]),
        pltpu.make_async_copy(du, w_dense.at[pl.ds(64, 64)], w_sem.at[1]),
        pltpu.make_async_copy(wg, w_gu.at[0, pl.ds(0, 2)], w_sem.at[2]),
        pltpu.make_async_copy(wu, w_gu.at[0, pl.ds(2, 2)], w_sem.at[3]),
    ]

    def columns(k, c):
        return pl.ds(pl.multiple_of((2 * k + c) * PART, PART), PART)

    for k in range(NY):
        loads.append(
            pltpu.make_async_copy(dd.at[:, columns(k, core)], dd_own.at[k], w_sem.at[4 + k])
        )
    for k in range(NY):
        loads.append(
            pltpu.make_async_copy(wd.at[:, :, columns(k, core)], wd_all.at[k, 0], w_sem.at[12 + k])
        )
    for load in smalls + loads:
        load.start()

    for load in smalls[0:3]:
        load.wait()
    lane = lax.broadcasted_iota(jnp.int32, (8, 256), 1)
    sub = lax.broadcasted_iota(jnp.int32, (8, 256), 0)
    expert = 2 * (lane // 8) + (lane // 2) % 2
    half = (lane // 4) % 2
    r0 = jnp.zeros((8, 256), jnp.int32)
    r1 = jnp.zeros((8, 256), jnp.int32)
    l0 = jnp.zeros((8, 256), F32)
    l1 = jnp.zeros((8, 256), F32)
    for t in range(8):
        r0 = jnp.where(sub == t, routes[0, t], r0)
        r1 = jnp.where(sub == t, routes[1, t], r1)
        l0 = jnp.where(sub == t, logits[0, t], l0)
        l1 = jnp.where(sub == t, logits[1, t], l1)
    top = jnp.maximum(l0, l1)
    e0, e1 = jnp.exp(l0 - top), jnp.exp(l1 - top)
    is0, is1 = (r0 == expert), (r1 == expert)
    hit = jnp.where(is0, 1.0, 0.0) + jnp.where(is1, 1.0, 0.0)
    before = jnp.zeros((8, 256), F32)
    for t in range(7):
        before = before + jnp.where(sub > t, hit[t : t + 1, :], 0.0)
    placed = jnp.where(before == (lane % 2).astype(F32), hit, 0.0)
    weight = (jnp.where(is0, e0, 0.0) + jnp.where(is1, e1, 0.0)) / (e0 + e1) * placed
    comb[0:8, :] = jnp.where(half == 0, weight, 0.0)
    comb[8:16, :] = jnp.where(half == 1, weight, 0.0)
    slots[...] = placed
    place[...] = jnp.concatenate(
        [jnp.where(half == 0, placed, 0.0), jnp.where(half == 1, placed, 0.0)], axis=0
    ).astype(BF16)

    def placed_rows(value):
        halves = jnp.concatenate(
            [value[:, 0:128].astype(F32), value[:, 128:256].astype(F32)], axis=0
        ).astype(BF16)
        rows = lax.dot_general(
            place[...], halves, (((0,), (0,)), ((), ())), preferred_element_type=F32
        )
        return rows.astype(BF16).reshape(NEP, 8, 128)

    tok_value = tok[...]
    a2a_out[...] = placed_rows(tok_value)
    a2a_in[me_e] = a2a_out[me_e]
    tok_all[me_t] = tok_value

    pl.semaphore_wait(barrier, NEP - 1 + NTP - 1)

    for step in y_order:
        for c in range(2):
            rcopy(
                tok, tok_all.at[me_t], tok_ssem, tok_rsem, (me_e, ys[step] * 2 + c)
            ).start()
    rcopy(tok, tok_all.at[me_t], tok_ssem, tok_rsem, partner).start()

    for peer in peers:
        rcopy(a2a_out.at[peer], a2a_in.at[me_e], a2a_ssem, a2a_rsem, (peer, me_t)).start()

    wparts = []
    for k in range(NY):
        copy = rcopy(
            dd.at[:, columns(k, other)], dd_par.at[k], wp_ssem.at[k], wp_rsem.at[k], partner
        )
        copy.start()
        wparts.append(copy)
    for k in range(NY):
        copy = rcopy(
            wd.at[:, :, columns(k, other)],
            wd_all.at[k, 1],
            wp_ssem.at[NY + k],
            wp_rsem.at[NY + k],
            partner,
        )
        copy.start()
        wparts.append(copy)
    for k, ref in enumerate((wg, wu)):
        copy = rcopy(
            ref,
            w_gu.at[1, pl.ds(2 * k, 2)],
            wp_ssem.at[2 * NY + k],
            wp_rsem.at[2 * NY + k],
            partner,
        )
        copy.start()
        wparts.append(copy)

    def arrived(src, dst, ssem, rsem, n):
        part = pl.ds(0, n)
        copy = rcopy(src.at[part], dst.at[part], ssem, rsem, partner)
        copy.wait_recv()
        return copy

    done = [arrived(tok_all, tok_all, tok_ssem, tok_rsem, NTP - 1)]
    squares = jnp.zeros((8, PART), F32)
    for j in range(NTP):
        v = tok_all[j].astype(F32)
        squares = squares + v * v
    scale = lax.rsqrt(jnp.sum(squares, axis=1, keepdims=True) / WIDTH + EPS)
    r_out[...] = jnp.sum(slots[...] * scale, axis=0, keepdims=True)
    for peer in peers:
        rcopy(r_out, r_in.at[me_e], r_ssem, r_rsem, (peer, me_t)).start()
    r_in[me_e] = r_out[...]
    for i, rel in enumerate(FAR):
        far_out[:, i] = placed_rows(tok_all[ys[rel] * 2 + core])
    for peer in peers:
        rcopy(far_out.at[peer], far_in.at[me_e], far_ssem, far_rsem, (peer, me_t)).start()
    far_in[me_e] = far_out[me_e]

    done.append(arrived(a2a_out, a2a_in, a2a_ssem, a2a_rsem, NEP - 1))
    sub3 = lax.broadcasted_iota(jnp.int32, (16, 8, 128), 1)

    def keep_rows(value, rel):
        pairs = value.astype(F32).reshape(16, 2, 8, 128)
        even, odd = pairs[:, 0], pairs[:, 1]
        left = jnp.where(sub3 < 4, even, pltpu.roll(odd, 4, 1)).reshape(ROWS, 128)
        right = jnp.where(sub3 < 4, pltpu.roll(even, 4, 1), odd).reshape(ROWS, 128)
        gathered[core, ys[rel], :, 0:128] = left.astype(BF16)
        gathered[core, ys[rel], :, 128:256] = right.astype(BF16)

    keep_rows(a2a_in[...], 0)

    sends = []

    def ag_copy(slot, k, rel, device):
        ref = gathered.at[core, ys[slot]]
        return rcopy(ref, ref, ag_ssem.at[k], ag_rsem.at[rel], device)

    for k, (rel, step) in enumerate(((6, 2), (2, -2), (7, 1), (1, -1))):
        copy = ag_copy(0, k, rel, ydev(step))
        copy.start()
        sends.append(copy)

    def pass_on(rel):
        ref = gathered.at[core, ys[rel]]
        copy = rcopy(ref, ref, pf_ssem.at[rel], pf_rsem.at[rel], partner)
        copy.start()
        sends.append(copy)

    def pass_wait(rel):
        ref = gathered.at[other, ys[rel]]
        rcopy(ref, ref, pf_ssem.at[rel], pf_rsem.at[rel], partner).wait_recv()

    pass_on(0)

    for load in smalls[3:6] + loads[0:2]:
        load.wait()
    act = jnp.zeros((8, 128), F32)
    mix_acc = jnp.zeros((8, PART), F32)
    for j in range(NTP):
        cols = slice(j * PART, (j + 1) * PART)
        n = (tok_all[j].astype(F32) * scale * gain[:, cols]).astype(BF16)
        mix_acc = mix_acc + n.astype(F32) * mixw[:, cols]
        act = act + nt_dot(n, w_dense[:, cols])
    gate_ref[...] = jnp.broadcast_to(
        jax.nn.sigmoid(jnp.sum(mix_acc, axis=1, keepdims=True)), (8, 128)
    )
    dh_own[...] = (silu(act[:, 0:64]) * act[:, 64:128]).astype(BF16)
    dh_copy = rcopy(dh_own, dh_par, dh_ssem, dh_rsem, partner)
    dh_copy.start()

    for load in loads[4:12]:
        load.wait()
    for copy in wparts[0:NY]:
        copy.wait_recv()
    dh_copy.wait_recv()
    for k in range(NY):
        dense_out[k] = jnp.dot(
            dh_own[...], dd_own[k], preferred_element_type=F32
        ) + jnp.dot(dh_par[...], dd_par[k], preferred_element_type=F32)
    dense_in[y] = dense_out[y]
    loads[2].wait()
    loads[3].wait()
    for copy in wparts[2 * NY :]:
        copy.wait_recv()
    for rel in (6, 2):
        ag_copy(rel, 0, rel, partner).wait_recv()
        pass_on(rel)
    done.append(arrived(r_in, r_in, r_ssem, r_rsem, NEP - 1))
    picked = (
        lax.broadcasted_iota(jnp.int32, (ROWS, NEP), 0) // 4
        == lax.broadcasted_iota(jnp.int32, (ROWS, NEP), 1)
    )
    spread = jnp.dot(
        jnp.where(picked, 1.0, 0.0),
        r_in[...].reshape(NEP, 256),
        preferred_element_type=F32,
        precision=lax.Precision.HIGHEST,
    )
    wanted = me_e * 8 + lax.broadcasted_iota(jnp.int32, (ROWS, 256), 0) % 4
    here = lax.broadcasted_iota(jnp.int32, (ROWS, 256), 1) == wanted
    row_scale = jnp.sum(jnp.where(here, spread, 0.0), axis=1, keepdims=True)

    def project(*slices, first=False):
        sums = [None, None]
        for c, rel in slices:
            cols = pl.ds(pl.multiple_of((2 * ys[rel] + c) * PART, PART), PART)
            n = (gathered[c, ys[rel]].astype(F32) * row_scale * gain[:, cols]).astype(BF16)
            for k in range(2):
                v = nt_dot(n, w_gu[k, :, :, cols].reshape(256, PART))
                sums[k] = v if sums[k] is None else sums[k] + v
        for k in range(2):
            acts[k] = sums[k] if first else acts[k] + sums[k]

    pass_wait(0)
    project((core, 0), (other, 0), (core, 6), (core, 2), first=True)
    for rel in (7, 1):
        ag_copy(rel, 0, rel, partner).wait_recv()
        pass_on(rel)
    for step in y_order:
        rcopy(
            dense_out.at[ys[step]], dense_in.at[y], dense_ssem, dense_rsem, ydev(step)
        ).start()
    pass_wait(6)
    pass_wait(2)
    project((core, 7), (core, 1), (other, 6), (other, 2))
    done.append(arrived(far_out, far_in, far_ssem, far_rsem, NEP - 1))
    for i, rel in enumerate(FAR):
        keep_rows(far_in[:, i], rel)
        pass_on(rel)
    pass_wait(7)
    pass_wait(1)
    project((other, 7), (other, 1), (core, 3), (core, 4), (core, 5))
    for rel in FAR:
        pass_wait(rel)
    project((other, 3), (other, 4), (other, 5))

    row = lax.broadcasted_iota(jnp.int32, (ROWS, 128), 0)
    col = lax.broadcasted_iota(jnp.int32, (ROWS, 128), 1)
    mine = (row // 2) % 2 == col // 64
    for k in range(2):
        v = acts[k]
        hidden = silu(v[:, 0:128]) * v[:, 128:256]
        hid[:, k * 128 : (k + 1) * 128] = jnp.where(mine, hidden, 0.0).astype(BF16)
    for load in loads[12:]:
        load.wait()
    for copy in wparts[NY : 2 * NY]:
        copy.wait_recv()

    diagonal = row == col

    def partial(rel):
        return jnp.dot(
            hid[...], wd_all[ys[rel]].reshape(256, PART), preferred_element_type=F32
        )

    def column(value):
        return jnp.sum(jnp.where(diagonal, value, 0.0), axis=0, keepdims=True)

    def messages(value):
        left = value[:, 0:128].reshape(16, 8, 128)
        right = value[:, 128:256].reshape(16, 8, 128)
        even = jnp.where(sub3 < 4, left, pltpu.roll(right, 4, 1))
        odd = jnp.where(sub3 < 4, pltpu.roll(left, 4, 1), right)
        return jnp.stack([even, odd], axis=1).reshape(NEP, 8, 128)

    def q_copies(k, device):
        return (
            rcopy(q_out.at[k], q_in.at[k], q_ssem.at[k], q_rsem.at[k], device),
            rcopy(s_out.at[k], s_in.at[k], sc_ssem.at[k], sc_rsem.at[k], device),
        )

    def q_send(k):
        value = partial(NEAR[k])
        most = jnp.maximum(jnp.max(jnp.abs(value), axis=1, keepdims=True), 1e-30)
        q_out[k] = jnp.round(value * (32767.0 / most)).astype(jnp.int16)
        s_out[k] = column(most * (1.0 / 32767.0))
        for copy in q_copies(k, ydev(NEAR[k])):
            copy.start()
            sends.append(copy)

    def q_get(k):
        for copy in q_copies(k, partner):
            copy.wait_recv()
        unit = jnp.sum(jnp.where(diagonal, s_in[k], 0.0), axis=1, keepdims=True)
        return q_in[k].astype(F32) * unit

    values = [partial(rel) for rel in FAR]
    most = jnp.maximum(jnp.maximum(jnp.abs(values[0]), jnp.abs(values[1])), jnp.abs(values[2]))
    most = jnp.maximum(jnp.max(most, axis=1, keepdims=True), 1e-30)
    fs_out[...] = column(most * (1.0 / 32767.0))
    for i in range(3):
        fq_out[:, i] = messages(jnp.round(values[i] * (32767.0 / most))).astype(jnp.int16)
    for peer in peers:
        rcopy(fq_out.at[peer], fq_in.at[me_e], fq_ssem, fq_rsem, (peer, me_t)).start()
        rcopy(fs_out, fs_in.at[me_e], fs_ssem, fs_rsem, (peer, me_t)).start()
    for k in range(4):
        q_send(k)
    fq_in[me_e] = fq_out[me_e]
    fs_in[me_e] = fs_out[...]
    kept[...] = partial(0)
    done.append(arrived(dense_out, dense_in, dense_ssem, dense_rsem, NY - 1))
    dense = dense_in[0]
    for k in range(1, NY):
        dense = dense + dense_in[k]
    gate = gate_ref[...]
    dense = jnp.concatenate([gate, gate], axis=1) * dense
    summed = kept[...]
    for k in (2, 3, 0, 1):
        summed = summed + q_get(k)
    ret_out[...] = messages(summed)
    for peer in peers:
        rcopy(ret_out.at[peer], ret_in.at[me_e], ret_ssem, ret_rsem, (peer, me_t)).start()
    ret_in[me_e] = ret_out[me_e]
    done.append(arrived(fq_out, fq_in, fq_ssem, fq_rsem, NEP - 1))
    done.append(arrived(fs_in, fs_in, fs_ssem, fs_rsem, NEP - 1))
    lane2 = lax.broadcasted_iota(jnp.int32, (128, 256), 1)
    mine4 = lax.broadcasted_iota(jnp.int32, (128, 256), 0) == me_e * 4 + lane2 % 4
    unit = jnp.dot(
        fs_in[...].reshape(NEP, 128),
        jnp.where(mine4, 1.0, 0.0),
        preferred_element_type=F32,
        precision=lax.Precision.HIGHEST,
    )
    source = lax.broadcasted_iota(jnp.int32, (NEP, 256), 0)
    source = source == lax.broadcasted_iota(jnp.int32, (NEP, 256), 1) // 8
    unit = jnp.sum(jnp.where(source, unit, 0.0), axis=0, keepdims=True)
    far_sum = jnp.dot(
        comb[...] * unit,
        jnp.concatenate(
            [fq_in[:, i].astype(F32).reshape(256, 128) for i in range(3)], axis=1
        ),
        preferred_element_type=F32,
        precision=lax.Precision.HIGHEST,
    )
    for i, rel in enumerate(FAR):
        cols = slice(i * 128, (i + 1) * 128)
        fy_out[i, :, 0:128] = far_sum[0:8, cols]
        fy_out[i, :, 128:256] = far_sum[8:16, cols]
        copy = rcopy(fy_out.at[i], fy_in.at[i], fy_ssem.at[i], fy_rsem.at[i], ydev(rel))
        copy.start()
        sends.append(copy)
    done.append(arrived(ret_out, ret_in, ret_ssem, ret_rsem, NEP - 1))
    mixed = jnp.dot(
        comb[...],
        ret_in[...].reshape(256, 128),
        preferred_element_type=F32,
        precision=lax.Precision.HIGHEST,
    )
    combined = jnp.concatenate([mixed[0:8], mixed[8:16]], axis=1) + dense
    for i in range(3):
        rcopy(fy_out.at[i], fy_in.at[i], fy_ssem.at[i], fy_rsem.at[i], partner).wait_recv()
        combined = combined + fy_in[i]
    token_diagonal = (
        lax.broadcasted_iota(jnp.int32, (8, 128), 0)
        == lax.broadcasted_iota(jnp.int32, (8, 128), 1)
    )
    own = jnp.sum(
        jnp.where(token_diagonal, jnp.sum(combined * combined, axis=1, keepdims=True), 0.0),
        axis=0,
        keepdims=True,
    )
    sq_out[...] = own
    for step in y_order:
        for c in range(2):
            rcopy(sq_out, sq_in.at[me_t], sq_ssem, sq_rsem, (me_e, ys[step] * 2 + c)).start()
    rcopy(sq_out, sq_in.at[me_t], sq_ssem, sq_rsem, partner).start()
    sq_in[me_t] = own
    done.append(arrived(sq_in, sq_in, sq_ssem, sq_rsem, NTP - 1))
    total_sq = sq_in[0]
    for j in range(1, NTP):
        total_sq = total_sq + sq_in[j]
    final = lax.rsqrt(
        jnp.sum(jnp.where(token_diagonal, total_sq, 0.0), axis=1, keepdims=True) / WIDTH + EPS
    )
    out[...] = (combined * final * ogain[...]).astype(BF16)

    for copy in wparts + sends + [dh_copy] + done:
        copy.wait_send()


def local(
    tokens,
    norm_gain,
    route_experts,
    route_logits,
    expert_gate,
    expert_up,
    expert_down,
    dense_gate,
    dense_up,
    dense_down,
    mix_weight,
    out_gain,
):
    vmem = pl.BlockSpec(memory_space=pltpu.VMEM)
    dma = pltpu.SemaphoreType.DMA
    return pl.pallas_call(
        kernel,
        out_shape=pltpu.VMEM((8, PART), BF16),
        in_specs=[pl.BlockSpec(memory_space=pl.ANY)] * 12,
        out_specs=vmem,
        scratch_shapes=[
            pltpu.VMEM((8, PART), BF16),
            pltpu.VMEM((1, WIDTH), F32),
            pltpu.SMEM((2, 8), jnp.int32),
            pltpu.SMEM((2, 8), F32),
            pltpu.VMEM((1, WIDTH), F32),
            pltpu.VMEM((1, PART), F32),
            pltpu.VMEM((2, 4, 64, WIDTH), BF16),
            pltpu.VMEM((NY, 2, 2, 64, PART), BF16),
            pltpu.VMEM((128, WIDTH), BF16),
            pltpu.VMEM((NY, 64, PART), BF16),
            pltpu.VMEM((NY, 64, PART), BF16),
            pltpu.VMEM((NEP, 8, 128), BF16),
            pltpu.VMEM((NEP, 8, 128), BF16),
            pltpu.VMEM((NEP, 3, 8, 128), BF16),
            pltpu.VMEM((NEP, 3, 8, 128), BF16),
            pltpu.VMEM((2, NY, ROWS, PART), BF16),
            pltpu.VMEM((NTP, 8, PART), BF16),
            pltpu.VMEM((NY, 8, PART), F32),
            pltpu.VMEM((NY, 8, PART), F32),
            pltpu.VMEM((8, 64), BF16),
            pltpu.VMEM((8, 64), BF16),
            pltpu.VMEM((16, 256), F32),
            pltpu.VMEM((16, 256), BF16),
            pltpu.VMEM((8, 256), F32),
            pltpu.VMEM((1, 256), F32),
            pltpu.VMEM((NEP, 1, 256), F32),
            pltpu.VMEM((2, ROWS, 256), F32),
            pltpu.VMEM((ROWS, 256), BF16),
            pltpu.VMEM((4, ROWS, PART), jnp.int16),
            pltpu.VMEM((4, ROWS, PART), jnp.int16),
            pltpu.VMEM((4, 1, 128), F32),
            pltpu.VMEM((4, 1, 128), F32),
            pltpu.VMEM((NEP, 3, 8, 128), jnp.int16),
            pltpu.VMEM((NEP, 3, 8, 128), jnp.int16),
            pltpu.VMEM((1, 128), F32),
            pltpu.VMEM((NEP, 1, 128), F32),
            pltpu.VMEM((3, 8, PART), F32),
            pltpu.VMEM((3, 8, PART), F32),
            pltpu.VMEM((ROWS, PART), F32),
            pltpu.VMEM((NEP, 8, 128), F32),
            pltpu.VMEM((NEP, 8, 128), F32),
            pltpu.VMEM((1, 128), F32),
            pltpu.VMEM((NTP, 1, 128), F32),
            pltpu.VMEM((8, 128), F32),
            dma((6,)),
            dma((20,)),
            dma((2 * NY + 2,)),
            dma((2 * NY + 2,)),
            dma,
            dma,
            dma,
            dma,
            dma,
            dma,
            dma,
            dma,
            dma,
            dma,
            dma((4,)),
            dma((8,)),
            dma((8,)),
            dma((8,)),
            dma,
            dma,
            dma((4,)),
            dma((4,)),
            dma((4,)),
            dma((4,)),
            dma,
            dma,
            dma,
            dma,
            dma((3,)),
            dma((3,)),
            dma,
            dma,
            dma,
            dma,
        ],
        compiler_params=pltpu.CompilerParams(
            collective_id=0, has_side_effects=True, vmem_limit_bytes=56650000
        ),
    )(
        tokens,
        norm_gain.reshape(1, WIDTH),
        route_experts.T,
        route_logits.T,
        jnp.swapaxes(expert_gate, 1, 2),
        jnp.swapaxes(expert_up, 1, 2),
        expert_down,
        dense_gate.T,
        dense_up.T,
        dense_down,
        mix_weight.reshape(1, WIDTH),
        out_gain.reshape(1, PART),
    )


def solution(mesh):
    tp = "tp"
    in_specs = (
        P("ep", tp),
        P(),
        P("ep", None),
        P("ep", None),
        P("ep", None, tp),
        P("ep", None, tp),
        P("ep", tp, None),
        P(None, tp),
        P(None, tp),
        P(tp, None),
        P(),
        P(tp),
    )
    return jax.shard_map(
        local, mesh=mesh, in_specs=in_specs, out_specs=P("ep", tp), check_vma=False
    )
```

```python
import functools

import jax
import jax.numpy as jnp
from jax import lax
from jax.experimental import pallas as pl
from jax.experimental.pallas import tpu as pltpu
from jax.sharding import PartitionSpec as P

MESH = pl.DeviceIdType.MESH
F32 = jnp.float32
BF16 = jnp.bfloat16
EPS = 1e-06

NX, NZ, NY = 4, 8, 8
NEP = NX * NZ
NTP = 2 * NY
ROWS = 128
FAR = (3, 4, 5)
NEAR = (6, 2, 7, 1)
PART = 256
WIDTH = 4096


def rcopy(src, dst, send_sem, recv_sem, device):
    return pltpu.make_async_remote_copy(
        src_ref=src,
        dst_ref=dst,
        send_sem=send_sem,
        recv_sem=recv_sem,
        device_id=device,
        device_id_type=MESH,
    )


def nt_dot(a, b):
    return lax.dot_general(a, b, (((1,), (1,)), ((), ())), preferred_element_type=F32)


def silu(v):
    return v / (1.0 + jnp.exp(-v))


def kernel(
    tok_hbm,
    gain_hbm,
    routes_hbm,
    logits_hbm,
    wg,
    wu,
    wd,
    dg,
    du,
    dd,
    mixw_hbm,
    ogain_hbm,
    out,
    tok,
    gain,
    routes,
    logits,
    mixw,
    ogain,
    w_gu,
    wd_own,
    wd_par,
    w_dense,
    dd_own,
    dd_par,
    a2a_out,
    a2a_in,
    far_out,
    far_in,
    far_par,
    gathered,
    tok_all,
    dense_out,
    dense_in,
    dh_own,
    dh_par,
    comb,
    place,
    slots,
    r_out,
    r_in,
    acts,
    hid,
    q_out,
    q_in,
    s_out,
    s_in,
    fq_out,
    fq_in,
    fs_out,
    fs_in,
    fy_out,
    fy_in,
    kept,
    ret_out,
    ret_in,
    sq_out,
    sq_in,
    gate_ref,
    i_sem,
    w_sem,
    wp_ssem,
    wp_rsem,
    a2a_ssem,
    a2a_rsem,
    far_ssem,
    far_rsem,
    tok_ssem,
    tok_rsem,
    dh_ssem,
    dh_rsem,
    dense_ssem,
    dense_rsem,
    ag_ssem,
    ag_rsem,
    pf_ssem,
    pf_rsem,
    fp_ssem,
    fp_rsem,
    r_ssem,
    r_rsem,
    q_ssem,
    q_rsem,
    sc_ssem,
    sc_rsem,
    fq_ssem,
    fq_rsem,
    fs_ssem,
    fs_rsem,
    fy_ssem,
    fy_rsem,
    ret_ssem,
    ret_rsem,
    sq_ssem,
    sq_rsem,
):
    me_e = lax.axis_index("ep")
    me_t = lax.axis_index("tp")
    z, x = lax.div(me_e, NX), lax.rem(me_e, NX)
    y, core = lax.div(me_t, 2), lax.rem(me_t, 2)
    other = 1 - core
    partner = (me_e, y * 2 + other)
    zs = [lax.rem(z + k, NZ) * NX for k in range(NZ)]
    xs = [lax.rem(x + k, NX) for k in range(NX)]
    ys = [lax.rem(y + k, NY) for k in range(NY)]
    peers = [zs[dz] + xs[dx] for dz in (4, 3, 5, 2, 6, 1, 7, 0) for dx in (2, 1, 3, 0)][:-1]
    y_order = (4, 3, 5, 2, 6, 1, 7)

    def ydev(step):
        return (me_e, ys[step % NY] * 2 + core)

    barrier = pltpu.get_barrier_semaphore()
    for peer in peers:
        pl.semaphore_signal(barrier, inc=1, device_id=(peer, me_t), device_id_type=MESH)
    for step in y_order:
        for c in range(2):
            pl.semaphore_signal(
                barrier, inc=1, device_id=(me_e, ys[step] * 2 + c), device_id_type=MESH
            )
    pl.semaphore_signal(barrier, inc=1, device_id=partner, device_id_type=MESH)

    smalls = [
        pltpu.make_async_copy(routes_hbm, routes, i_sem.at[0]),
        pltpu.make_async_copy(logits_hbm, logits, i_sem.at[1]),
        pltpu.make_async_copy(tok_hbm, tok, i_sem.at[2]),
        pltpu.make_async_copy(gain_hbm, gain, i_sem.at[3]),
        pltpu.make_async_copy(mixw_hbm, mixw, i_sem.at[4]),
        pltpu.make_async_copy(ogain_hbm, ogain, i_sem.at[5]),
    ]

    def columns(k, c):
        return pl.ds(pl.multiple_of((2 * k + c) * PART, PART), PART)

    def load(src, dst, k):
        pltpu.make_async_copy(src, dst, w_sem.at[k]).start()

    def loaded(dst, k):
        pltpu.make_async_copy(dst, dst, w_sem.at[k]).wait()

    for copy in smalls:
        copy.start()
    load(dg, w_dense.at[pl.ds(0, 64)], 0)
    load(du, w_dense.at[pl.ds(64, 64)], 0)
    for k in range(NY):
        load(dd.at[:, columns(k, core)], dd_own.at[k], 1)
    load(wg, w_gu.at[0, pl.ds(0, 2)], 2)
    load(wu, w_gu.at[0, pl.ds(2, 2)], 2)
    for k in range(NY):
        load(wd.at[:, :, columns(k, core)], wd_own.at[k], 3)

    for copy in smalls[0:3]:
        copy.wait()
    lane = lax.broadcasted_iota(jnp.int32, (8, 256), 1)
    sub = lax.broadcasted_iota(jnp.int32, (8, 256), 0)
    expert = 2 * (lane // 8) + (lane // 2) % 2
    half = (lane // 4) % 2
    r0 = jnp.zeros((8, 256), jnp.int32)
    r1 = jnp.zeros((8, 256), jnp.int32)
    l0 = jnp.zeros((8, 256), F32)
    l1 = jnp.zeros((8, 256), F32)
    for t in range(8):
        r0 = jnp.where(sub == t, routes[0, t], r0)
        r1 = jnp.where(sub == t, routes[1, t], r1)
        l0 = jnp.where(sub == t, logits[0, t], l0)
        l1 = jnp.where(sub == t, logits[1, t], l1)
    top = jnp.maximum(l0, l1)
    e0, e1 = jnp.exp(l0 - top), jnp.exp(l1 - top)
    is0, is1 = (r0 == expert), (r1 == expert)
    hit = jnp.where(is0, 1.0, 0.0) + jnp.where(is1, 1.0, 0.0)
    before = jnp.zeros((8, 256), F32)
    for t in range(7):
        before = before + jnp.where(sub > t, hit[t : t + 1, :], 0.0)
    placed = jnp.where(before == (lane % 2).astype(F32), hit, 0.0)
    weight = (jnp.where(is0, e0, 0.0) + jnp.where(is1, e1, 0.0)) / (e0 + e1) * placed
    comb[0:8, :] = jnp.where(half == 0, weight, 0.0)
    comb[8:16, :] = jnp.where(half == 1, weight, 0.0)
    slots[...] = placed
    place[...] = jnp.concatenate(
        [jnp.where(half == 0, placed, 0.0), jnp.where(half == 1, placed, 0.0)], axis=0
    ).astype(BF16)

    def placed_rows(value):
        halves = jnp.concatenate(
            [value[:, 0:128].astype(F32), value[:, 128:256].astype(F32)], axis=0
        ).astype(BF16)
        rows = lax.dot_general(
            place[...], halves, (((0,), (0,)), ((), ())), preferred_element_type=F32
        )
        return rows.astype(BF16).reshape(NEP, 8, 128)

    tok_value = tok[...]
    a2a_out[...] = placed_rows(tok_value)
    a2a_in[me_e] = a2a_out[me_e]
    tok_all[me_t] = tok_value

    pl.semaphore_wait(barrier, NEP - 1 + NTP - 1)

    for step in y_order:
        for c in range(2):
            rcopy(
                tok, tok_all.at[me_t], tok_ssem, tok_rsem, (me_e, ys[step] * 2 + c)
            ).start()
    rcopy(tok, tok_all.at[me_t], tok_ssem, tok_rsem, partner).start()

    for peer in peers:
        rcopy(a2a_out.at[peer], a2a_in.at[me_e], a2a_ssem, a2a_rsem, (peer, me_t)).start()

    for k in range(NY):
        rcopy(
            dd.at[:, columns(k, other)], dd_par.at[k], wp_ssem.at[0], wp_rsem.at[0], partner
        ).start()
    for k, ref in enumerate((wg, wu)):
        rcopy(
            ref, w_gu.at[1, pl.ds(2 * k, 2)], wp_ssem.at[1], wp_rsem.at[1], partner
        ).start()
    for k in range(NY):
        rcopy(
            wd.at[:, :, columns(k, other)], wd_par.at[k], wp_ssem.at[2], wp_rsem.at[2], partner
        ).start()
    parts = [
        rcopy(ref, ref, wp_ssem.at[k], wp_rsem.at[k], partner)
        for k, ref in enumerate((dd_par, w_gu.at[1], wd_par))
    ]

    def arrived(src, dst, ssem, rsem, n):
        part = pl.ds(0, n)
        copy = rcopy(src.at[part], dst.at[part], ssem, rsem, partner)
        copy.wait_recv()
        return copy

    done = [arrived(tok_all, tok_all, tok_ssem, tok_rsem, NTP - 1)]
    squares = jnp.zeros((8, PART), F32)
    for j in range(NTP):
        v = tok_all[j].astype(F32)
        squares = squares + v * v
    scale = lax.rsqrt(jnp.sum(squares, axis=1, keepdims=True) / WIDTH + EPS)
    r_out[...] = jnp.sum(slots[...] * scale, axis=0, keepdims=True)
    for i, rel in enumerate(FAR):
        far_out[:, i] = placed_rows(tok_all[ys[rel] * 2 + core])
    for peer in peers:
        rcopy(r_out, r_in.at[me_e], r_ssem, r_rsem, (peer, me_t)).start()
    for peer in peers:
        rcopy(far_out.at[peer], far_in.at[me_e], far_ssem, far_rsem, (peer, me_t)).start()
    r_in[me_e] = r_out[...]
    far_in[me_e] = far_out[me_e]

    done.append(arrived(a2a_out, a2a_in, a2a_ssem, a2a_rsem, NEP - 1))
    sub3 = lax.broadcasted_iota(jnp.int32, (16, 8, 128), 1)

    def keep_rows(value, c, rel):
        pairs = value.astype(F32).reshape(16, 2, 8, 128)
        even, odd = pairs[:, 0], pairs[:, 1]
        left = jnp.where(sub3 < 4, even, pltpu.roll(odd, 4, 1)).reshape(ROWS, 128)
        right = jnp.where(sub3 < 4, pltpu.roll(even, 4, 1), odd).reshape(ROWS, 128)
        gathered[c, ys[rel], :, 0:128] = left.astype(BF16)
        gathered[c, ys[rel], :, 128:256] = right.astype(BF16)

    keep_rows(a2a_in[...], core, 0)

    def ag_copy(slot, k, device):
        ref = gathered.at[core, ys[slot]]
        return rcopy(ref, ref, ag_ssem, ag_rsem.at[k], device)

    for k, step in enumerate((2, -2, 1, -1)):
        ag_copy(0, k, ydev(step)).start()

    def pass_copy(c, rel):
        ref = gathered.at[c, ys[rel]]
        k = ((0,) + NEAR).index(rel)
        return rcopy(ref, ref, pf_ssem, pf_rsem.at[k], partner)

    def pass_on(rel):
        pass_copy(core, rel).start()

    def pass_wait(rel):
        pass_copy(other, rel).wait_recv()

    pass_on(0)

    for copy in smalls[3:6]:
        copy.wait()
    loaded(w_dense, 0)
    act = jnp.zeros((8, 128), F32)
    mix_acc = jnp.zeros((8, PART), F32)
    for j in range(NTP):
        cols = slice(j * PART, (j + 1) * PART)
        n = (tok_all[j].astype(F32) * scale * gain[:, cols]).astype(BF16)
        mix_acc = mix_acc + n.astype(F32) * mixw[:, cols]
        act = act + nt_dot(n, w_dense[:, cols])
    gate_ref[...] = jnp.broadcast_to(
        jax.nn.sigmoid(jnp.sum(mix_acc, axis=1, keepdims=True)), (8, 128)
    )
    dh_own[...] = (silu(act[:, 0:64]) * act[:, 64:128]).astype(BF16)
    dh_copy = rcopy(dh_own, dh_par, dh_ssem, dh_rsem, partner)
    dh_copy.start()

    loaded(dd_own, 1)
    parts[0].wait_recv()
    dh_copy.wait_recv()
    for k in range(NY):
        dense_out[k] = jnp.dot(
            dh_own[...], dd_own[k], preferred_element_type=F32
        ) + jnp.dot(dh_par[...], dd_par[k], preferred_element_type=F32)
    dense_in[y] = dense_out[y]
    loaded(w_gu.at[0], 2)
    parts[1].wait_recv()
    for rel in (6, 2):
        ag_copy(rel, NEAR.index(rel), partner).wait_recv()
        pass_on(rel)
    done.append(arrived(r_in, r_in, r_ssem, r_rsem, NEP - 1))
    picked = (
        lax.broadcasted_iota(jnp.int32, (ROWS, NEP), 0) // 4
        == lax.broadcasted_iota(jnp.int32, (ROWS, NEP), 1)
    )
    spread = jnp.dot(
        jnp.where(picked, 1.0, 0.0),
        r_in[...].reshape(NEP, 256),
        preferred_element_type=F32,
        precision=lax.Precision.HIGHEST,
    )
    wanted = me_e * 8 + lax.broadcasted_iota(jnp.int32, (ROWS, 256), 0) % 4
    here = lax.broadcasted_iota(jnp.int32, (ROWS, 256), 1) == wanted
    row_scale = jnp.sum(jnp.where(here, spread, 0.0), axis=1, keepdims=True)

    def project(*slices, first=False):
        sums = [None, None]
        for c, rel in slices:
            cols = pl.ds(pl.multiple_of((2 * ys[rel] + c) * PART, PART), PART)
            n = (gathered[c, ys[rel]].astype(F32) * row_scale * gain[:, cols]).astype(BF16)
            for k in range(2):
                v = nt_dot(n, w_gu[k, :, :, cols].reshape(256, PART))
                sums[k] = v if sums[k] is None else sums[k] + v
        for k in range(2):
            acts[k] = sums[k] if first else acts[k] + sums[k]

    pass_wait(0)
    project((core, 0), (other, 0), (core, 6), (core, 2), first=True)
    for rel in (7, 1):
        ag_copy(rel, NEAR.index(rel), partner).wait_recv()
        pass_on(rel)
    for step in y_order:
        rcopy(
            dense_out.at[ys[step]], dense_in.at[y], dense_ssem, dense_rsem, ydev(step)
        ).start()
    pass_wait(6)
    pass_wait(2)
    project((core, 7), (core, 1), (other, 6), (other, 2))
    done.append(arrived(far_out, far_in, far_ssem, far_rsem, NEP - 1))
    raw = rcopy(far_in, far_par, fp_ssem, fp_rsem, partner)
    raw.start()
    for i, rel in enumerate(FAR):
        keep_rows(far_in[:, i], core, rel)
    pass_wait(7)
    pass_wait(1)
    project((other, 7), (other, 1), (core, 3), (core, 4), (core, 5))
    raw.wait_recv()
    for i, rel in enumerate(FAR):
        keep_rows(far_par[:, i], other, rel)
    project((other, 3), (other, 4), (other, 5))

    row = lax.broadcasted_iota(jnp.int32, (ROWS, 128), 0)
    col = lax.broadcasted_iota(jnp.int32, (ROWS, 128), 1)
    mine = (row // 2) % 2 == col // 64
    for k in range(2):
        v = acts[k]
        hidden = silu(v[:, 0:128]) * v[:, 128:256]
        hid[:, k * 128 : (k + 1) * 128] = jnp.where(mine, hidden, 0.0).astype(BF16)
    loaded(wd_own, 3)
    parts[2].wait_recv()

    diagonal = row == col

    def partial(rel):
        k = ys[rel]
        both = jnp.concatenate(
            [wd_own[k].reshape(128, PART), wd_par[k].reshape(128, PART)], axis=0
        )
        return jnp.dot(hid[...], both, preferred_element_type=F32)

    def column(value):
        return jnp.sum(jnp.where(diagonal, value, 0.0), axis=0, keepdims=True)

    def messages(value):
        left = value[:, 0:128].reshape(16, 8, 128)
        right = value[:, 128:256].reshape(16, 8, 128)
        even = jnp.where(sub3 < 4, left, pltpu.roll(right, 4, 1))
        odd = jnp.where(sub3 < 4, pltpu.roll(left, 4, 1), right)
        return jnp.stack([even, odd], axis=1).reshape(NEP, 8, 128)

    def q_copies(k, device):
        return (
            rcopy(q_out.at[k], q_in.at[k], q_ssem, q_rsem.at[k], device),
            rcopy(s_out.at[k], s_in.at[k], sc_ssem, sc_rsem.at[k], device),
        )

    def q_send(k):
        value = partial(NEAR[k])
        most = jnp.maximum(jnp.max(jnp.abs(value), axis=1, keepdims=True), 1e-30)
        q_out[k] = jnp.round(value * (32767.0 / most)).astype(jnp.int16)
        s_out[k] = column(most * (1.0 / 32767.0))
        for copy in q_copies(k, ydev(NEAR[k])):
            copy.start()

    def q_get(k):
        for copy in q_copies(k, partner):
            copy.wait_recv()
        unit = jnp.sum(jnp.where(diagonal, s_in[k], 0.0), axis=1, keepdims=True)
        return q_in[k].astype(F32) * unit

    values = [partial(rel) for rel in FAR]
    most = jnp.maximum(jnp.maximum(jnp.abs(values[0]), jnp.abs(values[1])), jnp.abs(values[2]))
    most = jnp.maximum(jnp.max(most, axis=1, keepdims=True), 1e-30)
    fs_out[...] = column(most * (1.0 / 32767.0))
    for i in range(3):
        fq_out[:, i] = messages(jnp.round(values[i] * (32767.0 / most))).astype(jnp.int16)
    for peer in peers:
        rcopy(fq_out.at[peer], fq_in.at[me_e], fq_ssem, fq_rsem, (peer, me_t)).start()
    for k in range(4):
        q_send(k)
    for peer in peers:
        rcopy(fs_out, fs_in.at[me_e], fs_ssem, fs_rsem, (peer, me_t)).start()
    fq_in[me_e] = fq_out[me_e]
    fs_in[me_e] = fs_out[...]
    kept[...] = partial(0)
    done.append(arrived(dense_out, dense_in, dense_ssem, dense_rsem, NY - 1))
    dense = dense_in[0]
    for k in range(1, NY):
        dense = dense + dense_in[k]
    gate = gate_ref[...]
    dense = jnp.concatenate([gate, gate], axis=1) * dense
    summed = kept[...]
    for k in range(4):
        summed = summed + q_get(k)
    ret_out[...] = messages(summed)
    for peer in peers:
        rcopy(ret_out.at[peer], ret_in.at[me_e], ret_ssem, ret_rsem, (peer, me_t)).start()
    ret_in[me_e] = ret_out[me_e]
    done.append(arrived(fq_out, fq_in, fq_ssem, fq_rsem, NEP - 1))
    done.append(arrived(fs_in, fs_in, fs_ssem, fs_rsem, NEP - 1))
    lane2 = lax.broadcasted_iota(jnp.int32, (128, 256), 1)
    mine4 = lax.broadcasted_iota(jnp.int32, (128, 256), 0) == me_e * 4 + lane2 % 4
    unit = jnp.dot(
        fs_in[...].reshape(NEP, 128),
        jnp.where(mine4, 1.0, 0.0),
        preferred_element_type=F32,
        precision=lax.Precision.HIGHEST,
    )
    source = lax.broadcasted_iota(jnp.int32, (NEP, 256), 0)
    source = source == lax.broadcasted_iota(jnp.int32, (NEP, 256), 1) // 8
    unit = jnp.sum(jnp.where(source, unit, 0.0), axis=0, keepdims=True)
    far_sum = jnp.dot(
        comb[...] * unit,
        jnp.concatenate(
            [fq_in[:, i].astype(F32).reshape(256, 128) for i in range(3)], axis=1
        ),
        preferred_element_type=F32,
        precision=lax.Precision.HIGHEST,
    )
    for i, rel in enumerate(FAR):
        cols = slice(i * 128, (i + 1) * 128)
        fy_out[i, :, 0:128] = far_sum[0:8, cols]
        fy_out[i, :, 128:256] = far_sum[8:16, cols]
        rcopy(fy_out.at[i], fy_in.at[i], fy_ssem, fy_rsem, ydev(rel)).start()
    done.append(arrived(ret_out, ret_in, ret_ssem, ret_rsem, NEP - 1))
    mixed = jnp.dot(
        comb[...],
        ret_in[...].reshape(256, 128),
        preferred_element_type=F32,
        precision=lax.Precision.HIGHEST,
    )
    combined = jnp.concatenate([mixed[0:8], mixed[8:16]], axis=1) + dense
    fy_copy = rcopy(fy_out, fy_in, fy_ssem, fy_rsem, partner)
    fy_copy.wait_recv()
    combined = combined + fy_in[0] + fy_in[1] + fy_in[2]
    token_diagonal = (
        lax.broadcasted_iota(jnp.int32, (8, 128), 0)
        == lax.broadcasted_iota(jnp.int32, (8, 128), 1)
    )
    own = jnp.sum(
        jnp.where(token_diagonal, jnp.sum(combined * combined, axis=1, keepdims=True), 0.0),
        axis=0,
        keepdims=True,
    )
    sq_out[...] = own
    for step in y_order:
        for c in range(2):
            rcopy(sq_out, sq_in.at[me_t], sq_ssem, sq_rsem, (me_e, ys[step] * 2 + c)).start()
    rcopy(sq_out, sq_in.at[me_t], sq_ssem, sq_rsem, partner).start()
    sq_in[me_t] = own
    done.append(arrived(sq_in, sq_in, sq_ssem, sq_rsem, NTP - 1))
    total_sq = sq_in[0]
    for j in range(1, NTP):
        total_sq = total_sq + sq_in[j]
    final = lax.rsqrt(
        jnp.sum(jnp.where(token_diagonal, total_sq, 0.0), axis=1, keepdims=True) / WIDTH + EPS
    )
    out[...] = (combined * final * ogain[...]).astype(BF16)

    near = gathered.at[core, pl.ds(0, 4)]
    done += [
        rcopy(near, near, ag_ssem, ag_rsem.at[0], partner),
        rcopy(q_out, q_in, q_ssem, q_rsem.at[0], partner),
        rcopy(s_out, s_in, sc_ssem, sc_rsem.at[0], partner),
    ]
    five = gathered.at[core, pl.ds(0, 5)]
    done.append(rcopy(five, five, pf_ssem, pf_rsem.at[0], partner))
    for copy in parts + [dh_copy, raw, fy_copy] + done:
        copy.wait_send()


def local(
    tokens,
    norm_gain,
    route_experts,
    route_logits,
    expert_gate,
    expert_up,
    expert_down,
    dense_gate,
    dense_up,
    dense_down,
    mix_weight,
    out_gain,
):
    vmem = pl.BlockSpec(memory_space=pltpu.VMEM)
    dma = pltpu.SemaphoreType.DMA
    return pl.pallas_call(
        kernel,
        out_shape=pltpu.VMEM((8, PART), BF16),
        in_specs=[pl.BlockSpec(memory_space=pl.ANY)] * 12,
        out_specs=vmem,
        scratch_shapes=[
            pltpu.VMEM((8, PART), BF16),
            pltpu.VMEM((1, WIDTH), F32),
            pltpu.SMEM((2, 8), jnp.int32),
            pltpu.SMEM((2, 8), F32),
            pltpu.VMEM((1, WIDTH), F32),
            pltpu.VMEM((1, PART), F32),
            pltpu.VMEM((2, 4, 64, WIDTH), BF16),
            pltpu.VMEM((NY, 2, 64, PART), BF16),
            pltpu.VMEM((NY, 2, 64, PART), BF16),
            pltpu.VMEM((128, WIDTH), BF16),
            pltpu.VMEM((NY, 64, PART), BF16),
            pltpu.VMEM((NY, 64, PART), BF16),
            pltpu.VMEM((NEP, 8, 128), BF16),
            pltpu.VMEM((NEP, 8, 128), BF16),
            pltpu.VMEM((NEP, 3, 8, 128), BF16),
            pltpu.VMEM((NEP, 3, 8, 128), BF16),
            pltpu.VMEM((NEP, 3, 8, 128), BF16),
            pltpu.VMEM((2, NY, ROWS, PART), BF16),
            pltpu.VMEM((NTP, 8, PART), BF16),
            pltpu.VMEM((NY, 8, PART), F32),
            pltpu.VMEM((NY, 8, PART), F32),
            pltpu.VMEM((8, 64), BF16),
            pltpu.VMEM((8, 64), BF16),
            pltpu.VMEM((16, 256), F32),
            pltpu.VMEM((16, 256), BF16),
            pltpu.VMEM((8, 256), F32),
            pltpu.VMEM((1, 256), F32),
            pltpu.VMEM((NEP, 1, 256), F32),
            pltpu.VMEM((2, ROWS, 256), F32),
            pltpu.VMEM((ROWS, 256), BF16),
            pltpu.VMEM((4, ROWS, PART), jnp.int16),
            pltpu.VMEM((4, ROWS, PART), jnp.int16),
            pltpu.VMEM((4, 1, 128), F32),
            pltpu.VMEM((4, 1, 128), F32),
            pltpu.VMEM((NEP, 3, 8, 128), jnp.int16),
            pltpu.VMEM((NEP, 3, 8, 128), jnp.int16),
            pltpu.VMEM((1, 128), F32),
            pltpu.VMEM((NEP, 1, 128), F32),
            pltpu.VMEM((3, 8, PART), F32),
            pltpu.VMEM((3, 8, PART), F32),
            pltpu.VMEM((ROWS, PART), F32),
            pltpu.VMEM((NEP, 8, 128), F32),
            pltpu.VMEM((NEP, 8, 128), F32),
            pltpu.VMEM((1, 128), F32),
            pltpu.VMEM((NTP, 1, 128), F32),
            pltpu.VMEM((8, 128), F32),
            dma((6,)),
            dma((4,)),
            dma((3,)),
            dma((3,)),
            dma,
            dma,
            dma,
            dma,
            dma,
            dma,
            dma,
            dma,
            dma,
            dma,
            dma,
            dma((4,)),
            dma,
            dma((5,)),
            dma,
            dma,
            dma,
            dma,
            dma,
            dma((4,)),
            dma,
            dma((4,)),
            dma,
            dma,
            dma,
            dma,
            dma,
            dma,
            dma,
            dma,
            dma,
            dma,
        ],
        compiler_params=pltpu.CompilerParams(
            collective_id=0, has_side_effects=True, vmem_limit_bytes=56650000
        ),
    )(
        tokens,
        norm_gain.reshape(1, WIDTH),
        route_experts.T,
        route_logits.T,
        jnp.swapaxes(expert_gate, 1, 2),
        jnp.swapaxes(expert_up, 1, 2),
        expert_down,
        dense_gate.T,
        dense_up.T,
        dense_down,
        mix_weight.reshape(1, WIDTH),
        out_gain.reshape(1, PART),
    )


def solution(mesh):
    tp = "tp"
    in_specs = (
        P("ep", tp),
        P(),
        P("ep", None),
        P("ep", None),
        P("ep", None, tp),
        P("ep", None, tp),
        P("ep", tp, None),
        P(None, tp),
        P(None, tp),
        P(tp, None),
        P(),
        P(tp),
    )
    return jax.shard_map(
        local, mesh=mesh, in_specs=in_specs, out_specs=P("ep", tp), check_vma=False
    )
```

```python
import functools

import jax
import jax.numpy as jnp
from jax import lax
from jax.experimental import pallas as pl
from jax.experimental.pallas import tpu as pltpu
from jax.sharding import PartitionSpec as P

MESH = pl.DeviceIdType.MESH
F32 = jnp.float32
BF16 = jnp.bfloat16
EPS = 1e-06

NX, NZ, NY = 4, 8, 8
NEP = NX * NZ
NTP = 2 * NY
ROWS = 128
HALF = ROWS // 2
FAR = (3, 4, 5)
NEAR = (6, 2, 7, 1)
PART = 256
WIDTH = 4096


def rcopy(src, dst, send_sem, recv_sem, device):
    return pltpu.make_async_remote_copy(
        src_ref=src,
        dst_ref=dst,
        send_sem=send_sem,
        recv_sem=recv_sem,
        device_id=device,
        device_id_type=MESH,
    )


def nt_dot(a, b):
    return lax.dot_general(a, b, (((1,), (1,)), ((), ())), preferred_element_type=F32)


def silu(v):
    return v / (1.0 + jnp.exp(-v))


def kernel(
    tok_hbm,
    gain_hbm,
    routes_hbm,
    logits_hbm,
    wg,
    wu,
    wd,
    dg,
    du,
    dd,
    mixw_hbm,
    ogain_hbm,
    out,
    tok,
    gain,
    routes,
    logits,
    mixw,
    ogain,
    w_gu,
    wd_own,
    wd_par,
    w_dense,
    dd_own,
    dd_par,
    a2a_out,
    a2a_in,
    far_out,
    far_in,
    far_par,
    gathered,
    tok_all,
    dense_out,
    dense_in,
    dh_own,
    dh_par,
    comb,
    place,
    slots,
    r_out,
    r_in,
    acts,
    hid,
    q_out,
    q_in,
    s_out,
    s_in,
    fq_out,
    fq_in,
    fs_out,
    fs_in,
    fy_out,
    fy_in,
    kept,
    ret_out,
    ret_in,
    sq_out,
    sq_in,
    gate_ref,
    i_sem,
    w_sem,
    wp_ssem,
    wp_rsem,
    a2a_ssem,
    a2a_rsem,
    far_ssem,
    far_rsem,
    tok_ssem,
    tok_rsem,
    dh_ssem,
    dh_rsem,
    dense_ssem,
    dense_rsem,
    ag_ssem,
    ag_rsem,
    pf_ssem,
    pf_rsem,
    fp_ssem,
    fp_rsem,
    r_ssem,
    r_rsem,
    q_ssem,
    q_rsem,
    sc_ssem,
    sc_rsem,
    fq_ssem,
    fq_rsem,
    fs_ssem,
    fs_rsem,
    fy_ssem,
    fy_rsem,
    ret_ssem,
    ret_rsem,
    sq_ssem,
    sq_rsem,
):
    me_e = lax.axis_index("ep")
    me_t = lax.axis_index("tp")
    z, x = lax.div(me_e, NX), lax.rem(me_e, NX)
    y, core = lax.div(me_t, 2), lax.rem(me_t, 2)
    other = 1 - core
    partner = (me_e, y * 2 + other)
    zs = [lax.rem(z + k, NZ) * NX for k in range(NZ)]
    xs = [lax.rem(x + k, NX) for k in range(NX)]
    ys = [lax.rem(y + k, NY) for k in range(NY)]
    peers = [zs[dz] + xs[dx] for dz in (4, 3, 5, 2, 6, 1, 7, 0) for dx in (2, 1, 3, 0)][:-1]
    y_order = (4, 3, 5, 2, 6, 1, 7)

    block = lax.div(z, 4)
    opposite = zs[4] + xs[0]
    z4 = [lax.rem(z + k, 4) * NX for k in range(4)]

    def to_block(b, send):
        for dz in (2, 1, 3, 0):
            for dx in (2, 1, 3, 0):
                if dz or dx:
                    send(4 * NX * b + z4[dz] + xs[dx])

        @pl.when(block != b)
        def _():
            send(opposite)

    def part(b, n):
        return pl.ds(b * n, n)

    def ydev(step):
        return (me_e, ys[step % NY] * 2 + core)

    barrier = pltpu.get_barrier_semaphore()
    for peer in peers:
        pl.semaphore_signal(barrier, inc=1, device_id=(peer, me_t), device_id_type=MESH)
    for step in y_order:
        for c in range(2):
            pl.semaphore_signal(
                barrier, inc=1, device_id=(me_e, ys[step] * 2 + c), device_id_type=MESH
            )
    pl.semaphore_signal(barrier, inc=1, device_id=partner, device_id_type=MESH)

    smalls = [
        pltpu.make_async_copy(routes_hbm, routes, i_sem.at[0]),
        pltpu.make_async_copy(logits_hbm, logits, i_sem.at[1]),
        pltpu.make_async_copy(tok_hbm, tok, i_sem.at[2]),
        pltpu.make_async_copy(gain_hbm, gain, i_sem.at[3]),
        pltpu.make_async_copy(mixw_hbm, mixw, i_sem.at[4]),
        pltpu.make_async_copy(ogain_hbm, ogain, i_sem.at[5]),
    ]

    def columns(k, c):
        return pl.ds(pl.multiple_of((2 * k + c) * PART, PART), PART)

    def load(src, dst, k):
        pltpu.make_async_copy(src, dst, w_sem.at[k]).start()

    def loaded(dst, k):
        pltpu.make_async_copy(dst, dst, w_sem.at[k]).wait()

    for copy in smalls:
        copy.start()
    load(dg, w_dense.at[pl.ds(0, 64)], 0)
    load(du, w_dense.at[pl.ds(64, 64)], 0)
    for k in range(NY):
        load(dd.at[:, columns(k, core)], dd_own.at[k], 1)
    load(wg, w_gu.at[0, pl.ds(0, 2)], 2)
    load(wu, w_gu.at[0, pl.ds(2, 2)], 2)
    for k in range(NY):
        load(wd.at[:, :, columns(k, core)], wd_own.at[k], 3)

    for copy in smalls[0:3]:
        copy.wait()
    lane = lax.broadcasted_iota(jnp.int32, (8, 256), 1)
    sub = lax.broadcasted_iota(jnp.int32, (8, 256), 0)
    expert = 2 * (lane // 8) + (lane // 2) % 2
    half = (lane // 4) % 2
    r0 = jnp.zeros((8, 256), jnp.int32)
    r1 = jnp.zeros((8, 256), jnp.int32)
    l0 = jnp.zeros((8, 256), F32)
    l1 = jnp.zeros((8, 256), F32)
    for t in range(8):
        r0 = jnp.where(sub == t, routes[0, t], r0)
        r1 = jnp.where(sub == t, routes[1, t], r1)
        l0 = jnp.where(sub == t, logits[0, t], l0)
        l1 = jnp.where(sub == t, logits[1, t], l1)
    top = jnp.maximum(l0, l1)
    e0, e1 = jnp.exp(l0 - top), jnp.exp(l1 - top)
    is0, is1 = (r0 == expert), (r1 == expert)
    hit = jnp.where(is0, 1.0, 0.0) + jnp.where(is1, 1.0, 0.0)
    before = jnp.zeros((8, 256), F32)
    for t in range(7):
        before = before + jnp.where(sub > t, hit[t : t + 1, :], 0.0)
    placed = jnp.where(before == (lane % 2).astype(F32), hit, 0.0)
    weight = (jnp.where(is0, e0, 0.0) + jnp.where(is1, e1, 0.0)) / (e0 + e1) * placed
    comb[0:8, :] = jnp.where(half == 0, weight, 0.0)
    comb[8:16, :] = jnp.where(half == 1, weight, 0.0)
    slots[...] = placed
    place[...] = jnp.concatenate(
        [jnp.where(half == 0, placed, 0.0), jnp.where(half == 1, placed, 0.0)], axis=0
    ).astype(BF16)

    def placed_rows(value):
        halves = jnp.concatenate(
            [value[:, 0:128].astype(F32), value[:, 128:256].astype(F32)], axis=0
        ).astype(BF16)
        rows = lax.dot_general(
            place[...], halves, (((0,), (0,)), ((), ())), preferred_element_type=F32
        )
        return rows.astype(BF16).reshape(NEP, 8, 128)

    tok_value = tok[...]
    a2a_out[...] = placed_rows(tok_value)
    a2a_in[me_e] = a2a_out[me_e]
    tok_all[me_t] = tok_value

    pl.semaphore_wait(barrier, NEP - 1 + NTP - 1)

    for step in y_order:
        for c in range(2):
            rcopy(
                tok, tok_all.at[me_t], tok_ssem, tok_rsem, (me_e, ys[step] * 2 + c)
            ).start()
    rcopy(tok, tok_all.at[me_t], tok_ssem, tok_rsem, partner).start()

    for peer in peers:
        rcopy(a2a_out.at[peer], a2a_in.at[me_e], a2a_ssem, a2a_rsem, (peer, me_t)).start()

    for k in range(NY):
        rcopy(
            dd.at[:, columns(k, other)], dd_par.at[k], wp_ssem.at[0], wp_rsem.at[0], partner
        ).start()
    for k, ref in enumerate((wg, wu)):
        rcopy(
            ref, w_gu.at[1, pl.ds(2 * k, 2)], wp_ssem.at[1], wp_rsem.at[1], partner
        ).start()
    for k in range(NY):
        rcopy(
            wd.at[:, :, columns(k, other)], wd_par.at[k], wp_ssem.at[2], wp_rsem.at[2], partner
        ).start()
    parts = [
        rcopy(ref, ref, wp_ssem.at[k], wp_rsem.at[k], partner)
        for k, ref in enumerate((dd_par, w_gu.at[1], wd_par))
    ]

    def arrived(src, dst, ssem, rsem, n):
        first = pl.ds(0, n)
        copy = rcopy(src.at[first], dst.at[first], ssem, rsem, partner)
        copy.wait_recv()
        return copy

    done = [arrived(tok_all, tok_all, tok_ssem, tok_rsem, NTP - 1)]
    squares = jnp.zeros((8, PART), F32)
    for j in range(NTP):
        v = tok_all[j].astype(F32)
        squares = squares + v * v
    scale = lax.rsqrt(jnp.sum(squares, axis=1, keepdims=True) / WIDTH + EPS)
    r_out[...] = jnp.sum(slots[...] * scale, axis=0, keepdims=True)
    for i, rel in enumerate(FAR):
        far_out[:, i] = placed_rows(tok_all[ys[rel] * 2 + core])
    for peer in peers:
        rcopy(r_out, r_in.at[me_e], r_ssem, r_rsem, (peer, me_t)).start()
    def send_far():
        for peer in peers:
            rcopy(
                far_out.at[peer], far_in.at[me_e], far_ssem, far_rsem.at[block], (peer, me_t)
            ).start()

    pl.when(block == 0)(send_far)
    far_self = pltpu.make_async_copy(
        far_out.at[me_e], far_in.at[me_e], far_rsem.at[block]
    )
    far_self.start()
    r_in[me_e] = r_out[...]

    done.append(arrived(a2a_out, a2a_in, a2a_ssem, a2a_rsem, NEP - 1))
    def low_half(n):
        return lax.broadcasted_iota(jnp.int32, (n, 8, 128), 1) < 4

    def keep_rows(value, c, rel, rows):
        n = value.shape[0] // 2
        low = low_half(n)
        pairs = value.astype(F32).reshape(n, 2, 8, 128)
        even, odd = pairs[:, 0], pairs[:, 1]
        left = jnp.where(low, even, pltpu.roll(odd, 4, 1)).reshape(8 * n, 128)
        right = jnp.where(low, pltpu.roll(even, 4, 1), odd).reshape(8 * n, 128)
        gathered[c, ys[rel], rows, 0:128] = left.astype(BF16)
        gathered[c, ys[rel], rows, 128:256] = right.astype(BF16)

    keep_rows(a2a_in[...], core, 0, slice(0, ROWS))

    def ag_copy(slot, k, device):
        ref = gathered.at[core, ys[slot]]
        return rcopy(ref, ref, ag_ssem, ag_rsem.at[k], device)

    for k, step in enumerate((2, -2, 1, -1)):
        ag_copy(0, k, ydev(step)).start()

    def pass_copy(c, rel):
        ref = gathered.at[c, ys[rel]]
        k = ((0,) + NEAR).index(rel)
        return rcopy(ref, ref, pf_ssem, pf_rsem.at[k], partner)

    def pass_on(rel):
        pass_copy(core, rel).start()

    def pass_wait(rel):
        pass_copy(other, rel).wait_recv()

    pass_on(0)

    for copy in smalls[3:6]:
        copy.wait()
    loaded(w_dense, 0)
    act = jnp.zeros((8, 128), F32)
    mix_acc = jnp.zeros((8, PART), F32)
    for j in range(NTP):
        cols = slice(j * PART, (j + 1) * PART)
        n = (tok_all[j].astype(F32) * scale * gain[:, cols]).astype(BF16)
        mix_acc = mix_acc + n.astype(F32) * mixw[:, cols]
        act = act + nt_dot(n, w_dense[:, cols])
    gate_ref[...] = jnp.broadcast_to(
        jax.nn.sigmoid(jnp.sum(mix_acc, axis=1, keepdims=True)), (8, 128)
    )
    dh_own[...] = (silu(act[:, 0:64]) * act[:, 64:128]).astype(BF16)
    dh_copy = rcopy(dh_own, dh_par, dh_ssem, dh_rsem, partner)
    dh_copy.start()
    pl.when(block == 1)(send_far)

    loaded(dd_own, 1)
    parts[0].wait_recv()
    dh_copy.wait_recv()
    for k in range(NY):
        dense_out[k] = jnp.dot(
            dh_own[...], dd_own[k], preferred_element_type=F32
        ) + jnp.dot(dh_par[...], dd_par[k], preferred_element_type=F32)
    dense_in[y] = dense_out[y]
    loaded(w_gu.at[0], 2)
    parts[1].wait_recv()
    for rel in (6, 2):
        ag_copy(rel, NEAR.index(rel), partner).wait_recv()
        pass_on(rel)
    done.append(arrived(r_in, r_in, r_ssem, r_rsem, NEP - 1))
    picked = (
        lax.broadcasted_iota(jnp.int32, (ROWS, NEP), 0) // 4
        == lax.broadcasted_iota(jnp.int32, (ROWS, NEP), 1)
    )
    spread = jnp.dot(
        jnp.where(picked, 1.0, 0.0),
        r_in[...].reshape(NEP, 256),
        preferred_element_type=F32,
        precision=lax.Precision.HIGHEST,
    )
    wanted = me_e * 8 + lax.broadcasted_iota(jnp.int32, (ROWS, 256), 0) % 4
    here = lax.broadcasted_iota(jnp.int32, (ROWS, 256), 1) == wanted
    row_scale = jnp.sum(jnp.where(here, spread, 0.0), axis=1, keepdims=True)

    def project(*slices, rows=slice(0, ROWS), first=False):
        sums = [None, None]
        for c, rel in slices:
            cols = pl.ds(pl.multiple_of((2 * ys[rel] + c) * PART, PART), PART)
            n = gathered[c, ys[rel], rows].astype(F32) * row_scale[rows] * gain[:, cols]
            n = n.astype(BF16)
            for k in range(2):
                v = nt_dot(n, w_gu[k, :, :, cols].reshape(256, PART))
                sums[k] = v if sums[k] is None else sums[k] + v
        for k in range(2):
            acts[k, rows] = sums[k] if first else acts[k, rows] + sums[k]

    pass_wait(0)
    project((core, 0), (other, 0), (core, 6), (core, 2), first=True)
    for rel in (7, 1):
        ag_copy(rel, NEAR.index(rel), partner).wait_recv()
        pass_on(rel)
    for step in y_order:
        rcopy(
            dense_out.at[ys[step]], dense_in.at[y], dense_ssem, dense_rsem, ydev(step)
        ).start()
    pass_wait(6)
    pass_wait(2)
    project((core, 7), (core, 1), (other, 6), (other, 2))
    row = lax.broadcasted_iota(jnp.int32, (HALF, 128), 0)
    col = lax.broadcasted_iota(jnp.int32, (HALF, 128), 1)
    mine = (row // 2) % 2 == col // 64
    diagonal = row == col

    def rows_of(b):
        return slice(b * HALF, (b + 1) * HALF)

    def far_wait(b):
        ref = far_in.at[part(b, 16)]
        rcopy(ref, ref, far_ssem, far_rsem.at[b], partner).wait_recv()
        copy = rcopy(ref, far_par.at[part(b, 16)], fp_ssem, fp_rsem.at[b], partner)
        copy.start()
        for i, rel in enumerate(FAR):
            keep_rows(far_in[b * 16 : (b + 1) * 16, i], core, rel, rows_of(b))
        return copy

    def far_other(b, copy):
        copy.wait_recv()
        for i, rel in enumerate(FAR):
            keep_rows(far_par[b * 16 : (b + 1) * 16, i], other, rel, rows_of(b))
        project((other, 3), (other, 4), (other, 5), rows=rows_of(b))

    def hide(b):
        for k in range(2):
            v = acts[k, rows_of(b)]
            hidden = silu(v[:, 0:128]) * v[:, 128:256]
            hid[rows_of(b), k * 128 : (k + 1) * 128] = jnp.where(mine, hidden, 0.0).astype(
                BF16
            )

    def partial(rel, b):
        k = ys[rel]
        both = jnp.concatenate(
            [wd_own[k].reshape(128, PART), wd_par[k].reshape(128, PART)], axis=0
        )
        return jnp.dot(hid[rows_of(b), :], both, preferred_element_type=F32)

    def column(value):
        return jnp.sum(jnp.where(diagonal, value, 0.0), axis=0, keepdims=True)

    def messages(value):
        n = value.shape[0] // 8
        low = low_half(n)
        left = value[:, 0:128].reshape(n, 8, 128)
        right = value[:, 128:256].reshape(n, 8, 128)
        even = jnp.where(low, left, pltpu.roll(right, 4, 1))
        odd = jnp.where(low, pltpu.roll(left, 4, 1), right)
        return jnp.stack([even, odd], axis=1).reshape(2 * n, 8, 128)

    def q_copies(k, b, device):
        at = (k, b)
        return (
            rcopy(q_out.at[at], q_in.at[at], q_ssem, q_rsem.at[at], device),
            rcopy(s_out.at[at], s_in.at[at], sc_ssem, sc_rsem.at[at], device),
        )

    def q_send(k, b):
        value = partial(NEAR[k], b)
        most = jnp.maximum(jnp.max(jnp.abs(value), axis=1, keepdims=True), 1e-30)
        q_out[k, b] = jnp.round(value * (32767.0 / most)).astype(jnp.int16)
        s_out[k, b] = column(most * (1.0 / 32767.0))
        for copy in q_copies(k, b, ydev(NEAR[k])):
            copy.start()

    def q_get(k, b):
        for copy in q_copies(k, b, partner):
            copy.wait_recv()
        unit = jnp.sum(jnp.where(diagonal, s_in[k, b], 0.0), axis=1, keepdims=True)
        return q_in[k, b].astype(F32) * unit

    def send_fq(peer):
        rcopy(fq_out.at[peer], fq_in.at[me_e], fq_ssem, fq_rsem, (peer, me_t)).start()

    def down(b):
        values = [partial(rel, b) for rel in FAR]
        most = jnp.maximum(
            jnp.maximum(jnp.abs(values[0]), jnp.abs(values[1])), jnp.abs(values[2])
        )
        most = jnp.maximum(jnp.max(most, axis=1, keepdims=True), 1e-30)
        fs_out[b] = column(most * (1.0 / 32767.0))
        for i in range(3):
            fq_out[b * 16 : (b + 1) * 16, i] = messages(
                jnp.round(values[i] * (32767.0 / most))
            ).astype(jnp.int16)
        to_block(b, send_fq)
        for k in range(4):
            q_send(k, b)

        def send_fs(peer):
            rcopy(fs_out.at[b], fs_in.at[me_e], fs_ssem, fs_rsem, (peer, me_t)).start()

        to_block(b, send_fs)
        kept[b] = partial(0, b)

    def send_ret(peer):
        rcopy(ret_out.at[peer], ret_in.at[me_e], ret_ssem, ret_rsem, (peer, me_t)).start()

    def give_back(b):
        summed = kept[b]
        for k in range(4):
            summed = summed + q_get(k, b)
        ret_out[b * 16 : (b + 1) * 16] = messages(summed)
        to_block(b, send_ret)

    raw0 = far_wait(0)
    pass_wait(7)
    pass_wait(1)
    project((other, 7), (other, 1))
    project((core, 3), (core, 4), (core, 5), rows=rows_of(0))
    far_other(0, raw0)
    hide(0)
    loaded(wd_own, 3)
    parts[2].wait_recv()
    down(0)
    raw1 = far_wait(1)
    project((core, 3), (core, 4), (core, 5), rows=rows_of(1))
    far_other(1, raw1)
    hide(1)
    down(1)
    fq_in[me_e] = fq_out[me_e]
    fs_in[me_e] = fs_out[block]
    done.append(arrived(dense_out, dense_in, dense_ssem, dense_rsem, NY - 1))
    dense = dense_in[0]
    for k in range(1, NY):
        dense = dense + dense_in[k]
    gate = gate_ref[...]
    dense = jnp.concatenate([gate, gate], axis=1) * dense
    give_back(0)
    done.append(arrived(fq_out, fq_in, fq_ssem, fq_rsem, NEP - 1))
    done.append(arrived(fs_in, fs_in, fs_ssem, fs_rsem, NEP - 1))
    lane2 = lax.broadcasted_iota(jnp.int32, (128, 256), 1)
    mine4 = lax.broadcasted_iota(jnp.int32, (128, 256), 0) == lax.rem(me_e, 16) * 4 + lane2 % 4
    unit = jnp.dot(
        fs_in[...].reshape(NEP, 128),
        jnp.where(mine4, 1.0, 0.0),
        preferred_element_type=F32,
        precision=lax.Precision.HIGHEST,
    )
    source = lax.broadcasted_iota(jnp.int32, (NEP, 256), 0)
    source = source == lax.broadcasted_iota(jnp.int32, (NEP, 256), 1) // 8
    unit = jnp.sum(jnp.where(source, unit, 0.0), axis=0, keepdims=True)
    far_sum = jnp.dot(
        comb[...] * unit,
        jnp.concatenate(
            [fq_in[:, i].astype(F32).reshape(256, 128) for i in range(3)], axis=1
        ),
        preferred_element_type=F32,
        precision=lax.Precision.HIGHEST,
    )
    for i, rel in enumerate(FAR):
        cols = slice(i * 128, (i + 1) * 128)
        fy_out[i, :, 0:128] = far_sum[0:8, cols]
        fy_out[i, :, 128:256] = far_sum[8:16, cols]
        rcopy(fy_out.at[i], fy_in.at[i], fy_ssem, fy_rsem, ydev(rel)).start()
    give_back(1)
    ret_in[me_e] = ret_out[me_e]
    done.append(arrived(ret_out, ret_in, ret_ssem, ret_rsem, NEP - 1))
    mixed = jnp.dot(
        comb[...],
        ret_in[...].reshape(256, 128),
        preferred_element_type=F32,
        precision=lax.Precision.HIGHEST,
    )
    combined = jnp.concatenate([mixed[0:8], mixed[8:16]], axis=1) + dense
    fy_copy = rcopy(fy_out, fy_in, fy_ssem, fy_rsem, partner)
    fy_copy.wait_recv()
    combined = combined + fy_in[0] + fy_in[1] + fy_in[2]
    token_diagonal = (
        lax.broadcasted_iota(jnp.int32, (8, 128), 0)
        == lax.broadcasted_iota(jnp.int32, (8, 128), 1)
    )
    own = jnp.sum(
        jnp.where(token_diagonal, jnp.sum(combined * combined, axis=1, keepdims=True), 0.0),
        axis=0,
        keepdims=True,
    )
    sq_out[...] = own
    for step in y_order:
        for c in range(2):
            rcopy(sq_out, sq_in.at[me_t], sq_ssem, sq_rsem, (me_e, ys[step] * 2 + c)).start()
    rcopy(sq_out, sq_in.at[me_t], sq_ssem, sq_rsem, partner).start()
    sq_in[me_t] = own
    done.append(arrived(sq_in, sq_in, sq_ssem, sq_rsem, NTP - 1))
    total_sq = sq_in[0]
    for j in range(1, NTP):
        total_sq = total_sq + sq_in[j]
    final = lax.rsqrt(
        jnp.sum(jnp.where(token_diagonal, total_sq, 0.0), axis=1, keepdims=True) / WIDTH + EPS
    )
    out[...] = (combined * final * ogain[...]).astype(BF16)

    near = gathered.at[core, pl.ds(0, 4)]
    most_far = far_in.at[pl.ds(0, NEP - 1)]
    done += [
        rcopy(near, near, ag_ssem, ag_rsem.at[0], partner),
        rcopy(q_out, q_in, q_ssem, q_rsem.at[0, 0], partner),
        rcopy(s_out, s_in, sc_ssem, sc_rsem.at[0, 0], partner),
        rcopy(most_far, most_far, far_ssem, far_rsem.at[0], partner),
    ]
    five = gathered.at[core, pl.ds(0, 5)]
    done.append(rcopy(five, five, pf_ssem, pf_rsem.at[0], partner))
    for copy in parts + [dh_copy, raw0, raw1, fy_copy] + done:
        copy.wait_send()


def local(
    tokens,
    norm_gain,
    route_experts,
    route_logits,
    expert_gate,
    expert_up,
    expert_down,
    dense_gate,
    dense_up,
    dense_down,
    mix_weight,
    out_gain,
):
    vmem = pl.BlockSpec(memory_space=pltpu.VMEM)
    dma = pltpu.SemaphoreType.DMA
    return pl.pallas_call(
        kernel,
        out_shape=pltpu.VMEM((8, PART), BF16),
        in_specs=[pl.BlockSpec(memory_space=pl.ANY)] * 12,
        out_specs=vmem,
        scratch_shapes=[
            pltpu.VMEM((8, PART), BF16),
            pltpu.VMEM((1, WIDTH), F32),
            pltpu.SMEM((2, 8), jnp.int32),
            pltpu.SMEM((2, 8), F32),
            pltpu.VMEM((1, WIDTH), F32),
            pltpu.VMEM((1, PART), F32),
            pltpu.VMEM((2, 4, 64, WIDTH), BF16),
            pltpu.VMEM((NY, 2, 64, PART), BF16),
            pltpu.VMEM((NY, 2, 64, PART), BF16),
            pltpu.VMEM((128, WIDTH), BF16),
            pltpu.VMEM((NY, 64, PART), BF16),
            pltpu.VMEM((NY, 64, PART), BF16),
            pltpu.VMEM((NEP, 8, 128), BF16),
            pltpu.VMEM((NEP, 8, 128), BF16),
            pltpu.VMEM((NEP, 3, 8, 128), BF16),
            pltpu.VMEM((NEP, 3, 8, 128), BF16),
            pltpu.VMEM((NEP, 3, 8, 128), BF16),
            pltpu.VMEM((2, NY, ROWS, PART), BF16),
            pltpu.VMEM((NTP, 8, PART), BF16),
            pltpu.VMEM((NY, 8, PART), F32),
            pltpu.VMEM((NY, 8, PART), F32),
            pltpu.VMEM((8, 64), BF16),
            pltpu.VMEM((8, 64), BF16),
            pltpu.VMEM((16, 256), F32),
            pltpu.VMEM((16, 256), BF16),
            pltpu.VMEM((8, 256), F32),
            pltpu.VMEM((1, 256), F32),
            pltpu.VMEM((NEP, 1, 256), F32),
            pltpu.VMEM((2, ROWS, 256), F32),
            pltpu.VMEM((ROWS, 256), BF16),
            pltpu.VMEM((4, 2, HALF, PART), jnp.int16),
            pltpu.VMEM((4, 2, HALF, PART), jnp.int16),
            pltpu.VMEM((4, 2, 1, 128), F32),
            pltpu.VMEM((4, 2, 1, 128), F32),
            pltpu.VMEM((NEP, 3, 8, 128), jnp.int16),
            pltpu.VMEM((NEP, 3, 8, 128), jnp.int16),
            pltpu.VMEM((2, 1, 128), F32),
            pltpu.VMEM((NEP, 1, 128), F32),
            pltpu.VMEM((3, 8, PART), F32),
            pltpu.VMEM((3, 8, PART), F32),
            pltpu.VMEM((2, HALF, PART), F32),
            pltpu.VMEM((NEP, 8, 128), F32),
            pltpu.VMEM((NEP, 8, 128), F32),
            pltpu.VMEM((1, 128), F32),
            pltpu.VMEM((NTP, 1, 128), F32),
            pltpu.VMEM((8, 128), F32),
            dma((6,)),
            dma((4,)),
            dma((3,)),
            dma((3,)),
            dma,
            dma,
            dma,
            dma((2,)),
            dma,
            dma,
            dma,
            dma,
            dma,
            dma,
            dma,
            dma((4,)),
            dma,
            dma((5,)),
            dma,
            dma((2,)),
            dma,
            dma,
            dma,
            dma((4, 2)),
            dma,
            dma((4, 2)),
            dma,
            dma,
            dma,
            dma,
            dma,
            dma,
            dma,
            dma,
            dma,
            dma,
        ],
        compiler_params=pltpu.CompilerParams(
            collective_id=0, has_side_effects=True, vmem_limit_bytes=56650000
        ),
    )(
        tokens,
        norm_gain.reshape(1, WIDTH),
        route_experts.T,
        route_logits.T,
        jnp.swapaxes(expert_gate, 1, 2),
        jnp.swapaxes(expert_up, 1, 2),
        expert_down,
        dense_gate.T,
        dense_up.T,
        dense_down,
        mix_weight.reshape(1, WIDTH),
        out_gain.reshape(1, PART),
    )


def solution(mesh):
    tp = "tp"
    in_specs = (
        P("ep", tp),
        P(),
        P("ep", None),
        P("ep", None),
        P("ep", None, tp),
        P("ep", None, tp),
        P("ep", tp, None),
        P(None, tp),
        P(None, tp),
        P(tp, None),
        P(),
        P(tp),
    )
    return jax.shard_map(
        local, mesh=mesh, in_specs=in_specs, out_specs=P("ep", tp), check_vma=False
    )
```

```python
import functools

import jax
import jax.numpy as jnp
from jax import lax
from jax.experimental import pallas as pl
from jax.experimental.pallas import tpu as pltpu
from jax.sharding import PartitionSpec as P

MESH = pl.DeviceIdType.MESH
F32 = jnp.float32
BF16 = jnp.bfloat16
EPS = 1e-06

NX, NZ, NY = 4, 8, 8
NEP = NX * NZ
NTP = 2 * NY
ROWS = 128
FAR = (3, 4, 5)
NEAR = (6, 2, 7, 1)
PART = 256
WIDTH = 4096


def rcopy(src, dst, send_sem, recv_sem, device):
    return pltpu.make_async_remote_copy(
        src_ref=src,
        dst_ref=dst,
        send_sem=send_sem,
        recv_sem=recv_sem,
        device_id=device,
        device_id_type=MESH,
    )


def nt_dot(a, b):
    return lax.dot_general(a, b, (((1,), (1,)), ((), ())), preferred_element_type=F32)


def silu(v):
    return v / (1.0 + jnp.exp(-v))


def kernel(
    tok_hbm,
    gain_hbm,
    routes_hbm,
    logits_hbm,
    wg,
    wu,
    wd,
    dg,
    du,
    dd,
    mixw_hbm,
    ogain_hbm,
    out,
    tok,
    gain,
    routes,
    logits,
    mixw,
    ogain,
    w_gu,
    wd_own,
    wd_par,
    w_dense,
    dd_own,
    dd_par,
    a2a_out,
    a2a_in,
    far_out,
    far_in,
    far_par,
    gathered,
    tok_all,
    dense_out,
    dense_in,
    dh_own,
    dh_par,
    comb,
    place,
    slots,
    r_out,
    r_in,
    acts,
    hid,
    q_out,
    q_in,
    s_out,
    s_in,
    fq_out,
    fq_in,
    fs_out,
    fs_in,
    fy_out,
    fy_in,
    kept,
    ret_out,
    ret_in,
    sq_out,
    sq_in,
    gate_ref,
    i_sem,
    w_sem,
    wp_ssem,
    wp_rsem,
    a2a_ssem,
    a2a_rsem,
    far_ssem,
    far_rsem,
    tok_ssem,
    tok_rsem,
    dh_ssem,
    dh_rsem,
    dense_ssem,
    dense_rsem,
    ag_ssem,
    ag_rsem,
    pf_ssem,
    pf_rsem,
    fp_ssem,
    fp_rsem,
    r_ssem,
    r_rsem,
    q_ssem,
    q_rsem,
    sc_ssem,
    sc_rsem,
    fq_ssem,
    fq_rsem,
    fs_ssem,
    fs_rsem,
    fy_ssem,
    fy_rsem,
    ret_ssem,
    ret_rsem,
    sq_ssem,
    sq_rsem,
):
    me_e = lax.axis_index("ep")
    me_t = lax.axis_index("tp")
    z, x = lax.div(me_e, NX), lax.rem(me_e, NX)
    y, core = lax.div(me_t, 2), lax.rem(me_t, 2)
    other = 1 - core
    partner = (me_e, y * 2 + other)
    zs = [lax.rem(z + k, NZ) * NX for k in range(NZ)]
    xs = [lax.rem(x + k, NX) for k in range(NX)]
    ys = [lax.rem(y + k, NY) for k in range(NY)]
    peers = [zs[dz] + xs[dx] for dz in (4, 3, 5, 2, 6, 1, 7, 0) for dx in (2, 1, 3, 0)][:-1]
    y_order = (4, 3, 5, 2, 6, 1, 7)
    owners = [k + lax.div(k - me_e + NEP, NEP) for k in range(NEP - 1)]

    def ydev(step):
        return (me_e, ys[step % NY] * 2 + core)

    barrier = pltpu.get_barrier_semaphore()
    for peer in peers:
        pl.semaphore_signal(barrier, inc=1, device_id=(peer, me_t), device_id_type=MESH)
    for step in y_order:
        for c in range(2):
            pl.semaphore_signal(
                barrier, inc=1, device_id=(me_e, ys[step] * 2 + c), device_id_type=MESH
            )
    pl.semaphore_signal(barrier, inc=1, device_id=partner, device_id_type=MESH)

    smalls = [
        pltpu.make_async_copy(routes_hbm, routes, i_sem.at[0]),
        pltpu.make_async_copy(logits_hbm, logits, i_sem.at[1]),
        pltpu.make_async_copy(tok_hbm, tok, i_sem.at[2]),
        pltpu.make_async_copy(gain_hbm, gain, i_sem.at[3]),
        pltpu.make_async_copy(mixw_hbm, mixw, i_sem.at[4]),
        pltpu.make_async_copy(ogain_hbm, ogain, i_sem.at[5]),
    ]

    def columns(k, c):
        return pl.ds(pl.multiple_of((2 * k + c) * PART, PART), PART)

    def load(src, dst, k):
        pltpu.make_async_copy(src, dst, w_sem.at[k]).start()

    def loaded(dst, k):
        pltpu.make_async_copy(dst, dst, w_sem.at[k]).wait()

    for copy in smalls:
        copy.start()
    load(dg, w_dense.at[pl.ds(0, 64)], 0)
    load(du, w_dense.at[pl.ds(64, 64)], 0)
    for k in range(NY):
        load(dd.at[:, columns(k, core)], dd_own.at[k], 1)
    load(wg, w_gu.at[0, pl.ds(0, 2)], 2)
    load(wu, w_gu.at[0, pl.ds(2, 2)], 2)
    for k in range(NY):
        load(wd.at[:, :, columns(k, core)], wd_own.at[k], 3)

    for copy in smalls[0:3]:
        copy.wait()
    lane = lax.broadcasted_iota(jnp.int32, (8, 256), 1)
    sub = lax.broadcasted_iota(jnp.int32, (8, 256), 0)
    expert = 2 * (lane // 8) + (lane // 2) % 2
    half = (lane // 4) % 2
    r0 = jnp.zeros((8, 256), jnp.int32)
    r1 = jnp.zeros((8, 256), jnp.int32)
    l0 = jnp.zeros((8, 256), F32)
    l1 = jnp.zeros((8, 256), F32)
    for t in range(8):
        r0 = jnp.where(sub == t, routes[0, t], r0)
        r1 = jnp.where(sub == t, routes[1, t], r1)
        l0 = jnp.where(sub == t, logits[0, t], l0)
        l1 = jnp.where(sub == t, logits[1, t], l1)
    top = jnp.maximum(l0, l1)
    e0, e1 = jnp.exp(l0 - top), jnp.exp(l1 - top)
    is0, is1 = (r0 == expert), (r1 == expert)
    hit = jnp.where(is0, 1.0, 0.0) + jnp.where(is1, 1.0, 0.0)
    before = jnp.zeros((8, 256), F32)
    for t in range(7):
        before = before + jnp.where(sub > t, hit[t : t + 1, :], 0.0)
    placed = jnp.where(before == (lane % 2).astype(F32), hit, 0.0)
    weight = (jnp.where(is0, e0, 0.0) + jnp.where(is1, e1, 0.0)) / (e0 + e1) * placed
    comb[0:8, :] = jnp.where(half == 0, weight, 0.0)
    comb[8:16, :] = jnp.where(half == 1, weight, 0.0)
    slots[...] = placed
    place[...] = jnp.concatenate(
        [jnp.where(half == 0, placed, 0.0), jnp.where(half == 1, placed, 0.0)], axis=0
    ).astype(BF16)

    def placed_rows(value):
        halves = jnp.concatenate(
            [value[:, 0:128].astype(F32), value[:, 128:256].astype(F32)], axis=0
        ).astype(BF16)
        rows = lax.dot_general(
            place[...], halves, (((0,), (0,)), ((), ())), preferred_element_type=F32
        )
        return rows.astype(BF16).reshape(NEP, 8, 128)

    tok_value = tok[...]
    a2a_out[...] = placed_rows(tok_value)
    a2a_in[me_e] = a2a_out[me_e]
    tok_all[me_t] = tok_value

    pl.semaphore_wait(barrier, NEP - 1 + NTP - 1)

    for step in y_order:
        for c in range(2):
            rcopy(
                tok, tok_all.at[me_t], tok_ssem, tok_rsem, (me_e, ys[step] * 2 + c)
            ).start()
    rcopy(tok, tok_all.at[me_t], tok_ssem, tok_rsem, partner).start()

    for peer in peers:
        rcopy(a2a_out.at[peer], a2a_in.at[me_e], a2a_ssem, a2a_rsem, (peer, me_t)).start()

    for k in range(NY):
        rcopy(
            dd.at[:, columns(k, other)], dd_par.at[k], wp_ssem.at[0], wp_rsem.at[0], partner
        ).start()
    for k, ref in enumerate((wg, wu)):
        rcopy(
            ref, w_gu.at[1, pl.ds(2 * k, 2)], wp_ssem.at[1], wp_rsem.at[1], partner
        ).start()
    for k in range(NY):
        rcopy(
            wd.at[:, :, columns(k, other)], wd_par.at[k], wp_ssem.at[2], wp_rsem.at[2], partner
        ).start()
    parts = [
        rcopy(ref, ref, wp_ssem.at[k], wp_rsem.at[k], partner)
        for k, ref in enumerate((dd_par, w_gu.at[1], wd_par))
    ]

    def arrived(src, dst, ssem, rsem, n):
        part = pl.ds(0, n)
        copy = rcopy(src.at[part], dst.at[part], ssem, rsem, partner)
        copy.wait_recv()
        return copy

    done = [arrived(tok_all, tok_all, tok_ssem, tok_rsem, NTP - 1)]
    squares = jnp.zeros((8, PART), F32)
    for j in range(NTP):
        v = tok_all[j].astype(F32)
        squares = squares + v * v
    scale = lax.rsqrt(jnp.sum(squares, axis=1, keepdims=True) / WIDTH + EPS)
    r_out[...] = jnp.sum(slots[...] * scale, axis=0, keepdims=True)
    for i, rel in enumerate(FAR):
        far_out[:, i] = placed_rows(tok_all[ys[rel] * 2 + core])
    for peer in peers:
        rcopy(r_out, r_in.at[me_e], r_ssem, r_rsem, (peer, me_t)).start()
    for peer in peers:
        rcopy(far_out.at[peer], far_in.at[me_e], far_ssem, far_rsem, (peer, me_t)).start()
    r_in[me_e] = r_out[...]
    far_in[me_e] = far_out[me_e]

    done.append(arrived(a2a_out, a2a_in, a2a_ssem, a2a_rsem, NEP - 1))
    sub3 = lax.broadcasted_iota(jnp.int32, (16, 8, 128), 1)

    def keep_rows(value, c, rel):
        pairs = value.astype(F32).reshape(16, 2, 8, 128)
        even, odd = pairs[:, 0], pairs[:, 1]
        left = jnp.where(sub3 < 4, even, pltpu.roll(odd, 4, 1)).reshape(ROWS, 128)
        right = jnp.where(sub3 < 4, pltpu.roll(even, 4, 1), odd).reshape(ROWS, 128)
        gathered[c, ys[rel], :, 0:128] = left.astype(BF16)
        gathered[c, ys[rel], :, 128:256] = right.astype(BF16)

    keep_rows(a2a_in[...], core, 0)

    def ag_copy(slot, k, device):
        ref = gathered.at[core, ys[slot]]
        return rcopy(ref, ref, ag_ssem, ag_rsem.at[k], device)

    for k, step in enumerate((2, -2, 1, -1)):
        ag_copy(0, k, ydev(step)).start()

    def pass_copy(c, rel):
        ref = gathered.at[c, ys[rel]]
        k = ((0,) + NEAR).index(rel)
        return rcopy(ref, ref, pf_ssem, pf_rsem.at[k], partner)

    def pass_on(rel):
        pass_copy(core, rel).start()

    def pass_wait(rel):
        pass_copy(other, rel).wait_recv()

    pass_on(0)

    for copy in smalls[3:6]:
        copy.wait()
    loaded(w_dense, 0)
    act = jnp.zeros((8, 128), F32)
    mix_acc = jnp.zeros((8, PART), F32)
    for j in range(NTP):
        cols = slice(j * PART, (j + 1) * PART)
        n = (tok_all[j].astype(F32) * scale * gain[:, cols]).astype(BF16)
        mix_acc = mix_acc + n.astype(F32) * mixw[:, cols]
        act = act + nt_dot(n, w_dense[:, cols])
    gate_ref[...] = jnp.broadcast_to(
        jax.nn.sigmoid(jnp.sum(mix_acc, axis=1, keepdims=True)), (8, 128)
    )
    dh_own[...] = (silu(act[:, 0:64]) * act[:, 64:128]).astype(BF16)
    dh_copy = rcopy(dh_own, dh_par, dh_ssem, dh_rsem, partner)
    dh_copy.start()

    loaded(dd_own, 1)
    parts[0].wait_recv()
    dh_copy.wait_recv()
    for k in range(NY):
        dense_out[k] = jnp.dot(
            dh_own[...], dd_own[k], preferred_element_type=F32
        ) + jnp.dot(dh_par[...], dd_par[k], preferred_element_type=F32)
    dense_in[y] = dense_out[y]
    loaded(w_gu.at[0], 2)
    parts[1].wait_recv()
    for rel in (6, 2):
        ag_copy(rel, NEAR.index(rel), partner).wait_recv()
        pass_on(rel)
    done.append(arrived(r_in, r_in, r_ssem, r_rsem, NEP - 1))
    picked = (
        lax.broadcasted_iota(jnp.int32, (ROWS, NEP), 0) // 4
        == lax.broadcasted_iota(jnp.int32, (ROWS, NEP), 1)
    )
    spread = jnp.dot(
        jnp.where(picked, 1.0, 0.0),
        r_in[...].reshape(NEP, 256),
        preferred_element_type=F32,
        precision=lax.Precision.HIGHEST,
    )
    wanted = me_e * 8 + lax.broadcasted_iota(jnp.int32, (ROWS, 256), 0) % 4
    here = lax.broadcasted_iota(jnp.int32, (ROWS, 256), 1) == wanted
    row_scale = jnp.sum(jnp.where(here, spread, 0.0), axis=1, keepdims=True)

    def project(*slices, first=False):
        sums = [None, None]
        for c, rel in slices:
            cols = pl.ds(pl.multiple_of((2 * ys[rel] + c) * PART, PART), PART)
            n = (gathered[c, ys[rel]].astype(F32) * row_scale * gain[:, cols]).astype(BF16)
            for k in range(2):
                v = nt_dot(n, w_gu[k, :, :, cols].reshape(256, PART))
                sums[k] = v if sums[k] is None else sums[k] + v
        for k in range(2):
            acts[k] = sums[k] if first else acts[k] + sums[k]

    pass_wait(0)
    project((core, 0), (other, 0), (core, 6), (core, 2), first=True)
    for rel in (7, 1):
        ag_copy(rel, NEAR.index(rel), partner).wait_recv()
        pass_on(rel)
    for step in y_order:
        rcopy(
            dense_out.at[ys[step]], dense_in.at[y], dense_ssem, dense_rsem, ydev(step)
        ).start()
    pass_wait(6)
    pass_wait(2)
    project((core, 7), (core, 1), (other, 6), (other, 2))
    done.append(arrived(far_out, far_in, far_ssem, far_rsem, NEP - 1))
    raw = rcopy(far_in, far_par, fp_ssem, fp_rsem, partner)
    raw.start()
    for i, rel in enumerate(FAR):
        keep_rows(far_in[:, i], core, rel)
    pass_wait(7)
    pass_wait(1)
    project((other, 7), (other, 1), (core, 3), (core, 4), (core, 5))
    raw.wait_recv()
    for i, rel in enumerate(FAR):
        keep_rows(far_par[:, i], other, rel)
    project((other, 3), (other, 4), (other, 5))

    row = lax.broadcasted_iota(jnp.int32, (ROWS, 128), 0)
    col = lax.broadcasted_iota(jnp.int32, (ROWS, 128), 1)
    mine = (row // 2) % 2 == col // 64
    for k in range(2):
        v = acts[k]
        hidden = silu(v[:, 0:128]) * v[:, 128:256]
        hid[:, k * 128 : (k + 1) * 128] = jnp.where(mine, hidden, 0.0).astype(BF16)
    loaded(wd_own, 3)
    parts[2].wait_recv()

    diagonal = row == col

    def partial(rel):
        k = ys[rel]
        both = jnp.concatenate(
            [wd_own[k].reshape(128, PART), wd_par[k].reshape(128, PART)], axis=0
        )
        return jnp.dot(hid[...], both, preferred_element_type=F32)

    def column(value):
        return jnp.sum(jnp.where(diagonal, value, 0.0), axis=0, keepdims=True)

    def messages(value):
        left = value[:, 0:128].reshape(16, 8, 128)
        right = value[:, 128:256].reshape(16, 8, 128)
        even = jnp.where(sub3 < 4, left, pltpu.roll(right, 4, 1))
        odd = jnp.where(sub3 < 4, pltpu.roll(left, 4, 1), right)
        return jnp.stack([even, odd], axis=1).reshape(NEP, 8, 128)

    def q_copies(k, device):
        return (
            rcopy(q_out.at[k], q_in.at[k], q_ssem, q_rsem.at[k], device),
            rcopy(s_out.at[k], s_in.at[k], sc_ssem, sc_rsem.at[k], device),
        )

    def q_send(k):
        value = partial(NEAR[k])
        most = jnp.maximum(jnp.max(jnp.abs(value), axis=1, keepdims=True), 1e-30)
        q_out[k] = jnp.round(value * (32767.0 / most)).astype(jnp.int16)
        s_out[k] = column(most * (1.0 / 32767.0))
        for copy in q_copies(k, ydev(NEAR[k])):
            copy.start()

    def q_get(k):
        for copy in q_copies(k, partner):
            copy.wait_recv()
        unit = jnp.sum(jnp.where(diagonal, s_in[k], 0.0), axis=1, keepdims=True)
        return q_in[k].astype(F32) * unit

    values = [partial(rel) for rel in FAR]
    most = jnp.maximum(jnp.maximum(jnp.abs(values[0]), jnp.abs(values[1])), jnp.abs(values[2]))
    most = jnp.maximum(jnp.max(most, axis=1, keepdims=True), 1e-30)
    fs_out[...] = column(most * (1.0 / 32767.0))
    for i in range(3):
        fq_out[:, i] = messages(jnp.round(values[i] * (32767.0 / most))).astype(jnp.int16)
    for peer in owners:
        rcopy(fq_out.at[peer], fq_in.at[me_e], fq_ssem, fq_rsem, (peer, me_t)).start()
    for k in range(4):
        q_send(k)
    for peer in owners:
        rcopy(fs_out, fs_in.at[me_e], fs_ssem, fs_rsem, (peer, me_t)).start()
    fq_in[me_e] = fq_out[me_e]
    fs_in[me_e] = fs_out[...]
    kept[...] = partial(0)
    done.append(arrived(dense_out, dense_in, dense_ssem, dense_rsem, NY - 1))
    dense = dense_in[0]
    for k in range(1, NY):
        dense = dense + dense_in[k]
    gate = gate_ref[...]
    dense = jnp.concatenate([gate, gate], axis=1) * dense
    summed = kept[...]
    for k in range(4):
        summed = summed + q_get(k)
    ret_out[...] = messages(summed)
    for peer in owners:
        rcopy(ret_out.at[peer], ret_in.at[me_e], ret_ssem, ret_rsem, (peer, me_t)).start()
    ret_in[me_e] = ret_out[me_e]
    done.append(arrived(fq_out, fq_in, fq_ssem, fq_rsem, NEP - 1))
    done.append(arrived(fs_in, fs_in, fs_ssem, fs_rsem, NEP - 1))
    lane2 = lax.broadcasted_iota(jnp.int32, (128, 256), 1)
    mine4 = lax.broadcasted_iota(jnp.int32, (128, 256), 0) == me_e * 4 + lane2 % 4
    unit = jnp.dot(
        fs_in[...].reshape(NEP, 128),
        jnp.where(mine4, 1.0, 0.0),
        preferred_element_type=F32,
        precision=lax.Precision.HIGHEST,
    )
    source = lax.broadcasted_iota(jnp.int32, (NEP, 256), 0)
    source = source == lax.broadcasted_iota(jnp.int32, (NEP, 256), 1) // 8
    unit = jnp.sum(jnp.where(source, unit, 0.0), axis=0, keepdims=True)
    far_sum = jnp.dot(
        comb[...] * unit,
        jnp.concatenate(
            [fq_in[:, i].astype(F32).reshape(256, 128) for i in range(3)], axis=1
        ),
        preferred_element_type=F32,
        precision=lax.Precision.HIGHEST,
    )
    for i, rel in enumerate(FAR):
        cols = slice(i * 128, (i + 1) * 128)
        fy_out[i, :, 0:128] = far_sum[0:8, cols]
        fy_out[i, :, 128:256] = far_sum[8:16, cols]
        rcopy(fy_out.at[i], fy_in.at[i], fy_ssem, fy_rsem, ydev(rel)).start()
    done.append(arrived(ret_out, ret_in, ret_ssem, ret_rsem, NEP - 1))
    mixed = jnp.dot(
        comb[...],
        ret_in[...].reshape(256, 128),
        preferred_element_type=F32,
        precision=lax.Precision.HIGHEST,
    )
    combined = jnp.concatenate([mixed[0:8], mixed[8:16]], axis=1) + dense
    fy_copy = rcopy(fy_out, fy_in, fy_ssem, fy_rsem, partner)
    fy_copy.wait_recv()
    combined = combined + fy_in[0] + fy_in[1] + fy_in[2]
    token_diagonal = (
        lax.broadcasted_iota(jnp.int32, (8, 128), 0)
        == lax.broadcasted_iota(jnp.int32, (8, 128), 1)
    )
    own = jnp.sum(
        jnp.where(token_diagonal, jnp.sum(combined * combined, axis=1, keepdims=True), 0.0),
        axis=0,
        keepdims=True,
    )
    sq_out[...] = own
    for step in y_order:
        for c in range(2):
            rcopy(sq_out, sq_in.at[me_t], sq_ssem, sq_rsem, (me_e, ys[step] * 2 + c)).start()
    rcopy(sq_out, sq_in.at[me_t], sq_ssem, sq_rsem, partner).start()
    sq_in[me_t] = own
    done.append(arrived(sq_in, sq_in, sq_ssem, sq_rsem, NTP - 1))
    total_sq = sq_in[0]
    for j in range(1, NTP):
        total_sq = total_sq + sq_in[j]
    final = lax.rsqrt(
        jnp.sum(jnp.where(token_diagonal, total_sq, 0.0), axis=1, keepdims=True) / WIDTH + EPS
    )
    out[...] = (combined * final * ogain[...]).astype(BF16)

    near = gathered.at[core, pl.ds(0, 4)]
    done += [
        rcopy(near, near, ag_ssem, ag_rsem.at[0], partner),
        rcopy(q_out, q_in, q_ssem, q_rsem.at[0], partner),
        rcopy(s_out, s_in, sc_ssem, sc_rsem.at[0], partner),
    ]
    five = gathered.at[core, pl.ds(0, 5)]
    done.append(rcopy(five, five, pf_ssem, pf_rsem.at[0], partner))
    for copy in parts + [dh_copy, raw, fy_copy] + done:
        copy.wait_send()


def local(
    tokens,
    norm_gain,
    route_experts,
    route_logits,
    expert_gate,
    expert_up,
    expert_down,
    dense_gate,
    dense_up,
    dense_down,
    mix_weight,
    out_gain,
):
    vmem = pl.BlockSpec(memory_space=pltpu.VMEM)
    dma = pltpu.SemaphoreType.DMA
    return pl.pallas_call(
        kernel,
        out_shape=pltpu.VMEM((8, PART), BF16),
        in_specs=[pl.BlockSpec(memory_space=pl.ANY)] * 12,
        out_specs=vmem,
        scratch_shapes=[
            pltpu.VMEM((8, PART), BF16),
            pltpu.VMEM((1, WIDTH), F32),
            pltpu.SMEM((2, 8), jnp.int32),
            pltpu.SMEM((2, 8), F32),
            pltpu.VMEM((1, WIDTH), F32),
            pltpu.VMEM((1, PART), F32),
            pltpu.VMEM((2, 4, 64, WIDTH), BF16),
            pltpu.VMEM((NY, 2, 64, PART), BF16),
            pltpu.VMEM((NY, 2, 64, PART), BF16),
            pltpu.VMEM((128, WIDTH), BF16),
            pltpu.VMEM((NY, 64, PART), BF16),
            pltpu.VMEM((NY, 64, PART), BF16),
            pltpu.VMEM((NEP, 8, 128), BF16),
            pltpu.VMEM((NEP, 8, 128), BF16),
            pltpu.VMEM((NEP, 3, 8, 128), BF16),
            pltpu.VMEM((NEP, 3, 8, 128), BF16),
            pltpu.VMEM((NEP, 3, 8, 128), BF16),
            pltpu.VMEM((2, NY, ROWS, PART), BF16),
            pltpu.VMEM((NTP, 8, PART), BF16),
            pltpu.VMEM((NY, 8, PART), F32),
            pltpu.VMEM((NY, 8, PART), F32),
            pltpu.VMEM((8, 64), BF16),
            pltpu.VMEM((8, 64), BF16),
            pltpu.VMEM((16, 256), F32),
            pltpu.VMEM((16, 256), BF16),
            pltpu.VMEM((8, 256), F32),
            pltpu.VMEM((1, 256), F32),
            pltpu.VMEM((NEP, 1, 256), F32),
            pltpu.VMEM((2, ROWS, 256), F32),
            pltpu.VMEM((ROWS, 256), BF16),
            pltpu.VMEM((4, ROWS, PART), jnp.int16),
            pltpu.VMEM((4, ROWS, PART), jnp.int16),
            pltpu.VMEM((4, 1, 128), F32),
            pltpu.VMEM((4, 1, 128), F32),
            pltpu.VMEM((NEP, 3, 8, 128), jnp.int16),
            pltpu.VMEM((NEP, 3, 8, 128), jnp.int16),
            pltpu.VMEM((1, 128), F32),
            pltpu.VMEM((NEP, 1, 128), F32),
            pltpu.VMEM((3, 8, PART), F32),
            pltpu.VMEM((3, 8, PART), F32),
            pltpu.VMEM((ROWS, PART), F32),
            pltpu.VMEM((NEP, 8, 128), F32),
            pltpu.VMEM((NEP, 8, 128), F32),
            pltpu.VMEM((1, 128), F32),
            pltpu.VMEM((NTP, 1, 128), F32),
            pltpu.VMEM((8, 128), F32),
            dma((6,)),
            dma((4,)),
            dma((3,)),
            dma((3,)),
            dma,
            dma,
            dma,
            dma,
            dma,
            dma,
            dma,
            dma,
            dma,
            dma,
            dma,
            dma((4,)),
            dma,
            dma((5,)),
            dma,
            dma,
            dma,
            dma,
            dma,
            dma((4,)),
            dma,
            dma((4,)),
            dma,
            dma,
            dma,
            dma,
            dma,
            dma,
            dma,
            dma,
            dma,
            dma,
        ],
        compiler_params=pltpu.CompilerParams(
            collective_id=0, has_side_effects=True, vmem_limit_bytes=56650000
        ),
    )(
        tokens,
        norm_gain.reshape(1, WIDTH),
        route_experts.T,
        route_logits.T,
        jnp.swapaxes(expert_gate, 1, 2),
        jnp.swapaxes(expert_up, 1, 2),
        expert_down,
        dense_gate.T,
        dense_up.T,
        dense_down,
        mix_weight.reshape(1, WIDTH),
        out_gain.reshape(1, PART),
    )


def solution(mesh):
    tp = "tp"
    in_specs = (
        P("ep", tp),
        P(),
        P("ep", None),
        P("ep", None),
        P("ep", None, tp),
        P("ep", None, tp),
        P("ep", tp, None),
        P(None, tp),
        P(None, tp),
        P(tp, None),
        P(),
        P(tp),
    )
    return jax.shard_map(
        local, mesh=mesh, in_specs=in_specs, out_specs=P("ep", tp), check_vma=False
    )
```

```python
import functools

import jax
import jax.numpy as jnp
from jax import lax
from jax.experimental import pallas as pl
from jax.experimental.pallas import tpu as pltpu
from jax.sharding import PartitionSpec as P

MESH = pl.DeviceIdType.MESH
F32 = jnp.float32
BF16 = jnp.bfloat16
EPS = 1e-06

NX, NZ, NY = 4, 8, 8
NEP = NX * NZ
NTP = 2 * NY
ROWS = 128
FAR = (3, 4, 5)
NEAR = (6, 2, 7, 1)
PART = 256
WIDTH = 4096


def rcopy(src, dst, send_sem, recv_sem, device):
    return pltpu.make_async_remote_copy(
        src_ref=src,
        dst_ref=dst,
        send_sem=send_sem,
        recv_sem=recv_sem,
        device_id=device,
        device_id_type=MESH,
    )


def nt_dot(a, b):
    return lax.dot_general(a, b, (((1,), (1,)), ((), ())), preferred_element_type=F32)


def pieces(value, axis):
    high = value.astype(BF16)
    rest = value - high.astype(F32)
    middle = rest.astype(BF16)
    low = (rest - middle.astype(F32)).astype(BF16)
    return jnp.concatenate([high, middle, low], axis=axis)


def silu(v):
    return v / (1.0 + jnp.exp(-v))


def kernel(
    tok_hbm,
    gain_hbm,
    routes_hbm,
    logits_hbm,
    wg,
    wu,
    wd,
    dg,
    du,
    dd,
    mixw_hbm,
    ogain_hbm,
    out,
    tok,
    gain,
    routes,
    logits,
    mixw,
    ogain,
    w_gu,
    wd_own,
    wd_par,
    w_dense,
    dd_own,
    dd_par,
    a2a_out,
    a2a_in,
    far_out,
    far_in,
    far_par,
    gathered,
    tok_all,
    dense_out,
    dense_in,
    dh_own,
    dh_par,
    comb,
    place,
    slots,
    r_out,
    r_in,
    acts,
    hid,
    q_out,
    q_in,
    s_out,
    s_in,
    fq_out,
    fq_in,
    fs_out,
    fs_in,
    fy_out,
    fy_in,
    kept,
    ret_out,
    ret_in,
    sq_out,
    sq_in,
    gate_ref,
    i_sem,
    w_sem,
    wp_ssem,
    wp_rsem,
    a2a_ssem,
    a2a_rsem,
    far_ssem,
    far_rsem,
    tok_ssem,
    tok_rsem,
    dh_ssem,
    dh_rsem,
    dense_ssem,
    dense_rsem,
    ag_ssem,
    ag_rsem,
    pf_ssem,
    pf_rsem,
    fp_ssem,
    fp_rsem,
    r_ssem,
    r_rsem,
    q_ssem,
    q_rsem,
    sc_ssem,
    sc_rsem,
    fq_ssem,
    fq_rsem,
    fs_ssem,
    fs_rsem,
    fy_ssem,
    fy_rsem,
    ret_ssem,
    ret_rsem,
    sq_ssem,
    sq_rsem,
):
    me_e = lax.axis_index("ep")
    me_t = lax.axis_index("tp")
    z, x = lax.div(me_e, NX), lax.rem(me_e, NX)
    y, core = lax.div(me_t, 2), lax.rem(me_t, 2)
    other = 1 - core
    partner = (me_e, y * 2 + other)
    zs = [lax.rem(z + k, NZ) * NX for k in range(NZ)]
    xs = [lax.rem(x + k, NX) for k in range(NX)]
    ys = [lax.rem(y + k, NY) for k in range(NY)]
    peers = [zs[dz] + xs[dx] for dz in (4, 3, 5, 2, 6, 1, 7, 0) for dx in (2, 1, 3, 0)][:-1]
    y_order = (4, 3, 5, 2, 6, 1, 7)

    def ydev(step):
        return (me_e, ys[step % NY] * 2 + core)

    barrier = pltpu.get_barrier_semaphore()
    for peer in peers:
        pl.semaphore_signal(barrier, inc=1, device_id=(peer, me_t), device_id_type=MESH)
    for step in y_order:
        for c in range(2):
            pl.semaphore_signal(
                barrier, inc=1, device_id=(me_e, ys[step] * 2 + c), device_id_type=MESH
            )
    pl.semaphore_signal(barrier, inc=1, device_id=partner, device_id_type=MESH)

    smalls = [
        pltpu.make_async_copy(routes_hbm, routes, i_sem.at[0]),
        pltpu.make_async_copy(logits_hbm, logits, i_sem.at[1]),
        pltpu.make_async_copy(tok_hbm, tok, i_sem.at[2]),
        pltpu.make_async_copy(gain_hbm, gain, i_sem.at[3]),
        pltpu.make_async_copy(mixw_hbm, mixw, i_sem.at[4]),
        pltpu.make_async_copy(ogain_hbm, ogain, i_sem.at[5]),
    ]

    def columns(k, c):
        return pl.ds(pl.multiple_of((2 * k + c) * PART, PART), PART)

    def load(src, dst, k):
        pltpu.make_async_copy(src, dst, w_sem.at[k]).start()

    def loaded(dst, k):
        pltpu.make_async_copy(dst, dst, w_sem.at[k]).wait()

    for copy in smalls:
        copy.start()
    load(dg, w_dense.at[pl.ds(0, 64)], 0)
    load(du, w_dense.at[pl.ds(64, 64)], 0)
    for k in range(NY):
        load(dd.at[:, columns(k, core)], dd_own.at[k], 1)
    load(wg, w_gu.at[0, pl.ds(0, 2)], 2)
    load(wu, w_gu.at[0, pl.ds(2, 2)], 2)
    for k in range(NY):
        load(wd.at[:, :, columns(k, core)], wd_own.at[k], 3)

    for copy in smalls[0:3]:
        copy.wait()
    lane = lax.broadcasted_iota(jnp.int32, (8, 256), 1)
    sub = lax.broadcasted_iota(jnp.int32, (8, 256), 0)
    expert = 2 * (lane // 8) + (lane // 2) % 2
    half = (lane // 4) % 2
    r0 = jnp.zeros((8, 256), jnp.int32)
    r1 = jnp.zeros((8, 256), jnp.int32)
    l0 = jnp.zeros((8, 256), F32)
    l1 = jnp.zeros((8, 256), F32)
    for t in range(8):
        r0 = jnp.where(sub == t, routes[0, t], r0)
        r1 = jnp.where(sub == t, routes[1, t], r1)
        l0 = jnp.where(sub == t, logits[0, t], l0)
        l1 = jnp.where(sub == t, logits[1, t], l1)
    top = jnp.maximum(l0, l1)
    e0, e1 = jnp.exp(l0 - top), jnp.exp(l1 - top)
    is0, is1 = (r0 == expert), (r1 == expert)
    hit = jnp.where(is0, 1.0, 0.0) + jnp.where(is1, 1.0, 0.0)
    before = jnp.zeros((8, 256), F32)
    for t in range(7):
        before = before + jnp.where(sub > t, hit[t : t + 1, :], 0.0)
    placed = jnp.where(before == (lane % 2).astype(F32), hit, 0.0)
    weight = (jnp.where(is0, e0, 0.0) + jnp.where(is1, e1, 0.0)) / (e0 + e1) * placed
    comb[0:8, :] = jnp.where(half == 0, weight, 0.0)
    comb[8:16, :] = jnp.where(half == 1, weight, 0.0)
    slots[...] = placed
    place[...] = jnp.concatenate(
        [jnp.where(half == 0, placed, 0.0), jnp.where(half == 1, placed, 0.0)], axis=0
    ).astype(BF16)

    def placed_rows(value):
        halves = jnp.concatenate(
            [value[:, 0:128].astype(F32), value[:, 128:256].astype(F32)], axis=0
        ).astype(BF16)
        rows = lax.dot_general(
            place[...], halves, (((0,), (0,)), ((), ())), preferred_element_type=F32
        )
        return rows.astype(BF16).reshape(NEP, 8, 128)

    tok_value = tok[...]
    a2a_out[...] = placed_rows(tok_value)
    a2a_in[me_e] = a2a_out[me_e]
    tok_all[me_t] = tok_value

    pl.semaphore_wait(barrier, NEP - 1 + NTP - 1)

    for step in y_order:
        for c in range(2):
            rcopy(
                tok, tok_all.at[me_t], tok_ssem, tok_rsem, (me_e, ys[step] * 2 + c)
            ).start()
    rcopy(tok, tok_all.at[me_t], tok_ssem, tok_rsem, partner).start()

    for peer in peers:
        rcopy(a2a_out.at[peer], a2a_in.at[me_e], a2a_ssem, a2a_rsem, (peer, me_t)).start()

    for k in range(NY):
        rcopy(
            dd.at[:, columns(k, other)], dd_par.at[k], wp_ssem.at[0], wp_rsem.at[0], partner
        ).start()
    for k, ref in enumerate((wg, wu)):
        rcopy(
            ref, w_gu.at[1, pl.ds(2 * k, 2)], wp_ssem.at[1], wp_rsem.at[1], partner
        ).start()
    for k in range(NY):
        rcopy(
            wd.at[:, :, columns(k, other)], wd_par.at[k], wp_ssem.at[2], wp_rsem.at[2], partner
        ).start()
    parts = [
        rcopy(ref, ref, wp_ssem.at[k], wp_rsem.at[k], partner)
        for k, ref in enumerate((dd_par, w_gu.at[1], wd_par))
    ]

    def arrived(src, dst, ssem, rsem, n):
        part = pl.ds(0, n)
        copy = rcopy(src.at[part], dst.at[part], ssem, rsem, partner)
        copy.wait_recv()
        return copy

    done = [arrived(tok_all, tok_all, tok_ssem, tok_rsem, NTP - 1)]
    squares = jnp.zeros((8, PART), F32)
    for j in range(NTP):
        v = tok_all[j].astype(F32)
        squares = squares + v * v
    scale = lax.rsqrt(jnp.sum(squares, axis=1, keepdims=True) / WIDTH + EPS)
    r_out[...] = jnp.sum(slots[...] * scale, axis=0, keepdims=True)
    for i, rel in enumerate(FAR):
        far_out[:, i] = placed_rows(tok_all[ys[rel] * 2 + core])
    for peer in peers:
        rcopy(r_out, r_in.at[me_e], r_ssem, r_rsem, (peer, me_t)).start()
    for peer in peers:
        rcopy(far_out.at[peer], far_in.at[me_e], far_ssem, far_rsem, (peer, me_t)).start()
    r_in[me_e] = r_out[...]
    far_in[me_e] = far_out[me_e]

    done.append(arrived(a2a_out, a2a_in, a2a_ssem, a2a_rsem, NEP - 1))
    sub3 = lax.broadcasted_iota(jnp.int32, (16, 8, 128), 1)

    def keep_rows(value, c, rel):
        pairs = value.astype(F32).reshape(16, 2, 8, 128)
        even, odd = pairs[:, 0], pairs[:, 1]
        left = jnp.where(sub3 < 4, even, pltpu.roll(odd, 4, 1)).reshape(ROWS, 128)
        right = jnp.where(sub3 < 4, pltpu.roll(even, 4, 1), odd).reshape(ROWS, 128)
        gathered[c, ys[rel], :, 0:128] = left.astype(BF16)
        gathered[c, ys[rel], :, 128:256] = right.astype(BF16)

    keep_rows(a2a_in[...], core, 0)

    def ag_copy(slot, k, device):
        ref = gathered.at[core, ys[slot]]
        return rcopy(ref, ref, ag_ssem, ag_rsem.at[k], device)

    for k, step in enumerate((2, -2, 1, -1)):
        ag_copy(0, k, ydev(step)).start()

    def pass_copy(c, rel):
        ref = gathered.at[c, ys[rel]]
        k = ((0,) + NEAR).index(rel)
        return rcopy(ref, ref, pf_ssem, pf_rsem.at[k], partner)

    def pass_on(rel):
        pass_copy(core, rel).start()

    def pass_wait(rel):
        pass_copy(other, rel).wait_recv()

    pass_on(0)

    for copy in smalls[3:6]:
        copy.wait()
    loaded(w_dense, 0)
    act = jnp.zeros((8, 128), F32)
    mix_acc = jnp.zeros((8, PART), F32)
    for j in range(NTP):
        cols = slice(j * PART, (j + 1) * PART)
        n = (tok_all[j].astype(F32) * scale * gain[:, cols]).astype(BF16)
        mix_acc = mix_acc + n.astype(F32) * mixw[:, cols]
        act = act + nt_dot(n, w_dense[:, cols])
    gate_ref[...] = jnp.broadcast_to(
        jax.nn.sigmoid(jnp.sum(mix_acc, axis=1, keepdims=True)), (8, 128)
    )
    dh_own[...] = (silu(act[:, 0:64]) * act[:, 64:128]).astype(BF16)
    dh_copy = rcopy(dh_own, dh_par, dh_ssem, dh_rsem, partner)
    dh_copy.start()

    loaded(dd_own, 1)
    parts[0].wait_recv()
    dh_copy.wait_recv()
    for k in range(NY):
        dense_out[k] = jnp.dot(
            dh_own[...], dd_own[k], preferred_element_type=F32
        ) + jnp.dot(dh_par[...], dd_par[k], preferred_element_type=F32)
    dense_in[y] = dense_out[y]
    loaded(w_gu.at[0], 2)
    parts[1].wait_recv()
    for rel in (6, 2):
        ag_copy(rel, NEAR.index(rel), partner).wait_recv()
        pass_on(rel)
    done.append(arrived(r_in, r_in, r_ssem, r_rsem, NEP - 1))
    picked = (
        lax.broadcasted_iota(jnp.int32, (ROWS, NEP), 0) // 4
        == lax.broadcasted_iota(jnp.int32, (ROWS, NEP), 1)
    )
    spread = jnp.dot(
        jnp.where(picked, 1.0, 0.0).astype(BF16),
        pieces(r_in[...].reshape(NEP, 256), 1),
        preferred_element_type=F32,
    )
    spread = spread[:, 0:256] + spread[:, 256:512] + spread[:, 512:768]
    wanted = me_e * 8 + lax.broadcasted_iota(jnp.int32, (ROWS, 256), 0) % 4
    here = lax.broadcasted_iota(jnp.int32, (ROWS, 256), 1) == wanted
    row_scale = jnp.sum(jnp.where(here, spread, 0.0), axis=1, keepdims=True)

    def project(*slices, first=False):
        total = None
        for c, rel in slices:
            cols = pl.ds(pl.multiple_of((2 * ys[rel] + c) * PART, PART), PART)
            n = (gathered[c, ys[rel]].astype(F32) * row_scale * gain[:, cols]).astype(BF16)
            v = nt_dot(n, w_gu[:, :, :, cols].reshape(512, PART))
            total = v if total is None else total + v
        acts[...] = total if first else acts[...] + total

    pass_wait(0)
    project((core, 0), (other, 0), (core, 6), (core, 2), first=True)
    for rel in (7, 1):
        ag_copy(rel, NEAR.index(rel), partner).wait_recv()
        pass_on(rel)
    for step in y_order:
        rcopy(
            dense_out.at[ys[step]], dense_in.at[y], dense_ssem, dense_rsem, ydev(step)
        ).start()
    pass_wait(6)
    pass_wait(2)
    project((core, 7), (core, 1), (other, 6), (other, 2))
    pass_wait(7)
    pass_wait(1)
    project((other, 7), (other, 1))
    done.append(arrived(far_out, far_in, far_ssem, far_rsem, NEP - 1))
    raw = rcopy(far_in, far_par, fp_ssem, fp_rsem, partner)
    raw.start()
    for i, rel in enumerate(FAR):
        keep_rows(far_in[:, i], core, rel)
    project((core, 3), (core, 4), (core, 5))
    raw.wait_recv()
    for i, rel in enumerate(FAR):
        keep_rows(far_par[:, i], other, rel)
    project((other, 3), (other, 4), (other, 5))

    row = lax.broadcasted_iota(jnp.int32, (ROWS, 128), 0)
    col = lax.broadcasted_iota(jnp.int32, (ROWS, 128), 1)
    mine = (row // 2) % 2 == col // 64
    for k in range(2):
        v = acts[:, k * 256 : (k + 1) * 256]
        hidden = silu(v[:, 0:128]) * v[:, 128:256]
        hid[:, k * 128 : (k + 1) * 128] = jnp.where(mine, hidden, 0.0).astype(BF16)
    loaded(wd_own, 3)
    parts[2].wait_recv()

    diagonal = row == col

    def partials(*rels):
        both = jnp.concatenate(
            [
                jnp.concatenate([w[ys[rel]].reshape(128, PART) for rel in rels], axis=1)
                for w in (wd_own, wd_par)
            ],
            axis=0,
        )
        v = jnp.dot(hid[...], both, preferred_element_type=F32)
        return [v[:, i * PART : (i + 1) * PART] for i in range(len(rels))]

    def column(value):
        return jnp.sum(jnp.where(diagonal, value, 0.0), axis=0, keepdims=True)

    def messages(value):
        left = value[:, 0:128].reshape(16, 8, 128)
        right = value[:, 128:256].reshape(16, 8, 128)
        even = jnp.where(sub3 < 4, left, pltpu.roll(right, 4, 1))
        odd = jnp.where(sub3 < 4, pltpu.roll(left, 4, 1), right)
        return jnp.stack([even, odd], axis=1).reshape(NEP, 8, 128)

    def q_copies(k, device):
        return (
            rcopy(q_out.at[k], q_in.at[k], q_ssem, q_rsem.at[k], device),
            rcopy(s_out.at[k], s_in.at[k], sc_ssem, sc_rsem.at[k], device),
        )

    def q_send(k, value):
        most = jnp.maximum(jnp.max(jnp.abs(value), axis=1, keepdims=True), 1e-30)
        q_out[k] = jnp.round(value * (32767.0 / most)).astype(jnp.int16)
        s_out[k] = column(most * (1.0 / 32767.0))
        for copy in q_copies(k, ydev(NEAR[k])):
            copy.start()

    def q_get(k):
        for copy in q_copies(k, partner):
            copy.wait_recv()
        unit = jnp.sum(jnp.where(diagonal, s_in[k], 0.0), axis=1, keepdims=True)
        return q_in[k].astype(F32) * unit

    values = partials(*FAR, 0)
    kept[...] = values[3]
    most = jnp.maximum(jnp.maximum(jnp.abs(values[0]), jnp.abs(values[1])), jnp.abs(values[2]))
    most = jnp.maximum(jnp.max(most, axis=1, keepdims=True), 1e-30)
    fs_out[...] = column(most * (1.0 / 32767.0))
    for i in range(3):
        fq_out[:, i] = messages(jnp.round(values[i] * (32767.0 / most))).astype(jnp.int16)
    for peer in peers:
        rcopy(fs_out, fs_in.at[me_e], fs_ssem, fs_rsem, (peer, me_t)).start()
    for peer in peers:
        rcopy(fq_out.at[peer], fq_in.at[me_e], fq_ssem, fq_rsem, (peer, me_t)).start()
    for k, value in enumerate(partials(*NEAR)):
        q_send(k, value)
    fq_in[me_e] = fq_out[me_e]
    fs_in[me_e] = fs_out[...]
    done.append(arrived(dense_out, dense_in, dense_ssem, dense_rsem, NY - 1))
    dense = dense_in[0]
    for k in range(1, NY):
        dense = dense + dense_in[k]
    gate = gate_ref[...]
    dense = jnp.concatenate([gate, gate], axis=1) * dense
    summed = kept[...]
    for k in range(4):
        summed = summed + q_get(k)
    ret_out[...] = messages(summed)
    for peer in peers:
        rcopy(ret_out.at[peer], ret_in.at[me_e], ret_ssem, ret_rsem, (peer, me_t)).start()
    ret_in[me_e] = ret_out[me_e]
    done.append(arrived(fs_in, fs_in, fs_ssem, fs_rsem, NEP - 1))
    lane2 = lax.broadcasted_iota(jnp.int32, (128, 256), 1)
    mine4 = lax.broadcasted_iota(jnp.int32, (128, 256), 0) == me_e * 4 + lane2 % 4
    unit = jnp.dot(
        pieces(fs_in[...].reshape(NEP, 128), 0),
        jnp.where(mine4, 1.0, 0.0).astype(BF16),
        preferred_element_type=F32,
    )
    unit = unit[0:NEP] + unit[NEP : 2 * NEP] + unit[2 * NEP : 3 * NEP]
    source = lax.broadcasted_iota(jnp.int32, (NEP, 256), 0)
    source = source == lax.broadcasted_iota(jnp.int32, (NEP, 256), 1) // 8
    unit = jnp.sum(jnp.where(source, unit, 0.0), axis=0, keepdims=True)
    far_comb = pieces(comb[...] * unit, 0)
    near_comb = pieces(comb[...], 0)
    done.append(arrived(fq_out, fq_in, fq_ssem, fq_rsem, NEP - 1))
    far_rows = jnp.concatenate(
        [fq_in[:, i].astype(F32).reshape(256, 128) for i in range(3)], axis=1
    )
    far_high = far_rows.astype(BF16)
    far_low = (far_rows - far_high.astype(F32)).astype(BF16)
    far_sum = jnp.dot(far_comb, far_high, preferred_element_type=F32) + jnp.dot(
        far_comb, far_low, preferred_element_type=F32
    )
    far_sum = far_sum[0:16] + far_sum[16:32] + far_sum[32:48]
    for i, rel in enumerate(FAR):
        cols = slice(i * 128, (i + 1) * 128)
        fy_out[i, :, 0:128] = far_sum[0:8, cols]
        fy_out[i, :, 128:256] = far_sum[8:16, cols]
        rcopy(fy_out.at[i], fy_in.at[i], fy_ssem, fy_rsem, ydev(rel)).start()
    done.append(arrived(ret_out, ret_in, ret_ssem, ret_rsem, NEP - 1))
    mixed = jnp.dot(
        near_comb, pieces(ret_in[...].reshape(256, 128), 1), preferred_element_type=F32
    )
    mixed = mixed[:, 0:128] + mixed[:, 128:256] + mixed[:, 256:384]
    mixed = mixed[0:16] + mixed[16:32] + mixed[32:48]
    combined = jnp.concatenate([mixed[0:8], mixed[8:16]], axis=1) + dense
    fy_copy = rcopy(fy_out, fy_in, fy_ssem, fy_rsem, partner)
    fy_copy.wait_recv()
    combined = combined + fy_in[0] + fy_in[1] + fy_in[2]
    token_diagonal = (
        lax.broadcasted_iota(jnp.int32, (8, 128), 0)
        == lax.broadcasted_iota(jnp.int32, (8, 128), 1)
    )
    own = jnp.sum(
        jnp.where(token_diagonal, jnp.sum(combined * combined, axis=1, keepdims=True), 0.0),
        axis=0,
        keepdims=True,
    )
    sq_out[...] = own
    for step in y_order:
        for c in range(2):
            rcopy(sq_out, sq_in.at[me_t], sq_ssem, sq_rsem, (me_e, ys[step] * 2 + c)).start()
    rcopy(sq_out, sq_in.at[me_t], sq_ssem, sq_rsem, partner).start()
    sq_in[me_t] = own
    done.append(arrived(sq_in, sq_in, sq_ssem, sq_rsem, NTP - 1))
    total_sq = sq_in[0]
    for j in range(1, NTP):
        total_sq = total_sq + sq_in[j]
    final = lax.rsqrt(
        jnp.sum(jnp.where(token_diagonal, total_sq, 0.0), axis=1, keepdims=True) / WIDTH + EPS
    )
    out[...] = (combined * final * ogain[...]).astype(BF16)

    near = gathered.at[core, pl.ds(0, 4)]
    done += [
        rcopy(near, near, ag_ssem, ag_rsem.at[0], partner),
        rcopy(q_out, q_in, q_ssem, q_rsem.at[0], partner),
        rcopy(s_out, s_in, sc_ssem, sc_rsem.at[0], partner),
    ]
    five = gathered.at[core, pl.ds(0, 5)]
    done.append(rcopy(five, five, pf_ssem, pf_rsem.at[0], partner))
    for copy in parts + [dh_copy, raw, fy_copy] + done:
        copy.wait_send()


def local(
    tokens,
    norm_gain,
    route_experts,
    route_logits,
    expert_gate,
    expert_up,
    expert_down,
    dense_gate,
    dense_up,
    dense_down,
    mix_weight,
    out_gain,
):
    vmem = pl.BlockSpec(memory_space=pltpu.VMEM)
    dma = pltpu.SemaphoreType.DMA
    return pl.pallas_call(
        kernel,
        out_shape=pltpu.VMEM((8, PART), BF16),
        in_specs=[pl.BlockSpec(memory_space=pl.ANY)] * 12,
        out_specs=vmem,
        scratch_shapes=[
            pltpu.VMEM((8, PART), BF16),
            pltpu.VMEM((1, WIDTH), F32),
            pltpu.SMEM((2, 8), jnp.int32),
            pltpu.SMEM((2, 8), F32),
            pltpu.VMEM((1, WIDTH), F32),
            pltpu.VMEM((1, PART), F32),
            pltpu.VMEM((2, 4, 64, WIDTH), BF16),
            pltpu.VMEM((NY, 2, 64, PART), BF16),
            pltpu.VMEM((NY, 2, 64, PART), BF16),
            pltpu.VMEM((128, WIDTH), BF16),
            pltpu.VMEM((NY, 64, PART), BF16),
            pltpu.VMEM((NY, 64, PART), BF16),
            pltpu.VMEM((NEP, 8, 128), BF16),
            pltpu.VMEM((NEP, 8, 128), BF16),
            pltpu.VMEM((NEP, 3, 8, 128), BF16),
            pltpu.VMEM((NEP, 3, 8, 128), BF16),
            pltpu.VMEM((NEP, 3, 8, 128), BF16),
            pltpu.VMEM((2, NY, ROWS, PART), BF16),
            pltpu.VMEM((NTP, 8, PART), BF16),
            pltpu.VMEM((NY, 8, PART), F32),
            pltpu.VMEM((NY, 8, PART), F32),
            pltpu.VMEM((8, 64), BF16),
            pltpu.VMEM((8, 64), BF16),
            pltpu.VMEM((16, 256), F32),
            pltpu.VMEM((16, 256), BF16),
            pltpu.VMEM((8, 256), F32),
            pltpu.VMEM((1, 256), F32),
            pltpu.VMEM((NEP, 1, 256), F32),
            pltpu.VMEM((ROWS, 512), F32),
            pltpu.VMEM((ROWS, 256), BF16),
            pltpu.VMEM((4, ROWS, PART), jnp.int16),
            pltpu.VMEM((4, ROWS, PART), jnp.int16),
            pltpu.VMEM((4, 1, 128), F32),
            pltpu.VMEM((4, 1, 128), F32),
            pltpu.VMEM((NEP, 3, 8, 128), jnp.int16),
            pltpu.VMEM((NEP, 3, 8, 128), jnp.int16),
            pltpu.VMEM((1, 128), F32),
            pltpu.VMEM((NEP, 1, 128), F32),
            pltpu.VMEM((3, 8, PART), F32),
            pltpu.VMEM((3, 8, PART), F32),
            pltpu.VMEM((ROWS, PART), F32),
            pltpu.VMEM((NEP, 8, 128), F32),
            pltpu.VMEM((NEP, 8, 128), F32),
            pltpu.VMEM((1, 128), F32),
            pltpu.VMEM((NTP, 1, 128), F32),
            pltpu.VMEM((8, 128), F32),
            dma((6,)),
            dma((4,)),
            dma((3,)),
            dma((3,)),
            dma,
            dma,
            dma,
            dma,
            dma,
            dma,
            dma,
            dma,
            dma,
            dma,
            dma,
            dma((4,)),
            dma,
            dma((5,)),
            dma,
            dma,
            dma,
            dma,
            dma,
            dma((4,)),
            dma,
            dma((4,)),
            dma,
            dma,
            dma,
            dma,
            dma,
            dma,
            dma,
            dma,
            dma,
            dma,
        ],
        compiler_params=pltpu.CompilerParams(
            collective_id=0, has_side_effects=True, vmem_limit_bytes=56650000
        ),
    )(
        tokens,
        norm_gain.reshape(1, WIDTH),
        route_experts.T,
        route_logits.T,
        jnp.swapaxes(expert_gate, 1, 2),
        jnp.swapaxes(expert_up, 1, 2),
        expert_down,
        dense_gate.T,
        dense_up.T,
        dense_down,
        mix_weight.reshape(1, WIDTH),
        out_gain.reshape(1, PART),
    )


def solution(mesh):
    tp = "tp"
    in_specs = (
        P("ep", tp),
        P(),
        P("ep", None),
        P("ep", None),
        P("ep", None, tp),
        P("ep", None, tp),
        P("ep", tp, None),
        P(None, tp),
        P(None, tp),
        P(tp, None),
        P(),
        P(tp),
    )
    return jax.shard_map(
        local, mesh=mesh, in_specs=in_specs, out_specs=P("ep", tp), check_vma=False
    )
```

```python
import functools

import jax
import jax.numpy as jnp
from jax import lax
from jax.experimental import pallas as pl
from jax.experimental.pallas import tpu as pltpu
from jax.sharding import PartitionSpec as P

MESH = pl.DeviceIdType.MESH
F32 = jnp.float32
BF16 = jnp.bfloat16
EPS = 1e-06

NX, NZ, NY = 4, 8, 8
NEP = NX * NZ
NTP = 2 * NY
ROWS = 128
FAR = (3, 4, 5)
NEAR = (6, 2, 7, 1)
PART = 256
WIDTH = 4096


def rcopy(src, dst, send_sem, recv_sem, device):
    return pltpu.make_async_remote_copy(
        src_ref=src,
        dst_ref=dst,
        send_sem=send_sem,
        recv_sem=recv_sem,
        device_id=device,
        device_id_type=MESH,
    )


def nt_dot(a, b):
    return lax.dot_general(a, b, (((1,), (1,)), ((), ())), preferred_element_type=F32)


def pieces(value, axis):
    high = value.astype(BF16)
    rest = value - high.astype(F32)
    middle = rest.astype(BF16)
    low = (rest - middle.astype(F32)).astype(BF16)
    return jnp.concatenate([high, middle, low], axis=axis)


def silu(v):
    return v / (1.0 + jnp.exp(-v))


def kernel(
    tok_hbm,
    gain_hbm,
    routes_hbm,
    logits_hbm,
    wg,
    wu,
    wd,
    dg,
    du,
    dd,
    mixw_hbm,
    ogain_hbm,
    out,
    tok,
    gain,
    routes,
    logits,
    mixw,
    ogain,
    w_gu,
    wd_own,
    wd_par,
    w_dense,
    dd_own,
    dd_par,
    a2a_out,
    a2a_in,
    far_out,
    far_in,
    far_par,
    gathered,
    tok_all,
    dense_out,
    dense_in,
    dh_own,
    dh_par,
    comb,
    place,
    slots,
    r_out,
    r_in,
    acts,
    hid,
    q_out,
    q_in,
    s_out,
    s_in,
    fq_out,
    fq_in,
    fs_out,
    fs_in,
    fy_out,
    fy_in,
    kept,
    ret_out,
    ret_in,
    sq_out,
    sq_in,
    gate_ref,
    i_sem,
    w_sem,
    wp_ssem,
    wp_rsem,
    a2a_ssem,
    a2a_rsem,
    far_ssem,
    far_rsem,
    tok_ssem,
    tok_rsem,
    dh_ssem,
    dh_rsem,
    dense_ssem,
    dense_rsem,
    ag_ssem,
    ag_rsem,
    pf_ssem,
    pf_rsem,
    fp_ssem,
    fp_rsem,
    r_ssem,
    r_rsem,
    q_ssem,
    q_rsem,
    sc_ssem,
    sc_rsem,
    fq_ssem,
    fq_rsem,
    fs_ssem,
    fs_rsem,
    fy_ssem,
    fy_rsem,
    ret_ssem,
    ret_rsem,
    sq_ssem,
    sq_rsem,
):
    me_e = lax.axis_index("ep")
    me_t = lax.axis_index("tp")
    z, x = lax.div(me_e, NX), lax.rem(me_e, NX)
    y, core = lax.div(me_t, 2), lax.rem(me_t, 2)
    other = 1 - core
    partner = (me_e, y * 2 + other)
    zs = [lax.rem(z + k, NZ) * NX for k in range(NZ)]
    xs = [lax.rem(x + k, NX) for k in range(NX)]
    ys = [lax.rem(y + k, NY) for k in range(NY)]
    peers = [zs[dz] + xs[dx] for dz in (4, 3, 5, 2, 6, 1, 7, 0) for dx in (2, 1, 3, 0)][:-1]
    y_order = (4, 3, 5, 2, 6, 1, 7)

    def ydev(step):
        return (me_e, ys[step % NY] * 2 + core)

    barrier = pltpu.get_barrier_semaphore()
    for peer in peers:
        pl.semaphore_signal(barrier, inc=1, device_id=(peer, me_t), device_id_type=MESH)
    for step in y_order:
        for c in range(2):
            pl.semaphore_signal(
                barrier, inc=1, device_id=(me_e, ys[step] * 2 + c), device_id_type=MESH
            )
    pl.semaphore_signal(barrier, inc=1, device_id=partner, device_id_type=MESH)

    smalls = [
        pltpu.make_async_copy(routes_hbm, routes, i_sem.at[0]),
        pltpu.make_async_copy(logits_hbm, logits, i_sem.at[1]),
        pltpu.make_async_copy(tok_hbm, tok, i_sem.at[2]),
        pltpu.make_async_copy(gain_hbm, gain, i_sem.at[3]),
        pltpu.make_async_copy(mixw_hbm, mixw, i_sem.at[4]),
        pltpu.make_async_copy(ogain_hbm, ogain, i_sem.at[5]),
    ]

    def columns(k, c):
        return pl.ds(pl.multiple_of((2 * k + c) * PART, PART), PART)

    def load(src, dst, k):
        pltpu.make_async_copy(src, dst, w_sem.at[k]).start()

    def loaded(dst, k):
        pltpu.make_async_copy(dst, dst, w_sem.at[k]).wait()

    for copy in smalls:
        copy.start()
    load(dg, w_dense.at[pl.ds(0, 64)], 0)
    load(du, w_dense.at[pl.ds(64, 64)], 0)
    for k in range(NY):
        load(dd.at[:, columns(k, core)], dd_own.at[k], 1)
    load(wg, w_gu.at[0, pl.ds(0, 2)], 2)
    load(wu, w_gu.at[0, pl.ds(2, 2)], 2)
    for k in range(NY):
        load(wd.at[:, :, columns(k, core)], wd_own.at[k], 3)

    for copy in smalls[0:3]:
        copy.wait()
    lane = lax.broadcasted_iota(jnp.int32, (8, 256), 1)
    sub = lax.broadcasted_iota(jnp.int32, (8, 256), 0)
    expert = 2 * (lane // 8) + (lane // 2) % 2
    half = (lane // 4) % 2
    r0 = jnp.zeros((8, 256), jnp.int32)
    r1 = jnp.zeros((8, 256), jnp.int32)
    l0 = jnp.zeros((8, 256), F32)
    l1 = jnp.zeros((8, 256), F32)
    for t in range(8):
        r0 = jnp.where(sub == t, routes[0, t], r0)
        r1 = jnp.where(sub == t, routes[1, t], r1)
        l0 = jnp.where(sub == t, logits[0, t], l0)
        l1 = jnp.where(sub == t, logits[1, t], l1)
    top = jnp.maximum(l0, l1)
    e0, e1 = jnp.exp(l0 - top), jnp.exp(l1 - top)
    is0, is1 = (r0 == expert), (r1 == expert)
    hit = jnp.where(is0, 1.0, 0.0) + jnp.where(is1, 1.0, 0.0)
    before = jnp.zeros((8, 256), F32)
    for t in range(7):
        before = before + jnp.where(sub > t, hit[t : t + 1, :], 0.0)
    placed = jnp.where(before == (lane % 2).astype(F32), hit, 0.0)
    weight = (jnp.where(is0, e0, 0.0) + jnp.where(is1, e1, 0.0)) / (e0 + e1) * placed
    comb[0:8, :] = jnp.where(half == 0, weight, 0.0)
    comb[8:16, :] = jnp.where(half == 1, weight, 0.0)
    left_half = lax.broadcasted_iota(jnp.int32, (256, 128), 0)
    slot = lax.broadcasted_iota(jnp.int32, (256, 128), 1)
    left_half = (left_half // 8 == slot // 4) & (left_half % 8 == slot % 4)
    slots[...] = jnp.dot(
        placed.astype(BF16),
        jnp.where(left_half, 1.0, 0.0).astype(BF16),
        preferred_element_type=F32,
    )
    place[...] = jnp.concatenate(
        [jnp.where(half == 0, placed, 0.0), jnp.where(half == 1, placed, 0.0)], axis=0
    ).astype(BF16)

    def placed_rows(value):
        halves = jnp.concatenate(
            [value[:, 0:128].astype(F32), value[:, 128:256].astype(F32)], axis=0
        ).astype(BF16)
        rows = lax.dot_general(
            place[...], halves, (((0,), (0,)), ((), ())), preferred_element_type=F32
        )
        return rows.astype(BF16).reshape(NEP, 8, 128)

    tok_value = tok[...]
    a2a_out[...] = placed_rows(tok_value)
    a2a_in[me_e] = a2a_out[me_e]
    tok_all[me_t] = tok_value

    pl.semaphore_wait(barrier, NEP - 1 + NTP - 1)

    for step in y_order:
        for c in range(2):
            rcopy(
                tok, tok_all.at[me_t], tok_ssem, tok_rsem, (me_e, ys[step] * 2 + c)
            ).start()
    rcopy(tok, tok_all.at[me_t], tok_ssem, tok_rsem, partner).start()

    for peer in peers:
        rcopy(a2a_out.at[peer], a2a_in.at[me_e], a2a_ssem, a2a_rsem, (peer, me_t)).start()

    for k in range(NY):
        rcopy(
            dd.at[:, columns(k, other)], dd_par.at[k], wp_ssem.at[0], wp_rsem.at[0], partner
        ).start()
    for k, ref in enumerate((wg, wu)):
        rcopy(
            ref, w_gu.at[1, pl.ds(2 * k, 2)], wp_ssem.at[1], wp_rsem.at[1], partner
        ).start()
    for k in range(NY):
        rcopy(
            wd.at[:, :, columns(k, other)], wd_par.at[k], wp_ssem.at[2], wp_rsem.at[2], partner
        ).start()
    parts = [
        rcopy(ref, ref, wp_ssem.at[k], wp_rsem.at[k], partner)
        for k, ref in enumerate((dd_par, w_gu.at[1], wd_par))
    ]

    def arrived(src, dst, ssem, rsem, n):
        part = pl.ds(0, n)
        copy = rcopy(src.at[part], dst.at[part], ssem, rsem, partner)
        copy.wait_recv()
        return copy

    done = [arrived(tok_all, tok_all, tok_ssem, tok_rsem, NTP - 1)]
    squares = jnp.zeros((8, PART), F32)
    for j in range(NTP):
        v = tok_all[j].astype(F32)
        squares = squares + v * v
    scale = lax.rsqrt(jnp.sum(squares, axis=1, keepdims=True) / WIDTH + EPS)
    r_out[...] = jnp.sum(slots[...] * scale, axis=0, keepdims=True)
    for i, rel in enumerate(FAR):
        far_out[:, i] = placed_rows(tok_all[ys[rel] * 2 + core])
    for peer in peers:
        rcopy(r_out, r_in.at[me_e], r_ssem, r_rsem, (peer, me_t)).start()
    for peer in peers:
        rcopy(far_out.at[peer], far_in.at[me_e], far_ssem, far_rsem, (peer, me_t)).start()
    r_in[me_e] = r_out[...]
    far_in[me_e] = far_out[me_e]

    done.append(arrived(a2a_out, a2a_in, a2a_ssem, a2a_rsem, NEP - 1))
    sub3 = lax.broadcasted_iota(jnp.int32, (16, 8, 128), 1)

    def keep_rows(value, c, rel):
        pairs = value.astype(F32).reshape(16, 2, 8, 128)
        even, odd = pairs[:, 0], pairs[:, 1]
        left = jnp.where(sub3 < 4, even, pltpu.roll(odd, 4, 1)).reshape(ROWS, 128)
        right = jnp.where(sub3 < 4, pltpu.roll(even, 4, 1), odd).reshape(ROWS, 128)
        gathered[c, ys[rel], :, 0:128] = left.astype(BF16)
        gathered[c, ys[rel], :, 128:256] = right.astype(BF16)

    keep_rows(a2a_in[...], core, 0)

    def ag_copy(slot, k, device):
        ref = gathered.at[core, ys[slot]]
        return rcopy(ref, ref, ag_ssem, ag_rsem.at[k], device)

    for k, step in enumerate((2, -2, 1, -1)):
        ag_copy(0, k, ydev(step)).start()

    def pass_copy(c, rel):
        ref = gathered.at[c, ys[rel]]
        k = ((0,) + NEAR).index(rel)
        return rcopy(ref, ref, pf_ssem, pf_rsem.at[k], partner)

    def pass_on(rel):
        pass_copy(core, rel).start()

    def pass_wait(rel):
        pass_copy(other, rel).wait_recv()

    pass_on(0)

    for copy in smalls[3:6]:
        copy.wait()
    loaded(w_dense, 0)
    act = jnp.zeros((8, 128), F32)
    mix_acc = jnp.zeros((8, PART), F32)
    for j in range(NTP):
        cols = slice(j * PART, (j + 1) * PART)
        n = (tok_all[j].astype(F32) * scale * gain[:, cols]).astype(BF16)
        mix_acc = mix_acc + n.astype(F32) * mixw[:, cols]
        act = act + nt_dot(n, w_dense[:, cols])
    gate_ref[...] = jnp.broadcast_to(
        jax.nn.sigmoid(jnp.sum(mix_acc, axis=1, keepdims=True)), (8, 128)
    )
    dh_own[...] = (silu(act[:, 0:64]) * act[:, 64:128]).astype(BF16)
    dh_copy = rcopy(dh_own, dh_par, dh_ssem, dh_rsem, partner)
    dh_copy.start()

    loaded(dd_own, 1)
    parts[0].wait_recv()
    dh_copy.wait_recv()
    for k in range(NY):
        dense_out[k] = jnp.dot(
            dh_own[...], dd_own[k], preferred_element_type=F32
        ) + jnp.dot(dh_par[...], dd_par[k], preferred_element_type=F32)
    dense_in[y] = dense_out[y]
    loaded(w_gu.at[0], 2)
    parts[1].wait_recv()
    for rel in (6, 2):
        ag_copy(rel, NEAR.index(rel), partner).wait_recv()
        pass_on(rel)
    done.append(arrived(r_in, r_in, r_ssem, r_rsem, NEP - 1))
    picked = (
        lax.broadcasted_iota(jnp.int32, (ROWS, NEP), 0) // 4
        == lax.broadcasted_iota(jnp.int32, (ROWS, NEP), 1)
    )
    spread = jnp.dot(
        jnp.where(picked, 1.0, 0.0).astype(BF16),
        pieces(r_in[...].reshape(NEP, 128), 1),
        preferred_element_type=F32,
    )
    spread = spread[:, 0:128] + spread[:, 128:256] + spread[:, 256:384]
    wanted = me_e * 4 + lax.broadcasted_iota(jnp.int32, (ROWS, 128), 0) % 4
    here = lax.broadcasted_iota(jnp.int32, (ROWS, 128), 1) == wanted
    row_scale = jnp.sum(jnp.where(here, spread, 0.0), axis=1, keepdims=True)

    def project(*slices, first=False):
        total = None
        for c, rel in slices:
            cols = pl.ds(pl.multiple_of((2 * ys[rel] + c) * PART, PART), PART)
            n = (gathered[c, ys[rel]].astype(F32) * row_scale * gain[:, cols]).astype(BF16)
            v = nt_dot(n, w_gu[:, :, :, cols].reshape(512, PART))
            total = v if total is None else total + v
        acts[...] = total if first else acts[...] + total

    pass_wait(0)
    project((core, 0), (other, 0), (core, 6), (core, 2), first=True)
    for rel in (7, 1):
        ag_copy(rel, NEAR.index(rel), partner).wait_recv()
        pass_on(rel)
    for step in y_order:
        rcopy(
            dense_out.at[ys[step]], dense_in.at[y], dense_ssem, dense_rsem, ydev(step)
        ).start()
    pass_wait(6)
    pass_wait(2)
    project((core, 7), (core, 1), (other, 6), (other, 2))
    done.append(arrived(far_out, far_in, far_ssem, far_rsem, NEP - 1))
    raws = [
        rcopy(far_in.at[:, i], far_par.at[:, i], fp_ssem, fp_rsem.at[i], partner)
        for i in range(3)
    ]
    for copy in raws:
        copy.start()
    for i, rel in enumerate(FAR):
        keep_rows(far_in[:, i], core, rel)
    project((core, 3), (core, 4), (core, 5))
    pass_wait(7)
    pass_wait(1)
    project((other, 7), (other, 1))
    for i in range(2):
        raws[i].wait_recv()
        keep_rows(far_par[:, i], other, FAR[i])
    project((other, 3), (other, 4))
    raws[2].wait_recv()
    keep_rows(far_par[:, 2], other, FAR[2])
    project((other, 5))

    row = lax.broadcasted_iota(jnp.int32, (ROWS, 128), 0)
    col = lax.broadcasted_iota(jnp.int32, (ROWS, 128), 1)
    mine = (row // 2) % 2 == col // 64
    for k in range(2):
        v = acts[:, k * 256 : (k + 1) * 256]
        hidden = silu(v[:, 0:128]) * v[:, 128:256]
        hid[:, k * 128 : (k + 1) * 128] = jnp.where(mine, hidden, 0.0).astype(BF16)
    loaded(wd_own, 3)
    parts[2].wait_recv()

    diagonal = row == col

    def partials(*rels):
        both = jnp.concatenate(
            [
                jnp.concatenate([w[ys[rel]].reshape(128, PART) for rel in rels], axis=1)
                for w in (wd_own, wd_par)
            ],
            axis=0,
        )
        v = jnp.dot(hid[...], both, preferred_element_type=F32)
        return [v[:, i * PART : (i + 1) * PART] for i in range(len(rels))]

    def column(value):
        return jnp.sum(jnp.where(diagonal, value, 0.0), axis=0, keepdims=True)

    def messages(value):
        left = value[:, 0:128].reshape(16, 8, 128)
        right = value[:, 128:256].reshape(16, 8, 128)
        even = jnp.where(sub3 < 4, left, pltpu.roll(right, 4, 1))
        odd = jnp.where(sub3 < 4, pltpu.roll(left, 4, 1), right)
        return jnp.stack([even, odd], axis=1).reshape(NEP, 8, 128)

    def q_copies(k, device):
        return (
            rcopy(q_out.at[k], q_in.at[k], q_ssem, q_rsem.at[k], device),
            rcopy(s_out.at[k], s_in.at[k], sc_ssem, sc_rsem.at[k], device),
        )

    def q_send(k, value):
        most = jnp.maximum(jnp.max(jnp.abs(value), axis=1, keepdims=True), 1e-30)
        q_out[k] = jnp.round(value * (32767.0 / most)).astype(jnp.int16)
        s_out[k] = column(most * (1.0 / 32767.0))
        for copy in q_copies(k, ydev(NEAR[k])):
            copy.start()

    def q_get(k):
        for copy in q_copies(k, partner):
            copy.wait_recv()
        unit = jnp.sum(jnp.where(diagonal, s_in[k], 0.0), axis=1, keepdims=True)
        return q_in[k].astype(F32) * unit

    for k, value in enumerate(partials(NEAR[0], NEAR[1])):
        q_send(k, value)

    values = partials(*FAR, 0)
    kept[...] = values[3]
    most = jnp.maximum(jnp.maximum(jnp.abs(values[0]), jnp.abs(values[1])), jnp.abs(values[2]))
    most = jnp.maximum(jnp.max(most, axis=1, keepdims=True), 1e-30)
    fs_out[...] = column(most * (1.0 / 32767.0))
    for i in range(3):
        fq_out[:, i] = messages(jnp.round(values[i] * (32767.0 / most))).astype(jnp.int16)
    for peer in peers:
        rcopy(fs_out, fs_in.at[me_e], fs_ssem, fs_rsem, (peer, me_t)).start()
    for peer in peers:
        rcopy(fq_out.at[peer], fq_in.at[me_e], fq_ssem, fq_rsem, (peer, me_t)).start()
    for k, value in enumerate(partials(NEAR[2], NEAR[3])):
        q_send(2 + k, value)
    fq_in[me_e] = fq_out[me_e]
    fs_in[me_e] = fs_out[...]
    done.append(arrived(dense_out, dense_in, dense_ssem, dense_rsem, NY - 1))
    dense = dense_in[0]
    for k in range(1, NY):
        dense = dense + dense_in[k]
    gate = gate_ref[...]
    dense = jnp.concatenate([gate, gate], axis=1) * dense
    summed = kept[...]
    for k in range(4):
        summed = summed + q_get(k)
    ret_out[...] = messages(summed)
    for peer in peers:
        rcopy(ret_out.at[peer], ret_in.at[me_e], ret_ssem, ret_rsem, (peer, me_t)).start()
    ret_in[me_e] = ret_out[me_e]
    done.append(arrived(fs_in, fs_in, fs_ssem, fs_rsem, NEP - 1))
    lane2 = lax.broadcasted_iota(jnp.int32, (128, 256), 1)
    mine4 = lax.broadcasted_iota(jnp.int32, (128, 256), 0) == me_e * 4 + lane2 % 4
    unit = jnp.dot(
        pieces(fs_in[...].reshape(NEP, 128), 0),
        jnp.where(mine4, 1.0, 0.0).astype(BF16),
        preferred_element_type=F32,
    )
    unit = unit[0:NEP] + unit[NEP : 2 * NEP] + unit[2 * NEP : 3 * NEP]
    source = lax.broadcasted_iota(jnp.int32, (NEP, 256), 0)
    source = source == lax.broadcasted_iota(jnp.int32, (NEP, 256), 1) // 8
    unit = jnp.sum(jnp.where(source, unit, 0.0), axis=0, keepdims=True)
    far_comb = pieces(comb[...] * unit, 0)
    near_comb = pieces(comb[...], 0)
    done.append(arrived(fq_out, fq_in, fq_ssem, fq_rsem, NEP - 1))
    far_rows = jnp.concatenate(
        [fq_in[:, i].astype(F32).reshape(256, 128) for i in range(3)], axis=1
    )
    far_high = far_rows.astype(BF16)
    far_low = (far_rows - far_high.astype(F32)).astype(BF16)
    far_sum = jnp.dot(far_comb, far_high, preferred_element_type=F32) + jnp.dot(
        far_comb, far_low, preferred_element_type=F32
    )
    far_sum = far_sum[0:16] + far_sum[16:32] + far_sum[32:48]
    for i, rel in enumerate(FAR):
        cols = slice(i * 128, (i + 1) * 128)
        fy_out[i, :, 0:128] = far_sum[0:8, cols]
        fy_out[i, :, 128:256] = far_sum[8:16, cols]
        rcopy(fy_out.at[i], fy_in.at[i], fy_ssem, fy_rsem, ydev(rel)).start()
    done.append(arrived(ret_out, ret_in, ret_ssem, ret_rsem, NEP - 1))
    mixed = jnp.dot(
        near_comb, pieces(ret_in[...].reshape(256, 128), 1), preferred_element_type=F32
    )
    mixed = mixed[:, 0:128] + mixed[:, 128:256] + mixed[:, 256:384]
    mixed = mixed[0:16] + mixed[16:32] + mixed[32:48]
    combined = jnp.concatenate([mixed[0:8], mixed[8:16]], axis=1) + dense
    fy_copy = rcopy(fy_out, fy_in, fy_ssem, fy_rsem, partner)
    fy_copy.wait_recv()
    combined = combined + fy_in[0] + fy_in[1] + fy_in[2]
    token_diagonal = (
        lax.broadcasted_iota(jnp.int32, (8, 128), 0)
        == lax.broadcasted_iota(jnp.int32, (8, 128), 1)
    )
    own = jnp.sum(
        jnp.where(token_diagonal, jnp.sum(combined * combined, axis=1, keepdims=True), 0.0),
        axis=0,
        keepdims=True,
    )
    sq_out[...] = own
    for step in y_order:
        for c in range(2):
            rcopy(sq_out, sq_in.at[me_t], sq_ssem, sq_rsem, (me_e, ys[step] * 2 + c)).start()
    rcopy(sq_out, sq_in.at[me_t], sq_ssem, sq_rsem, partner).start()
    sq_in[me_t] = own
    done.append(arrived(sq_in, sq_in, sq_ssem, sq_rsem, NTP - 1))
    total_sq = sq_in[0]
    for j in range(1, NTP):
        total_sq = total_sq + sq_in[j]
    final = lax.rsqrt(
        jnp.sum(jnp.where(token_diagonal, total_sq, 0.0), axis=1, keepdims=True) / WIDTH + EPS
    )
    out[...] = (combined * final * ogain[...]).astype(BF16)

    near = gathered.at[core, pl.ds(0, 4)]
    done += [
        rcopy(near, near, ag_ssem, ag_rsem.at[0], partner),
        rcopy(q_out, q_in, q_ssem, q_rsem.at[0], partner),
        rcopy(s_out, s_in, sc_ssem, sc_rsem.at[0], partner),
    ]
    five = gathered.at[core, pl.ds(0, 5)]
    done.append(rcopy(five, five, pf_ssem, pf_rsem.at[0], partner))
    for copy in parts + [dh_copy, fy_copy] + raws + done:
        copy.wait_send()


def local(
    tokens,
    norm_gain,
    route_experts,
    route_logits,
    expert_gate,
    expert_up,
    expert_down,
    dense_gate,
    dense_up,
    dense_down,
    mix_weight,
    out_gain,
):
    vmem = pl.BlockSpec(memory_space=pltpu.VMEM)
    dma = pltpu.SemaphoreType.DMA
    return pl.pallas_call(
        kernel,
        out_shape=pltpu.VMEM((8, PART), BF16),
        in_specs=[pl.BlockSpec(memory_space=pl.ANY)] * 12,
        out_specs=vmem,
        scratch_shapes=[
            pltpu.VMEM((8, PART), BF16),
            pltpu.VMEM((1, WIDTH), F32),
            pltpu.SMEM((2, 8), jnp.int32),
            pltpu.SMEM((2, 8), F32),
            pltpu.VMEM((1, WIDTH), F32),
            pltpu.VMEM((1, PART), F32),
            pltpu.VMEM((2, 4, 64, WIDTH), BF16),
            pltpu.VMEM((NY, 2, 64, PART), BF16),
            pltpu.VMEM((NY, 2, 64, PART), BF16),
            pltpu.VMEM((128, WIDTH), BF16),
            pltpu.VMEM((NY, 64, PART), BF16),
            pltpu.VMEM((NY, 64, PART), BF16),
            pltpu.VMEM((NEP, 8, 128), BF16),
            pltpu.VMEM((NEP, 8, 128), BF16),
            pltpu.VMEM((NEP, 3, 8, 128), BF16),
            pltpu.VMEM((NEP, 3, 8, 128), BF16),
            pltpu.VMEM((NEP, 3, 8, 128), BF16),
            pltpu.VMEM((2, NY, ROWS, PART), BF16),
            pltpu.VMEM((NTP, 8, PART), BF16),
            pltpu.VMEM((NY, 8, PART), F32),
            pltpu.VMEM((NY, 8, PART), F32),
            pltpu.VMEM((8, 64), BF16),
            pltpu.VMEM((8, 64), BF16),
            pltpu.VMEM((16, 256), F32),
            pltpu.VMEM((16, 256), BF16),
            pltpu.VMEM((8, 128), F32),
            pltpu.VMEM((1, 128), F32),
            pltpu.VMEM((NEP, 1, 128), F32),
            pltpu.VMEM((ROWS, 512), F32),
            pltpu.VMEM((ROWS, 256), BF16),
            pltpu.VMEM((4, ROWS, PART), jnp.int16),
            pltpu.VMEM((4, ROWS, PART), jnp.int16),
            pltpu.VMEM((4, 1, 128), F32),
            pltpu.VMEM((4, 1, 128), F32),
            pltpu.VMEM((NEP, 3, 8, 128), jnp.int16),
            pltpu.VMEM((NEP, 3, 8, 128), jnp.int16),
            pltpu.VMEM((1, 128), F32),
            pltpu.VMEM((NEP, 1, 128), F32),
            pltpu.VMEM((3, 8, PART), F32),
            pltpu.VMEM((3, 8, PART), F32),
            pltpu.VMEM((ROWS, PART), F32),
            pltpu.VMEM((NEP, 8, 128), F32),
            pltpu.VMEM((NEP, 8, 128), F32),
            pltpu.VMEM((1, 128), F32),
            pltpu.VMEM((NTP, 1, 128), F32),
            pltpu.VMEM((8, 128), F32),
            dma((6,)),
            dma((4,)),
            dma((3,)),
            dma((3,)),
            dma,
            dma,
            dma,
            dma,
            dma,
            dma,
            dma,
            dma,
            dma,
            dma,
            dma,
            dma((4,)),
            dma,
            dma((5,)),
            dma,
            dma((3,)),
            dma,
            dma,
            dma,
            dma((4,)),
            dma,
            dma((4,)),
            dma,
            dma,
            dma,
            dma,
            dma,
            dma,
            dma,
            dma,
            dma,
            dma,
        ],
        compiler_params=pltpu.CompilerParams(
            collective_id=0, has_side_effects=True, vmem_limit_bytes=56650000
        ),
    )(
        tokens,
        norm_gain.reshape(1, WIDTH),
        route_experts.T,
        route_logits.T,
        jnp.swapaxes(expert_gate, 1, 2),
        jnp.swapaxes(expert_up, 1, 2),
        expert_down,
        dense_gate.T,
        dense_up.T,
        dense_down,
        mix_weight.reshape(1, WIDTH),
        out_gain.reshape(1, PART),
    )


def solution(mesh):
    tp = "tp"
    in_specs = (
        P("ep", tp),
        P(),
        P("ep", None),
        P("ep", None),
        P("ep", None, tp),
        P("ep", None, tp),
        P("ep", tp, None),
        P(None, tp),
        P(None, tp),
        P(tp, None),
        P(),
        P(tp),
    )
    return jax.shard_map(
        local, mesh=mesh, in_specs=in_specs, out_specs=P("ep", tp), check_vma=False
    )
```

```python
import functools

import jax
import jax.numpy as jnp
from jax import lax
from jax.experimental import pallas as pl
from jax.experimental.pallas import tpu as pltpu
from jax.sharding import PartitionSpec as P

MESH = pl.DeviceIdType.MESH
F32 = jnp.float32
BF16 = jnp.bfloat16
EPS = 1e-06

NX, NZ, NY = 4, 8, 8
NEP = NX * NZ
NTP = 2 * NY
ROWS = 128
FAR = (3, 4, 5)
NEAR = (6, 2, 7, 1)
PART = 256
WIDTH = 4096


def rcopy(src, dst, send_sem, recv_sem, device):
    return pltpu.make_async_remote_copy(
        src_ref=src,
        dst_ref=dst,
        send_sem=send_sem,
        recv_sem=recv_sem,
        device_id=device,
        device_id_type=MESH,
    )


def nt_dot(a, b):
    return lax.dot_general(a, b, (((1,), (1,)), ((), ())), preferred_element_type=F32)


def pieces(value, axis):
    high = value.astype(BF16)
    rest = value - high.astype(F32)
    middle = rest.astype(BF16)
    low = (rest - middle.astype(F32)).astype(BF16)
    return jnp.concatenate([high, middle, low], axis=axis)


def silu(v):
    return v / (1.0 + jnp.exp(-v))


def kernel(
    tok_hbm,
    gain_hbm,
    routes_hbm,
    logits_hbm,
    wg,
    wu,
    wd,
    dg,
    du,
    dd,
    mixw_hbm,
    ogain_hbm,
    out,
    tok,
    gain,
    routes,
    logits,
    mixw,
    ogain,
    w_gu,
    wd_own,
    wd_par,
    w_dense,
    dd_own,
    dd_par,
    a2a_out,
    a2a_in,
    far_out,
    far_in,
    far_par,
    gathered,
    tok_all,
    dense_out,
    dense_in,
    dh_own,
    dh_par,
    comb,
    place,
    slots,
    r_out,
    r_in,
    acts,
    hid,
    q_out,
    q_in,
    s_out,
    s_in,
    fq_out,
    fq_in,
    fs_out,
    fs_in,
    fy_out,
    fy_in,
    kept,
    ret_out,
    ret_in,
    sq_out,
    sq_in,
    gate_ref,
    i_sem,
    w_sem,
    wp_ssem,
    wp_rsem,
    a2a_ssem,
    a2a_rsem,
    far_ssem,
    far_rsem,
    tok_ssem,
    tok_rsem,
    dh_ssem,
    dh_rsem,
    dense_ssem,
    dense_rsem,
    ag_ssem,
    ag_rsem,
    pf_ssem,
    pf_rsem,
    fp_ssem,
    fp_rsem,
    r_ssem,
    r_rsem,
    q_ssem,
    q_rsem,
    sc_ssem,
    sc_rsem,
    fq_ssem,
    fq_rsem,
    fs_ssem,
    fs_rsem,
    fy_ssem,
    fy_rsem,
    ret_ssem,
    ret_rsem,
    sq_ssem,
    sq_rsem,
):
    me_e = lax.axis_index("ep")
    me_t = lax.axis_index("tp")
    z, x = lax.div(me_e, NX), lax.rem(me_e, NX)
    y, core = lax.div(me_t, 2), lax.rem(me_t, 2)
    other = 1 - core
    partner = (me_e, y * 2 + other)
    zs = [lax.rem(z + k, NZ) * NX for k in range(NZ)]
    xs = [lax.rem(x + k, NX) for k in range(NX)]
    ys = [lax.rem(y + k, NY) for k in range(NY)]
    peers = [zs[dz] + xs[dx] for dz in (4, 3, 5, 2, 6, 1, 7, 0) for dx in (2, 1, 3, 0)][:-1]
    y_order = (4, 3, 5, 2, 6, 1, 7)

    def ydev(step):
        return (me_e, ys[step % NY] * 2 + core)

    barrier = pltpu.get_barrier_semaphore()
    for peer in peers:
        pl.semaphore_signal(barrier, inc=1, device_id=(peer, me_t), device_id_type=MESH)
    for step in y_order:
        for c in range(2):
            pl.semaphore_signal(
                barrier, inc=1, device_id=(me_e, ys[step] * 2 + c), device_id_type=MESH
            )
    pl.semaphore_signal(barrier, inc=1, device_id=partner, device_id_type=MESH)

    smalls = [
        pltpu.make_async_copy(routes_hbm, routes, i_sem.at[0]),
        pltpu.make_async_copy(logits_hbm, logits, i_sem.at[1]),
        pltpu.make_async_copy(tok_hbm, tok, i_sem.at[2]),
        pltpu.make_async_copy(gain_hbm, gain, i_sem.at[3]),
        pltpu.make_async_copy(mixw_hbm, mixw, i_sem.at[4]),
        pltpu.make_async_copy(ogain_hbm, ogain, i_sem.at[5]),
    ]

    def columns(k, c):
        return pl.ds(pl.multiple_of((2 * k + c) * PART, PART), PART)

    def load(src, dst, k):
        pltpu.make_async_copy(src, dst, w_sem.at[k]).start()

    def loaded(dst, k):
        pltpu.make_async_copy(dst, dst, w_sem.at[k]).wait()

    for copy in smalls:
        copy.start()
    load(dg, w_dense.at[pl.ds(0, 64)], 0)
    load(du, w_dense.at[pl.ds(64, 64)], 0)
    for k in range(NY):
        load(dd.at[:, columns(k, core)], dd_own.at[k], 1)
    load(wg, w_gu.at[0, pl.ds(0, 2)], 2)
    load(wu, w_gu.at[0, pl.ds(2, 2)], 2)
    for k in range(NY):
        load(wd.at[:, :, columns(k, core)], wd_own.at[k], 3)

    for copy in smalls[0:3]:
        copy.wait()
    lane = lax.broadcasted_iota(jnp.int32, (8, 256), 1)
    sub = lax.broadcasted_iota(jnp.int32, (8, 256), 0)
    expert = 2 * (lane // 8) + (lane // 2) % 2
    half = (lane // 4) % 2
    r0 = jnp.zeros((8, 256), jnp.int32)
    r1 = jnp.zeros((8, 256), jnp.int32)
    l0 = jnp.zeros((8, 256), F32)
    l1 = jnp.zeros((8, 256), F32)
    for t in range(8):
        r0 = jnp.where(sub == t, routes[0, t], r0)
        r1 = jnp.where(sub == t, routes[1, t], r1)
        l0 = jnp.where(sub == t, logits[0, t], l0)
        l1 = jnp.where(sub == t, logits[1, t], l1)
    top = jnp.maximum(l0, l1)
    e0, e1 = jnp.exp(l0 - top), jnp.exp(l1 - top)
    is0, is1 = (r0 == expert), (r1 == expert)
    hit = jnp.where(is0, 1.0, 0.0) + jnp.where(is1, 1.0, 0.0)
    before = jnp.zeros((8, 256), F32)
    for t in range(7):
        before = before + jnp.where(sub > t, hit[t : t + 1, :], 0.0)
    placed = jnp.where(before == (lane % 2).astype(F32), hit, 0.0)
    weight = (jnp.where(is0, e0, 0.0) + jnp.where(is1, e1, 0.0)) / (e0 + e1) * placed
    comb[0:8, :] = jnp.where(half == 0, weight, 0.0)
    comb[8:16, :] = jnp.where(half == 1, weight, 0.0)
    left_half = lax.broadcasted_iota(jnp.int32, (256, 128), 0)
    slot = lax.broadcasted_iota(jnp.int32, (256, 128), 1)
    left_half = (left_half // 8 == slot // 4) & (left_half % 8 == slot % 4)
    slots[...] = jnp.dot(
        placed.astype(BF16),
        jnp.where(left_half, 1.0, 0.0).astype(BF16),
        preferred_element_type=F32,
    )
    place[...] = jnp.concatenate(
        [jnp.where(half == 0, placed, 0.0), jnp.where(half == 1, placed, 0.0)], axis=0
    ).astype(BF16)

    def placed_rows(value):
        halves = jnp.concatenate(
            [value[:, 0:128].astype(F32), value[:, 128:256].astype(F32)], axis=0
        ).astype(BF16)
        rows = lax.dot_general(
            place[...], halves, (((0,), (0,)), ((), ())), preferred_element_type=F32
        )
        return rows.astype(BF16).reshape(NEP, 8, 128)

    tok_value = tok[...]
    a2a_out[...] = placed_rows(tok_value)
    a2a_in[me_e] = a2a_out[me_e]
    tok_all[me_t] = tok_value

    pl.semaphore_wait(barrier, NEP - 1 + NTP - 1)

    for step in y_order:
        for c in range(2):
            rcopy(
                tok, tok_all.at[me_t], tok_ssem, tok_rsem, (me_e, ys[step] * 2 + c)
            ).start()
    rcopy(tok, tok_all.at[me_t], tok_ssem, tok_rsem, partner).start()

    for peer in peers:
        rcopy(a2a_out.at[peer], a2a_in.at[me_e], a2a_ssem, a2a_rsem, (peer, me_t)).start()

    for k in range(NY):
        rcopy(
            dd.at[:, columns(k, other)], dd_par.at[k], wp_ssem.at[0], wp_rsem.at[0], partner
        ).start()
    for k, ref in enumerate((wg, wu)):
        rcopy(
            ref, w_gu.at[1, pl.ds(2 * k, 2)], wp_ssem.at[1], wp_rsem.at[1], partner
        ).start()
    for k in range(NY):
        rcopy(
            wd.at[:, :, columns(k, other)], wd_par.at[k], wp_ssem.at[2], wp_rsem.at[2], partner
        ).start()
    parts = [
        rcopy(ref, ref, wp_ssem.at[k], wp_rsem.at[k], partner)
        for k, ref in enumerate((dd_par, w_gu.at[1], wd_par))
    ]

    def arrived(src, dst, ssem, rsem, n):
        part = pl.ds(0, n)
        copy = rcopy(src.at[part], dst.at[part], ssem, rsem, partner)
        copy.wait_recv()
        return copy

    done = [arrived(tok_all, tok_all, tok_ssem, tok_rsem, NTP - 1)]
    squares = jnp.zeros((8, PART), F32)
    for j in range(NTP):
        v = tok_all[j].astype(F32)
        squares = squares + v * v
    scale = lax.rsqrt(jnp.sum(squares, axis=1, keepdims=True) / WIDTH + EPS)
    r_out[...] = jnp.sum(slots[...] * scale, axis=0, keepdims=True)
    for i, rel in enumerate(FAR):
        far_out[:, i] = placed_rows(tok_all[ys[rel] * 2 + core])
    for peer in peers:
        rcopy(r_out, r_in.at[me_e], r_ssem, r_rsem, (peer, me_t)).start()
    for peer in peers:
        rcopy(far_out.at[peer], far_in.at[me_e], far_ssem, far_rsem, (peer, me_t)).start()
    r_in[me_e] = r_out[...]
    far_in[me_e] = far_out[me_e]

    done.append(arrived(a2a_out, a2a_in, a2a_ssem, a2a_rsem, NEP - 1))
    sub3 = lax.broadcasted_iota(jnp.int32, (16, 8, 128), 1)

    def keep_rows(value, c, rel):
        pairs = value.astype(F32).reshape(16, 2, 8, 128)
        even, odd = pairs[:, 0], pairs[:, 1]
        left = jnp.where(sub3 < 4, even, pltpu.roll(odd, 4, 1)).reshape(ROWS, 128)
        right = jnp.where(sub3 < 4, pltpu.roll(even, 4, 1), odd).reshape(ROWS, 128)
        gathered[c, ys[rel], :, 0:128] = left.astype(BF16)
        gathered[c, ys[rel], :, 128:256] = right.astype(BF16)

    keep_rows(a2a_in[...], core, 0)

    def ag_copy(slot, k, device):
        ref = gathered.at[core, ys[slot]]
        return rcopy(ref, ref, ag_ssem, ag_rsem.at[k], device)

    for k, step in enumerate((2, -2, 1, -1)):
        ag_copy(0, k, ydev(step)).start()

    def pass_copy(c, rel):
        ref = gathered.at[c, ys[rel]]
        k = ((0,) + NEAR).index(rel)
        return rcopy(ref, ref, pf_ssem, pf_rsem.at[k], partner)

    def pass_on(rel):
        pass_copy(core, rel).start()

    def pass_wait(rel):
        pass_copy(other, rel).wait_recv()

    pass_on(0)

    for copy in smalls[3:6]:
        copy.wait()
    loaded(w_dense, 0)
    act = jnp.zeros((8, 128), F32)
    mix_acc = jnp.zeros((8, PART), F32)
    for j in range(NTP):
        cols = slice(j * PART, (j + 1) * PART)
        n = (tok_all[j].astype(F32) * scale * gain[:, cols]).astype(BF16)
        mix_acc = mix_acc + n.astype(F32) * mixw[:, cols]
        act = act + nt_dot(n, w_dense[:, cols])
    gate_ref[...] = jnp.broadcast_to(
        jax.nn.sigmoid(jnp.sum(mix_acc, axis=1, keepdims=True)), (8, 128)
    )
    dh_own[...] = (silu(act[:, 0:64]) * act[:, 64:128]).astype(BF16)
    dh_copy = rcopy(dh_own, dh_par, dh_ssem, dh_rsem, partner)
    dh_copy.start()

    loaded(dd_own, 1)
    parts[0].wait_recv()
    dh_copy.wait_recv()
    for k in range(NY):
        dense_out[k] = jnp.dot(
            dh_own[...], dd_own[k], preferred_element_type=F32
        ) + jnp.dot(dh_par[...], dd_par[k], preferred_element_type=F32)
    dense_in[y] = dense_out[y]
    loaded(w_gu.at[0], 2)
    parts[1].wait_recv()
    for rel in (6, 2):
        ag_copy(rel, NEAR.index(rel), partner).wait_recv()
        pass_on(rel)
    done.append(arrived(r_in, r_in, r_ssem, r_rsem, NEP - 1))
    picked = (
        lax.broadcasted_iota(jnp.int32, (ROWS, NEP), 0) // 4
        == lax.broadcasted_iota(jnp.int32, (ROWS, NEP), 1)
    )
    spread = jnp.dot(
        jnp.where(picked, 1.0, 0.0).astype(BF16),
        pieces(r_in[...].reshape(NEP, 128), 1),
        preferred_element_type=F32,
    )
    spread = spread[:, 0:128] + spread[:, 128:256] + spread[:, 256:384]
    wanted = me_e * 4 + lax.broadcasted_iota(jnp.int32, (ROWS, 128), 0) % 4
    here = lax.broadcasted_iota(jnp.int32, (ROWS, 128), 1) == wanted
    row_scale = jnp.sum(jnp.where(here, spread, 0.0), axis=1, keepdims=True)

    def project(*slices, first=False):
        total = None
        for c, rel in slices:
            cols = pl.ds(pl.multiple_of((2 * ys[rel] + c) * PART, PART), PART)
            n = (gathered[c, ys[rel]].astype(F32) * row_scale * gain[:, cols]).astype(BF16)
            v = nt_dot(n, w_gu[:, :, :, cols].reshape(512, PART))
            total = v if total is None else total + v
        acts[...] = total if first else acts[...] + total

    pass_wait(0)
    project((core, 0), (other, 0), (core, 6), (core, 2), first=True)
    for rel in (7, 1):
        ag_copy(rel, NEAR.index(rel), partner).wait_recv()
        pass_on(rel)
    for step in y_order:
        rcopy(
            dense_out.at[ys[step]], dense_in.at[y], dense_ssem, dense_rsem, ydev(step)
        ).start()
    pass_wait(6)
    pass_wait(2)
    project((core, 7), (core, 1), (other, 6), (other, 2))
    done.append(arrived(far_out, far_in, far_ssem, far_rsem, NEP - 1))
    raws = [
        rcopy(far_in.at[:, i], far_par.at[:, i], fp_ssem, fp_rsem.at[i], partner)
        for i in range(3)
    ]
    for copy in raws:
        copy.start()
    for i, rel in enumerate(FAR):
        keep_rows(far_in[:, i], core, rel)
    project((core, 3), (core, 4), (core, 5))
    pass_wait(7)
    pass_wait(1)
    project((other, 7), (other, 1))
    for i in range(2):
        raws[i].wait_recv()
        keep_rows(far_par[:, i], other, FAR[i])
    project((other, 3), (other, 4))
    raws[2].wait_recv()
    keep_rows(far_par[:, 2], other, FAR[2])
    project((other, 5))

    row = lax.broadcasted_iota(jnp.int32, (ROWS, 128), 0)
    col = lax.broadcasted_iota(jnp.int32, (ROWS, 128), 1)
    mine = (row // 2) % 2 == col // 64
    for k in range(2):
        v = acts[:, k * 256 : (k + 1) * 256]
        hidden = silu(v[:, 0:128]) * v[:, 128:256]
        hid[:, k * 128 : (k + 1) * 128] = jnp.where(mine, hidden, 0.0).astype(BF16)
    loaded(wd_own, 3)
    parts[2].wait_recv()

    diagonal = row == col

    def partials(*rels):
        both = jnp.concatenate(
            [
                jnp.concatenate([w[ys[rel]].reshape(128, PART) for rel in rels], axis=1)
                for w in (wd_own, wd_par)
            ],
            axis=0,
        )
        v = jnp.dot(hid[...], both, preferred_element_type=F32)
        return [v[:, i * PART : (i + 1) * PART] for i in range(len(rels))]

    def column(value):
        return jnp.sum(jnp.where(diagonal, value, 0.0), axis=0, keepdims=True)

    def messages(value):
        left = value[:, 0:128].reshape(16, 8, 128)
        right = value[:, 128:256].reshape(16, 8, 128)
        even = jnp.where(sub3 < 4, left, pltpu.roll(right, 4, 1))
        odd = jnp.where(sub3 < 4, pltpu.roll(left, 4, 1), right)
        return jnp.stack([even, odd], axis=1).reshape(NEP, 8, 128)

    def q_copies(k, device):
        return (
            rcopy(q_out.at[k], q_in.at[k], q_ssem, q_rsem.at[k], device),
            rcopy(s_out.at[k], s_in.at[k], sc_ssem, sc_rsem.at[k], device),
        )

    def q_pack(k, value):
        most = jnp.maximum(jnp.max(jnp.abs(value), axis=1, keepdims=True), 1e-30)
        q_out[k] = jnp.round(value * (32767.0 / most)).astype(jnp.int16)
        s_out[k] = column(most * (1.0 / 32767.0))

    def q_send(k):
        for copy in q_copies(k, ydev(NEAR[k])):
            copy.start()

    def q_get(k):
        for copy in q_copies(k, partner):
            copy.wait_recv()
        unit = jnp.sum(jnp.where(diagonal, s_in[k], 0.0), axis=1, keepdims=True)
        return q_in[k].astype(F32) * unit

    near2 = partials(NEAR[0], NEAR[1])
    values = partials(*FAR, 0)
    q_pack(0, near2[0])
    q_pack(1, near2[1])
    kept[...] = values[3]
    most = jnp.maximum(jnp.maximum(jnp.abs(values[0]), jnp.abs(values[1])), jnp.abs(values[2]))
    most = jnp.maximum(jnp.max(most, axis=1, keepdims=True), 1e-30)
    fs_out[...] = column(most * (1.0 / 32767.0))
    for i in range(3):
        fq_out[:, i] = messages(jnp.round(values[i] * (32767.0 / most))).astype(jnp.int16)
    q_send(0)
    q_send(1)
    for peer in peers:
        rcopy(fs_out, fs_in.at[me_e], fs_ssem, fs_rsem, (peer, me_t)).start()
    for peer in peers:
        rcopy(fq_out.at[peer], fq_in.at[me_e], fq_ssem, fq_rsem, (peer, me_t)).start()
    near1 = partials(NEAR[2], NEAR[3])
    q_pack(2, near1[0])
    q_pack(3, near1[1])
    q_send(2)
    q_send(3)
    fq_in[me_e] = fq_out[me_e]
    fs_in[me_e] = fs_out[...]
    done.append(arrived(dense_out, dense_in, dense_ssem, dense_rsem, NY - 1))
    dense = dense_in[0]
    for k in range(1, NY):
        dense = dense + dense_in[k]
    gate = gate_ref[...]
    dense = jnp.concatenate([gate, gate], axis=1) * dense
    summed = kept[...]
    for k in range(4):
        summed = summed + q_get(k)
    ret_out[...] = messages(summed)
    for peer in peers:
        rcopy(ret_out.at[peer], ret_in.at[me_e], ret_ssem, ret_rsem, (peer, me_t)).start()
    ret_in[me_e] = ret_out[me_e]
    done.append(arrived(fs_in, fs_in, fs_ssem, fs_rsem, NEP - 1))
    lane2 = lax.broadcasted_iota(jnp.int32, (128, 256), 1)
    mine4 = lax.broadcasted_iota(jnp.int32, (128, 256), 0) == me_e * 4 + lane2 % 4
    unit = jnp.dot(
        pieces(fs_in[...].reshape(NEP, 128), 0),
        jnp.where(mine4, 1.0, 0.0).astype(BF16),
        preferred_element_type=F32,
    )
    unit = unit[0:NEP] + unit[NEP : 2 * NEP] + unit[2 * NEP : 3 * NEP]
    source = lax.broadcasted_iota(jnp.int32, (NEP, 256), 0)
    source = source == lax.broadcasted_iota(jnp.int32, (NEP, 256), 1) // 8
    unit = jnp.sum(jnp.where(source, unit, 0.0), axis=0, keepdims=True)
    far_comb = pieces(comb[...] * unit, 0)
    near_comb = pieces(comb[...], 0)
    done.append(arrived(fq_out, fq_in, fq_ssem, fq_rsem, NEP - 1))
    far_rows = jnp.concatenate(
        [fq_in[:, i].astype(F32).reshape(256, 128) for i in range(3)], axis=1
    )
    far_high = far_rows.astype(BF16)
    far_low = (far_rows - far_high.astype(F32)).astype(BF16)
    far_sum = jnp.dot(far_comb, far_high, preferred_element_type=F32) + jnp.dot(
        far_comb, far_low, preferred_element_type=F32
    )
    far_sum = far_sum[0:16] + far_sum[16:32] + far_sum[32:48]
    for i, rel in enumerate(FAR):
        cols = slice(i * 128, (i + 1) * 128)
        fy_out[i, :, 0:128] = far_sum[0:8, cols]
        fy_out[i, :, 128:256] = far_sum[8:16, cols]
        rcopy(fy_out.at[i], fy_in.at[i], fy_ssem, fy_rsem, ydev(rel)).start()
    done.append(arrived(ret_out, ret_in, ret_ssem, ret_rsem, NEP - 1))
    mixed = jnp.dot(
        near_comb, pieces(ret_in[...].reshape(256, 128), 1), preferred_element_type=F32
    )
    mixed = mixed[:, 0:128] + mixed[:, 128:256] + mixed[:, 256:384]
    mixed = mixed[0:16] + mixed[16:32] + mixed[32:48]
    combined = jnp.concatenate([mixed[0:8], mixed[8:16]], axis=1) + dense
    fy_copy = rcopy(fy_out, fy_in, fy_ssem, fy_rsem, partner)
    fy_copy.wait_recv()
    combined = combined + fy_in[0] + fy_in[1] + fy_in[2]
    token_diagonal = (
        lax.broadcasted_iota(jnp.int32, (8, 128), 0)
        == lax.broadcasted_iota(jnp.int32, (8, 128), 1)
    )
    own = jnp.sum(
        jnp.where(token_diagonal, jnp.sum(combined * combined, axis=1, keepdims=True), 0.0),
        axis=0,
        keepdims=True,
    )
    sq_out[...] = own
    for step in y_order:
        for c in range(2):
            rcopy(sq_out, sq_in.at[me_t], sq_ssem, sq_rsem, (me_e, ys[step] * 2 + c)).start()
    rcopy(sq_out, sq_in.at[me_t], sq_ssem, sq_rsem, partner).start()
    sq_in[me_t] = own
    done.append(arrived(sq_in, sq_in, sq_ssem, sq_rsem, NTP - 1))
    total_sq = sq_in[0]
    for j in range(1, NTP):
        total_sq = total_sq + sq_in[j]
    final = lax.rsqrt(
        jnp.sum(jnp.where(token_diagonal, total_sq, 0.0), axis=1, keepdims=True) / WIDTH + EPS
    )
    out[...] = (combined * final * ogain[...]).astype(BF16)

    near = gathered.at[core, pl.ds(0, 4)]
    done += [
        rcopy(near, near, ag_ssem, ag_rsem.at[0], partner),
        rcopy(q_out, q_in, q_ssem, q_rsem.at[0], partner),
        rcopy(s_out, s_in, sc_ssem, sc_rsem.at[0], partner),
    ]
    five = gathered.at[core, pl.ds(0, 5)]
    done.append(rcopy(five, five, pf_ssem, pf_rsem.at[0], partner))
    for copy in parts + [dh_copy, fy_copy] + raws + done:
        copy.wait_send()


def local(
    tokens,
    norm_gain,
    route_experts,
    route_logits,
    expert_gate,
    expert_up,
    expert_down,
    dense_gate,
    dense_up,
    dense_down,
    mix_weight,
    out_gain,
):
    vmem = pl.BlockSpec(memory_space=pltpu.VMEM)
    dma = pltpu.SemaphoreType.DMA
    return pl.pallas_call(
        kernel,
        out_shape=pltpu.VMEM((8, PART), BF16),
        in_specs=[pl.BlockSpec(memory_space=pl.ANY)] * 12,
        out_specs=vmem,
        scratch_shapes=[
            pltpu.VMEM((8, PART), BF16),
            pltpu.VMEM((1, WIDTH), F32),
            pltpu.SMEM((2, 8), jnp.int32),
            pltpu.SMEM((2, 8), F32),
            pltpu.VMEM((1, WIDTH), F32),
            pltpu.VMEM((1, PART), F32),
            pltpu.VMEM((2, 4, 64, WIDTH), BF16),
            pltpu.VMEM((NY, 2, 64, PART), BF16),
            pltpu.VMEM((NY, 2, 64, PART), BF16),
            pltpu.VMEM((128, WIDTH), BF16),
            pltpu.VMEM((NY, 64, PART), BF16),
            pltpu.VMEM((NY, 64, PART), BF16),
            pltpu.VMEM((NEP, 8, 128), BF16),
            pltpu.VMEM((NEP, 8, 128), BF16),
            pltpu.VMEM((NEP, 3, 8, 128), BF16),
            pltpu.VMEM((NEP, 3, 8, 128), BF16),
            pltpu.VMEM((NEP, 3, 8, 128), BF16),
            pltpu.VMEM((2, NY, ROWS, PART), BF16),
            pltpu.VMEM((NTP, 8, PART), BF16),
            pltpu.VMEM((NY, 8, PART), F32),
            pltpu.VMEM((NY, 8, PART), F32),
            pltpu.VMEM((8, 64), BF16),
            pltpu.VMEM((8, 64), BF16),
            pltpu.VMEM((16, 256), F32),
            pltpu.VMEM((16, 256), BF16),
            pltpu.VMEM((8, 128), F32),
            pltpu.VMEM((1, 128), F32),
            pltpu.VMEM((NEP, 1, 128), F32),
            pltpu.VMEM((ROWS, 512), F32),
            pltpu.VMEM((ROWS, 256), BF16),
            pltpu.VMEM((4, ROWS, PART), jnp.int16),
            pltpu.VMEM((4, ROWS, PART), jnp.int16),
            pltpu.VMEM((4, 1, 128), F32),
            pltpu.VMEM((4, 1, 128), F32),
            pltpu.VMEM((NEP, 3, 8, 128), jnp.int16),
            pltpu.VMEM((NEP, 3, 8, 128), jnp.int16),
            pltpu.VMEM((1, 128), F32),
            pltpu.VMEM((NEP, 1, 128), F32),
            pltpu.VMEM((3, 8, PART), F32),
            pltpu.VMEM((3, 8, PART), F32),
            pltpu.VMEM((ROWS, PART), F32),
            pltpu.VMEM((NEP, 8, 128), F32),
            pltpu.VMEM((NEP, 8, 128), F32),
            pltpu.VMEM((1, 128), F32),
            pltpu.VMEM((NTP, 1, 128), F32),
            pltpu.VMEM((8, 128), F32),
            dma((6,)),
            dma((4,)),
            dma((3,)),
            dma((3,)),
            dma,
            dma,
            dma,
            dma,
            dma,
            dma,
            dma,
            dma,
            dma,
            dma,
            dma,
            dma((4,)),
            dma,
            dma((5,)),
            dma,
            dma((3,)),
            dma,
            dma,
            dma,
            dma((4,)),
            dma,
            dma((4,)),
            dma,
            dma,
            dma,
            dma,
            dma,
            dma,
            dma,
            dma,
            dma,
            dma,
        ],
        compiler_params=pltpu.CompilerParams(
            collective_id=0, has_side_effects=True, vmem_limit_bytes=56650000
        ),
    )(
        tokens,
        norm_gain.reshape(1, WIDTH),
        route_experts.T,
        route_logits.T,
        jnp.swapaxes(expert_gate, 1, 2),
        jnp.swapaxes(expert_up, 1, 2),
        expert_down,
        dense_gate.T,
        dense_up.T,
        dense_down,
        mix_weight.reshape(1, WIDTH),
        out_gain.reshape(1, PART),
    )


def solution(mesh):
    tp = "tp"
    in_specs = (
        P("ep", tp),
        P(),
        P("ep", None),
        P("ep", None),
        P("ep", None, tp),
        P("ep", None, tp),
        P("ep", tp, None),
        P(None, tp),
        P(None, tp),
        P(tp, None),
        P(),
        P(tp),
    )
    return jax.shard_map(
        local, mesh=mesh, in_specs=in_specs, out_specs=P("ep", tp), check_vma=False
    )
```

```python
import functools

import jax
import jax.numpy as jnp
from jax import lax
from jax.experimental import pallas as pl
from jax.experimental.pallas import tpu as pltpu
from jax.sharding import PartitionSpec as P

MESH = pl.DeviceIdType.MESH
F32 = jnp.float32
BF16 = jnp.bfloat16
EPS = 1e-06

NX, NZ, NY = 4, 8, 8
NEP = NX * NZ
NTP = 2 * NY
ROWS = 128
FAR = (3, 4, 5)
NEAR = (6, 2, 7, 1)
PART = 256
WIDTH = 4096


def rcopy(src, dst, send_sem, recv_sem, device):
    return pltpu.make_async_remote_copy(
        src_ref=src,
        dst_ref=dst,
        send_sem=send_sem,
        recv_sem=recv_sem,
        device_id=device,
        device_id_type=MESH,
    )


def nt_dot(a, b):
    return lax.dot_general(a, b, (((1,), (1,)), ((), ())), preferred_element_type=F32)


def pieces(value, axis):
    high = value.astype(BF16)
    rest = value - high.astype(F32)
    middle = rest.astype(BF16)
    low = (rest - middle.astype(F32)).astype(BF16)
    return jnp.concatenate([high, middle, low], axis=axis)


def silu(v):
    return v / (1.0 + jnp.exp(-v))


def kernel(
    tok_hbm,
    gain_hbm,
    routes_hbm,
    logits_hbm,
    wg,
    wu,
    wd,
    dg,
    du,
    dd,
    mixw_hbm,
    ogain_hbm,
    out,
    tok,
    gain,
    routes,
    logits,
    mixw,
    ogain,
    w_gu,
    wd_own,
    wd_par,
    w_dense,
    dd_own,
    dd_par,
    a2a_out,
    a2a_in,
    far_out,
    far_in,
    far_par,
    gathered,
    tok_all,
    ss_out,
    ss_in,
    dense_out,
    dense_in,
    dh_own,
    dh_par,
    comb,
    place,
    slots,
    r_out,
    r_in,
    acts,
    hid,
    q_out,
    q_in,
    s_out,
    s_in,
    fq_out,
    fq_in,
    fs_out,
    fs_in,
    fy_out,
    fy_in,
    kept,
    ret_out,
    ret_in,
    sq_out,
    sq_in,
    gate_ref,
    i_sem,
    w_sem,
    wp_ssem,
    wp_rsem,
    a2a_ssem,
    a2a_rsem,
    far_ssem,
    far_rsem,
    tok_ssem,
    tok_rsem,
    tp_ssem,
    tp_rsem,
    ss_ssem,
    ss_rsem,
    dh_ssem,
    dh_rsem,
    dense_ssem,
    dense_rsem,
    ag_ssem,
    ag_rsem,
    pf_ssem,
    pf_rsem,
    fp_ssem,
    fp_rsem,
    r_ssem,
    r_rsem,
    q_ssem,
    q_rsem,
    sc_ssem,
    sc_rsem,
    fq_ssem,
    fq_rsem,
    fs_ssem,
    fs_rsem,
    fy_ssem,
    fy_rsem,
    ret_ssem,
    ret_rsem,
    sq_ssem,
    sq_rsem,
):
    me_e = lax.axis_index("ep")
    me_t = lax.axis_index("tp")
    z, x = lax.div(me_e, NX), lax.rem(me_e, NX)
    y, core = lax.div(me_t, 2), lax.rem(me_t, 2)
    other = 1 - core
    partner = (me_e, y * 2 + other)
    zs = [lax.rem(z + k, NZ) * NX for k in range(NZ)]
    xs = [lax.rem(x + k, NX) for k in range(NX)]
    ys = [lax.rem(y + k, NY) for k in range(NY)]
    peers = [zs[dz] + xs[dx] for dz in (4, 3, 5, 2, 6, 1, 7, 0) for dx in (2, 1, 3, 0)][:-1]
    y_order = (4, 3, 5, 2, 6, 1, 7)

    def ydev(step):
        return (me_e, ys[step % NY] * 2 + core)

    barrier = pltpu.get_barrier_semaphore()
    for peer in peers:
        pl.semaphore_signal(barrier, inc=1, device_id=(peer, me_t), device_id_type=MESH)
    for step in y_order:
        for c in range(2):
            pl.semaphore_signal(
                barrier, inc=1, device_id=(me_e, ys[step] * 2 + c), device_id_type=MESH
            )
    pl.semaphore_signal(barrier, inc=1, device_id=partner, device_id_type=MESH)

    smalls = [
        pltpu.make_async_copy(routes_hbm, routes, i_sem.at[0]),
        pltpu.make_async_copy(logits_hbm, logits, i_sem.at[1]),
        pltpu.make_async_copy(tok_hbm, tok, i_sem.at[2]),
        pltpu.make_async_copy(gain_hbm, gain, i_sem.at[3]),
        pltpu.make_async_copy(mixw_hbm, mixw, i_sem.at[4]),
        pltpu.make_async_copy(ogain_hbm, ogain, i_sem.at[5]),
    ]

    def columns(k, c):
        return pl.ds(pl.multiple_of((2 * k + c) * PART, PART), PART)

    def load(src, dst, k):
        pltpu.make_async_copy(src, dst, w_sem.at[k]).start()

    def loaded(dst, k):
        pltpu.make_async_copy(dst, dst, w_sem.at[k]).wait()

    for copy in smalls:
        copy.start()
    load(dg, w_dense.at[pl.ds(0, 64)], 0)
    load(du, w_dense.at[pl.ds(64, 64)], 0)
    for k in range(NY):
        load(dd.at[:, columns(k, core)], dd_own.at[k], 1)
    load(wg, w_gu.at[0, pl.ds(0, 2)], 2)
    load(wu, w_gu.at[0, pl.ds(2, 2)], 2)
    for k in range(NY):
        load(wd.at[:, :, columns(k, core)], wd_own.at[k], 3)

    for copy in smalls[0:3]:
        copy.wait()
    lane = lax.broadcasted_iota(jnp.int32, (8, 256), 1)
    sub = lax.broadcasted_iota(jnp.int32, (8, 256), 0)
    expert = 2 * (lane // 8) + (lane // 2) % 2
    half = (lane // 4) % 2
    r0 = jnp.zeros((8, 256), jnp.int32)
    r1 = jnp.zeros((8, 256), jnp.int32)
    l0 = jnp.zeros((8, 256), F32)
    l1 = jnp.zeros((8, 256), F32)
    for t in range(8):
        r0 = jnp.where(sub == t, routes[0, t], r0)
        r1 = jnp.where(sub == t, routes[1, t], r1)
        l0 = jnp.where(sub == t, logits[0, t], l0)
        l1 = jnp.where(sub == t, logits[1, t], l1)
    top = jnp.maximum(l0, l1)
    e0, e1 = jnp.exp(l0 - top), jnp.exp(l1 - top)
    is0, is1 = (r0 == expert), (r1 == expert)
    hit = jnp.where(is0, 1.0, 0.0) + jnp.where(is1, 1.0, 0.0)
    before = jnp.zeros((8, 256), F32)
    for t in range(7):
        before = before + jnp.where(sub > t, hit[t : t + 1, :], 0.0)
    placed = jnp.where(before == (lane % 2).astype(F32), hit, 0.0)
    weight = (jnp.where(is0, e0, 0.0) + jnp.where(is1, e1, 0.0)) / (e0 + e1) * placed
    comb[0:8, :] = jnp.where(half == 0, weight, 0.0)
    comb[8:16, :] = jnp.where(half == 1, weight, 0.0)
    left_half = lax.broadcasted_iota(jnp.int32, (256, 128), 0)
    slot = lax.broadcasted_iota(jnp.int32, (256, 128), 1)
    left_half = (left_half // 8 == slot // 4) & (left_half % 8 == slot % 4)
    slots[...] = jnp.dot(
        placed.astype(BF16),
        jnp.where(left_half, 1.0, 0.0).astype(BF16),
        preferred_element_type=F32,
    )
    place[...] = jnp.concatenate(
        [jnp.where(half == 0, placed, 0.0), jnp.where(half == 1, placed, 0.0)], axis=0
    ).astype(BF16)

    def placed_rows(value):
        halves = jnp.concatenate(
            [value[:, 0:128].astype(F32), value[:, 128:256].astype(F32)], axis=0
        ).astype(BF16)
        rows = lax.dot_general(
            place[...], halves, (((0,), (0,)), ((), ())), preferred_element_type=F32
        )
        return rows.astype(BF16).reshape(NEP, 8, 128)

    tok_value = tok[...]
    a2a_out[...] = placed_rows(tok_value)
    a2a_in[me_e] = a2a_out[me_e]
    tok_all[core, y] = tok_value
    token_diagonal = (
        lax.broadcasted_iota(jnp.int32, (8, 128), 0)
        == lax.broadcasted_iota(jnp.int32, (8, 128), 1)
    )

    def to_row(value):
        return jnp.sum(jnp.where(token_diagonal, value, 0.0), axis=0, keepdims=True)

    def to_column(value):
        return jnp.sum(jnp.where(token_diagonal, value, 0.0), axis=1, keepdims=True)

    wide = tok_value.astype(F32)
    ss_out[...] = to_row(jnp.sum(wide * wide, axis=1, keepdims=True))
    ss_in[me_t] = ss_out[...]

    pl.semaphore_wait(barrier, NEP - 1 + NTP - 1)

    for step in y_order:
        rcopy(tok, tok_all.at[core, y], tok_ssem, tok_rsem, ydev(step)).start()
        for c in range(2):
            rcopy(
                ss_out, ss_in.at[me_t], ss_ssem, ss_rsem, (me_e, ys[step] * 2 + c)
            ).start()
    rcopy(ss_out, ss_in.at[me_t], ss_ssem, ss_rsem, partner).start()

    for peer in peers:
        rcopy(a2a_out.at[peer], a2a_in.at[me_e], a2a_ssem, a2a_rsem, (peer, me_t)).start()

    for k in range(NY):
        rcopy(
            dd.at[:, columns(k, other)], dd_par.at[k], wp_ssem.at[0], wp_rsem.at[0], partner
        ).start()
    for k, ref in enumerate((wg, wu)):
        rcopy(
            ref, w_gu.at[1, pl.ds(2 * k, 2)], wp_ssem.at[1], wp_rsem.at[1], partner
        ).start()
    for k in range(NY):
        rcopy(
            wd.at[:, :, columns(k, other)], wd_par.at[k], wp_ssem.at[2], wp_rsem.at[2], partner
        ).start()
    parts = [
        rcopy(ref, ref, wp_ssem.at[k], wp_rsem.at[k], partner)
        for k, ref in enumerate((dd_par, w_gu.at[1], wd_par))
    ]

    def arrived(src, dst, ssem, rsem, n):
        part = pl.ds(0, n)
        copy = rcopy(src.at[part], dst.at[part], ssem, rsem, partner)
        copy.wait_recv()
        return copy

    done = [arrived(ss_in, ss_in, ss_ssem, ss_rsem, NTP - 1)]
    some = tok_all.at[0, pl.ds(0, NY - 1)]
    tok_copy = rcopy(some, some, tok_ssem, tok_rsem, partner)
    tok_copy.wait_recv()
    squares = ss_in[0]
    for j in range(1, NTP):
        squares = squares + ss_in[j]
    scale = lax.rsqrt(to_column(squares) / WIDTH + EPS)
    r_out[...] = jnp.sum(slots[...] * scale, axis=0, keepdims=True)
    for i, rel in enumerate(FAR):
        far_out[:, i] = placed_rows(tok_all[core, ys[rel]])
    for peer in peers:
        rcopy(r_out, r_in.at[me_e], r_ssem, r_rsem, (peer, me_t)).start()
    for peer in peers:
        rcopy(far_out.at[peer], far_in.at[me_e], far_ssem, far_rsem, (peer, me_t)).start()
    tok_pass = rcopy(tok_all.at[core], tok_all.at[core], tp_ssem, tp_rsem, partner)
    tok_pass.start()
    r_in[me_e] = r_out[...]
    far_in[me_e] = far_out[me_e]

    done.append(arrived(a2a_out, a2a_in, a2a_ssem, a2a_rsem, NEP - 1))
    sub3 = lax.broadcasted_iota(jnp.int32, (16, 8, 128), 1)

    def keep_rows(value, c, rel):
        pairs = value.astype(F32).reshape(16, 2, 8, 128)
        even, odd = pairs[:, 0], pairs[:, 1]
        left = jnp.where(sub3 < 4, even, pltpu.roll(odd, 4, 1)).reshape(ROWS, 128)
        right = jnp.where(sub3 < 4, pltpu.roll(even, 4, 1), odd).reshape(ROWS, 128)
        gathered[c, ys[rel], :, 0:128] = left.astype(BF16)
        gathered[c, ys[rel], :, 128:256] = right.astype(BF16)

    keep_rows(a2a_in[...], core, 0)

    def ag_copy(slot, k, device):
        ref = gathered.at[core, ys[slot]]
        return rcopy(ref, ref, ag_ssem, ag_rsem.at[k], device)

    for k, step in enumerate((2, -2, 1, -1)):
        ag_copy(0, k, ydev(step)).start()

    def pass_copy(c, rel):
        ref = gathered.at[c, ys[rel]]
        k = ((0,) + NEAR).index(rel)
        return rcopy(ref, ref, pf_ssem, pf_rsem.at[k], partner)

    def pass_on(rel):
        pass_copy(core, rel).start()

    def pass_wait(rel):
        pass_copy(other, rel).wait_recv()

    pass_on(0)

    for copy in smalls[3:6]:
        copy.wait()
    loaded(w_dense, 0)
    rcopy(tok_all.at[other], tok_all.at[other], tp_ssem, tp_rsem, partner).wait_recv()
    act = jnp.zeros((8, 128), F32)
    mix_acc = jnp.zeros((8, PART), F32)
    for j in range(NTP):
        cols = slice(j * PART, (j + 1) * PART)
        n = (tok_all[j % 2, j // 2].astype(F32) * scale * gain[:, cols]).astype(BF16)
        mix_acc = mix_acc + n.astype(F32) * mixw[:, cols]
        act = act + nt_dot(n, w_dense[:, cols])
    gate_ref[...] = jnp.broadcast_to(
        jax.nn.sigmoid(jnp.sum(mix_acc, axis=1, keepdims=True)), (8, 128)
    )
    dh_own[...] = (silu(act[:, 0:64]) * act[:, 64:128]).astype(BF16)
    dh_copy = rcopy(dh_own, dh_par, dh_ssem, dh_rsem, partner)
    dh_copy.start()

    loaded(dd_own, 1)
    parts[0].wait_recv()
    dh_copy.wait_recv()
    for k in range(NY):
        dense_out[k] = jnp.dot(
            dh_own[...], dd_own[k], preferred_element_type=F32
        ) + jnp.dot(dh_par[...], dd_par[k], preferred_element_type=F32)
    dense_in[y] = dense_out[y]
    loaded(w_gu.at[0], 2)
    parts[1].wait_recv()
    for rel in (6, 2):
        ag_copy(rel, NEAR.index(rel), partner).wait_recv()
        pass_on(rel)
    done.append(arrived(r_in, r_in, r_ssem, r_rsem, NEP - 1))
    picked = (
        lax.broadcasted_iota(jnp.int32, (ROWS, NEP), 0) // 4
        == lax.broadcasted_iota(jnp.int32, (ROWS, NEP), 1)
    )
    spread = jnp.dot(
        jnp.where(picked, 1.0, 0.0).astype(BF16),
        pieces(r_in[...].reshape(NEP, 128), 1),
        preferred_element_type=F32,
    )
    spread = spread[:, 0:128] + spread[:, 128:256] + spread[:, 256:384]
    wanted = me_e * 4 + lax.broadcasted_iota(jnp.int32, (ROWS, 128), 0) % 4
    here = lax.broadcasted_iota(jnp.int32, (ROWS, 128), 1) == wanted
    row_scale = jnp.sum(jnp.where(here, spread, 0.0), axis=1, keepdims=True)

    def project(*slices, first=False):
        total = None
        for c, rel in slices:
            cols = pl.ds(pl.multiple_of((2 * ys[rel] + c) * PART, PART), PART)
            n = (gathered[c, ys[rel]].astype(F32) * row_scale * gain[:, cols]).astype(BF16)
            v = nt_dot(n, w_gu[:, :, :, cols].reshape(512, PART))
            total = v if total is None else total + v
        acts[...] = total if first else acts[...] + total

    pass_wait(0)
    project((core, 0), (other, 0), (core, 6), (core, 2), first=True)
    for rel in (7, 1):
        ag_copy(rel, NEAR.index(rel), partner).wait_recv()
        pass_on(rel)
    for step in y_order:
        rcopy(
            dense_out.at[ys[step]], dense_in.at[y], dense_ssem, dense_rsem, ydev(step)
        ).start()
    pass_wait(6)
    pass_wait(2)
    project((core, 7), (core, 1), (other, 6), (other, 2))
    done.append(arrived(far_out, far_in, far_ssem, far_rsem, NEP - 1))
    raws = [
        rcopy(far_in.at[:, i], far_par.at[:, i], fp_ssem, fp_rsem.at[i], partner)
        for i in range(3)
    ]
    for copy in raws:
        copy.start()
    for i, rel in enumerate(FAR):
        keep_rows(far_in[:, i], core, rel)
    project((core, 3), (core, 4), (core, 5))
    pass_wait(7)
    pass_wait(1)
    project((other, 7), (other, 1))
    for i in range(2):
        raws[i].wait_recv()
        keep_rows(far_par[:, i], other, FAR[i])
    project((other, 3), (other, 4))
    raws[2].wait_recv()
    keep_rows(far_par[:, 2], other, FAR[2])
    project((other, 5))

    row = lax.broadcasted_iota(jnp.int32, (ROWS, 128), 0)
    col = lax.broadcasted_iota(jnp.int32, (ROWS, 128), 1)
    mine = (row // 2) % 2 == col // 64
    for k in range(2):
        v = acts[:, k * 256 : (k + 1) * 256]
        hidden = silu(v[:, 0:128]) * v[:, 128:256]
        hid[:, k * 128 : (k + 1) * 128] = jnp.where(mine, hidden, 0.0).astype(BF16)
    loaded(wd_own, 3)
    parts[2].wait_recv()

    diagonal = row == col

    def partials(*rels):
        both = jnp.concatenate(
            [
                jnp.concatenate([w[ys[rel]].reshape(128, PART) for rel in rels], axis=1)
                for w in (wd_own, wd_par)
            ],
            axis=0,
        )
        v = jnp.dot(hid[...], both, preferred_element_type=F32)
        return [v[:, i * PART : (i + 1) * PART] for i in range(len(rels))]

    def column(value):
        return jnp.sum(jnp.where(diagonal, value, 0.0), axis=0, keepdims=True)

    def messages(value):
        left = value[:, 0:128].reshape(16, 8, 128)
        right = value[:, 128:256].reshape(16, 8, 128)
        even = jnp.where(sub3 < 4, left, pltpu.roll(right, 4, 1))
        odd = jnp.where(sub3 < 4, pltpu.roll(left, 4, 1), right)
        return jnp.stack([even, odd], axis=1).reshape(NEP, 8, 128)

    def q_copies(k, device):
        return (
            rcopy(q_out.at[k], q_in.at[k], q_ssem, q_rsem.at[k], device),
            rcopy(s_out.at[k], s_in.at[k], sc_ssem, sc_rsem.at[k], device),
        )

    def q_pack(k, value):
        most = jnp.maximum(jnp.max(jnp.abs(value), axis=1, keepdims=True), 1e-30)
        q_out[k] = jnp.round(value * (32767.0 / most)).astype(jnp.int16)
        s_out[k] = column(most * (1.0 / 32767.0))

    def q_send(k):
        for copy in q_copies(k, ydev(NEAR[k])):
            copy.start()

    def q_get(k):
        for copy in q_copies(k, partner):
            copy.wait_recv()
        unit = jnp.sum(jnp.where(diagonal, s_in[k], 0.0), axis=1, keepdims=True)
        return q_in[k].astype(F32) * unit

    near2 = partials(NEAR[0], NEAR[1])
    values = partials(*FAR, 0)
    q_pack(0, near2[0])
    q_pack(1, near2[1])
    kept[...] = values[3]
    most = jnp.maximum(jnp.maximum(jnp.abs(values[0]), jnp.abs(values[1])), jnp.abs(values[2]))
    most = jnp.maximum(jnp.max(most, axis=1, keepdims=True), 1e-30)
    fs_out[...] = column(most * (1.0 / 32767.0))
    for i in range(3):
        fq_out[:, i] = messages(jnp.round(values[i] * (32767.0 / most))).astype(jnp.int16)
    q_send(0)
    q_send(1)
    for peer in peers:
        rcopy(fs_out, fs_in.at[me_e], fs_ssem, fs_rsem, (peer, me_t)).start()
    for peer in peers:
        rcopy(fq_out.at[peer], fq_in.at[me_e], fq_ssem, fq_rsem, (peer, me_t)).start()
    near1 = partials(NEAR[2], NEAR[3])
    q_pack(2, near1[0])
    q_pack(3, near1[1])
    q_send(2)
    q_send(3)
    fq_in[me_e] = fq_out[me_e]
    fs_in[me_e] = fs_out[...]
    done.append(arrived(dense_out, dense_in, dense_ssem, dense_rsem, NY - 1))
    dense = dense_in[0]
    for k in range(1, NY):
        dense = dense + dense_in[k]
    gate = gate_ref[...]
    dense = jnp.concatenate([gate, gate], axis=1) * dense
    summed = kept[...]
    for k in range(4):
        summed = summed + q_get(k)
    ret_out[...] = messages(summed)
    for peer in peers:
        rcopy(ret_out.at[peer], ret_in.at[me_e], ret_ssem, ret_rsem, (peer, me_t)).start()
    ret_in[me_e] = ret_out[me_e]
    done.append(arrived(fs_in, fs_in, fs_ssem, fs_rsem, NEP - 1))
    lane2 = lax.broadcasted_iota(jnp.int32, (128, 256), 1)
    mine4 = lax.broadcasted_iota(jnp.int32, (128, 256), 0) == me_e * 4 + lane2 % 4
    unit = jnp.dot(
        pieces(fs_in[...].reshape(NEP, 128), 0),
        jnp.where(mine4, 1.0, 0.0).astype(BF16),
        preferred_element_type=F32,
    )
    unit = unit[0:NEP] + unit[NEP : 2 * NEP] + unit[2 * NEP : 3 * NEP]
    source = lax.broadcasted_iota(jnp.int32, (NEP, 256), 0)
    source = source == lax.broadcasted_iota(jnp.int32, (NEP, 256), 1) // 8
    unit = jnp.sum(jnp.where(source, unit, 0.0), axis=0, keepdims=True)
    far_comb = pieces(comb[...] * unit, 0)
    near_comb = pieces(comb[...], 0)
    done.append(arrived(fq_out, fq_in, fq_ssem, fq_rsem, NEP - 1))
    far_rows = jnp.concatenate(
        [fq_in[:, i].astype(F32).reshape(256, 128) for i in range(3)], axis=1
    )
    far_high = far_rows.astype(BF16)
    far_low = (far_rows - far_high.astype(F32)).astype(BF16)
    far_sum = jnp.dot(far_comb, far_high, preferred_element_type=F32) + jnp.dot(
        far_comb, far_low, preferred_element_type=F32
    )
    far_sum = far_sum[0:16] + far_sum[16:32] + far_sum[32:48]
    for i, rel in enumerate(FAR):
        cols = slice(i * 128, (i + 1) * 128)
        fy_out[i, :, 0:128] = far_sum[0:8, cols]
        fy_out[i, :, 128:256] = far_sum[8:16, cols]
        rcopy(fy_out.at[i], fy_in.at[i], fy_ssem, fy_rsem, ydev(rel)).start()
    done.append(arrived(ret_out, ret_in, ret_ssem, ret_rsem, NEP - 1))
    mixed = jnp.dot(
        near_comb, pieces(ret_in[...].reshape(256, 128), 1), preferred_element_type=F32
    )
    mixed = mixed[:, 0:128] + mixed[:, 128:256] + mixed[:, 256:384]
    mixed = mixed[0:16] + mixed[16:32] + mixed[32:48]
    combined = jnp.concatenate([mixed[0:8], mixed[8:16]], axis=1) + dense
    fy_copy = rcopy(fy_out, fy_in, fy_ssem, fy_rsem, partner)
    fy_copy.wait_recv()
    combined = combined + fy_in[0] + fy_in[1] + fy_in[2]
    own = to_row(jnp.sum(combined * combined, axis=1, keepdims=True))
    sq_out[...] = own
    for step in y_order:
        for c in range(2):
            rcopy(sq_out, sq_in.at[me_t], sq_ssem, sq_rsem, (me_e, ys[step] * 2 + c)).start()
    rcopy(sq_out, sq_in.at[me_t], sq_ssem, sq_rsem, partner).start()
    sq_in[me_t] = own
    done.append(arrived(sq_in, sq_in, sq_ssem, sq_rsem, NTP - 1))
    total_sq = sq_in[0]
    for j in range(1, NTP):
        total_sq = total_sq + sq_in[j]
    final = lax.rsqrt(to_column(total_sq) / WIDTH + EPS)
    out[...] = (combined * final * ogain[...]).astype(BF16)

    near = gathered.at[core, pl.ds(0, 4)]
    done += [
        rcopy(near, near, ag_ssem, ag_rsem.at[0], partner),
        rcopy(q_out, q_in, q_ssem, q_rsem.at[0], partner),
        rcopy(s_out, s_in, sc_ssem, sc_rsem.at[0], partner),
    ]
    five = gathered.at[core, pl.ds(0, 5)]
    done.append(rcopy(five, five, pf_ssem, pf_rsem.at[0], partner))
    for copy in parts + [tok_copy, tok_pass, dh_copy, fy_copy] + raws + done:
        copy.wait_send()


def local(
    tokens,
    norm_gain,
    route_experts,
    route_logits,
    expert_gate,
    expert_up,
    expert_down,
    dense_gate,
    dense_up,
    dense_down,
    mix_weight,
    out_gain,
):
    vmem = pl.BlockSpec(memory_space=pltpu.VMEM)
    dma = pltpu.SemaphoreType.DMA
    return pl.pallas_call(
        kernel,
        out_shape=pltpu.VMEM((8, PART), BF16),
        in_specs=[pl.BlockSpec(memory_space=pl.ANY)] * 12,
        out_specs=vmem,
        scratch_shapes=[
            pltpu.VMEM((8, PART), BF16),
            pltpu.VMEM((1, WIDTH), F32),
            pltpu.SMEM((2, 8), jnp.int32),
            pltpu.SMEM((2, 8), F32),
            pltpu.VMEM((1, WIDTH), F32),
            pltpu.VMEM((1, PART), F32),
            pltpu.VMEM((2, 4, 64, WIDTH), BF16),
            pltpu.VMEM((NY, 2, 64, PART), BF16),
            pltpu.VMEM((NY, 2, 64, PART), BF16),
            pltpu.VMEM((128, WIDTH), BF16),
            pltpu.VMEM((NY, 64, PART), BF16),
            pltpu.VMEM((NY, 64, PART), BF16),
            pltpu.VMEM((NEP, 8, 128), BF16),
            pltpu.VMEM((NEP, 8, 128), BF16),
            pltpu.VMEM((NEP, 3, 8, 128), BF16),
            pltpu.VMEM((NEP, 3, 8, 128), BF16),
            pltpu.VMEM((NEP, 3, 8, 128), BF16),
            pltpu.VMEM((2, NY, ROWS, PART), BF16),
            pltpu.VMEM((2, NY, 8, PART), BF16),
            pltpu.VMEM((1, 128), F32),
            pltpu.VMEM((NTP, 1, 128), F32),
            pltpu.VMEM((NY, 8, PART), F32),
            pltpu.VMEM((NY, 8, PART), F32),
            pltpu.VMEM((8, 64), BF16),
            pltpu.VMEM((8, 64), BF16),
            pltpu.VMEM((16, 256), F32),
            pltpu.VMEM((16, 256), BF16),
            pltpu.VMEM((8, 128), F32),
            pltpu.VMEM((1, 128), F32),
            pltpu.VMEM((NEP, 1, 128), F32),
            pltpu.VMEM((ROWS, 512), F32),
            pltpu.VMEM((ROWS, 256), BF16),
            pltpu.VMEM((4, ROWS, PART), jnp.int16),
            pltpu.VMEM((4, ROWS, PART), jnp.int16),
            pltpu.VMEM((4, 1, 128), F32),
            pltpu.VMEM((4, 1, 128), F32),
            pltpu.VMEM((NEP, 3, 8, 128), jnp.int16),
            pltpu.VMEM((NEP, 3, 8, 128), jnp.int16),
            pltpu.VMEM((1, 128), F32),
            pltpu.VMEM((NEP, 1, 128), F32),
            pltpu.VMEM((3, 8, PART), F32),
            pltpu.VMEM((3, 8, PART), F32),
            pltpu.VMEM((ROWS, PART), F32),
            pltpu.VMEM((NEP, 8, 128), F32),
            pltpu.VMEM((NEP, 8, 128), F32),
            pltpu.VMEM((1, 128), F32),
            pltpu.VMEM((NTP, 1, 128), F32),
            pltpu.VMEM((8, 128), F32),
            dma((6,)),
            dma((4,)),
            dma((3,)),
            dma((3,)),
            dma,
            dma,
            dma,
            dma,
            dma,
            dma,
            dma,
            dma,
            dma,
            dma,
            dma,
            dma,
            dma,
            dma,
            dma,
            dma((4,)),
            dma,
            dma((5,)),
            dma,
            dma((3,)),
            dma,
            dma,
            dma,
            dma((4,)),
            dma,
            dma((4,)),
            dma,
            dma,
            dma,
            dma,
            dma,
            dma,
            dma,
            dma,
            dma,
            dma,
        ],
        compiler_params=pltpu.CompilerParams(
            collective_id=0, has_side_effects=True, vmem_limit_bytes=56650000
        ),
    )(
        tokens,
        norm_gain.reshape(1, WIDTH),
        route_experts.T,
        route_logits.T,
        jnp.swapaxes(expert_gate, 1, 2),
        jnp.swapaxes(expert_up, 1, 2),
        expert_down,
        dense_gate.T,
        dense_up.T,
        dense_down,
        mix_weight.reshape(1, WIDTH),
        out_gain.reshape(1, PART),
    )


def solution(mesh):
    tp = "tp"
    in_specs = (
        P("ep", tp),
        P(),
        P("ep", None),
        P("ep", None),
        P("ep", None, tp),
        P("ep", None, tp),
        P("ep", tp, None),
        P(None, tp),
        P(None, tp),
        P(tp, None),
        P(),
        P(tp),
    )
    return jax.shard_map(
        local, mesh=mesh, in_specs=in_specs, out_specs=P("ep", tp), check_vma=False
    )
```

```python
import functools

import jax
import jax.numpy as jnp
from jax import lax
from jax.experimental import pallas as pl
from jax.experimental.pallas import tpu as pltpu
from jax.sharding import PartitionSpec as P

MESH = pl.DeviceIdType.MESH
F32 = jnp.float32
BF16 = jnp.bfloat16
EPS = 1e-06

NX, NZ, NY = 4, 8, 8
NEP = NX * NZ
NTP = 2 * NY
ROWS = 128
FAR = (4, 3, 5)
NEAR = (6, 2, 7, 1)
PART = 256
WIDTH = 4096


def rcopy(src, dst, send_sem, recv_sem, device):
    return pltpu.make_async_remote_copy(
        src_ref=src,
        dst_ref=dst,
        send_sem=send_sem,
        recv_sem=recv_sem,
        device_id=device,
        device_id_type=MESH,
    )


def nt_dot(a, b):
    return lax.dot_general(a, b, (((1,), (1,)), ((), ())), preferred_element_type=F32)


def pieces(value, axis):
    high = value.astype(BF16)
    rest = value - high.astype(F32)
    middle = rest.astype(BF16)
    low = (rest - middle.astype(F32)).astype(BF16)
    return jnp.concatenate([high, middle, low], axis=axis)


def silu(v):
    return v / (1.0 + jnp.exp(-v))


def kernel(
    tok_hbm,
    gain_hbm,
    routes_hbm,
    logits_hbm,
    wg,
    wu,
    wd,
    dg,
    du,
    dd,
    mixw_hbm,
    ogain_hbm,
    out,
    tok,
    gain,
    routes,
    logits,
    mixw,
    ogain,
    w_gu,
    wd_own,
    wd_par,
    w_dense,
    dd_own,
    dd_par,
    a2a_out,
    a2a_in,
    far_out,
    far_in,
    far_par,
    gathered,
    tok_all,
    dense_out,
    dense_in,
    dh_own,
    dh_par,
    comb,
    place,
    slots,
    r_out,
    r_in,
    acts,
    hid,
    q_out,
    q_in,
    s_out,
    s_in,
    fq_out,
    fq_in,
    fs_out,
    fs_in,
    fy_out,
    fy_in,
    kept,
    ret_out,
    ret_in,
    sq_out,
    sq_in,
    gate_ref,
    i_sem,
    w_sem,
    wp_ssem,
    wp_rsem,
    a2a_ssem,
    a2a_rsem,
    far_ssem,
    far_rsem,
    tok_ssem,
    tok_rsem,
    dh_ssem,
    dh_rsem,
    dense_ssem,
    dense_rsem,
    ag_ssem,
    ag_rsem,
    pf_ssem,
    pf_rsem,
    fp_ssem,
    fp_rsem,
    r_ssem,
    r_rsem,
    q_ssem,
    q_rsem,
    sc_ssem,
    sc_rsem,
    fq_ssem,
    fq_rsem,
    fs_ssem,
    fs_rsem,
    fy_ssem,
    fy_rsem,
    ret_ssem,
    ret_rsem,
    sq_ssem,
    sq_rsem,
):
    me_e = lax.axis_index("ep")
    me_t = lax.axis_index("tp")
    z, x = lax.div(me_e, NX), lax.rem(me_e, NX)
    y, core = lax.div(me_t, 2), lax.rem(me_t, 2)
    other = 1 - core
    partner = (me_e, y * 2 + other)
    zs = [lax.rem(z + k, NZ) * NX for k in range(NZ)]
    xs = [lax.rem(x + k, NX) for k in range(NX)]
    ys = [lax.rem(y + k, NY) for k in range(NY)]
    peers = [zs[dz] + xs[dx] for dz in (4, 3, 5, 2, 6, 1, 7, 0) for dx in (2, 1, 3, 0)][:-1]
    y_order = (4, 3, 5, 2, 6, 1, 7)

    def ydev(step):
        return (me_e, ys[step % NY] * 2 + core)

    barrier = pltpu.get_barrier_semaphore()
    for peer in peers:
        pl.semaphore_signal(barrier, inc=1, device_id=(peer, me_t), device_id_type=MESH)
    for step in y_order:
        for c in range(2):
            pl.semaphore_signal(
                barrier, inc=1, device_id=(me_e, ys[step] * 2 + c), device_id_type=MESH
            )
    pl.semaphore_signal(barrier, inc=1, device_id=partner, device_id_type=MESH)

    smalls = [
        pltpu.make_async_copy(routes_hbm, routes, i_sem.at[0]),
        pltpu.make_async_copy(logits_hbm, logits, i_sem.at[1]),
        pltpu.make_async_copy(tok_hbm, tok, i_sem.at[2]),
        pltpu.make_async_copy(gain_hbm, gain, i_sem.at[3]),
        pltpu.make_async_copy(mixw_hbm, mixw, i_sem.at[4]),
        pltpu.make_async_copy(ogain_hbm, ogain, i_sem.at[5]),
    ]

    def columns(k, c):
        return pl.ds(pl.multiple_of((2 * k + c) * PART, PART), PART)

    def load(src, dst, k):
        pltpu.make_async_copy(src, dst, w_sem.at[k]).start()

    def loaded(dst, k):
        pltpu.make_async_copy(dst, dst, w_sem.at[k]).wait()

    for copy in smalls:
        copy.start()
    load(dg, w_dense.at[pl.ds(0, 64)], 0)
    load(du, w_dense.at[pl.ds(64, 64)], 0)
    for k in range(NY):
        load(dd.at[:, columns(k, core)], dd_own.at[k], 1)
    load(wg, w_gu.at[0, pl.ds(0, 2)], 2)
    load(wu, w_gu.at[0, pl.ds(2, 2)], 2)
    for k in range(NY):
        load(wd.at[:, :, columns(k, core)], wd_own.at[k], 3)

    for copy in smalls[0:3]:
        copy.wait()
    lane = lax.broadcasted_iota(jnp.int32, (8, 256), 1)
    sub = lax.broadcasted_iota(jnp.int32, (8, 256), 0)
    expert = 2 * (lane // 8) + (lane // 2) % 2
    half = (lane // 4) % 2
    r0 = jnp.zeros((8, 256), jnp.int32)
    r1 = jnp.zeros((8, 256), jnp.int32)
    l0 = jnp.zeros((8, 256), F32)
    l1 = jnp.zeros((8, 256), F32)
    for t in range(8):
        r0 = jnp.where(sub == t, routes[0, t], r0)
        r1 = jnp.where(sub == t, routes[1, t], r1)
        l0 = jnp.where(sub == t, logits[0, t], l0)
        l1 = jnp.where(sub == t, logits[1, t], l1)
    top = jnp.maximum(l0, l1)
    e0, e1 = jnp.exp(l0 - top), jnp.exp(l1 - top)
    is0, is1 = (r0 == expert), (r1 == expert)
    hit = jnp.where(is0, 1.0, 0.0) + jnp.where(is1, 1.0, 0.0)
    before = jnp.zeros((8, 256), F32)
    for t in range(7):
        before = before + jnp.where(sub > t, hit[t : t + 1, :], 0.0)
    placed = jnp.where(before == (lane % 2).astype(F32), hit, 0.0)
    weight = (jnp.where(is0, e0, 0.0) + jnp.where(is1, e1, 0.0)) / (e0 + e1) * placed
    comb[0:8, :] = jnp.where(half == 0, weight, 0.0)
    comb[8:16, :] = jnp.where(half == 1, weight, 0.0)
    left_half = lax.broadcasted_iota(jnp.int32, (256, 128), 0)
    slot = lax.broadcasted_iota(jnp.int32, (256, 128), 1)
    left_half = (left_half // 8 == slot // 4) & (left_half % 8 == slot % 4)
    slots[...] = jnp.dot(
        placed.astype(BF16),
        jnp.where(left_half, 1.0, 0.0).astype(BF16),
        preferred_element_type=F32,
    )
    place[...] = jnp.concatenate(
        [jnp.where(half == 0, placed, 0.0), jnp.where(half == 1, placed, 0.0)], axis=0
    ).astype(BF16)

    def placed_rows(value):
        halves = jnp.concatenate(
            [value[:, 0:128].astype(F32), value[:, 128:256].astype(F32)], axis=0
        ).astype(BF16)
        rows = lax.dot_general(
            place[...], halves, (((0,), (0,)), ((), ())), preferred_element_type=F32
        )
        return rows.astype(BF16).reshape(NEP, 8, 128)

    tok_value = tok[...]
    a2a_out[...] = placed_rows(tok_value)
    a2a_in[me_e] = a2a_out[me_e]
    tok_all[me_t] = tok_value

    pl.semaphore_wait(barrier, NEP - 1 + NTP - 1)

    for step in y_order:
        for c in range(2):
            rcopy(
                tok, tok_all.at[me_t], tok_ssem, tok_rsem, (me_e, ys[step] * 2 + c)
            ).start()
    rcopy(tok, tok_all.at[me_t], tok_ssem, tok_rsem, partner).start()

    for peer in peers:
        rcopy(a2a_out.at[peer], a2a_in.at[me_e], a2a_ssem, a2a_rsem, (peer, me_t)).start()

    for k in range(NY):
        rcopy(
            dd.at[:, columns(k, other)], dd_par.at[k], wp_ssem.at[0], wp_rsem.at[0], partner
        ).start()
    for k, ref in enumerate((wg, wu)):
        rcopy(
            ref, w_gu.at[1, pl.ds(2 * k, 2)], wp_ssem.at[1], wp_rsem.at[1], partner
        ).start()
    for k in range(NY):
        rcopy(
            wd.at[:, :, columns(k, other)], wd_par.at[k], wp_ssem.at[2], wp_rsem.at[2], partner
        ).start()
    parts = [
        rcopy(ref, ref, wp_ssem.at[k], wp_rsem.at[k], partner)
        for k, ref in enumerate((dd_par, w_gu.at[1], wd_par))
    ]

    def arrived(src, dst, ssem, rsem, n):
        part = pl.ds(0, n)
        copy = rcopy(src.at[part], dst.at[part], ssem, rsem, partner)
        copy.wait_recv()
        return copy

    done = [arrived(tok_all, tok_all, tok_ssem, tok_rsem, NTP - 1)]
    squares = jnp.zeros((8, PART), F32)
    for j in range(NTP):
        v = tok_all[j].astype(F32)
        squares = squares + v * v
    scale = lax.rsqrt(jnp.sum(squares, axis=1, keepdims=True) / WIDTH + EPS)
    r_out[...] = jnp.sum(slots[...] * scale, axis=0, keepdims=True)
    for i, rel in enumerate(FAR):
        far_out[:, i] = placed_rows(tok_all[ys[rel] * 2 + core])
    for peer in peers:
        rcopy(r_out, r_in.at[me_e], r_ssem, r_rsem, (peer, me_t)).start()
    for peer in peers:
        rcopy(far_out.at[peer], far_in.at[me_e], far_ssem, far_rsem, (peer, me_t)).start()
    r_in[me_e] = r_out[...]
    far_in[me_e] = far_out[me_e]

    done.append(arrived(a2a_out, a2a_in, a2a_ssem, a2a_rsem, NEP - 1))
    sub3 = lax.broadcasted_iota(jnp.int32, (16, 8, 128), 1)

    def keep_rows(value, c, rel):
        pairs = value.astype(F32).reshape(16, 2, 8, 128)
        even, odd = pairs[:, 0], pairs[:, 1]
        left = jnp.where(sub3 < 4, even, pltpu.roll(odd, 4, 1)).reshape(ROWS, 128)
        right = jnp.where(sub3 < 4, pltpu.roll(even, 4, 1), odd).reshape(ROWS, 128)
        gathered[c, ys[rel], :, 0:128] = left.astype(BF16)
        gathered[c, ys[rel], :, 128:256] = right.astype(BF16)

    keep_rows(a2a_in[...], core, 0)

    def ag_copy(slot, k, device):
        ref = gathered.at[core, ys[slot]]
        return rcopy(ref, ref, ag_ssem, ag_rsem.at[k], device)

    for k, step in enumerate((2, -2, 1, -1)):
        ag_copy(0, k, ydev(step)).start()

    def pass_copy(c, rel):
        ref = gathered.at[c, ys[rel]]
        k = ((0,) + NEAR).index(rel)
        return rcopy(ref, ref, pf_ssem, pf_rsem.at[k], partner)

    def pass_on(rel):
        pass_copy(core, rel).start()

    def pass_wait(rel):
        pass_copy(other, rel).wait_recv()

    pass_on(0)

    for copy in smalls[3:6]:
        copy.wait()
    loaded(w_dense, 0)
    act = jnp.zeros((8, 128), F32)
    mix_acc = jnp.zeros((8, PART), F32)
    for j in range(NTP):
        cols = slice(j * PART, (j + 1) * PART)
        n = (tok_all[j].astype(F32) * scale * gain[:, cols]).astype(BF16)
        mix_acc = mix_acc + n.astype(F32) * mixw[:, cols]
        act = act + nt_dot(n, w_dense[:, cols])
    gate_ref[...] = jnp.broadcast_to(
        jax.nn.sigmoid(jnp.sum(mix_acc, axis=1, keepdims=True)), (8, 128)
    )
    dh_own[...] = (silu(act[:, 0:64]) * act[:, 64:128]).astype(BF16)
    dh_copy = rcopy(dh_own, dh_par, dh_ssem, dh_rsem, partner)
    dh_copy.start()

    loaded(dd_own, 1)
    parts[0].wait_recv()
    dh_copy.wait_recv()
    for k in range(NY):
        dense_out[k] = jnp.dot(
            dh_own[...], dd_own[k], preferred_element_type=F32
        ) + jnp.dot(dh_par[...], dd_par[k], preferred_element_type=F32)
    dense_in[y] = dense_out[y]
    loaded(w_gu.at[0], 2)
    parts[1].wait_recv()
    for rel in (6, 2):
        ag_copy(rel, NEAR.index(rel), partner).wait_recv()
        pass_on(rel)
    done.append(arrived(r_in, r_in, r_ssem, r_rsem, NEP - 1))
    picked = (
        lax.broadcasted_iota(jnp.int32, (ROWS, NEP), 0) // 4
        == lax.broadcasted_iota(jnp.int32, (ROWS, NEP), 1)
    )
    spread = jnp.dot(
        jnp.where(picked, 1.0, 0.0).astype(BF16),
        pieces(r_in[...].reshape(NEP, 128), 1),
        preferred_element_type=F32,
    )
    spread = spread[:, 0:128] + spread[:, 128:256] + spread[:, 256:384]
    wanted = me_e * 4 + lax.broadcasted_iota(jnp.int32, (ROWS, 128), 0) % 4
    here = lax.broadcasted_iota(jnp.int32, (ROWS, 128), 1) == wanted
    row_scale = jnp.sum(jnp.where(here, spread, 0.0), axis=1, keepdims=True)

    def project(*slices, first=False):
        total = None
        for c, rel in slices:
            cols = pl.ds(pl.multiple_of((2 * ys[rel] + c) * PART, PART), PART)
            n = (gathered[c, ys[rel]].astype(F32) * row_scale * gain[:, cols]).astype(BF16)
            v = nt_dot(n, w_gu[:, :, :, cols].reshape(512, PART))
            total = v if total is None else total + v
        acts[...] = total if first else acts[...] + total

    pass_wait(0)
    project((core, 0), (other, 0), (core, 6), (core, 2), first=True)
    for rel in (7, 1):
        ag_copy(rel, NEAR.index(rel), partner).wait_recv()
        pass_on(rel)
    for step in y_order:
        rcopy(
            dense_out.at[ys[step]], dense_in.at[y], dense_ssem, dense_rsem, ydev(step)
        ).start()
    pass_wait(6)
    pass_wait(2)
    project((core, 7), (core, 1), (other, 6), (other, 2))
    done.append(arrived(far_out, far_in, far_ssem, far_rsem, NEP - 1))
    raws = [
        rcopy(far_in.at[:, i], far_par.at[:, i], fp_ssem, fp_rsem.at[i], partner)
        for i in range(3)
    ]
    for copy in raws:
        copy.start()
    for i, rel in enumerate(FAR):
        keep_rows(far_in[:, i], core, rel)
    project((core, 3), (core, 4), (core, 5))
    pass_wait(7)
    pass_wait(1)
    project((other, 7), (other, 1))
    for i in range(2):
        raws[i].wait_recv()
        keep_rows(far_par[:, i], other, FAR[i])
    project((other, 3), (other, 4))
    raws[2].wait_recv()
    keep_rows(far_par[:, 2], other, FAR[2])
    project((other, 5))

    row = lax.broadcasted_iota(jnp.int32, (ROWS, 128), 0)
    col = lax.broadcasted_iota(jnp.int32, (ROWS, 128), 1)
    mine = (row // 2) % 2 == col // 64
    for k in range(2):
        v = acts[:, k * 256 : (k + 1) * 256]
        hidden = silu(v[:, 0:128]) * v[:, 128:256]
        hid[:, k * 128 : (k + 1) * 128] = jnp.where(mine, hidden, 0.0).astype(BF16)
    loaded(wd_own, 3)
    parts[2].wait_recv()

    diagonal = row == col

    def partials(*rels):
        both = jnp.concatenate(
            [
                jnp.concatenate([w[ys[rel]].reshape(128, PART) for rel in rels], axis=1)
                for w in (wd_own, wd_par)
            ],
            axis=0,
        )
        v = jnp.dot(hid[...], both, preferred_element_type=F32)
        return [v[:, i * PART : (i + 1) * PART] for i in range(len(rels))]

    def column(value):
        return jnp.sum(jnp.where(diagonal, value, 0.0), axis=0, keepdims=True)

    def messages(value):
        left = value[:, 0:128].reshape(16, 8, 128)
        right = value[:, 128:256].reshape(16, 8, 128)
        even = jnp.where(sub3 < 4, left, pltpu.roll(right, 4, 1))
        odd = jnp.where(sub3 < 4, pltpu.roll(left, 4, 1), right)
        return jnp.stack([even, odd], axis=1).reshape(NEP, 8, 128)

    def q_copies(k, device):
        return (
            rcopy(q_out.at[k], q_in.at[k], q_ssem, q_rsem.at[k], device),
            rcopy(s_out.at[k], s_in.at[k], sc_ssem, sc_rsem.at[k], device),
        )

    def q_pack(k, value):
        most = jnp.maximum(jnp.max(jnp.abs(value), axis=1, keepdims=True), 1e-30)
        q_out[k] = jnp.round(value * (32767.0 / most)).astype(jnp.int16)
        s_out[k] = column(most * (1.0 / 32767.0))

    def q_send(k):
        for copy in q_copies(k, ydev(NEAR[k])):
            copy.start()

    def q_get(k):
        for copy in q_copies(k, partner):
            copy.wait_recv()
        unit = jnp.sum(jnp.where(diagonal, s_in[k], 0.0), axis=1, keepdims=True)
        return q_in[k].astype(F32) * unit

    near2 = partials(NEAR[0], NEAR[1])
    values = partials(*FAR, 0)
    q_pack(0, near2[0])
    q_pack(1, near2[1])
    kept[...] = values[3]
    most = jnp.maximum(jnp.maximum(jnp.abs(values[0]), jnp.abs(values[1])), jnp.abs(values[2]))
    most = jnp.maximum(jnp.max(most, axis=1, keepdims=True), 1e-30)
    fs_out[...] = column(most * (1.0 / 32767.0))
    for i in range(3):
        fq_out[:, i] = messages(jnp.round(values[i] * (32767.0 / most))).astype(jnp.int16)
    q_send(0)
    q_send(1)
    for peer in peers:
        rcopy(fs_out, fs_in.at[me_e], fs_ssem, fs_rsem, (peer, me_t)).start()
    for peer in peers:
        rcopy(fq_out.at[peer], fq_in.at[me_e], fq_ssem, fq_rsem, (peer, me_t)).start()
    near1 = partials(NEAR[2], NEAR[3])
    q_pack(2, near1[0])
    q_pack(3, near1[1])
    q_send(2)
    q_send(3)
    fq_in[me_e] = fq_out[me_e]
    fs_in[me_e] = fs_out[...]
    done.append(arrived(dense_out, dense_in, dense_ssem, dense_rsem, NY - 1))
    dense = dense_in[0]
    for k in range(1, NY):
        dense = dense + dense_in[k]
    gate = gate_ref[...]
    dense = jnp.concatenate([gate, gate], axis=1) * dense
    summed = kept[...]
    for k in range(4):
        summed = summed + q_get(k)
    ret_out[...] = messages(summed)
    for peer in peers:
        rcopy(ret_out.at[peer], ret_in.at[me_e], ret_ssem, ret_rsem, (peer, me_t)).start()
    ret_in[me_e] = ret_out[me_e]
    done.append(arrived(fs_in, fs_in, fs_ssem, fs_rsem, NEP - 1))
    lane2 = lax.broadcasted_iota(jnp.int32, (128, 256), 1)
    mine4 = lax.broadcasted_iota(jnp.int32, (128, 256), 0) == me_e * 4 + lane2 % 4
    unit = jnp.dot(
        pieces(fs_in[...].reshape(NEP, 128), 0),
        jnp.where(mine4, 1.0, 0.0).astype(BF16),
        preferred_element_type=F32,
    )
    unit = unit[0:NEP] + unit[NEP : 2 * NEP] + unit[2 * NEP : 3 * NEP]
    source = lax.broadcasted_iota(jnp.int32, (NEP, 256), 0)
    source = source == lax.broadcasted_iota(jnp.int32, (NEP, 256), 1) // 8
    unit = jnp.sum(jnp.where(source, unit, 0.0), axis=0, keepdims=True)
    far_comb = pieces(comb[...] * unit, 0)
    near_comb = pieces(comb[...], 0)
    done.append(arrived(fq_out, fq_in, fq_ssem, fq_rsem, NEP - 1))
    far_rows = jnp.concatenate(
        [fq_in[:, i].astype(F32).reshape(256, 128) for i in range(3)], axis=1
    )
    far_high = far_rows.astype(BF16)
    far_low = (far_rows - far_high.astype(F32)).astype(BF16)
    far_sum = jnp.dot(far_comb, far_high, preferred_element_type=F32) + jnp.dot(
        far_comb, far_low, preferred_element_type=F32
    )
    far_sum = far_sum[0:16] + far_sum[16:32] + far_sum[32:48]
    for i, rel in enumerate(FAR):
        cols = slice(i * 128, (i + 1) * 128)
        fy_out[i, :, 0:128] = far_sum[0:8, cols]
        fy_out[i, :, 128:256] = far_sum[8:16, cols]
        rcopy(fy_out.at[i], fy_in.at[i], fy_ssem, fy_rsem, ydev(rel)).start()
    done.append(arrived(ret_out, ret_in, ret_ssem, ret_rsem, NEP - 1))
    mixed = jnp.dot(
        near_comb, pieces(ret_in[...].reshape(256, 128), 1), preferred_element_type=F32
    )
    mixed = mixed[:, 0:128] + mixed[:, 128:256] + mixed[:, 256:384]
    mixed = mixed[0:16] + mixed[16:32] + mixed[32:48]
    combined = jnp.concatenate([mixed[0:8], mixed[8:16]], axis=1) + dense
    fy_copy = rcopy(fy_out, fy_in, fy_ssem, fy_rsem, partner)
    fy_copy.wait_recv()
    combined = combined + fy_in[0] + fy_in[1] + fy_in[2]
    token_diagonal = (
        lax.broadcasted_iota(jnp.int32, (8, 128), 0)
        == lax.broadcasted_iota(jnp.int32, (8, 128), 1)
    )
    own = jnp.sum(
        jnp.where(token_diagonal, jnp.sum(combined * combined, axis=1, keepdims=True), 0.0),
        axis=0,
        keepdims=True,
    )
    sq_out[...] = own
    for step in y_order:
        for c in range(2):
            rcopy(sq_out, sq_in.at[me_t], sq_ssem, sq_rsem, (me_e, ys[step] * 2 + c)).start()
    rcopy(sq_out, sq_in.at[me_t], sq_ssem, sq_rsem, partner).start()
    sq_in[me_t] = own
    done.append(arrived(sq_in, sq_in, sq_ssem, sq_rsem, NTP - 1))
    total_sq = sq_in[0]
    for j in range(1, NTP):
        total_sq = total_sq + sq_in[j]
    final = lax.rsqrt(
        jnp.sum(jnp.where(token_diagonal, total_sq, 0.0), axis=1, keepdims=True) / WIDTH + EPS
    )
    out[...] = (combined * final * ogain[...]).astype(BF16)

    near = gathered.at[core, pl.ds(0, 4)]
    done += [
        rcopy(near, near, ag_ssem, ag_rsem.at[0], partner),
        rcopy(q_out, q_in, q_ssem, q_rsem.at[0], partner),
        rcopy(s_out, s_in, sc_ssem, sc_rsem.at[0], partner),
    ]
    five = gathered.at[core, pl.ds(0, 5)]
    done.append(rcopy(five, five, pf_ssem, pf_rsem.at[0], partner))
    for copy in parts + [dh_copy, fy_copy] + raws + done:
        copy.wait_send()


def local(
    tokens,
    norm_gain,
    route_experts,
    route_logits,
    expert_gate,
    expert_up,
    expert_down,
    dense_gate,
    dense_up,
    dense_down,
    mix_weight,
    out_gain,
):
    vmem = pl.BlockSpec(memory_space=pltpu.VMEM)
    dma = pltpu.SemaphoreType.DMA
    return pl.pallas_call(
        kernel,
        out_shape=pltpu.VMEM((8, PART), BF16),
        in_specs=[pl.BlockSpec(memory_space=pl.ANY)] * 12,
        out_specs=vmem,
        scratch_shapes=[
            pltpu.VMEM((8, PART), BF16),
            pltpu.VMEM((1, WIDTH), F32),
            pltpu.SMEM((2, 8), jnp.int32),
            pltpu.SMEM((2, 8), F32),
            pltpu.VMEM((1, WIDTH), F32),
            pltpu.VMEM((1, PART), F32),
            pltpu.VMEM((2, 4, 64, WIDTH), BF16),
            pltpu.VMEM((NY, 2, 64, PART), BF16),
            pltpu.VMEM((NY, 2, 64, PART), BF16),
            pltpu.VMEM((128, WIDTH), BF16),
            pltpu.VMEM((NY, 64, PART), BF16),
            pltpu.VMEM((NY, 64, PART), BF16),
            pltpu.VMEM((NEP, 8, 128), BF16),
            pltpu.VMEM((NEP, 8, 128), BF16),
            pltpu.VMEM((NEP, 3, 8, 128), BF16),
            pltpu.VMEM((NEP, 3, 8, 128), BF16),
            pltpu.VMEM((NEP, 3, 8, 128), BF16),
            pltpu.VMEM((2, NY, ROWS, PART), BF16),
            pltpu.VMEM((NTP, 8, PART), BF16),
            pltpu.VMEM((NY, 8, PART), F32),
            pltpu.VMEM((NY, 8, PART), F32),
            pltpu.VMEM((8, 64), BF16),
            pltpu.VMEM((8, 64), BF16),
            pltpu.VMEM((16, 256), F32),
            pltpu.VMEM((16, 256), BF16),
            pltpu.VMEM((8, 128), F32),
            pltpu.VMEM((1, 128), F32),
            pltpu.VMEM((NEP, 1, 128), F32),
            pltpu.VMEM((ROWS, 512), F32),
            pltpu.VMEM((ROWS, 256), BF16),
            pltpu.VMEM((4, ROWS, PART), jnp.int16),
            pltpu.VMEM((4, ROWS, PART), jnp.int16),
            pltpu.VMEM((4, 1, 128), F32),
            pltpu.VMEM((4, 1, 128), F32),
            pltpu.VMEM((NEP, 3, 8, 128), jnp.int16),
            pltpu.VMEM((NEP, 3, 8, 128), jnp.int16),
            pltpu.VMEM((1, 128), F32),
            pltpu.VMEM((NEP, 1, 128), F32),
            pltpu.VMEM((3, 8, PART), F32),
            pltpu.VMEM((3, 8, PART), F32),
            pltpu.VMEM((ROWS, PART), F32),
            pltpu.VMEM((NEP, 8, 128), F32),
            pltpu.VMEM((NEP, 8, 128), F32),
            pltpu.VMEM((1, 128), F32),
            pltpu.VMEM((NTP, 1, 128), F32),
            pltpu.VMEM((8, 128), F32),
            dma((6,)),
            dma((4,)),
            dma((3,)),
            dma((3,)),
            dma,
            dma,
            dma,
            dma,
            dma,
            dma,
            dma,
            dma,
            dma,
            dma,
            dma,
            dma((4,)),
            dma,
            dma((5,)),
            dma,
            dma((3,)),
            dma,
            dma,
            dma,
            dma((4,)),
            dma,
            dma((4,)),
            dma,
            dma,
            dma,
            dma,
            dma,
            dma,
            dma,
            dma,
            dma,
            dma,
        ],
        compiler_params=pltpu.CompilerParams(
            collective_id=0, has_side_effects=True, vmem_limit_bytes=56650000
        ),
    )(
        tokens,
        norm_gain.reshape(1, WIDTH),
        route_experts.T,
        route_logits.T,
        jnp.swapaxes(expert_gate, 1, 2),
        jnp.swapaxes(expert_up, 1, 2),
        expert_down,
        dense_gate.T,
        dense_up.T,
        dense_down,
        mix_weight.reshape(1, WIDTH),
        out_gain.reshape(1, PART),
    )


def solution(mesh):
    tp = "tp"
    in_specs = (
        P("ep", tp),
        P(),
        P("ep", None),
        P("ep", None),
        P("ep", None, tp),
        P("ep", None, tp),
        P("ep", tp, None),
        P(None, tp),
        P(None, tp),
        P(tp, None),
        P(),
        P(tp),
    )
    return jax.shard_map(
        local, mesh=mesh, in_specs=in_specs, out_specs=P("ep", tp), check_vma=False
    )
```

```python
import functools

import jax
import jax.numpy as jnp
from jax import lax
from jax.experimental import pallas as pl
from jax.experimental.pallas import tpu as pltpu
from jax.sharding import PartitionSpec as P

MESH = pl.DeviceIdType.MESH
F32 = jnp.float32
BF16 = jnp.bfloat16
EPS = 1e-06

NX, NZ, NY = 4, 8, 8
NEP = NX * NZ
NTP = 2 * NY
ROWS = 128
FAR = (3, 4, 5)
NEAR = (6, 2, 7, 1)
PART = 256
WIDTH = 4096


def rcopy(src, dst, send_sem, recv_sem, device):
    return pltpu.make_async_remote_copy(
        src_ref=src,
        dst_ref=dst,
        send_sem=send_sem,
        recv_sem=recv_sem,
        device_id=device,
        device_id_type=MESH,
    )


def nt_dot(a, b):
    return lax.dot_general(a, b, (((1,), (1,)), ((), ())), preferred_element_type=F32)


def pieces(value, axis):
    high = value.astype(BF16)
    rest = value - high.astype(F32)
    middle = rest.astype(BF16)
    low = (rest - middle.astype(F32)).astype(BF16)
    return jnp.concatenate([high, middle, low], axis=axis)


def silu(v):
    return v / (1.0 + jnp.exp(-v))


def kernel(
    tok_hbm,
    gain_hbm,
    routes_hbm,
    logits_hbm,
    wg,
    wu,
    wd,
    dg,
    du,
    dd,
    mixw_hbm,
    ogain_hbm,
    out,
    tok,
    gain,
    routes,
    logits,
    mixw,
    ogain,
    w_gu,
    wd_own,
    wd_par,
    w_dense,
    dd_own,
    dd_par,
    a2a_out,
    a2a_in,
    far_out,
    far_in,
    far_par,
    gathered,
    tok_all,
    dense_out,
    dense_in,
    dh_own,
    dh_par,
    comb,
    place,
    slots,
    r_out,
    r_in,
    acts,
    hid,
    q_out,
    q_in,
    s_out,
    s_in,
    fq_out,
    fq_in,
    fs_out,
    fs_in,
    fy_out,
    fy_in,
    kept,
    ret_out,
    ret_in,
    sq_out,
    sq_in,
    gate_ref,
    i_sem,
    w_sem,
    wp_ssem,
    wp_rsem,
    a2a_ssem,
    a2a_rsem,
    far_ssem,
    far_rsem,
    tok_ssem,
    tok_rsem,
    dh_ssem,
    dh_rsem,
    dense_ssem,
    dense_rsem,
    ag_ssem,
    ag_rsem,
    pf_ssem,
    pf_rsem,
    fp_ssem,
    fp_rsem,
    r_ssem,
    r_rsem,
    q_ssem,
    q_rsem,
    sc_ssem,
    sc_rsem,
    fq_ssem,
    fq_rsem,
    fs_ssem,
    fs_rsem,
    fy_ssem,
    fy_rsem,
    ret_ssem,
    ret_rsem,
    sq_ssem,
    sq_rsem,
):
    me_e = lax.axis_index("ep")
    me_t = lax.axis_index("tp")
    z, x = lax.div(me_e, NX), lax.rem(me_e, NX)
    y, core = lax.div(me_t, 2), lax.rem(me_t, 2)
    other = 1 - core
    partner = (me_e, y * 2 + other)
    zs = [lax.rem(z + k, NZ) * NX for k in range(NZ)]
    xs = [lax.rem(x + k, NX) for k in range(NX)]
    ys = [lax.rem(y + k, NY) for k in range(NY)]
    peers = [zs[dz] + xs[dx] for dz in (4, 3, 5, 2, 6, 1, 7, 0) for dx in (2, 1, 3, 0)][:-1]
    y_order = (4, 3, 5, 2, 6, 1, 7)

    def ydev(step):
        return (me_e, ys[step % NY] * 2 + core)

    barrier = pltpu.get_barrier_semaphore()
    for peer in peers:
        pl.semaphore_signal(barrier, inc=1, device_id=(peer, me_t), device_id_type=MESH)
    for step in y_order:
        for c in range(2):
            pl.semaphore_signal(
                barrier, inc=1, device_id=(me_e, ys[step] * 2 + c), device_id_type=MESH
            )
    pl.semaphore_signal(barrier, inc=1, device_id=partner, device_id_type=MESH)

    smalls = [
        pltpu.make_async_copy(routes_hbm, routes, i_sem.at[0]),
        pltpu.make_async_copy(logits_hbm, logits, i_sem.at[1]),
        pltpu.make_async_copy(tok_hbm, tok, i_sem.at[2]),
        pltpu.make_async_copy(gain_hbm, gain, i_sem.at[3]),
        pltpu.make_async_copy(mixw_hbm, mixw, i_sem.at[4]),
        pltpu.make_async_copy(ogain_hbm, ogain, i_sem.at[5]),
    ]

    def columns(k, c):
        return pl.ds(pl.multiple_of((2 * k + c) * PART, PART), PART)

    def load(src, dst, k):
        pltpu.make_async_copy(src, dst, w_sem.at[k]).start()

    def loaded(dst, k):
        pltpu.make_async_copy(dst, dst, w_sem.at[k]).wait()

    for copy in smalls:
        copy.start()
    load(dg, w_dense.at[pl.ds(0, 64)], 0)
    load(du, w_dense.at[pl.ds(64, 64)], 0)
    for k in range(NY):
        load(dd.at[:, columns(k, core)], dd_own.at[k], 1)
    load(wg, w_gu.at[0, pl.ds(0, 2)], 2)
    load(wu, w_gu.at[0, pl.ds(2, 2)], 2)
    for k in range(NY):
        load(wd.at[:, :, columns(k, core)], wd_own.at[k], 3)

    for copy in smalls[0:3]:
        copy.wait()
    lane = lax.broadcasted_iota(jnp.int32, (8, 256), 1)
    sub = lax.broadcasted_iota(jnp.int32, (8, 256), 0)
    expert = 2 * (lane // 8) + (lane // 2) % 2
    half = (lane // 4) % 2
    r0 = jnp.zeros((8, 256), jnp.int32)
    r1 = jnp.zeros((8, 256), jnp.int32)
    l0 = jnp.zeros((8, 256), F32)
    l1 = jnp.zeros((8, 256), F32)
    for t in range(8):
        r0 = jnp.where(sub == t, routes[0, t], r0)
        r1 = jnp.where(sub == t, routes[1, t], r1)
        l0 = jnp.where(sub == t, logits[0, t], l0)
        l1 = jnp.where(sub == t, logits[1, t], l1)
    top = jnp.maximum(l0, l1)
    e0, e1 = jnp.exp(l0 - top), jnp.exp(l1 - top)
    is0, is1 = (r0 == expert), (r1 == expert)
    hit = jnp.where(is0, 1.0, 0.0) + jnp.where(is1, 1.0, 0.0)
    before = jnp.zeros((8, 256), F32)
    for t in range(7):
        before = before + jnp.where(sub > t, hit[t : t + 1, :], 0.0)
    placed = jnp.where(before == (lane % 2).astype(F32), hit, 0.0)
    weight = (jnp.where(is0, e0, 0.0) + jnp.where(is1, e1, 0.0)) / (e0 + e1) * placed
    comb[0:8, :] = jnp.where(half == 0, weight, 0.0)
    comb[8:16, :] = jnp.where(half == 1, weight, 0.0)
    left_half = lax.broadcasted_iota(jnp.int32, (256, 128), 0)
    slot = lax.broadcasted_iota(jnp.int32, (256, 128), 1)
    left_half = (left_half // 8 == slot // 4) & (left_half % 8 == slot % 4)
    slots[...] = jnp.dot(
        placed.astype(BF16),
        jnp.where(left_half, 1.0, 0.0).astype(BF16),
        preferred_element_type=F32,
    )
    place[...] = jnp.concatenate(
        [jnp.where(half == 0, placed, 0.0), jnp.where(half == 1, placed, 0.0)], axis=0
    ).astype(BF16)

    def placed_rows(value):
        halves = jnp.concatenate(
            [value[:, 0:128].astype(F32), value[:, 128:256].astype(F32)], axis=0
        ).astype(BF16)
        rows = lax.dot_general(
            place[...], halves, (((0,), (0,)), ((), ())), preferred_element_type=F32
        )
        return rows.astype(BF16).reshape(NEP, 8, 128)

    tok_value = tok[...]
    a2a_out[...] = placed_rows(tok_value)
    a2a_in[me_e] = a2a_out[me_e]
    tok_all[me_t] = tok_value

    pl.semaphore_wait(barrier, NEP - 1 + NTP - 1)

    for step in y_order:
        for c in range(2):
            rcopy(
                tok, tok_all.at[me_t], tok_ssem, tok_rsem, (me_e, ys[step] * 2 + c)
            ).start()
    rcopy(tok, tok_all.at[me_t], tok_ssem, tok_rsem, partner).start()

    for peer in peers:
        rcopy(a2a_out.at[peer], a2a_in.at[me_e], a2a_ssem, a2a_rsem, (peer, me_t)).start()

    for k in range(NY):
        rcopy(
            dd.at[:, columns(k, other)], dd_par.at[k], wp_ssem.at[0], wp_rsem.at[0], partner
        ).start()
    for k, ref in enumerate((wg, wu)):
        rcopy(
            ref, w_gu.at[1, pl.ds(2 * k, 2)], wp_ssem.at[1], wp_rsem.at[1], partner
        ).start()
    for k in range(NY):
        rcopy(
            wd.at[:, :, columns(k, other)], wd_par.at[k], wp_ssem.at[2], wp_rsem.at[2], partner
        ).start()
    parts = [
        rcopy(ref, ref, wp_ssem.at[k], wp_rsem.at[k], partner)
        for k, ref in enumerate((dd_par, w_gu.at[1], wd_par))
    ]

    def arrived(src, dst, ssem, rsem, n):
        part = pl.ds(0, n)
        copy = rcopy(src.at[part], dst.at[part], ssem, rsem, partner)
        copy.wait_recv()
        return copy

    done = [arrived(tok_all, tok_all, tok_ssem, tok_rsem, NTP - 1)]
    squares = jnp.zeros((8, PART), F32)
    for j in range(NTP):
        v = tok_all[j].astype(F32)
        squares = squares + v * v
    scale = lax.rsqrt(jnp.sum(squares, axis=1, keepdims=True) / WIDTH + EPS)
    r_out[...] = jnp.sum(slots[...] * scale, axis=0, keepdims=True)
    for i, rel in enumerate(FAR):
        far_out[:, i] = placed_rows(tok_all[ys[rel] * 2 + core])
    for peer in peers:
        rcopy(r_out, r_in.at[me_e], r_ssem, r_rsem, (peer, me_t)).start()
    for peer in peers:
        rcopy(far_out.at[peer], far_in.at[me_e], far_ssem, far_rsem, (peer, me_t)).start()
    r_in[me_e] = r_out[...]
    far_in[me_e] = far_out[me_e]

    done.append(arrived(a2a_out, a2a_in, a2a_ssem, a2a_rsem, NEP - 1))
    sub3 = lax.broadcasted_iota(jnp.int32, (16, 8, 128), 1)

    def keep_rows(value, c, rel):
        pairs = value.astype(F32).reshape(16, 2, 8, 128)
        even, odd = pairs[:, 0], pairs[:, 1]
        left = jnp.where(sub3 < 4, even, pltpu.roll(odd, 4, 1)).reshape(ROWS, 128)
        right = jnp.where(sub3 < 4, pltpu.roll(even, 4, 1), odd).reshape(ROWS, 128)
        gathered[c, ys[rel], :, 0:128] = left.astype(BF16)
        gathered[c, ys[rel], :, 128:256] = right.astype(BF16)

    keep_rows(a2a_in[...], core, 0)

    def ag_copy(slot, k, device):
        ref = gathered.at[core, ys[slot]]
        return rcopy(ref, ref, ag_ssem, ag_rsem.at[k], device)

    for k, step in enumerate((2, -2, 1, -1)):
        ag_copy(0, k, ydev(step)).start()

    def pass_copy(c, rel):
        ref = gathered.at[c, ys[rel]]
        k = ((0,) + NEAR).index(rel)
        return rcopy(ref, ref, pf_ssem, pf_rsem.at[k], partner)

    def pass_on(rel):
        pass_copy(core, rel).start()

    def pass_wait(rel):
        pass_copy(other, rel).wait_recv()

    pass_on(0)

    for copy in smalls[3:6]:
        copy.wait()
    loaded(w_dense, 0)
    act = jnp.zeros((8, 128), F32)
    mix_acc = jnp.zeros((8, PART), F32)
    for j in range(NTP):
        cols = slice(j * PART, (j + 1) * PART)
        n = (tok_all[j].astype(F32) * scale * gain[:, cols]).astype(BF16)
        mix_acc = mix_acc + n.astype(F32) * mixw[:, cols]
        act = act + nt_dot(n, w_dense[:, cols])
    gate_ref[...] = jnp.broadcast_to(
        jax.nn.sigmoid(jnp.sum(mix_acc, axis=1, keepdims=True)), (8, 128)
    )
    dh_own[...] = (silu(act[:, 0:64]) * act[:, 64:128]).astype(BF16)
    dh_copy = rcopy(dh_own, dh_par, dh_ssem, dh_rsem, partner)
    dh_copy.start()

    loaded(dd_own, 1)
    parts[0].wait_recv()
    dh_copy.wait_recv()
    for k in range(NY):
        dense_out[k] = jnp.dot(
            dh_own[...], dd_own[k], preferred_element_type=F32
        ) + jnp.dot(dh_par[...], dd_par[k], preferred_element_type=F32)
    dense_in[y] = dense_out[y]
    loaded(w_gu.at[0], 2)
    parts[1].wait_recv()
    for rel in (6, 2):
        ag_copy(rel, NEAR.index(rel), partner).wait_recv()
        pass_on(rel)
    done.append(arrived(r_in, r_in, r_ssem, r_rsem, NEP - 1))
    picked = (
        lax.broadcasted_iota(jnp.int32, (ROWS, NEP), 0) // 4
        == lax.broadcasted_iota(jnp.int32, (ROWS, NEP), 1)
    )
    spread = jnp.dot(
        jnp.where(picked, 1.0, 0.0).astype(BF16),
        pieces(r_in[...].reshape(NEP, 128), 1),
        preferred_element_type=F32,
    )
    spread = spread[:, 0:128] + spread[:, 128:256] + spread[:, 256:384]
    wanted = me_e * 4 + lax.broadcasted_iota(jnp.int32, (ROWS, 128), 0) % 4
    here = lax.broadcasted_iota(jnp.int32, (ROWS, 128), 1) == wanted
    row_scale = jnp.sum(jnp.where(here, spread, 0.0), axis=1, keepdims=True)

    def project(*slices, first=False):
        total = None
        for c, rel in slices:
            cols = pl.ds(pl.multiple_of((2 * ys[rel] + c) * PART, PART), PART)
            n = (gathered[c, ys[rel]].astype(F32) * row_scale * gain[:, cols]).astype(BF16)
            v = nt_dot(n, w_gu[:, :, :, cols].reshape(512, PART))
            total = v if total is None else total + v
        acts[...] = total if first else acts[...] + total

    pass_wait(0)
    project((core, 0), (other, 0), (core, 6), (core, 2), first=True)
    for rel in (7, 1):
        ag_copy(rel, NEAR.index(rel), partner).wait_recv()
        pass_on(rel)
    for step in y_order:
        rcopy(
            dense_out.at[ys[step]], dense_in.at[y], dense_ssem, dense_rsem, ydev(step)
        ).start()
    pass_wait(6)
    pass_wait(2)
    project((core, 7), (core, 1), (other, 6), (other, 2))
    done.append(arrived(far_out, far_in, far_ssem, far_rsem, NEP - 1))
    raws = [
        rcopy(far_in.at[:, i], far_par.at[:, i], fp_ssem, fp_rsem.at[i], partner)
        for i in range(3)
    ]
    for copy in raws:
        copy.start()
    for i, rel in enumerate(FAR):
        keep_rows(far_in[:, i], core, rel)
    project((core, 3), (core, 4), (core, 5))
    pass_wait(7)
    pass_wait(1)
    project((other, 7), (other, 1))
    for i in range(2):
        raws[i].wait_recv()
        keep_rows(far_par[:, i], other, FAR[i])
    project((other, 3), (other, 4))
    raws[2].wait_recv()
    keep_rows(far_par[:, 2], other, FAR[2])
    project((other, 5))

    row = lax.broadcasted_iota(jnp.int32, (ROWS, 128), 0)
    col = lax.broadcasted_iota(jnp.int32, (ROWS, 128), 1)
    mine = (row // 2) % 2 == col // 64
    for k in range(2):
        v = acts[:, k * 256 : (k + 1) * 256]
        hidden = silu(v[:, 0:128]) * v[:, 128:256]
        hid[:, k * 128 : (k + 1) * 128] = jnp.where(mine, hidden, 0.0).astype(BF16)
    loaded(wd_own, 3)
    parts[2].wait_recv()

    diagonal = row == col

    def partials(*rels):
        both = jnp.concatenate(
            [
                jnp.concatenate([w[ys[rel]].reshape(128, PART) for rel in rels], axis=1)
                for w in (wd_own, wd_par)
            ],
            axis=0,
        )
        v = jnp.dot(hid[...], both, preferred_element_type=F32)
        return [v[:, i * PART : (i + 1) * PART] for i in range(len(rels))]

    def column(value):
        return jnp.sum(jnp.where(diagonal, value, 0.0), axis=0, keepdims=True)

    def messages(value):
        left = value[:, 0:128].reshape(16, 8, 128)
        right = value[:, 128:256].reshape(16, 8, 128)
        even = jnp.where(sub3 < 4, left, pltpu.roll(right, 4, 1))
        odd = jnp.where(sub3 < 4, pltpu.roll(left, 4, 1), right)
        return jnp.stack([even, odd], axis=1).reshape(NEP, 8, 128)

    def q_copies(k, device):
        return (
            rcopy(q_out.at[k], q_in.at[k], q_ssem, q_rsem.at[k], device),
            rcopy(s_out.at[k], s_in.at[k], sc_ssem, sc_rsem.at[k], device),
        )

    def q_pack(k, value):
        most = jnp.maximum(jnp.max(jnp.abs(value), axis=1, keepdims=True), 1e-30)
        q_out[k] = jnp.round(value * (32767.0 / most)).astype(jnp.int16)
        s_out[k] = column(most * (1.0 / 32767.0))

    def q_send(k):
        for copy in q_copies(k, ydev(NEAR[k])):
            copy.start()

    def q_get(k):
        for copy in q_copies(k, partner):
            copy.wait_recv()
        unit = jnp.sum(jnp.where(diagonal, s_in[k], 0.0), axis=1, keepdims=True)
        return q_in[k].astype(F32) * unit

    values = partials(*FAR, 0)
    kept[...] = values[3]
    most = jnp.maximum(jnp.maximum(jnp.abs(values[0]), jnp.abs(values[1])), jnp.abs(values[2]))
    most = jnp.maximum(jnp.max(most, axis=1, keepdims=True), 1e-30)
    fs_out[...] = column(most * (1.0 / 32767.0))
    for i in range(3):
        fq_out[:, i] = messages(jnp.round(values[i] * (32767.0 / most))).astype(jnp.int16)
    for peer in peers:
        rcopy(fs_out, fs_in.at[me_e], fs_ssem, fs_rsem, (peer, me_t)).start()
    for peer in peers:
        rcopy(fq_out.at[peer], fq_in.at[me_e], fq_ssem, fq_rsem, (peer, me_t)).start()
    for k, value in enumerate(partials(*NEAR)):
        q_pack(k, value)
    for k in range(4):
        q_send(k)
    fq_in[me_e] = fq_out[me_e]
    fs_in[me_e] = fs_out[...]
    done.append(arrived(dense_out, dense_in, dense_ssem, dense_rsem, NY - 1))
    dense = dense_in[0]
    for k in range(1, NY):
        dense = dense + dense_in[k]
    gate = gate_ref[...]
    dense = jnp.concatenate([gate, gate], axis=1) * dense
    summed = kept[...]
    for k in range(4):
        summed = summed + q_get(k)
    ret_out[...] = messages(summed)
    for peer in peers:
        rcopy(ret_out.at[peer], ret_in.at[me_e], ret_ssem, ret_rsem, (peer, me_t)).start()
    ret_in[me_e] = ret_out[me_e]
    done.append(arrived(fs_in, fs_in, fs_ssem, fs_rsem, NEP - 1))
    lane2 = lax.broadcasted_iota(jnp.int32, (128, 256), 1)
    mine4 = lax.broadcasted_iota(jnp.int32, (128, 256), 0) == me_e * 4 + lane2 % 4
    unit = jnp.dot(
        pieces(fs_in[...].reshape(NEP, 128), 0),
        jnp.where(mine4, 1.0, 0.0).astype(BF16),
        preferred_element_type=F32,
    )
    unit = unit[0:NEP] + unit[NEP : 2 * NEP] + unit[2 * NEP : 3 * NEP]
    source = lax.broadcasted_iota(jnp.int32, (NEP, 256), 0)
    source = source == lax.broadcasted_iota(jnp.int32, (NEP, 256), 1) // 8
    unit = jnp.sum(jnp.where(source, unit, 0.0), axis=0, keepdims=True)
    far_comb = pieces(comb[...] * unit, 0)
    near_comb = pieces(comb[...], 0)
    done.append(arrived(fq_out, fq_in, fq_ssem, fq_rsem, NEP - 1))
    far_rows = jnp.concatenate(
        [fq_in[:, i].astype(F32).reshape(256, 128) for i in range(3)], axis=1
    )
    far_high = far_rows.astype(BF16)
    far_low = (far_rows - far_high.astype(F32)).astype(BF16)
    far_sum = jnp.dot(far_comb, far_high, preferred_element_type=F32) + jnp.dot(
        far_comb, far_low, preferred_element_type=F32
    )
    far_sum = far_sum[0:16] + far_sum[16:32] + far_sum[32:48]
    for i, rel in enumerate(FAR):
        cols = slice(i * 128, (i + 1) * 128)
        fy_out[i, :, 0:128] = far_sum[0:8, cols]
        fy_out[i, :, 128:256] = far_sum[8:16, cols]
        rcopy(fy_out.at[i], fy_in.at[i], fy_ssem, fy_rsem, ydev(rel)).start()
    done.append(arrived(ret_out, ret_in, ret_ssem, ret_rsem, NEP - 1))
    mixed = jnp.dot(
        near_comb, pieces(ret_in[...].reshape(256, 128), 1), preferred_element_type=F32
    )
    mixed = mixed[:, 0:128] + mixed[:, 128:256] + mixed[:, 256:384]
    mixed = mixed[0:16] + mixed[16:32] + mixed[32:48]
    combined = jnp.concatenate([mixed[0:8], mixed[8:16]], axis=1) + dense
    fy_copy = rcopy(fy_out, fy_in, fy_ssem, fy_rsem, partner)
    fy_copy.wait_recv()
    combined = combined + fy_in[0] + fy_in[1] + fy_in[2]
    token_diagonal = (
        lax.broadcasted_iota(jnp.int32, (8, 128), 0)
        == lax.broadcasted_iota(jnp.int32, (8, 128), 1)
    )
    own = jnp.sum(
        jnp.where(token_diagonal, jnp.sum(combined * combined, axis=1, keepdims=True), 0.0),
        axis=0,
        keepdims=True,
    )
    sq_out[...] = own
    for step in y_order:
        for c in range(2):
            rcopy(sq_out, sq_in.at[me_t], sq_ssem, sq_rsem, (me_e, ys[step] * 2 + c)).start()
    rcopy(sq_out, sq_in.at[me_t], sq_ssem, sq_rsem, partner).start()
    sq_in[me_t] = own
    done.append(arrived(sq_in, sq_in, sq_ssem, sq_rsem, NTP - 1))
    total_sq = sq_in[0]
    for j in range(1, NTP):
        total_sq = total_sq + sq_in[j]
    final = lax.rsqrt(
        jnp.sum(jnp.where(token_diagonal, total_sq, 0.0), axis=1, keepdims=True) / WIDTH + EPS
    )
    out[...] = (combined * final * ogain[...]).astype(BF16)

    near = gathered.at[core, pl.ds(0, 4)]
    done += [
        rcopy(near, near, ag_ssem, ag_rsem.at[0], partner),
        rcopy(q_out, q_in, q_ssem, q_rsem.at[0], partner),
        rcopy(s_out, s_in, sc_ssem, sc_rsem.at[0], partner),
    ]
    five = gathered.at[core, pl.ds(0, 5)]
    done.append(rcopy(five, five, pf_ssem, pf_rsem.at[0], partner))
    for copy in parts + [dh_copy, fy_copy] + raws + done:
        copy.wait_send()


def local(
    tokens,
    norm_gain,
    route_experts,
    route_logits,
    expert_gate,
    expert_up,
    expert_down,
    dense_gate,
    dense_up,
    dense_down,
    mix_weight,
    out_gain,
):
    vmem = pl.BlockSpec(memory_space=pltpu.VMEM)
    dma = pltpu.SemaphoreType.DMA
    return pl.pallas_call(
        kernel,
        out_shape=pltpu.VMEM((8, PART), BF16),
        in_specs=[pl.BlockSpec(memory_space=pl.ANY)] * 12,
        out_specs=vmem,
        scratch_shapes=[
            pltpu.VMEM((8, PART), BF16),
            pltpu.VMEM((1, WIDTH), F32),
            pltpu.SMEM((2, 8), jnp.int32),
            pltpu.SMEM((2, 8), F32),
            pltpu.VMEM((1, WIDTH), F32),
            pltpu.VMEM((1, PART), F32),
            pltpu.VMEM((2, 4, 64, WIDTH), BF16),
            pltpu.VMEM((NY, 2, 64, PART), BF16),
            pltpu.VMEM((NY, 2, 64, PART), BF16),
            pltpu.VMEM((128, WIDTH), BF16),
            pltpu.VMEM((NY, 64, PART), BF16),
            pltpu.VMEM((NY, 64, PART), BF16),
            pltpu.VMEM((NEP, 8, 128), BF16),
            pltpu.VMEM((NEP, 8, 128), BF16),
            pltpu.VMEM((NEP, 3, 8, 128), BF16),
            pltpu.VMEM((NEP, 3, 8, 128), BF16),
            pltpu.VMEM((NEP, 3, 8, 128), BF16),
            pltpu.VMEM((2, NY, ROWS, PART), BF16),
            pltpu.VMEM((NTP, 8, PART), BF16),
            pltpu.VMEM((NY, 8, PART), F32),
            pltpu.VMEM((NY, 8, PART), F32),
            pltpu.VMEM((8, 64), BF16),
            pltpu.VMEM((8, 64), BF16),
            pltpu.VMEM((16, 256), F32),
            pltpu.VMEM((16, 256), BF16),
            pltpu.VMEM((8, 128), F32),
            pltpu.VMEM((1, 128), F32),
            pltpu.VMEM((NEP, 1, 128), F32),
            pltpu.VMEM((ROWS, 512), F32),
            pltpu.VMEM((ROWS, 256), BF16),
            pltpu.VMEM((4, ROWS, PART), jnp.int16),
            pltpu.VMEM((4, ROWS, PART), jnp.int16),
            pltpu.VMEM((4, 1, 128), F32),
            pltpu.VMEM((4, 1, 128), F32),
            pltpu.VMEM((NEP, 3, 8, 128), jnp.int16),
            pltpu.VMEM((NEP, 3, 8, 128), jnp.int16),
            pltpu.VMEM((1, 128), F32),
            pltpu.VMEM((NEP, 1, 128), F32),
            pltpu.VMEM((3, 8, PART), F32),
            pltpu.VMEM((3, 8, PART), F32),
            pltpu.VMEM((ROWS, PART), F32),
            pltpu.VMEM((NEP, 8, 128), F32),
            pltpu.VMEM((NEP, 8, 128), F32),
            pltpu.VMEM((1, 128), F32),
            pltpu.VMEM((NTP, 1, 128), F32),
            pltpu.VMEM((8, 128), F32),
            dma((6,)),
            dma((4,)),
            dma((3,)),
            dma((3,)),
            dma,
            dma,
            dma,
            dma,
            dma,
            dma,
            dma,
            dma,
            dma,
            dma,
            dma,
            dma((4,)),
            dma,
            dma((5,)),
            dma,
            dma((3,)),
            dma,
            dma,
            dma,
            dma((4,)),
            dma,
            dma((4,)),
            dma,
            dma,
            dma,
            dma,
            dma,
            dma,
            dma,
            dma,
            dma,
            dma,
        ],
        compiler_params=pltpu.CompilerParams(
            collective_id=0, has_side_effects=True, vmem_limit_bytes=56650000
        ),
    )(
        tokens,
        norm_gain.reshape(1, WIDTH),
        route_experts.T,
        route_logits.T,
        jnp.swapaxes(expert_gate, 1, 2),
        jnp.swapaxes(expert_up, 1, 2),
        expert_down,
        dense_gate.T,
        dense_up.T,
        dense_down,
        mix_weight.reshape(1, WIDTH),
        out_gain.reshape(1, PART),
    )


def solution(mesh):
    tp = "tp"
    in_specs = (
        P("ep", tp),
        P(),
        P("ep", None),
        P("ep", None),
        P("ep", None, tp),
        P("ep", None, tp),
        P("ep", tp, None),
        P(None, tp),
        P(None, tp),
        P(tp, None),
        P(),
        P(tp),
    )
    return jax.shard_map(
        local, mesh=mesh, in_specs=in_specs, out_specs=P("ep", tp), check_vma=False
    )
```

```python
import functools

import jax
import jax.numpy as jnp
from jax import lax
from jax.experimental import pallas as pl
from jax.experimental.pallas import tpu as pltpu
from jax.sharding import PartitionSpec as P

MESH = pl.DeviceIdType.MESH
F32 = jnp.float32
BF16 = jnp.bfloat16
EPS = 1e-06

NX, NZ, NY = 4, 8, 8
NEP = NX * NZ
NTP = 2 * NY
ROWS = 128
FAR = (3, 4, 5)
NEAR = (6, 2, 7, 1)
PART = 256
WIDTH = 4096


def rcopy(src, dst, send_sem, recv_sem, device):
    return pltpu.make_async_remote_copy(
        src_ref=src,
        dst_ref=dst,
        send_sem=send_sem,
        recv_sem=recv_sem,
        device_id=device,
        device_id_type=MESH,
    )


def nt_dot(a, b):
    return lax.dot_general(a, b, (((1,), (1,)), ((), ())), preferred_element_type=F32)


def pieces(value, axis):
    high = value.astype(BF16)
    rest = value - high.astype(F32)
    middle = rest.astype(BF16)
    low = (rest - middle.astype(F32)).astype(BF16)
    return jnp.concatenate([high, middle, low], axis=axis)


def silu(v):
    return v / (1.0 + jnp.exp(-v))


def kernel(
    tok_hbm,
    gain_hbm,
    routes_hbm,
    logits_hbm,
    wg,
    wu,
    wd,
    dg,
    du,
    dd,
    mixw_hbm,
    ogain_hbm,
    out,
    tok,
    gain,
    routes,
    logits,
    mixw,
    ogain,
    w_gu,
    wd_own,
    wd_par,
    w_dense,
    dd_own,
    dd_par,
    a2a_out,
    a2a_in,
    far_out,
    far_in,
    far_par,
    gathered,
    tok_all,
    dense_out,
    dense_in,
    dh_own,
    dh_par,
    comb,
    place,
    slots,
    r_out,
    r_in,
    acts,
    hid,
    q_out,
    q_in,
    s_out,
    s_in,
    fq_out,
    fq_in,
    fs_out,
    fs_in,
    fy_out,
    fy_in,
    kept,
    ret_out,
    ret_in,
    sq_out,
    sq_in,
    gate_ref,
    i_sem,
    w_sem,
    wp_ssem,
    wp_rsem,
    a2a_ssem,
    a2a_rsem,
    far_ssem,
    far_rsem,
    tok_ssem,
    tok_rsem,
    dh_ssem,
    dh_rsem,
    dense_ssem,
    dense_rsem,
    ag_ssem,
    ag_rsem,
    pf_ssem,
    pf_rsem,
    fp_ssem,
    fp_rsem,
    r_ssem,
    r_rsem,
    q_ssem,
    q_rsem,
    sc_ssem,
    sc_rsem,
    fq_ssem,
    fq_rsem,
    fs_ssem,
    fs_rsem,
    fy_ssem,
    fy_rsem,
    ret_ssem,
    ret_rsem,
    sq_ssem,
    sq_rsem,
):
    me_e = lax.axis_index("ep")
    me_t = lax.axis_index("tp")
    z, x = lax.div(me_e, NX), lax.rem(me_e, NX)
    y, core = lax.div(me_t, 2), lax.rem(me_t, 2)
    other = 1 - core
    partner = (me_e, y * 2 + other)
    zs = [lax.rem(z + k, NZ) * NX for k in range(NZ)]
    xs = [lax.rem(x + k, NX) for k in range(NX)]
    ys = [lax.rem(y + k, NY) for k in range(NY)]
    peers = [zs[dz] + xs[dx] for dz in (4, 3, 5, 2, 6, 1, 7, 0) for dx in (2, 1, 3, 0)][:-1]
    y_order = (4, 3, 5, 2, 6, 1, 7)

    def ydev(step):
        return (me_e, ys[step % NY] * 2 + core)

    barrier = pltpu.get_barrier_semaphore()
    for peer in peers:
        pl.semaphore_signal(barrier, inc=1, device_id=(peer, me_t), device_id_type=MESH)
    for step in y_order:
        for c in range(2):
            pl.semaphore_signal(
                barrier, inc=1, device_id=(me_e, ys[step] * 2 + c), device_id_type=MESH
            )
    pl.semaphore_signal(barrier, inc=1, device_id=partner, device_id_type=MESH)

    smalls = [
        pltpu.make_async_copy(routes_hbm, routes, i_sem.at[0]),
        pltpu.make_async_copy(logits_hbm, logits, i_sem.at[1]),
        pltpu.make_async_copy(tok_hbm, tok, i_sem.at[2]),
        pltpu.make_async_copy(gain_hbm, gain, i_sem.at[3]),
        pltpu.make_async_copy(mixw_hbm, mixw, i_sem.at[4]),
        pltpu.make_async_copy(ogain_hbm, ogain, i_sem.at[5]),
    ]

    def columns(k, c):
        return pl.ds(pl.multiple_of((2 * k + c) * PART, PART), PART)

    def load(src, dst, k):
        pltpu.make_async_copy(src, dst, w_sem.at[k]).start()

    def loaded(dst, k):
        pltpu.make_async_copy(dst, dst, w_sem.at[k]).wait()

    for copy in smalls:
        copy.start()
    load(dg, w_dense.at[pl.ds(0, 64)], 0)
    load(du, w_dense.at[pl.ds(64, 64)], 0)
    for k in range(NY):
        load(dd.at[:, columns(k, core)], dd_own.at[k], 1)
    load(wg, w_gu.at[0, pl.ds(0, 2)], 2)
    load(wu, w_gu.at[0, pl.ds(2, 2)], 2)
    for k in range(NY):
        load(wd.at[:, :, columns(k, core)], wd_own.at[k], 3)

    for copy in smalls[0:3]:
        copy.wait()
    lane = lax.broadcasted_iota(jnp.int32, (8, 256), 1)
    sub = lax.broadcasted_iota(jnp.int32, (8, 256), 0)
    expert = 2 * (lane // 8) + (lane // 2) % 2
    half = (lane // 4) % 2
    r0 = jnp.zeros((8, 256), jnp.int32)
    r1 = jnp.zeros((8, 256), jnp.int32)
    l0 = jnp.zeros((8, 256), F32)
    l1 = jnp.zeros((8, 256), F32)
    for t in range(8):
        r0 = jnp.where(sub == t, routes[0, t], r0)
        r1 = jnp.where(sub == t, routes[1, t], r1)
        l0 = jnp.where(sub == t, logits[0, t], l0)
        l1 = jnp.where(sub == t, logits[1, t], l1)
    top = jnp.maximum(l0, l1)
    e0, e1 = jnp.exp(l0 - top), jnp.exp(l1 - top)
    is0, is1 = (r0 == expert), (r1 == expert)
    hit = jnp.where(is0, 1.0, 0.0) + jnp.where(is1, 1.0, 0.0)
    before = jnp.zeros((8, 256), F32)
    for t in range(7):
        before = before + jnp.where(sub > t, hit[t : t + 1, :], 0.0)
    placed = jnp.where(before == (lane % 2).astype(F32), hit, 0.0)
    weight = (jnp.where(is0, e0, 0.0) + jnp.where(is1, e1, 0.0)) / (e0 + e1) * placed
    comb[0:8, :] = jnp.where(half == 0, weight, 0.0)
    comb[8:16, :] = jnp.where(half == 1, weight, 0.0)
    left_half = lax.broadcasted_iota(jnp.int32, (256, 128), 0)
    slot = lax.broadcasted_iota(jnp.int32, (256, 128), 1)
    left_half = (left_half // 8 == slot // 4) & (left_half % 8 == slot % 4)
    slots[...] = jnp.dot(
        placed.astype(BF16),
        jnp.where(left_half, 1.0, 0.0).astype(BF16),
        preferred_element_type=F32,
    )
    place[...] = jnp.concatenate(
        [jnp.where(half == 0, placed, 0.0), jnp.where(half == 1, placed, 0.0)], axis=0
    ).astype(BF16)

    def placed_rows(value):
        halves = jnp.concatenate(
            [value[:, 0:128].astype(F32), value[:, 128:256].astype(F32)], axis=0
        ).astype(BF16)
        rows = lax.dot_general(
            place[...], halves, (((0,), (0,)), ((), ())), preferred_element_type=F32
        )
        return rows.astype(BF16).reshape(NEP, 8, 128)

    tok_value = tok[...]
    a2a_out[...] = placed_rows(tok_value)
    a2a_in[me_e] = a2a_out[me_e]
    tok_all[me_t] = tok_value

    pl.semaphore_wait(barrier, NEP - 1 + NTP - 1)

    for step in y_order:
        for c in range(2):
            rcopy(
                tok, tok_all.at[me_t], tok_ssem, tok_rsem, (me_e, ys[step] * 2 + c)
            ).start()
    rcopy(tok, tok_all.at[me_t], tok_ssem, tok_rsem, partner).start()

    for peer in peers:
        rcopy(a2a_out.at[peer], a2a_in.at[me_e], a2a_ssem, a2a_rsem, (peer, me_t)).start()

    for k in range(NY):
        rcopy(
            dd.at[:, columns(k, other)], dd_par.at[k], wp_ssem.at[0], wp_rsem.at[0], partner
        ).start()
    for k, ref in enumerate((wg, wu)):
        rcopy(
            ref, w_gu.at[1, pl.ds(2 * k, 2)], wp_ssem.at[1], wp_rsem.at[1], partner
        ).start()
    for k in range(NY):
        rcopy(
            wd.at[:, :, columns(k, other)], wd_par.at[k], wp_ssem.at[2], wp_rsem.at[2], partner
        ).start()
    parts = [
        rcopy(ref, ref, wp_ssem.at[k], wp_rsem.at[k], partner)
        for k, ref in enumerate((dd_par, w_gu.at[1], wd_par))
    ]

    def arrived(src, dst, ssem, rsem, n):
        part = pl.ds(0, n)
        copy = rcopy(src.at[part], dst.at[part], ssem, rsem, partner)
        copy.wait_recv()
        return copy

    done = [arrived(tok_all, tok_all, tok_ssem, tok_rsem, NTP - 1)]
    squares = jnp.zeros((8, PART), F32)
    for j in range(NTP):
        v = tok_all[j].astype(F32)
        squares = squares + v * v
    scale = lax.rsqrt(jnp.sum(squares, axis=1, keepdims=True) / WIDTH + EPS)
    r_out[...] = jnp.sum(slots[...] * scale, axis=0, keepdims=True)
    for i, rel in enumerate(FAR):
        far_out[:, i] = placed_rows(tok_all[ys[rel] * 2 + core])
    for peer in peers:
        rcopy(r_out, r_in.at[me_e], r_ssem, r_rsem, (peer, me_t)).start()
    for peer in peers:
        rcopy(far_out.at[peer], far_in.at[me_e], far_ssem, far_rsem, (peer, me_t)).start()
    r_in[me_e] = r_out[...]
    far_in[me_e] = far_out[me_e]

    done.append(arrived(a2a_out, a2a_in, a2a_ssem, a2a_rsem, NEP - 1))
    sub3 = lax.broadcasted_iota(jnp.int32, (16, 8, 128), 1)

    def keep_rows(value, c, rel):
        pairs = value.astype(F32).reshape(16, 2, 8, 128)
        even, odd = pairs[:, 0], pairs[:, 1]
        left = jnp.where(sub3 < 4, even, pltpu.roll(odd, 4, 1)).reshape(ROWS, 128)
        right = jnp.where(sub3 < 4, pltpu.roll(even, 4, 1), odd).reshape(ROWS, 128)
        gathered[c, ys[rel], :, 0:128] = left.astype(BF16)
        gathered[c, ys[rel], :, 128:256] = right.astype(BF16)

    keep_rows(a2a_in[...], core, 0)

    def ag_copy(slot, k, device):
        ref = gathered.at[core, ys[slot]]
        return rcopy(ref, ref, ag_ssem, ag_rsem.at[k], device)

    for k, step in enumerate((2, -2, 1, -1)):
        ag_copy(0, k, ydev(step)).start()

    def pass_copy(c, rel):
        ref = gathered.at[c, ys[rel]]
        k = ((0,) + NEAR).index(rel)
        return rcopy(ref, ref, pf_ssem, pf_rsem.at[k], partner)

    def pass_on(rel):
        pass_copy(core, rel).start()

    def pass_wait(rel):
        pass_copy(other, rel).wait_recv()

    pass_on(0)

    for copy in smalls[3:6]:
        copy.wait()
    loaded(w_dense, 0)
    act = jnp.zeros((8, 128), F32)
    mix_acc = jnp.zeros((8, PART), F32)
    for j in range(NTP):
        cols = slice(j * PART, (j + 1) * PART)
        n = (tok_all[j].astype(F32) * scale * gain[:, cols]).astype(BF16)
        mix_acc = mix_acc + n.astype(F32) * mixw[:, cols]
        act = act + nt_dot(n, w_dense[:, cols])
    gate_ref[...] = jnp.broadcast_to(
        jax.nn.sigmoid(jnp.sum(mix_acc, axis=1, keepdims=True)), (8, 128)
    )
    dh_own[...] = (silu(act[:, 0:64]) * act[:, 64:128]).astype(BF16)
    dh_copy = rcopy(dh_own, dh_par, dh_ssem, dh_rsem, partner)
    dh_copy.start()

    loaded(dd_own, 1)
    parts[0].wait_recv()
    dh_copy.wait_recv()
    for k in range(NY):
        dense_out[k] = jnp.dot(
            dh_own[...], dd_own[k], preferred_element_type=F32
        ) + jnp.dot(dh_par[...], dd_par[k], preferred_element_type=F32)
    dense_in[y] = dense_out[y]
    loaded(w_gu.at[0], 2)
    parts[1].wait_recv()
    for rel in (6, 2):
        ag_copy(rel, NEAR.index(rel), partner).wait_recv()
        pass_on(rel)
    done.append(arrived(r_in, r_in, r_ssem, r_rsem, NEP - 1))
    picked = (
        lax.broadcasted_iota(jnp.int32, (ROWS, NEP), 0) // 4
        == lax.broadcasted_iota(jnp.int32, (ROWS, NEP), 1)
    )
    spread = jnp.dot(
        jnp.where(picked, 1.0, 0.0).astype(BF16),
        pieces(r_in[...].reshape(NEP, 128), 1),
        preferred_element_type=F32,
    )
    spread = spread[:, 0:128] + spread[:, 128:256] + spread[:, 256:384]
    wanted = me_e * 4 + lax.broadcasted_iota(jnp.int32, (ROWS, 128), 0) % 4
    here = lax.broadcasted_iota(jnp.int32, (ROWS, 128), 1) == wanted
    row_scale = jnp.sum(jnp.where(here, spread, 0.0), axis=1, keepdims=True)

    def project(*slices, first=False):
        total = None
        for c, rel in slices:
            cols = pl.ds(pl.multiple_of((2 * ys[rel] + c) * PART, PART), PART)
            n = (gathered[c, ys[rel]].astype(F32) * row_scale * gain[:, cols]).astype(BF16)
            v = nt_dot(n, w_gu[:, :, :, cols].reshape(512, PART))
            total = v if total is None else total + v
        acts[...] = total if first else acts[...] + total

    pass_wait(0)
    project((core, 0), (other, 0), (core, 6), (core, 2), first=True)
    for rel in (7, 1):
        ag_copy(rel, NEAR.index(rel), partner).wait_recv()
        pass_on(rel)
    pass_wait(6)
    pass_wait(2)
    project((core, 7), (core, 1), (other, 6), (other, 2))
    done.append(arrived(far_out, far_in, far_ssem, far_rsem, NEP - 1))
    raws = [
        rcopy(far_in.at[:, i], far_par.at[:, i], fp_ssem, fp_rsem.at[i], partner)
        for i in range(3)
    ]
    for copy in raws:
        copy.start()
    for step in y_order:
        rcopy(
            dense_out.at[ys[step]], dense_in.at[y], dense_ssem, dense_rsem, ydev(step)
        ).start()
    for i, rel in enumerate(FAR):
        keep_rows(far_in[:, i], core, rel)
    project((core, 3), (core, 4), (core, 5))
    pass_wait(7)
    pass_wait(1)
    project((other, 7), (other, 1))
    for i in range(2):
        raws[i].wait_recv()
        keep_rows(far_par[:, i], other, FAR[i])
    project((other, 3), (other, 4))
    raws[2].wait_recv()
    keep_rows(far_par[:, 2], other, FAR[2])
    project((other, 5))

    row = lax.broadcasted_iota(jnp.int32, (ROWS, 128), 0)
    col = lax.broadcasted_iota(jnp.int32, (ROWS, 128), 1)
    mine = (row // 2) % 2 == col // 64
    for k in range(2):
        v = acts[:, k * 256 : (k + 1) * 256]
        hidden = silu(v[:, 0:128]) * v[:, 128:256]
        hid[:, k * 128 : (k + 1) * 128] = jnp.where(mine, hidden, 0.0).astype(BF16)
    loaded(wd_own, 3)
    parts[2].wait_recv()

    diagonal = row == col

    def partials(*rels):
        both = jnp.concatenate(
            [
                jnp.concatenate([w[ys[rel]].reshape(128, PART) for rel in rels], axis=1)
                for w in (wd_own, wd_par)
            ],
            axis=0,
        )
        v = jnp.dot(hid[...], both, preferred_element_type=F32)
        return [v[:, i * PART : (i + 1) * PART] for i in range(len(rels))]

    def column(value):
        return jnp.sum(jnp.where(diagonal, value, 0.0), axis=0, keepdims=True)

    def messages(value):
        left = value[:, 0:128].reshape(16, 8, 128)
        right = value[:, 128:256].reshape(16, 8, 128)
        even = jnp.where(sub3 < 4, left, pltpu.roll(right, 4, 1))
        odd = jnp.where(sub3 < 4, pltpu.roll(left, 4, 1), right)
        return jnp.stack([even, odd], axis=1).reshape(NEP, 8, 128)

    def q_copies(k, device):
        return (
            rcopy(q_out.at[k], q_in.at[k], q_ssem, q_rsem.at[k], device),
            rcopy(s_out.at[k], s_in.at[k], sc_ssem, sc_rsem.at[k], device),
        )

    def q_pack(k, value):
        most = jnp.maximum(jnp.max(jnp.abs(value), axis=1, keepdims=True), 1e-30)
        q_out[k] = jnp.round(value * (32767.0 / most)).astype(jnp.int16)
        s_out[k] = column(most * (1.0 / 32767.0))

    def q_send(k):
        for copy in q_copies(k, ydev(NEAR[k])):
            copy.start()

    def q_get(k):
        for copy in q_copies(k, partner):
            copy.wait_recv()
        unit = jnp.sum(jnp.where(diagonal, s_in[k], 0.0), axis=1, keepdims=True)
        return q_in[k].astype(F32) * unit

    near2 = partials(NEAR[0], NEAR[1])
    values = partials(*FAR, 0)
    q_pack(0, near2[0])
    q_pack(1, near2[1])
    kept[...] = values[3]
    most = jnp.maximum(jnp.maximum(jnp.abs(values[0]), jnp.abs(values[1])), jnp.abs(values[2]))
    most = jnp.maximum(jnp.max(most, axis=1, keepdims=True), 1e-30)
    fs_out[...] = column(most * (1.0 / 32767.0))
    for i in range(3):
        fq_out[:, i] = messages(jnp.round(values[i] * (32767.0 / most))).astype(jnp.int16)
    q_send(0)
    q_send(1)
    for peer in peers:
        rcopy(fs_out, fs_in.at[me_e], fs_ssem, fs_rsem, (peer, me_t)).start()
    for peer in peers:
        rcopy(fq_out.at[peer], fq_in.at[me_e], fq_ssem, fq_rsem, (peer, me_t)).start()
    near1 = partials(NEAR[2], NEAR[3])
    q_pack(2, near1[0])
    q_pack(3, near1[1])
    q_send(2)
    q_send(3)
    fq_in[me_e] = fq_out[me_e]
    fs_in[me_e] = fs_out[...]
    done.append(arrived(dense_out, dense_in, dense_ssem, dense_rsem, NY - 1))
    dense = dense_in[0]
    for k in range(1, NY):
        dense = dense + dense_in[k]
    gate = gate_ref[...]
    dense = jnp.concatenate([gate, gate], axis=1) * dense
    summed = kept[...]
    for k in range(4):
        summed = summed + q_get(k)
    ret_out[...] = messages(summed)
    for peer in peers:
        rcopy(ret_out.at[peer], ret_in.at[me_e], ret_ssem, ret_rsem, (peer, me_t)).start()
    ret_in[me_e] = ret_out[me_e]
    done.append(arrived(fs_in, fs_in, fs_ssem, fs_rsem, NEP - 1))
    lane2 = lax.broadcasted_iota(jnp.int32, (128, 256), 1)
    mine4 = lax.broadcasted_iota(jnp.int32, (128, 256), 0) == me_e * 4 + lane2 % 4
    unit = jnp.dot(
        pieces(fs_in[...].reshape(NEP, 128), 0),
        jnp.where(mine4, 1.0, 0.0).astype(BF16),
        preferred_element_type=F32,
    )
    unit = unit[0:NEP] + unit[NEP : 2 * NEP] + unit[2 * NEP : 3 * NEP]
    source = lax.broadcasted_iota(jnp.int32, (NEP, 256), 0)
    source = source == lax.broadcasted_iota(jnp.int32, (NEP, 256), 1) // 8
    unit = jnp.sum(jnp.where(source, unit, 0.0), axis=0, keepdims=True)
    far_comb = pieces(comb[...] * unit, 0)
    near_comb = pieces(comb[...], 0)
    done.append(arrived(fq_out, fq_in, fq_ssem, fq_rsem, NEP - 1))
    far_rows = jnp.concatenate(
        [fq_in[:, i].astype(F32).reshape(256, 128) for i in range(3)], axis=1
    )
    far_high = far_rows.astype(BF16)
    far_low = (far_rows - far_high.astype(F32)).astype(BF16)
    far_sum = jnp.dot(far_comb, far_high, preferred_element_type=F32) + jnp.dot(
        far_comb, far_low, preferred_element_type=F32
    )
    far_sum = far_sum[0:16] + far_sum[16:32] + far_sum[32:48]
    for i, rel in enumerate(FAR):
        cols = slice(i * 128, (i + 1) * 128)
        fy_out[i, :, 0:128] = far_sum[0:8, cols]
        fy_out[i, :, 128:256] = far_sum[8:16, cols]
        rcopy(fy_out.at[i], fy_in.at[i], fy_ssem, fy_rsem, ydev(rel)).start()
    done.append(arrived(ret_out, ret_in, ret_ssem, ret_rsem, NEP - 1))
    mixed = jnp.dot(
        near_comb, pieces(ret_in[...].reshape(256, 128), 1), preferred_element_type=F32
    )
    mixed = mixed[:, 0:128] + mixed[:, 128:256] + mixed[:, 256:384]
    mixed = mixed[0:16] + mixed[16:32] + mixed[32:48]
    combined = jnp.concatenate([mixed[0:8], mixed[8:16]], axis=1) + dense
    fy_copy = rcopy(fy_out, fy_in, fy_ssem, fy_rsem, partner)
    fy_copy.wait_recv()
    combined = combined + fy_in[0] + fy_in[1] + fy_in[2]
    token_diagonal = (
        lax.broadcasted_iota(jnp.int32, (8, 128), 0)
        == lax.broadcasted_iota(jnp.int32, (8, 128), 1)
    )
    own = jnp.sum(
        jnp.where(token_diagonal, jnp.sum(combined * combined, axis=1, keepdims=True), 0.0),
        axis=0,
        keepdims=True,
    )
    sq_out[...] = own
    for step in y_order:
        for c in range(2):
            rcopy(sq_out, sq_in.at[me_t], sq_ssem, sq_rsem, (me_e, ys[step] * 2 + c)).start()
    rcopy(sq_out, sq_in.at[me_t], sq_ssem, sq_rsem, partner).start()
    sq_in[me_t] = own
    done.append(arrived(sq_in, sq_in, sq_ssem, sq_rsem, NTP - 1))
    total_sq = sq_in[0]
    for j in range(1, NTP):
        total_sq = total_sq + sq_in[j]
    final = lax.rsqrt(
        jnp.sum(jnp.where(token_diagonal, total_sq, 0.0), axis=1, keepdims=True) / WIDTH + EPS
    )
    out[...] = (combined * final * ogain[...]).astype(BF16)

    near = gathered.at[core, pl.ds(0, 4)]
    done += [
        rcopy(near, near, ag_ssem, ag_rsem.at[0], partner),
        rcopy(q_out, q_in, q_ssem, q_rsem.at[0], partner),
        rcopy(s_out, s_in, sc_ssem, sc_rsem.at[0], partner),
    ]
    five = gathered.at[core, pl.ds(0, 5)]
    done.append(rcopy(five, five, pf_ssem, pf_rsem.at[0], partner))
    for copy in parts + [dh_copy, fy_copy] + raws + done:
        copy.wait_send()


def local(
    tokens,
    norm_gain,
    route_experts,
    route_logits,
    expert_gate,
    expert_up,
    expert_down,
    dense_gate,
    dense_up,
    dense_down,
    mix_weight,
    out_gain,
):
    vmem = pl.BlockSpec(memory_space=pltpu.VMEM)
    dma = pltpu.SemaphoreType.DMA
    return pl.pallas_call(
        kernel,
        out_shape=pltpu.VMEM((8, PART), BF16),
        in_specs=[pl.BlockSpec(memory_space=pl.ANY)] * 12,
        out_specs=vmem,
        scratch_shapes=[
            pltpu.VMEM((8, PART), BF16),
            pltpu.VMEM((1, WIDTH), F32),
            pltpu.SMEM((2, 8), jnp.int32),
            pltpu.SMEM((2, 8), F32),
            pltpu.VMEM((1, WIDTH), F32),
            pltpu.VMEM((1, PART), F32),
            pltpu.VMEM((2, 4, 64, WIDTH), BF16),
            pltpu.VMEM((NY, 2, 64, PART), BF16),
            pltpu.VMEM((NY, 2, 64, PART), BF16),
            pltpu.VMEM((128, WIDTH), BF16),
            pltpu.VMEM((NY, 64, PART), BF16),
            pltpu.VMEM((NY, 64, PART), BF16),
            pltpu.VMEM((NEP, 8, 128), BF16),
            pltpu.VMEM((NEP, 8, 128), BF16),
            pltpu.VMEM((NEP, 3, 8, 128), BF16),
            pltpu.VMEM((NEP, 3, 8, 128), BF16),
            pltpu.VMEM((NEP, 3, 8, 128), BF16),
            pltpu.VMEM((2, NY, ROWS, PART), BF16),
            pltpu.VMEM((NTP, 8, PART), BF16),
            pltpu.VMEM((NY, 8, PART), F32),
            pltpu.VMEM((NY, 8, PART), F32),
            pltpu.VMEM((8, 64), BF16),
            pltpu.VMEM((8, 64), BF16),
            pltpu.VMEM((16, 256), F32),
            pltpu.VMEM((16, 256), BF16),
            pltpu.VMEM((8, 128), F32),
            pltpu.VMEM((1, 128), F32),
            pltpu.VMEM((NEP, 1, 128), F32),
            pltpu.VMEM((ROWS, 512), F32),
            pltpu.VMEM((ROWS, 256), BF16),
            pltpu.VMEM((4, ROWS, PART), jnp.int16),
            pltpu.VMEM((4, ROWS, PART), jnp.int16),
            pltpu.VMEM((4, 1, 128), F32),
            pltpu.VMEM((4, 1, 128), F32),
            pltpu.VMEM((NEP, 3, 8, 128), jnp.int16),
            pltpu.VMEM((NEP, 3, 8, 128), jnp.int16),
            pltpu.VMEM((1, 128), F32),
            pltpu.VMEM((NEP, 1, 128), F32),
            pltpu.VMEM((3, 8, PART), F32),
            pltpu.VMEM((3, 8, PART), F32),
            pltpu.VMEM((ROWS, PART), F32),
            pltpu.VMEM((NEP, 8, 128), F32),
            pltpu.VMEM((NEP, 8, 128), F32),
            pltpu.VMEM((1, 128), F32),
            pltpu.VMEM((NTP, 1, 128), F32),
            pltpu.VMEM((8, 128), F32),
            dma((6,)),
            dma((4,)),
            dma((3,)),
            dma((3,)),
            dma,
            dma,
            dma,
            dma,
            dma,
            dma,
            dma,
            dma,
            dma,
            dma,
            dma,
            dma((4,)),
            dma,
            dma((5,)),
            dma,
            dma((3,)),
            dma,
            dma,
            dma,
            dma((4,)),
            dma,
            dma((4,)),
            dma,
            dma,
            dma,
            dma,
            dma,
            dma,
            dma,
            dma,
            dma,
            dma,
        ],
        compiler_params=pltpu.CompilerParams(
            collective_id=0, has_side_effects=True, vmem_limit_bytes=56650000
        ),
    )(
        tokens,
        norm_gain.reshape(1, WIDTH),
        route_experts.T,
        route_logits.T,
        jnp.swapaxes(expert_gate, 1, 2),
        jnp.swapaxes(expert_up, 1, 2),
        expert_down,
        dense_gate.T,
        dense_up.T,
        dense_down,
        mix_weight.reshape(1, WIDTH),
        out_gain.reshape(1, PART),
    )


def solution(mesh):
    tp = "tp"
    in_specs = (
        P("ep", tp),
        P(),
        P("ep", None),
        P("ep", None),
        P("ep", None, tp),
        P("ep", None, tp),
        P("ep", tp, None),
        P(None, tp),
        P(None, tp),
        P(tp, None),
        P(),
        P(tp),
    )
    return jax.shard_map(
        local, mesh=mesh, in_specs=in_specs, out_specs=P("ep", tp), check_vma=False
    )
```
